32 devices in a mesh: sp: 16 (over z, y, x), tp: 2 (over core).
Axes of the slice: x: 2, y: 2, z: 4, core: 2. Of those that a mesh axis runs over, the one named last changes fastest.
Arguments:
- tokens: bfloat16 [6144, 4096], P(('sp', 'tp')), may hold values from -6 to 6
- norm_gain: float32 [4096], replicated, may hold values from 0.1 to 1.9
- conv_val_w: bfloat16 [4096, 1024], P('sp', 'tp'), may hold values from -0.09375 to 0.09375
- conv_gate_w: bfloat16 [4096, 1024], P('sp', 'tp'), may hold values from -0.09375 to 0.09375
- rec_gate_w: bfloat16 [4096, 1536], P('sp', 'tp'), may hold values from -0.09375 to 0.09375
- rec_in_w: bfloat16 [4096, 1536], P('sp', 'tp'), may hold values from -0.09375 to 0.09375
- conv_taps: bfloat16 [31, 1024], P(None, 'tp'), may hold values from -3 to 3
- conv_bias: float32 [1024], P('tp'), may hold values from 1 to 15
- conv_gain: float32 [1024], P('tp'), may hold values from 0.1 to 1.9
- short_taps: bfloat16 [4, 1536], P(None, 'tp'), may hold values from -3 to 3
- decay_map: bfloat16 [24, 64, 64], P('tp'), may hold values from -0.75 to 0.75
- input_map: bfloat16 [24, 64, 64], P('tp'), may hold values from -0.75 to 0.75
- decay_base: float32 [1536], P('tp'), may hold values from 3.5 to 17
- decay_jump: float32 [6144, 1536], P('sp', 'tp'), may hold values from -1.5 to 0
- out_conv_w: bfloat16 [1024, 4096], P('tp', 'sp'), may hold values from -0.125 to 0.125
- out_rec_w: bfloat16 [1536, 4096], P('tp', 'sp'), may hold values from -0.125 to 0.125
Outputs:
- mixed: bfloat16 [6144, 4096], P(('sp', 'tp'))
The draws below stay inside these ranges and needn't reach their ends.
All inputs are finite; a program needn't handle non-finite values.
Results may differ from the reference program's by a relative error of at most 0.015.
Values may be sent and summed in bfloat16 or wider, within the bound.
A program may use at most 128 MiB of HBM per device.

```python
import math
import jax
import jax.numpy as jnp
from jax import lax

D = 4096
HEAD_SIZE = 64
LRU_HEADS = 24
TAPS = 31
SHORT_TAPS = 4
CONV_WIDTH = 1024
LRU_WIDTH = 1536
TOKENS = 6144
N_TP = 2


def draw_conv_taps(key, part):
    key_base, key_jitter = jax.random.split(jax.random.fold_in(key, 31))
    channel = jnp.arange(CONV_WIDTH, dtype=jnp.float32) / CONV_WIDTH
    jitter = jnp.exp(jax.random.uniform(key_jitter, (CONV_WIDTH,), jnp.float32, math.log(0.8), math.log(1.25)))
    base = jnp.clip(jax.random.normal(key_base, (TAPS, CONV_WIDTH), jnp.float32), -4.0, 4.0)
    rising = jnp.exp(math.log(3.0) * channel)
    return (base * (rising * jitter)[None, :] * (1.0 / math.sqrt(TAPS))).astype(jnp.bfloat16)


def draw_conv_bias(key, part):
    key_jitter = jax.random.fold_in(key, 37)
    channel = jnp.arange(CONV_WIDTH, dtype=jnp.float32) / CONV_WIDTH
    jitter = jnp.exp(jax.random.uniform(key_jitter, (CONV_WIDTH,), jnp.float32, math.log(0.8), math.log(1.25)))
    rising = jnp.exp(math.log(4.0) * channel)
    return 1.5 * rising * jitter


def draw_decay_base(key, part):
    key_kind, key_slow, key_fast = jax.random.split(jax.random.fold_in(key, 29), 3)
    keep_share = 0.5
    slow = jax.random.uniform(key_kind, (LRU_WIDTH,), jnp.float32) < keep_share
    slow_rate = jnp.exp(jax.random.uniform(key_slow, (LRU_WIDTH,), jnp.float32, math.log(0.01), math.log(0.05))) / TOKENS
    fast_rate = jnp.exp(jax.random.uniform(key_fast, (LRU_WIDTH,), jnp.float32, math.log(0.0075), math.log(0.025)))
    rate = jnp.where(slow, slow_rate, fast_rate)
    return -jnp.log(jnp.expm1(rate))


def draw_decay_jump(key, part):
    key_leak, key_where, key_drop = jax.random.split(jax.random.fold_in(key, 23), 3)
    blocks = (TOKENS + 63) // 64
    lowest, highest = (0.05, 0.5)
    leak = jnp.exp(jax.random.uniform(key_leak, (blocks,), jnp.float32, math.log(lowest), math.log(highest))) / TOKENS
    position_leak = jnp.repeat(leak, 64)[:TOKENS]
    places = jax.random.randint(key_where, (2,), 0, TOKENS)
    hits = (jnp.arange(TOKENS)[:, None] == places[None, :]).astype(jnp.float32)
    drops = jnp.log1p(-jax.random.uniform(key_drop, (2, LRU_WIDTH), jnp.float32, 0.2, 0.5))
    return jnp.dot(hits, drops, precision=lax.Precision.HIGHEST) - position_leak[:, None]


def block_levels(stream_key, shape, pieces, low, high):
    level = 1.0
    for axis_at, blocks in pieces:
        heights = jax.random.uniform(jax.random.fold_in(jax.random.fold_in(stream_key, 6), axis_at), (blocks,), jnp.float32, low / len(pieces), high / len(pieces))
        level = level * jnp.repeat(jnp.exp(heights), shape[axis_at] // blocks).reshape((-1,) + (1,) * (len(shape) - 1 - axis_at))
    return level


def gaussian(key, shape, width, most, pieces=(), kind=jnp.bfloat16):
    level = block_levels(key, shape, pieces, -0.22, 0.18) if pieces else 1.0
    drawn = jax.random.normal(key, shape, jnp.float32) * width * level
    return jnp.minimum(jnp.maximum(drawn, -most), most).astype(kind)


def setup_inputs(seed: int = 0) -> dict:
    key_list = jax.random.split(jax.random.key(seed), 17)
    return {
        "tokens": gaussian(key_list[0], (TOKENS, D), 1.0, 6.0, ((0, 32),)),
        "norm_gain": jnp.clip(1.0 + 0.18 * jax.random.normal(key_list[1], (D,), jnp.float32), 0.1, 1.9),
        "conv_val_w": gaussian(key_list[2], (D, CONV_WIDTH), D ** -0.5, 0.09375, ((0, 16), (1, 2))),
        "conv_gate_w": gaussian(key_list[3], (D, CONV_WIDTH), D ** -0.5, 0.09375, ((0, 16), (1, 2))),
        "rec_gate_w": gaussian(key_list[4], (D, LRU_WIDTH), D ** -0.5, 0.09375, ((0, 16), (1, 2))),
        "rec_in_w": gaussian(key_list[5], (D, LRU_WIDTH), D ** -0.5, 0.09375, ((0, 16), (1, 2))),
        "conv_taps": draw_conv_taps(jax.random.fold_in(key_list[16], 71), 0),
        "conv_bias": draw_conv_bias(jax.random.fold_in(key_list[16], 71), 0),
        "conv_gain": jnp.clip(1.0 + 0.18 * jax.random.normal(key_list[8], (CONV_WIDTH,), jnp.float32), 0.1, 1.9),
        "short_taps": gaussian(key_list[9], (SHORT_TAPS, LRU_WIDTH), SHORT_TAPS ** -0.5, 3.0, ((1, 2),)),
        "decay_map": gaussian(key_list[10], (LRU_HEADS, HEAD_SIZE, HEAD_SIZE), HEAD_SIZE ** -0.5, 0.75, ((0, 2),)),
        "input_map": gaussian(key_list[11], (LRU_HEADS, HEAD_SIZE, HEAD_SIZE), HEAD_SIZE ** -0.5, 0.75, ((0, 2),)),
        "decay_base": draw_decay_base(jax.random.fold_in(key_list[16], 71), 0),
        "decay_jump": draw_decay_jump(jax.random.fold_in(key_list[16], 71), 0),
        "out_conv_w": gaussian(key_list[14], (CONV_WIDTH, D), (CONV_WIDTH + LRU_WIDTH) ** -0.5, 0.125, ((0, 2), (1, 16))),
        "out_rec_w": gaussian(key_list[15], (LRU_WIDTH, D), (CONV_WIDTH + LRU_WIDTH) ** -0.5, 0.125, ((0, 2), (1, 16))),
    }


RATE_SCALE = 8.0

def norm_rows(values, gain):
    widened = values.astype(jnp.float32)
    inverse = lax.rsqrt(lax.optimization_barrier(jnp.mean(widened * widened, axis=-1, keepdims=True)) + 1e-06)
    return (widened * inverse * gain).astype(jnp.bfloat16)

def causal_filter(signal, weights):
    lags = weights.shape[0]
    length = signal.shape[0]
    padded = jnp.pad(signal, ((lags - 1, 0), (0, 0)))
    result = jnp.zeros_like(signal)
    for lag_index in range(lags):
        result = result + weights[lag_index][None, :] * padded[lag_index:lag_index + length]
    return result

def chain_step(earlier, latter):
    return (earlier[0] * latter[0], latter[0] * earlier[1] + latter[1])

def reference(tokens, norm_gain, conv_val_w, conv_gate_w, rec_gate_w, rec_in_w, conv_taps, conv_bias, conv_gain, short_taps, decay_map, input_map, decay_base, decay_jump, out_conv_w, out_rec_w):
    normed = norm_rows(tokens, norm_gain)
    conv_val = jnp.dot(normed, conv_val_w, preferred_element_type=jnp.float32).astype(jnp.bfloat16)
    conv_gate = jnp.dot(normed, conv_gate_w, preferred_element_type=jnp.float32).astype(jnp.bfloat16)
    rec_gate = jnp.dot(normed, rec_gate_w, preferred_element_type=jnp.float32).astype(jnp.bfloat16)
    rec_in = jnp.dot(normed, rec_in_w, preferred_element_type=jnp.float32).astype(jnp.bfloat16)
    glu = (conv_val.astype(jnp.float32) * jax.nn.sigmoid(conv_gate.astype(jnp.float32))).astype(jnp.bfloat16)
    filtered = causal_filter(glu.astype(jnp.float32), conv_taps.astype(jnp.float32)) + conv_bias[None, :]
    centered = filtered - lax.optimization_barrier(jnp.mean(filtered, axis=1, keepdims=True))
    spread = lax.optimization_barrier(jnp.mean(centered * centered, axis=1, keepdims=True))
    conv_out = jax.nn.silu(centered * lax.rsqrt(spread + 1e-05) * conv_gain).astype(jnp.bfloat16)
    smoothed = causal_filter(rec_in.astype(jnp.float32), short_taps.astype(jnp.float32)).astype(jnp.bfloat16)
    grouped = smoothed.astype(jnp.float32).reshape(TOKENS, LRU_HEADS, HEAD_SIZE)
    retain = jax.nn.sigmoid(jnp.einsum('thi,hio->tho', grouped, decay_map.astype(jnp.float32)).reshape(TOKENS, LRU_WIDTH))
    admit = jax.nn.sigmoid(jnp.einsum('thi,hio->tho', grouped, input_map.astype(jnp.float32)).reshape(TOKENS, LRU_WIDTH))
    log_decay = -RATE_SCALE * retain * jax.nn.softplus(-decay_base)[None, :] + decay_jump
    decay = jnp.exp(log_decay)
    inflow = jnp.sqrt(-jnp.expm1(2.0 * log_decay)) * admit * smoothed.astype(jnp.float32)
    products, state = lax.associative_scan(chain_step, (decay, inflow), axis=0)
    rec_out = (jax.nn.gelu(rec_gate.astype(jnp.float32)) * state).astype(jnp.bfloat16)
    conv_block = CONV_WIDTH // N_TP
    rec_block = LRU_WIDTH // N_TP
    mixed = jnp.zeros((TOKENS, D), jnp.float32)
    for block_index in range(N_TP):
        conv_cols = slice(block_index * conv_block, (block_index + 1) * conv_block)
        rec_cols = slice(block_index * rec_block, (block_index + 1) * rec_block)
        term = jnp.dot(conv_out[:, conv_cols], out_conv_w[conv_cols], preferred_element_type=jnp.float32)
        term = term + jnp.dot(rec_out[:, rec_cols], out_rec_w[rec_cols], preferred_element_type=jnp.float32)
        mixed = mixed + lax.optimization_barrier(term.astype(jnp.bfloat16)).astype(jnp.float32)
    return mixed.astype(jnp.bfloat16)
```

```python
import functools

import jax
import jax.numpy as jnp
from jax import lax
from jax.experimental import pallas as pl
from jax.experimental.pallas import tpu as pltpu
from jax.sharding import PartitionSpec as P

CONV_WIDTH = 1024


RATE_SCALE = 8.0


def passed_along(value, axis, by):
    count = lax.axis_size(axis)
    pairs = [(i, i + by) for i in range(count) if 0 <= i + by < count]
    return lax.ppermute(value, axis, pairs)


def prefix(part, axis, combine, identity):
    place = lax.axis_index(axis)
    gathered = jax.tree.map(lambda a: lax.all_gather(a, axis), part)
    state = jax.tree.map(lambda a, e: jnp.zeros_like(a) + jnp.asarray(e, a.dtype), part, identity)

    def one(step, state):
        return combine(
            state, jax.tree.map(lambda a: lax.dynamic_index_in_dim(a, step, 0, False), gathered)
        )

    return lax.fori_loop(0, place, one, state)


def norm_rows(values, gain):
    widened = values.astype(jnp.float32)
    inverse = lax.rsqrt(jnp.mean(widened * widened, axis=-1, keepdims=True) + 1e-06)
    return (widened * inverse * gain).astype(jnp.bfloat16)


def causal_window(edge, current, weights):
    extended = jnp.concatenate([edge, current], axis=0).astype(jnp.float32)
    taps_wide = weights.astype(jnp.float32)
    length = current.shape[0]
    result = jnp.zeros((length, current.shape[1]), jnp.float32)
    for lag_index in range(weights.shape[0]):
        result = result + taps_wide[lag_index][None, :] * extended[lag_index : lag_index + length]
    return result


def chain_step(earlier, latter):
    return (earlier[0] * latter[0], latter[0] * earlier[1] + latter[1])


def glu_of(conv_val, conv_gate):
    return (conv_val.astype(jnp.float32) * jax.nn.sigmoid(conv_gate.astype(jnp.float32))).astype(
        jnp.bfloat16
    )


def shards(
    tokens,
    norm_gain,
    conv_val_w,
    conv_gate_w,
    rec_gate_w,
    rec_in_w,
    conv_taps,
    conv_bias,
    conv_gain,
    short_taps,
    decay_map,
    input_map,
    decay_base,
    decay_jump,
    out_conv_w,
    out_rec_w,
):
    rec_cols = rec_in_w.shape[1]
    conv_lags = conv_taps.shape[0] - 1
    short_lags = short_taps.shape[0] - 1
    normed = norm_rows(tokens, norm_gain)
    val_full, gate_full = (
        lax.all_gather(conv_val_w, "sp", axis=0, tiled=True),
        lax.all_gather(conv_gate_w, "sp", axis=0, tiled=True),
    )
    all_rows = lax.all_gather(normed, "tp", axis=0, tiled=True)
    conv_val = jnp.dot(all_rows, val_full, preferred_element_type=jnp.float32).astype(jnp.bfloat16)
    conv_gate = jnp.dot(all_rows, gate_full, preferred_element_type=jnp.float32).astype(
        jnp.bfloat16
    )
    glu = glu_of(conv_val, conv_gate)
    conv_edge = passed_along(glu[-conv_lags:], "sp", 1)
    rgate_full, rin_full = (
        lax.all_gather(rec_gate_w, "sp", axis=0, tiled=True),
        lax.all_gather(rec_in_w, "sp", axis=0, tiled=True),
    )
    rec_gate = jnp.dot(all_rows, rgate_full, preferred_element_type=jnp.float32).astype(
        jnp.bfloat16
    )
    rec_in = jnp.dot(all_rows, rin_full, preferred_element_type=jnp.float32).astype(jnp.bfloat16)
    rec_edge = passed_along(rec_in[-short_lags:], "sp", 1)
    filtered = causal_window(conv_edge, glu, conv_taps) + conv_bias[None, :]
    row_total = lax.psum(jnp.sum(filtered, axis=1), "tp")
    centered = filtered - (row_total / CONV_WIDTH)[:, None]
    spread = lax.psum(jnp.sum(centered * centered, axis=1), "tp") / CONV_WIDTH
    conv_out = jax.nn.silu(centered * lax.rsqrt(spread + 1e-05)[:, None] * conv_gain).astype(
        jnp.bfloat16
    )
    smoothed = causal_window(rec_edge, rec_in, short_taps).astype(jnp.bfloat16)
    length = smoothed.shape[0]
    grouped = smoothed.reshape(length, decay_map.shape[0], decay_map.shape[1])
    retain = jax.nn.sigmoid(
        jnp.einsum("thi,hio->tho", grouped, decay_map, preferred_element_type=jnp.float32).reshape(
            length, rec_cols
        )
    )
    admit = jax.nn.sigmoid(
        jnp.einsum("thi,hio->tho", grouped, input_map, preferred_element_type=jnp.float32).reshape(
            length, rec_cols
        )
    )
    log_decay = -RATE_SCALE * retain * jax.nn.softplus(-decay_base)[None, :] + decay_jump
    decay = jnp.exp(log_decay)
    inflow = jnp.sqrt(-jnp.expm1(2.0 * log_decay)) * admit * smoothed.astype(jnp.float32)
    products, local_state = lax.associative_scan(chain_step, (decay, inflow), axis=0)
    entering = prefix(
        (products[-1], local_state[-1]),
        "sp",
        chain_step,
        (jnp.ones((rec_cols,), jnp.float32), jnp.zeros((rec_cols,), jnp.float32)),
    )
    state = local_state + products * entering[1][None, :]
    rec_out = (jax.nn.gelu(rec_gate.astype(jnp.float32)) * state).astype(jnp.bfloat16)
    conv_full, rec_full = (
        lax.all_gather(out_conv_w, "sp", axis=1, tiled=True),
        lax.all_gather(out_rec_w, "sp", axis=1, tiled=True),
    )
    return lax.psum_scatter(
        (
            jnp.dot(conv_out, conv_full, preferred_element_type=jnp.float32)
            + jnp.dot(rec_out, rec_full, preferred_element_type=jnp.float32)
        ).astype(jnp.bfloat16),
        "tp",
        scatter_dimension=0,
        tiled=True,
    )


MESH = pl.DeviceIdType.MESH
ANY = pl.BlockSpec(memory_space=pl.ANY)
VMEM = pl.BlockSpec(memory_space=pltpu.VMEM)
SEGMENTS = 8


class Spot:
    def __init__(self, planes):
        self.s, self.c = lax.axis_index("sp"), lax.axis_index("tp")
        self.z, self.q = self.s // 4, self.s % 4
        self.qx = self.q + 1 - 2 * (self.q % 2)
        self.qy = (self.q + 2) % 4
        self.qd = 3 - self.q
        self.has_up, self.has_down = self.z < planes - 1, self.z > 0
        self.up, self.down = self.at(self.s + 4, self.c), self.at(self.s - 4, self.c)
        self.partner = self.at(self.s, 1 - self.c)

    def at(self, s, c):
        return {"sp": s, "tp": c}

    def mate(self, q):
        return self.at(self.z * 4 + q, self.c)


class Mail:
    def __init__(self, send_sem):
        self.send_sem, self.count, self.open = send_sem, 0, []

    def send(self, src, dst, recv, device, when=None):
        copy = pltpu.make_async_remote_copy(
            src_ref=src, dst_ref=dst, send_sem=self.send_sem.at[self.count],
            recv_sem=recv, device_id=device, device_id_type=MESH,
        )
        self.count += 1
        self.open.append((copy.wait_send, when))
        if when is None:
            copy.start()
        else:
            pl.when(when)(copy.start)

    def local(self, src, dst):
        copy = pltpu.make_async_copy(src, dst, self.send_sem.at[self.count])
        self.count += 1
        copy.start()
        self.open.append((copy.wait, None))
        return self.open[-1]

    def arrived(self, dst, recv, device):
        pltpu.make_async_remote_copy(
            src_ref=dst, dst_ref=dst, send_sem=self.send_sem.at[0],
            recv_sem=recv, device_id=device, device_id_type=MESH,
        ).wait_recv()

    def finish(self):
        for wait, when in self.open:
            if when is None:
                wait()
            else:
                pl.when(when)(wait)


def greet(me, devices, line):
    barrier = pltpu.get_barrier_semaphore()
    for device in devices:
        pl.semaphore_signal(barrier, inc=1, device_id=device, device_id_type=MESH)
    amount = len(devices)
    if line:
        for has, device in ((me.has_up, me.up), (me.has_down, me.down)):
            @pl.when(has)
            def _():
                pl.semaphore_signal(barrier, inc=1, device_id=device, device_id_type=MESH)
        amount = amount + me.has_up.astype(jnp.int32) + me.has_down.astype(jnp.int32)
    pl.semaphore_wait(barrier, amount)


class PlaneGather:
    def __init__(self, me, mail, own, slot, recv, recv_pair):
        self.me, self.mail, self.own, self.slot = me, mail, own, slot
        self.recv, self.recv_pair = recv, recv_pair

    def start(self):
        me, mail = self.me, self.mail
        for h in (0, 1):
            for q, half in ((me.qx, h), (me.qy, 1 - h)):
                mail.send(self.own(half), self.slot(me.q, me.c, half), self.recv.at[me.q, half], me.mate(q))
        for half in (0, 1):
            mail.send(self.own(half), self.slot(me.q, me.c, half), self.recv_pair.at[me.q, half], me.partner)

    def took(self, q, half):
        me, mail = self.me, self.mail
        here = self.slot(q, me.c, half)
        mail.arrived(here, self.recv.at[q, half], me.partner)
        return here

    def share(self, q, half, here):
        self.mail.send(here, here, self.recv_pair.at[q, half], self.me.partner)

    def first(self):
        me = self.me
        for q, half, to in ((me.qx, 0, me.qy), (me.qy, 1, me.qx)):
            here = self.took(q, half)
            self.mail.send(here, here, self.recv.at[q, half], me.mate(to))
            self.share(q, half, here)

    def second(self):
        for q, half in ((self.me.qx, 1), (self.me.qy, 0)):
            self.share(q, half, self.took(q, half))

    def third(self):
        for half in (0, 1):
            self.share(self.me.qd, half, self.took(self.me.qd, half))

    def last(self, origins):
        me = self.me
        for q in origins:
            for half in (0, 1):
                self.mail.arrived(self.slot(q, 1 - me.c, half), self.recv_pair.at[q, half], me.partner)


def minus_expm1(y):
    series = 1.0 + y * (1.0 / 8.0)
    for n in (7.0, 6.0, 5.0, 4.0, 3.0, 2.0):
        series = 1.0 + y * (1.0 / n) * series
    return jnp.where(y > -0.35, -y * series, 1.0 - jnp.exp(y))


def gelu(v):
    return 0.5 * v * (1.0 + jnp.tanh(0.7978845608028654 * (v + 0.044715 * v * v * v)))


class Line:
    def __init__(self, me, mail, planes, slot, recv, seen=None):
        self.me, self.mail, self.planes = me, mail, planes
        self.slot, self.recv, self.seen = slot, recv, seen

    def own(self, piece, src, up=True, down=True):
        me = self.me
        for wanted, has, device in ((up, me.has_up, me.up), (down, me.has_down, me.down)):
            if wanted:
                self.mail.send(src, self.slot(me.z, piece), self.recv.at[me.z, piece], device, has)

    def relay(self, k, piece, up=True, down=True):
        me = self.me
        for wanted, origin, there, on, more in (
            (up, me.z - k, me.z >= k, me.up, me.has_up),
            (down, me.z + k, me.z + k < self.planes, me.down, me.has_down),
        ):
            if wanted:
                here, sem = self.slot(origin, piece), self.recv.at[origin, piece]
                pl.when(there)(functools.partial(self.mail.arrived, here, sem, me.partner))
                if k < self.planes - 1:
                    self.mail.send(here, here, sem, on, jnp.logical_and(there, more))
                if self.seen is not None:
                    self.seen(origin, piece, there)


OUT_PARTS = 4


def layer_kernel(
    planes, lags, x_ref, gain, wr, wc, jb, cpar, rpar, dmap, imap, w_ref,
    out, xall, rwall, cwall, projr, jall, wz, wp, yall, cbuf, gext, rext, filt, dec, inf, maps, stat,
    st_all, carry, cr_all,
    send, rx, rpx, rwr, rwc, zr, zc, zo, rj, ry, rp, rv, rq, rw, rh, rs, rc, ls, lr,
):
    me = Spot(planes)
    mail = Mail(send)
    c_lags, s_lags = lags
    f32, bf16 = jnp.float32, jnp.bfloat16
    rows, depth = x_ref.shape[0], wr.shape[1]
    length = xall.shape[0]
    cw, rwid = gext.shape[1], rpar.shape[2]
    seg = length // SEGMENTS
    top = gext.shape[0] - length
    rtop = rext.shape[0] - length
    fold = dec.shape[0]
    part = planes // 2
    width = yall.shape[1] // 8
    mine = me.q * 2 + me.c
    others = (me.qx, me.qy, me.qd)
    pieces = (me.q,) + others
    parts = tuple(range(OUT_PARTS))
    tall = w_ref.shape[0] // OUT_PARTS
    last = planes - 1
    mates = [me.at(me.z * 4 + (me.q + dq) % 4, c) for dq in range(4) for c in (me.c, 1 - me.c)][1:]
    lined = [me.at((me.s + 4 * k) % (4 * planes), me.c) for k in range(1, planes)]
    greet(me, mates + lined, False)

    def of_rows(ref):
        def slot(origin, piece):
            return ref.at[pl.ds(pl.multiple_of((origin * 4 + piece) * depth, depth), depth)]

        return slot

    def theirs_too(origin, piece, when):
        theirs = jnp.logical_and(origin // part != me.c, when)
        place = origin - (1 - me.c) * part
        rest = pl.ds(piece * tall, tall)
        mail.send(wz.at[origin, rest], wp.at[place, rest], rw.at[place, piece], me.partner, theirs)

    rl = Line(me, mail, planes, of_rows(rwall), zr)
    cl = Line(me, mail, planes, of_rows(cwall), zc)
    ol = Line(me, mail, planes, lambda origin, p: wz.at[origin, pl.ds(p * tall, tall)], zo, theirs_too)

    def out_own(p):
        ol.own(p, w_ref.at[pl.ds(p * tall, tall)])

    for q in others:
        mail.send(wr.at[q], rl.slot(me.z, me.q), rwr.at[me.q], me.mate(q))
    rl.own(me.q, wr.at[me.q])

    first_row = mine * rows

    @pl.loop(0, rows // 16)
    def _(i):
        values = x_ref[pl.ds(pl.multiple_of(i * 16, 16), 16)].astype(f32)
        inverse = lax.rsqrt(jnp.mean(values * values, axis=1, keepdims=True) + 1e-06)
        place = pl.ds(pl.multiple_of(first_row + i * 16, 16), 16)
        xall[place] = (values * inverse * gain[...]).astype(bf16)

    half_rows = rows // 2

    def xslot(q, c, h):
        return xall.at[pl.ds(pl.multiple_of((q * 2 + c) * rows + h * half_rows, 16), half_rows)]

    xg = PlaneGather(me, mail, lambda h: xslot(me.q, me.c, h), xslot, rx, rpx)
    xg.start()
    for q in others:
        mail.send(wc.at[q], cl.slot(me.z, me.q), rwc.at[me.q], me.mate(q))
    out_own(0)
    kept_here = [
        mail.local(wr.at[me.q], rl.slot(me.z, me.q)),
        mail.local(wc.at[me.q], cl.slot(me.z, me.q)),
        mail.local(w_ref, wz.at[me.z]),
        mail.local(jb.at[me.q], jall.at[me.q]),
    ]
    for entry in kept_here:
        mail.open.remove(entry)
        entry[0]()
    for p in parts:
        rest = pl.ds(p * tall, tall)
        place = me.z - (1 - me.c) * part
        mail.send(w_ref.at[rest], wp.at[place, rest], rw.at[place, p], me.partner, me.z // part != me.c)

    maps[...] = jnp.zeros_like(maps)
    size = dmap.shape[1]
    heads = rwid // size
    for h in range(heads):
        spot = pl.ds(h * size, size)
        maps[spot, pl.ds(h * size, size)] = dmap[me.q * heads + h]
        maps[spot, pl.ds(fold * 128 + h * size, size)] = imap[me.q * heads + h]

    for q in others:
        here = rl.slot(me.z, q)
        mail.arrived(here, rwr.at[q], me.partner)
        rl.own(q, here)
    for p in pieces:
        rl.relay(1, p)
    cl.own(me.q, wc.at[me.q])
    xg.first()
    for q in others:
        mail.send(jb.at[q], jall.at[me.q], rj.at[me.q], me.mate(q))
    for k in range(2, last):
        for p in pieces:
            rl.relay(k, p)
    xg.second()
    for q in others:
        here = cl.slot(me.z, q)
        mail.arrived(here, rwc.at[q], me.partner)
        cl.own(q, here)
    for p in pieces:
        rl.relay(last, p)
    xg.last(pieces[:3])

    tile = length // 4

    def project_rec(q):
        at = pl.ds(pl.multiple_of(q * tile, tile), tile)
        product = jnp.dot(xall[at], rwall[...], preferred_element_type=f32).astype(bf16)
        projr[at] = product
        rext[pl.ds(pl.multiple_of(q * tile + rtop, 16), tile)] = product[:, :rwid].astype(f32)

    @pl.loop(0, 3)
    def _(i):
        project_rec((me.q // 2 + i // 2) % 2 * 2 + (me.q % 2 + i % 2) % 2)

    for n, p in enumerate(pieces):
        cl.relay(1, p, n < 2, True)
    xg.third()
    xg.last(pieces[3:])
    project_rec(me.qd)

    mail.send(rext.at[pl.ds(length, rtop)], rext.at[pl.ds(0, rtop)], rh.at[0], me.up, me.has_up)
    for p in pieces[2:]:
        cl.relay(1, p, True, False)
    for k in range(2, last):
        for n, p in enumerate(pieces):
            cl.relay(k, p, n < 1, True)

    @pl.when(jnp.logical_not(me.has_down))
    def _():
        rext[pl.ds(0, rtop)] = jnp.zeros((rtop, rwid), f32)
        gext[pl.ds(0, top)] = jnp.zeros((top, cw), f32)

    for q in others:
        mail.arrived(jall.at[q], rj.at[q], me.partner)

    softened = rpar[me.q, pl.ds(s_lags + 1, 1), :]

    @pl.loop(0, SEGMENTS)
    def _(n):
        i = SEGMENTS - 1 - n

        @pl.when(jnp.logical_and(i == 0, me.has_down))
        def _():
            mail.arrived(rext.at[pl.ds(0, rtop)], rh.at[0], me.partner)

        base = pl.multiple_of(i * seg, 8)
        window = rext[pl.ds(pl.multiple_of(base + rtop - 8, 8), seg + 8)]
        smooth = jnp.zeros((seg, rwid), f32)
        for k in range(s_lags + 1):
            smooth = smooth + rpar[me.q, pl.ds(k, 1), :] * window[8 - s_lags + k : 8 - s_lags + k + seg]
        smooth = smooth.astype(bf16)
        gates = jax.nn.sigmoid(jnp.dot(smooth, maps[...], preferred_element_type=f32))
        retain, admit = gates[:, :rwid], gates[:, fold * 128 : fold * 128 + rwid]
        wide = jall[i // 2].astype(f32)
        moved = jnp.where(i % 2 == 0, wide[:, :rwid], wide[:, rwid:])
        log_decay = moved - retain * softened
        decay = jnp.exp(log_decay)
        inflow = jnp.sqrt(minus_expm1(2.0 * log_decay)) * admit * smooth.astype(f32)
        for f in range(fold):
            w = min(128, rwid - f * 128)
            dec[f, pl.ds(base, seg), pl.ds(0, w)] = decay[:, f * 128 : f * 128 + w]
            inf[f, pl.ds(base, seg), pl.ds(0, w)] = inflow[:, f * 128 : f * 128 + w]

    def one(i, held):
        after = []
        for f in range(fold):
            at = pl.ds(i, SEGMENTS, stride=seg)
            d = dec.at[f][at, :]
            product, state = held[2 * f] * d, held[2 * f + 1] * d + inf.at[f][at, :]
            dec.at[f][at, :] = product
            inf.at[f][at, :] = state
            after += [product, state]
        return tuple(after)

    flat = (SEGMENTS, 128)
    ends = lax.fori_loop(0, seg, one, (jnp.ones(flat, f32), jnp.zeros(flat, f32)) * fold, unroll=8)
    for f in range(fold):
        product, state = jnp.ones((1, 128), f32), jnp.zeros((1, 128), f32)
        for i in range(SEGMENTS):
            p, s = ends[2 * f][i : i + 1], ends[2 * f + 1][i : i + 1]
            product, state = product * p, p * state + s
        carry[pl.ds(2 * f, 1)] = product
        carry[pl.ds(2 * f + 1, 1)] = state
    for k in range(1, planes):
        mail.send(carry, cr_all.at[me.z], rc.at[me.z], lined[k - 1], me.z + k < planes)
    for k in range(2, last):
        for p in pieces[1:]:
            cl.relay(k, p, True, False)
    for p in parts[1:]:
        out_own(p)

    for k in range(1, planes):
        z = me.z - k
        pl.when(z >= 0)(functools.partial(mail.arrived, cr_all.at[z], rc.at[z], me.partner))
    entering = []
    for f in range(fold):
        held = jnp.zeros((1, 128), f32)
        for j in range(planes - 1):
            after = cr_all[j, pl.ds(2 * f, 1)] * held + cr_all[j, pl.ds(2 * f + 1, 1)]
            held = jnp.where(j < me.z, after, held)
        for i in range(SEGMENTS):
            entering.append(held)
            held = ends[2 * f][i : i + 1] * held + ends[2 * f + 1][i : i + 1]
    own_at = pl.multiple_of(mine * width, 128)
    for i in range(SEGMENTS):
        here = pl.ds(i * seg, seg)
        state = [dec[f, here] * entering[f * SEGMENTS + i] + inf[f, here] for f in range(fold)]
        state = jnp.concatenate(state, axis=1)[:, :rwid]
        result = gelu(projr[here, pl.ds(rwid, rwid)].astype(f32)) * state
        fill = jnp.zeros((seg, width - cw - rwid), f32)
        yall[here, pl.ds(pl.multiple_of(own_at + cw, 128), width - cw)] = jnp.concatenate([result, fill], axis=1).astype(bf16)

    half_length = length // 2

    def gather(lane, lanes, recv, recv_pair):
        def slot(q, c, h):
            spot = pl.ds(pl.multiple_of((q * 2 + c) * width + lane, 128), lanes)
            return yall.at[pl.ds(h * half_length, half_length), spot]

        return PlaneGather(me, mail, lambda h: slot(me.q, me.c, h), slot, recv, recv_pair)

    vg = gather(cw, width - cw, rv, rq)
    vg.start()
    for p in pieces:
        cl.relay(last, p)

    @pl.loop(0, 4)
    def _(i):
        at = pl.ds(pl.multiple_of(i * tile, tile), tile)
        product = jnp.dot(xall[at], cwall[...], preferred_element_type=f32).astype(bf16).astype(f32)
        glu = (product[:, :cw] * jax.nn.sigmoid(product[:, cw:])).astype(bf16).astype(f32)
        gext[pl.ds(pl.multiple_of(i * tile + top, 8), tile)] = glu

    mail.send(gext.at[pl.ds(length, top)], gext.at[pl.ds(0, top)], rh.at[1], me.up, me.has_up)
    for p in parts:
        ol.relay(1, p)
    strips = length // 64

    def filter_strip(n):
        i = strips - 1 - n

        @pl.when(jnp.logical_and(i == 0, me.has_down))
        def _():
            mail.arrived(gext.at[pl.ds(0, top)], rh.at[1], me.partner)

        base = pl.multiple_of(i * 64, 8)
        window = gext[pl.ds(base, 64 + top)]
        total = jnp.zeros((64, cw), f32) + cpar[pl.ds(c_lags + 1, 1), :]
        for k in range(c_lags + 1):
            begin = top - c_lags + k
            total = total + cpar[pl.ds(k, 1), :] * window[begin : begin + 64]
        filt[pl.ds(base, 64)] = total
        part_sum = jnp.sum(total, axis=1, keepdims=True)
        off = total - part_sum * (1.0 / cw)
        lane = lax.broadcasted_iota(jnp.int32, (64, 128), 1)
        spread = jnp.sum(off * off, axis=1, keepdims=True)
        stat[pl.ds(base, 64)] = jnp.where(lane == 0, part_sum, spread)

    pl.loop(0, strips // 4)(filter_strip)
    vg.first()
    pl.loop(strips // 4, strips)(filter_strip)

    packed = stat[...].T
    st_all[mine] = packed[0:8]
    for device in mates:
        mail.send(st_all.at[mine], st_all.at[mine], rs.at[mine], device)

    for k in range(1, 8):
        d = (mine + k) % 8
        mail.arrived(st_all.at[d], rs.at[d], me.partner)
    total = sum(st_all[d, 0:1, :] for d in range(8))
    mean = total * (1.0 / (8 * cw))
    spread = jnp.zeros_like(mean)
    for d in range(8):
        shift = st_all[d, 0:1, :] * (1.0 / cw) - mean
        spread = spread + st_all[d, 1:2, :] + cw * shift * shift
    scale = lax.rsqrt(spread * (1.0 / (8 * cw)) + 1e-05)
    row = lax.broadcasted_iota(jnp.int32, (128, length), 0)
    stat[...] = jnp.where(row == 0, mean, scale).T

    @pl.loop(0, SEGMENTS)
    def _(i):
        here = pl.ds(pl.multiple_of(i * seg, 16), seg)
        pair = stat[here]
        v = (filt[here] - pair[:, 0:1]) * pair[:, 1:2] * cpar[pl.ds(c_lags + 2, 1), :]
        yall[here, pl.ds(own_at, cw)] = (v * jax.nn.sigmoid(v)).astype(bf16)

    yg = gather(0, cw, ry, rp)
    yg.start()
    vg.second()
    yg.first()
    for k in range(2, last):
        for p in parts:
            ol.relay(k, p)
    vg.third()
    yg.second()
    yg.third()
    vg.last(pieces)
    yg.last(pieces)

    used, cols = cw + rwid, w_ref.shape[1]
    tile_rows = length // 8
    upward = me.z < part

    def multiply(d, k):
        here = pl.ds(pl.multiple_of(d * tile_rows, 16), tile_rows)
        total = jnp.zeros((tile_rows, cols), f32)
        for q in range(4):
            for c, block in ((me.c, wz.at[me.c * part + k]), (1 - me.c, wp.at[k])):
                left = yall[here, pl.ds(pl.multiple_of((q * 2 + c) * width, 128), width)]
                total = total + jnp.dot(
                    left[:, :used], block[pl.ds(q * used, used)], preferred_element_type=f32
                )
        cbuf[d, k] = total.astype(bf16)

    def place(q, c, k):
        return out.at[:, pl.ds(pl.multiple_of(((c * part + k) * 4 + q) * cols, 128), cols)]

    def target(i):
        flip = 3 - i // 2
        q = (me.q // 2 + flip // 2) % 2 * 2 + (me.q % 2 + flip % 2) % 2
        return q, (me.c + 1 + i) % 2

    def parcel(i, k):
        q, c = target(i)
        return pltpu.make_async_remote_copy(
            src_ref=cbuf.at[q * 2 + c, k], dst_ref=place(me.q, me.c, k), send_sem=ls.at[i, k],
            recv_sem=lr.at[mine, k], device_id=me.at(me.z * 4 + q, c), device_id_type=MESH,
        )

    def kept(k):
        return pltpu.make_async_copy(cbuf.at[mine, k], place(me.q, me.c, k), ls.at[7, k])

    def round_of(n):
        k = jnp.where(upward, n, part - 1 - n)

        @pl.loop(0, 7)
        def _(i):
            q, c = target(i)
            multiply(q * 2 + c, k)
            parcel(i, k).start()

        multiply(mine, k)
        kept(k).start()

    for n in range(part):
        k = jnp.where(upward, n, part - 1 - n)
        if n == part - 1:
            for p in parts:
                ol.relay(last, p)
        for p in parts:
            mail.arrived(wp.at[k, pl.ds(p * tall, tall)], rw.at[k, p], me.partner)
        round_of(n)

    @pl.loop(0, 7)
    def _(i):
        q, c = target(i)
        for k in range(part):
            mail.arrived(place(q, c, k), lr.at[q * 2 + c, k], me.partner)
            parcel(i, k).wait_send()

    for k in range(part):
        kept(k).wait()
    mail.finish()


def layer(planes, tokens, gain, wr, wc, jb, cpar, rpar, dmap, imap, weights, lags):
    rows, width_in = tokens.shape
    length = 8 * rows
    cw, rwid = wc.shape[2] // 2, rpar.shape[2]
    depth = wr.shape[1]
    used, cols = cw + rwid, weights.shape[1]
    width = used + -used % 128
    fold = (rwid + 127) // 128
    f32, bf16 = jnp.float32, jnp.bfloat16
    dma, vmem = pltpu.SemaphoreType.DMA, pltpu.VMEM
    top = lags[0] + -lags[0] % 16
    rtop = lags[1] + -lags[1] % 16
    part = planes // 2
    deep = planes * 4 * depth
    return pl.pallas_call(
        functools.partial(layer_kernel, planes, lags),
        out_shape=jax.ShapeDtypeStruct((rows, planes * 4 * cols), bf16),
        in_specs=[VMEM] * 10,
        out_specs=ANY,
        scratch_shapes=[
            vmem((length, width_in), bf16),
            vmem((deep, wr.shape[2]), bf16),
            vmem((deep, wc.shape[2]), bf16),
            vmem((length, wr.shape[2]), bf16),
            vmem(jb.shape, bf16),
            vmem((planes,) + weights.shape, bf16),
            vmem((part,) + weights.shape, bf16),
            vmem((length, 8 * width), bf16),
            vmem((8, part, rows, cols), bf16),
            vmem((top + length, cw), f32),
            vmem((rtop + length, rwid), f32),
            vmem((length, cw), f32),
            vmem((fold, length, 128), f32),
            vmem((fold, length, 128), f32),
            vmem((rwid, 2 * fold * 128), bf16),
            vmem((length, 128), f32),
            vmem((8, 8, length), f32),
            vmem((8, 128), f32),
            vmem((planes, 8, 128), f32),
            dma((100 + 20 * planes,)), dma((4, 2)), dma((4, 2)), dma((4,)), dma((4,)),
            dma((planes, 4)), dma((planes, 4)), dma((planes, OUT_PARTS)), dma((4,)),
            dma((4, 2)), dma((4, 2)), dma((4, 2)), dma((4, 2)), dma((part, OUT_PARTS)),
            dma((2,)), dma((8,)), dma((planes,)), dma((8, part)), dma((8, part)),
        ],
        compiler_params=pltpu.CompilerParams(
            collective_id=0, has_side_effects=True, vmem_limit_bytes=60 * 1024 * 1024
        ),
    )(tokens, gain, wr, wc, jb, cpar, rpar, dmap, imap, weights)


def plane_shards(
    planes,
    tokens,
    norm_gain,
    conv_val_w,
    conv_gate_w,
    rec_gate_w,
    rec_in_w,
    conv_taps,
    conv_bias,
    conv_gain,
    short_taps,
    decay_map,
    input_map,
    decay_base,
    decay_jump,
    out_conv_w,
    out_rec_w,
):
    s = lax.axis_index("sp")
    q = s % 4
    f32 = jnp.float32

    def by_mate(a):
        return a.reshape(a.shape[0], 4, a.shape[1] // 4).transpose(1, 0, 2)

    def mine(a, axis):
        size = a.shape[axis] // 4
        return lax.dynamic_slice_in_dim(a, q * size, size, axis)

    wr = jnp.concatenate([by_mate(w) for w in (rec_in_w, rec_gate_w)], axis=2)
    wc = jnp.concatenate([by_mate(w) for w in (conv_val_w, conv_gate_w)], axis=2)
    half = decay_jump.shape[0] // 2
    cw, rw = conv_val_w.shape[1] // 4, rec_in_w.shape[1] // 4
    jb = decay_jump.astype(jnp.bfloat16).reshape(2, half, 4, rw).transpose(2, 1, 0, 3).reshape(4, half, 2 * rw)
    cols = out_conv_w.shape[1]
    rows_by_mate = jnp.concatenate(
        [out_conv_w.reshape(4, cw, cols), out_rec_w.reshape(4, rw, cols)], axis=1
    ).reshape(-1, cols)
    cpar = mine(jnp.concatenate([conv_taps.astype(f32), conv_bias[None], conv_gain[None]]), 1)
    rpar = by_mate(jnp.concatenate([short_taps.astype(f32), RATE_SCALE * jax.nn.softplus(-decay_base)[None]]))
    lags = (conv_taps.shape[0] - 1, short_taps.shape[0] - 1)
    return layer(
        planes, tokens, norm_gain[None], wr, wc, jb, cpar, rpar, decay_map, input_map, rows_by_mate, lags
    )


def solution(mesh):
    in_specs = (
        P(("sp", "tp"), None),
        P(),
        P("sp", "tp"),
        P("sp", "tp"),
        P("sp", "tp"),
        P("sp", "tp"),
        P(None, "tp"),
        P("tp"),
        P("tp"),
        P(None, "tp"),
        P("tp", None, None),
        P("tp", None, None),
        P("tp"),
        P("sp", "tp"),
        P("tp", "sp"),
        P("tp", "sp"),
    )
    out_specs = P(("sp", "tp"), None)
    count = mesh.shape["sp"]
    planar = mesh.shape["tp"] == 2 and count % 8 == 0 and count >= 16
    body = functools.partial(plane_shards, count // 4) if planar else shards
    return jax.shard_map(body, mesh=mesh, in_specs=in_specs, out_specs=out_specs, check_vma=False)
```

```python
import functools

import jax
import jax.numpy as jnp
from jax import lax
from jax.experimental import pallas as pl
from jax.experimental.pallas import tpu as pltpu
from jax.sharding import PartitionSpec as P

CONV_WIDTH = 1024


RATE_SCALE = 8.0


def passed_along(value, axis, by):
    count = lax.axis_size(axis)
    pairs = [(i, i + by) for i in range(count) if 0 <= i + by < count]
    return lax.ppermute(value, axis, pairs)


def prefix(part, axis, combine, identity):
    place = lax.axis_index(axis)
    gathered = jax.tree.map(lambda a: lax.all_gather(a, axis), part)
    state = jax.tree.map(lambda a, e: jnp.zeros_like(a) + jnp.asarray(e, a.dtype), part, identity)

    def one(step, state):
        return combine(
            state, jax.tree.map(lambda a: lax.dynamic_index_in_dim(a, step, 0, False), gathered)
        )

    return lax.fori_loop(0, place, one, state)


def norm_rows(values, gain):
    widened = values.astype(jnp.float32)
    inverse = lax.rsqrt(jnp.mean(widened * widened, axis=-1, keepdims=True) + 1e-06)
    return (widened * inverse * gain).astype(jnp.bfloat16)


def causal_window(edge, current, weights):
    extended = jnp.concatenate([edge, current], axis=0).astype(jnp.float32)
    taps_wide = weights.astype(jnp.float32)
    length = current.shape[0]
    result = jnp.zeros((length, current.shape[1]), jnp.float32)
    for lag_index in range(weights.shape[0]):
        result = result + taps_wide[lag_index][None, :] * extended[lag_index : lag_index + length]
    return result


def chain_step(earlier, latter):
    return (earlier[0] * latter[0], latter[0] * earlier[1] + latter[1])


def glu_of(conv_val, conv_gate):
    return (conv_val.astype(jnp.float32) * jax.nn.sigmoid(conv_gate.astype(jnp.float32))).astype(
        jnp.bfloat16
    )


def shards(
    tokens,
    norm_gain,
    conv_val_w,
    conv_gate_w,
    rec_gate_w,
    rec_in_w,
    conv_taps,
    conv_bias,
    conv_gain,
    short_taps,
    decay_map,
    input_map,
    decay_base,
    decay_jump,
    out_conv_w,
    out_rec_w,
):
    rec_cols = rec_in_w.shape[1]
    conv_lags = conv_taps.shape[0] - 1
    short_lags = short_taps.shape[0] - 1
    normed = norm_rows(tokens, norm_gain)
    val_full, gate_full = (
        lax.all_gather(conv_val_w, "sp", axis=0, tiled=True),
        lax.all_gather(conv_gate_w, "sp", axis=0, tiled=True),
    )
    all_rows = lax.all_gather(normed, "tp", axis=0, tiled=True)
    conv_val = jnp.dot(all_rows, val_full, preferred_element_type=jnp.float32).astype(jnp.bfloat16)
    conv_gate = jnp.dot(all_rows, gate_full, preferred_element_type=jnp.float32).astype(
        jnp.bfloat16
    )
    glu = glu_of(conv_val, conv_gate)
    conv_edge = passed_along(glu[-conv_lags:], "sp", 1)
    rgate_full, rin_full = (
        lax.all_gather(rec_gate_w, "sp", axis=0, tiled=True),
        lax.all_gather(rec_in_w, "sp", axis=0, tiled=True),
    )
    rec_gate = jnp.dot(all_rows, rgate_full, preferred_element_type=jnp.float32).astype(
        jnp.bfloat16
    )
    rec_in = jnp.dot(all_rows, rin_full, preferred_element_type=jnp.float32).astype(jnp.bfloat16)
    rec_edge = passed_along(rec_in[-short_lags:], "sp", 1)
    filtered = causal_window(conv_edge, glu, conv_taps) + conv_bias[None, :]
    row_total = lax.psum(jnp.sum(filtered, axis=1), "tp")
    centered = filtered - (row_total / CONV_WIDTH)[:, None]
    spread = lax.psum(jnp.sum(centered * centered, axis=1), "tp") / CONV_WIDTH
    conv_out = jax.nn.silu(centered * lax.rsqrt(spread + 1e-05)[:, None] * conv_gain).astype(
        jnp.bfloat16
    )
    smoothed = causal_window(rec_edge, rec_in, short_taps).astype(jnp.bfloat16)
    length = smoothed.shape[0]
    grouped = smoothed.reshape(length, decay_map.shape[0], decay_map.shape[1])
    retain = jax.nn.sigmoid(
        jnp.einsum("thi,hio->tho", grouped, decay_map, preferred_element_type=jnp.float32).reshape(
            length, rec_cols
        )
    )
    admit = jax.nn.sigmoid(
        jnp.einsum("thi,hio->tho", grouped, input_map, preferred_element_type=jnp.float32).reshape(
            length, rec_cols
        )
    )
    log_decay = -RATE_SCALE * retain * jax.nn.softplus(-decay_base)[None, :] + decay_jump
    decay = jnp.exp(log_decay)
    inflow = jnp.sqrt(-jnp.expm1(2.0 * log_decay)) * admit * smoothed.astype(jnp.float32)
    products, local_state = lax.associative_scan(chain_step, (decay, inflow), axis=0)
    entering = prefix(
        (products[-1], local_state[-1]),
        "sp",
        chain_step,
        (jnp.ones((rec_cols,), jnp.float32), jnp.zeros((rec_cols,), jnp.float32)),
    )
    state = local_state + products * entering[1][None, :]
    rec_out = (jax.nn.gelu(rec_gate.astype(jnp.float32)) * state).astype(jnp.bfloat16)
    conv_full, rec_full = (
        lax.all_gather(out_conv_w, "sp", axis=1, tiled=True),
        lax.all_gather(out_rec_w, "sp", axis=1, tiled=True),
    )
    return lax.psum_scatter(
        (
            jnp.dot(conv_out, conv_full, preferred_element_type=jnp.float32)
            + jnp.dot(rec_out, rec_full, preferred_element_type=jnp.float32)
        ).astype(jnp.bfloat16),
        "tp",
        scatter_dimension=0,
        tiled=True,
    )


MESH = pl.DeviceIdType.MESH
ANY = pl.BlockSpec(memory_space=pl.ANY)
VMEM = pl.BlockSpec(memory_space=pltpu.VMEM)
SEGMENTS = 8


class Spot:
    def __init__(self, planes):
        self.s, self.c = lax.axis_index("sp"), lax.axis_index("tp")
        self.z, self.q = self.s // 4, self.s % 4
        self.qx = self.q + 1 - 2 * (self.q % 2)
        self.qy = (self.q + 2) % 4
        self.qd = 3 - self.q
        self.has_up, self.has_down = self.z < planes - 1, self.z > 0
        self.up, self.down = self.at(self.s + 4, self.c), self.at(self.s - 4, self.c)
        self.partner = self.at(self.s, 1 - self.c)

    def at(self, s, c):
        return {"sp": s, "tp": c}

    def mate(self, q):
        return self.at(self.z * 4 + q, self.c)


class Mail:
    def __init__(self, send_sem):
        self.send_sem, self.count, self.open = send_sem, 0, []

    def send(self, src, dst, recv, device, when=None):
        copy = pltpu.make_async_remote_copy(
            src_ref=src, dst_ref=dst, send_sem=self.send_sem.at[self.count],
            recv_sem=recv, device_id=device, device_id_type=MESH,
        )
        self.count += 1
        self.open.append((copy.wait_send, when))
        if when is None:
            copy.start()
        else:
            pl.when(when)(copy.start)

    def local(self, src, dst):
        copy = pltpu.make_async_copy(src, dst, self.send_sem.at[self.count])
        self.count += 1
        copy.start()
        self.open.append((copy.wait, None))
        return self.open[-1]

    def arrived(self, dst, recv, device):
        pltpu.make_async_remote_copy(
            src_ref=dst, dst_ref=dst, send_sem=self.send_sem.at[0],
            recv_sem=recv, device_id=device, device_id_type=MESH,
        ).wait_recv()

    def finish(self):
        for wait, when in self.open:
            if when is None:
                wait()
            else:
                pl.when(when)(wait)


def greet(me, devices, line):
    barrier = pltpu.get_barrier_semaphore()
    for device in devices:
        pl.semaphore_signal(barrier, inc=1, device_id=device, device_id_type=MESH)
    amount = len(devices)
    if line:
        for has, device in ((me.has_up, me.up), (me.has_down, me.down)):
            @pl.when(has)
            def _():
                pl.semaphore_signal(barrier, inc=1, device_id=device, device_id_type=MESH)
        amount = amount + me.has_up.astype(jnp.int32) + me.has_down.astype(jnp.int32)
    pl.semaphore_wait(barrier, amount)


class PlaneGather:
    def __init__(self, me, mail, slot, recv, recv_pair):
        self.me, self.mail, self.slot = me, mail, slot
        self.recv, self.recv_pair = recv, recv_pair
        self.parts = recv.shape[1]
        self.half = self.parts // 2

    def start(self):
        me, mail = self.me, self.mail
        for h in range(self.parts):
            for q, part in ((me.qx, h), (me.qy, (h + self.half) % self.parts)):
                own = self.slot(me.q, me.c, part)
                mail.send(own, own, self.recv.at[me.q, part], me.mate(q))
        for part in range(self.parts):
            self.share(me.q, part, self.slot(me.q, me.c, part))

    def took(self, q, part):
        here = self.slot(q, self.me.c, part)
        self.mail.arrived(here, self.recv.at[q, part], self.me.partner)
        return here

    def share(self, q, part, here):
        self.mail.send(here, here, self.recv_pair.at[q, part], self.me.partner)

    def first(self, i):
        me = self.me
        for q, part, to in ((me.qx, i, me.qy), (me.qy, self.half + i, me.qx)):
            here = self.took(q, part)
            self.mail.send(here, here, self.recv.at[q, part], me.mate(to))
            self.share(q, part, here)

    def second(self):
        for i in range(self.half):
            for q, part in ((self.me.qx, self.half + i), (self.me.qy, i)):
                self.share(q, part, self.took(q, part))

    def third(self):
        for i in range(self.half):
            for part in (i, self.half + i):
                self.share(self.me.qd, part, self.took(self.me.qd, part))

    def last(self, origins):
        me = self.me
        for q in origins:
            for part in range(self.parts):
                self.mail.arrived(self.slot(q, 1 - me.c, part), self.recv_pair.at[q, part], me.partner)


def minus_expm1(y):
    series = 1.0 + y * (1.0 / 8.0)
    for n in (7.0, 6.0, 5.0, 4.0, 3.0, 2.0):
        series = 1.0 + y * (1.0 / n) * series
    return jnp.where(y > -0.35, -y * series, 1.0 - jnp.exp(y))


def gelu(v):
    return 0.5 * v * (1.0 + jnp.tanh(0.7978845608028654 * (v + 0.044715 * v * v * v)))


class Line:
    def __init__(self, me, mail, planes, slot, recv, seen=None):
        self.me, self.mail, self.planes = me, mail, planes
        self.slot, self.recv, self.seen = slot, recv, seen

    def own(self, piece, src, up=True, down=True):
        me = self.me
        for wanted, has, device in ((up, me.has_up, me.up), (down, me.has_down, me.down)):
            if wanted:
                self.mail.send(src, self.slot(me.z, piece), self.recv.at[me.z, piece], device, has)

    def ways(self, k):
        me = self.me
        return (
            (me.z - k, me.z >= k, me.up, me.has_up),
            (me.z + k, me.z + k < self.planes, me.down, me.has_down),
        )

    def take(self, origin, piece, when):
        here, sem = self.slot(origin, piece), self.recv.at[origin, piece]
        pl.when(when)(functools.partial(self.mail.arrived, here, sem, self.me.partner))
        if self.seen is not None:
            self.seen(origin, piece, when)
        return here, sem

    def relay(self, k, piece, up=True, down=True):
        for wanted, (origin, there, on, more) in zip((up, down), self.ways(k)):
            if wanted:
                when = jnp.logical_and(there, more)
                here, sem = self.take(origin, piece, when)
                self.mail.send(here, here, sem, on, when)

    def settle(self, k, piece):
        for origin, there, _, more in self.ways(k):
            self.take(origin, piece, jnp.logical_and(there, jnp.logical_not(more)))


def small_softplus(v):
    u = jnp.exp(-jnp.abs(v))
    series = jnp.zeros_like(u)
    for n in (8.0, 7.0, 6.0, 5.0, 4.0, 3.0, 2.0, 1.0):
        series = 1.0 / n - u * series
    return jnp.maximum(v, 0.0) + jnp.where(u < 0.1, u * series, jnp.log(1.0 + u))


OUT_PARTS = 4


def layer_kernel(
    planes, lags, tokens, gain_in, val_w, gate_w, rgate_w, rin_w, taps_in, bias_in, cgain_in, staps_in,
    dmap_in, imap_in, base_in, jump_in, ocw, orw,
    out, x_ref, gain, rin_s, rgate_s, wr, wc, taps, bias, cgain, staps, dmap, imap, rbase, jump, jb, cpar, rpar,
    ld, xall, rwall, cwall, projr, jall, wz, wp, yall, cbuf, gext, rext, filt, dec, inf, maps, stat,
    st_all, carry, cr_all,
    send, rx, rpx, rwr, rwc, zr, zc, zo, rj, ry, rp, rv, rq, rw, rh, rs, rc, ls, lr,
):
    me = Spot(planes)
    mail = Mail(send)
    c_lags, s_lags = lags
    f32, bf16 = jnp.float32, jnp.bfloat16
    rows, depth = x_ref.shape[0], wr.shape[1]
    length = xall.shape[0]
    cw, rwid = gext.shape[1], rpar.shape[1]
    seg = length // SEGMENTS
    top = gext.shape[0] - length
    rtop = rext.shape[0] - length
    fold = dec.shape[0]
    part = planes // 2
    width = yall.shape[1] // 8
    mine = me.q * 2 + me.c
    others = (me.qx, me.qy, me.qd)
    pieces = (me.q,) + others
    parts = tuple(range(OUT_PARTS))
    tall = wz.shape[1] // OUT_PARTS
    last = planes - 1
    mates = [me.at(me.z * 4 + (me.q + dq) % 4, c) for dq in range(4) for c in (me.c, 1 - me.c)][1:]
    lined = [me.at((me.s + 4 * k) % (4 * planes), me.c) for k in range(1, planes)]
    loads = []

    def load(src, dst):
        copy = pltpu.make_async_copy(src, dst, ld.at[len(loads)])
        loads.append(copy)
        copy.start()
        return copy

    got_rec = [load(rin_w, rin_s), load(rgate_w, rgate_s)]
    got_x = [load(tokens, x_ref), load(gain_in, gain)]
    got_conv = []
    for q in range(4):
        got_conv.append(load(val_w.at[:, pl.ds(q * cw, cw)], wc.at[q, :, pl.ds(0, cw)]))
        got_conv.append(load(gate_w.at[:, pl.ds(q * cw, cw)], wc.at[q, :, pl.ds(cw, cw)]))
    got_out = []
    for q in range(4):
        at = q * (cw + rwid)
        got_out.append(load(ocw.at[pl.ds(q * cw, cw)], wz.at[me.z, pl.ds(at, cw)]))
        got_out.append(load(orw.at[pl.ds(q * rwid, rwid)], wz.at[me.z, pl.ds(at + cw, rwid)]))
    got_jump = [load(jump_in, jump)]
    got_small = [
        load(src, dst)
        for src, dst in (
            (taps_in, taps), (bias_in, bias), (cgain_in, cgain), (staps_in, staps),
            (dmap_in, dmap), (imap_in, imap), (base_in, rbase),
        )
    ]
    greet(me, mates + lined, False)
    for copy in got_rec:
        copy.wait()
    for q in range(4):
        lanes = slice(q * rwid, (q + 1) * rwid)
        wr[q] = jnp.concatenate([rin_s[:, lanes], rgate_s[:, lanes]], axis=1)

    def of_rows(ref):
        def slot(origin, piece):
            return ref.at[pl.ds(pl.multiple_of((origin * 4 + piece) * depth, depth), depth)]

        return slot

    def theirs_too(origin, piece, when):
        theirs = jnp.logical_and(origin // part != me.c, when)
        place = origin - (1 - me.c) * part
        rest = pl.ds(piece * tall, tall)
        mail.send(wz.at[origin, rest], wp.at[place, rest], rw.at[place, piece], me.partner, theirs)

    rl = Line(me, mail, planes, of_rows(rwall), zr)
    cl = Line(me, mail, planes, of_rows(cwall), zc)
    ol = Line(me, mail, planes, lambda origin, p: wz.at[origin, pl.ds(p * tall, tall)], zo, theirs_too)

    def out_own(p):
        ol.own(p, wz.at[me.z, pl.ds(p * tall, tall)])

    for q in others:
        mail.send(wr.at[q], rl.slot(me.z, me.q), rwr.at[me.q], me.mate(q))
    rl.own(me.q, wr.at[me.q])

    for copy in got_x:
        copy.wait()
    first_row = mine * rows

    @pl.loop(0, rows // 16)
    def _(i):
        values = x_ref[pl.ds(pl.multiple_of(i * 16, 16), 16)].astype(f32)
        inverse = lax.rsqrt(jnp.mean(values * values, axis=1, keepdims=True) + 1e-06)
        place = pl.ds(pl.multiple_of(first_row + i * 16, 16), 16)
        xall[place] = (values * inverse * gain[...]).astype(bf16)

    part_rows = rows // rx.shape[1]

    def xslot(q, c, h):
        return xall.at[pl.ds(pl.multiple_of((q * 2 + c) * rows + h * part_rows, 16), part_rows)]

    xg = PlaneGather(me, mail, xslot, rx, rpx)
    xg.start()
    for copy in got_conv + got_out:
        copy.wait()
    for q in others:
        mail.send(wc.at[q], cl.slot(me.z, me.q), rwc.at[me.q], me.mate(q))
    out_own(0)
    out_own(1)
    kept_here = [mail.local(wr.at[me.q], rl.slot(me.z, me.q)), mail.local(wc.at[me.q], cl.slot(me.z, me.q))]
    for entry in kept_here:
        mail.open.remove(entry)
        entry[0]()
    for p in parts:
        theirs_too(me.z, p, True)
    for copy in got_jump + got_small:
        copy.wait()
    half = jump.shape[0] // 2
    for q in range(4):
        lanes = slice(q * rwid, (q + 1) * rwid)
        jb[q] = jnp.concatenate([jump[:half, lanes], jump[half:, lanes]], axis=1).astype(bf16)
    jall[me.q] = jb[me.q]
    own_lanes = pl.ds(pl.multiple_of(me.q * cw, 128), cw)
    cpar[pl.ds(0, c_lags + 1)] = taps[:, own_lanes].astype(f32)
    cpar[pl.ds(c_lags + 1, 1)] = bias[:, own_lanes]
    cpar[pl.ds(c_lags + 2, 1)] = cgain[:, own_lanes]
    window = -(-rwid // 128) * 128
    wide_lanes = pl.ds(pl.multiple_of(me.q * rwid // 128 * 128, 128), window)

    def own_rec(values):
        moved = values[:, :rwid]
        for lead in sorted({q * rwid % 128 for q in range(4)} - {0}):
            moved = jnp.where(me.q * rwid % 128 == lead, values[:, lead : lead + rwid], moved)
        return moved

    rpar[pl.ds(0, s_lags + 1)] = own_rec(staps[:, wide_lanes].astype(f32))
    rpar[pl.ds(s_lags + 1, 1)] = own_rec(RATE_SCALE * small_softplus(-rbase[:, wide_lanes]))

    maps[...] = jnp.zeros_like(maps)
    size = dmap.shape[1]
    heads = rwid // size
    for h in range(heads):
        spot = pl.ds(h * size, size)
        maps[spot, pl.ds(h * size, size)] = dmap[me.q * heads + h]
        maps[spot, pl.ds(fold * 128 + h * size, size)] = imap[me.q * heads + h]

    for q in others:
        here = rl.slot(me.z, q)
        mail.arrived(here, rwr.at[q], me.partner)
        rl.own(q, here)
    for p in pieces:
        rl.relay(1, p)
    cl.own(me.q, wc.at[me.q])
    for i in range(xg.half):
        xg.first(i)
    for q in others:
        mail.send(jb.at[q], jall.at[me.q], rj.at[me.q], me.mate(q))
    for k in range(2, last):
        for p in pieces:
            rl.relay(k, p)
    xg.second()
    for q in others:
        here = cl.slot(me.z, q)
        mail.arrived(here, rwc.at[q], me.partner)
        cl.own(q, here)
    for k in range(1, planes):
        for p in pieces:
            rl.settle(k, p)
    xg.last(pieces[:3])

    tile = length // 4

    def project_rec(q):
        at = pl.ds(pl.multiple_of(q * tile, tile), tile)
        product = jnp.dot(xall[at], rwall[...], preferred_element_type=f32).astype(bf16)
        projr[at] = product
        rext[pl.ds(pl.multiple_of(q * tile + rtop, 16), tile)] = product[:, :rwid].astype(f32)

    @pl.loop(0, 3)
    def _(i):
        project_rec((me.q // 2 + i // 2) % 2 * 2 + (me.q % 2 + i % 2) % 2)

    for n, p in enumerate(pieces):
        cl.relay(1, p, n < 2, True)
    xg.third()
    xg.last(pieces[3:])
    project_rec(me.qd)

    mail.send(rext.at[pl.ds(length, rtop)], rext.at[pl.ds(0, rtop)], rh.at[0], me.up, me.has_up)
    for p in pieces[2:]:
        cl.relay(1, p, True, False)
    for k in range(2, last):
        for n, p in enumerate(pieces):
            cl.relay(k, p, n < 1, True)

    @pl.when(jnp.logical_not(me.has_down))
    def _():
        rext[pl.ds(0, rtop)] = jnp.zeros((rtop, rwid), f32)
        gext[pl.ds(0, top)] = jnp.zeros((top, cw), f32)

    softened = rpar[pl.ds(s_lags + 1, 1), :]

    @pl.loop(0, SEGMENTS)
    def _(n):
        i = SEGMENTS - 1 - n

        @pl.when(jnp.logical_and(i == 0, me.has_down))
        def _():
            mail.arrived(rext.at[pl.ds(0, rtop)], rh.at[0], me.partner)

        @pl.when(jnp.logical_and(i % 2 == 1, i // 2 != me.q))
        def _():
            mail.arrived(jall.at[i // 2], rj.at[i // 2], me.partner)

        base = pl.multiple_of(i * seg, 8)
        window = rext[pl.ds(pl.multiple_of(base + rtop - 8, 8), seg + 8)]
        smooth = jnp.zeros((seg, rwid), f32)
        for k in range(s_lags + 1):
            smooth = smooth + rpar[pl.ds(k, 1), :] * window[8 - s_lags + k : 8 - s_lags + k + seg]
        smooth = smooth.astype(bf16)
        gates = jax.nn.sigmoid(jnp.dot(smooth, maps[...], preferred_element_type=f32))
        retain, admit = gates[:, :rwid], gates[:, fold * 128 : fold * 128 + rwid]
        wide = jall[i // 2].astype(f32)
        moved = jnp.where(i % 2 == 0, wide[:, :rwid], wide[:, rwid:])
        log_decay = moved - retain * softened
        decay = jnp.exp(log_decay)
        inflow = jnp.sqrt(minus_expm1(2.0 * log_decay)) * admit * smooth.astype(f32)
        for f in range(fold):
            w = min(128, rwid - f * 128)
            dec[f, pl.ds(base, seg), pl.ds(0, w)] = decay[:, f * 128 : f * 128 + w]
            inf[f, pl.ds(base, seg), pl.ds(0, w)] = inflow[:, f * 128 : f * 128 + w]

    def one(i, held):
        after = []
        for f in range(fold):
            at = pl.ds(i, SEGMENTS, stride=seg)
            d = dec.at[f][at, :]
            product, state = held[2 * f] * d, held[2 * f + 1] * d + inf.at[f][at, :]
            dec.at[f][at, :] = product
            inf.at[f][at, :] = state
            after += [product, state]
        return tuple(after)

    flat = (SEGMENTS, 128)
    ends = lax.fori_loop(0, seg, one, (jnp.ones(flat, f32), jnp.zeros(flat, f32)) * fold, unroll=8)
    for f in range(fold):
        product, state = jnp.ones((1, 128), f32), jnp.zeros((1, 128), f32)
        for i in range(SEGMENTS):
            p, s = ends[2 * f][i : i + 1], ends[2 * f + 1][i : i + 1]
            product, state = product * p, p * state + s
        carry[pl.ds(2 * f, 1)] = product
        carry[pl.ds(2 * f + 1, 1)] = state
    for k in range(1, planes):
        mail.send(carry, cr_all.at[me.z], rc.at[me.z], lined[k - 1], me.z + k < planes)
    for k in range(2, last):
        for p in pieces[1:]:
            cl.relay(k, p, True, False)
    for p in parts[2:]:
        out_own(p)

    for k in range(1, planes):
        z = me.z - k
        pl.when(z >= 0)(functools.partial(mail.arrived, cr_all.at[z], rc.at[z], me.partner))
    entering = []
    for f in range(fold):
        held = jnp.zeros((1, 128), f32)
        for j in range(planes - 1):
            after = cr_all[j, pl.ds(2 * f, 1)] * held + cr_all[j, pl.ds(2 * f + 1, 1)]
            held = jnp.where(j < me.z, after, held)
        for i in range(SEGMENTS):
            entering.append(held)
            held = ends[2 * f][i : i + 1] * held + ends[2 * f + 1][i : i + 1]
    own_at = pl.multiple_of(mine * width, 128)
    for i in range(SEGMENTS):
        here = pl.ds(i * seg, seg)
        state = [dec[f, here] * entering[f * SEGMENTS + i] + inf[f, here] for f in range(fold)]
        state = jnp.concatenate(state, axis=1)[:, :rwid]
        result = gelu(projr[here, pl.ds(rwid, rwid)].astype(f32)) * state
        fill = jnp.zeros((seg, width - cw - rwid), f32)
        yall[here, pl.ds(pl.multiple_of(own_at + cw, 128), width - cw)] = jnp.concatenate([result, fill], axis=1).astype(bf16)

    part_length = length // rv.shape[1]

    def gather(lane, lanes, recv, recv_pair):
        def slot(q, c, h):
            spot = pl.ds(pl.multiple_of((q * 2 + c) * width + lane, 128), lanes)
            return yall.at[pl.ds(h * part_length, part_length), spot]

        return PlaneGather(me, mail, slot, recv, recv_pair)

    vg = gather(cw, width - cw, rv, rq)
    vg.start()
    for k in range(1, planes):
        for p in pieces:
            cl.settle(k, p)

    @pl.loop(0, 4)
    def _(i):
        at = pl.ds(pl.multiple_of(i * tile, tile), tile)
        product = jnp.dot(xall[at], cwall[...], preferred_element_type=f32).astype(bf16).astype(f32)
        glu = (product[:, :cw] * jax.nn.sigmoid(product[:, cw:])).astype(bf16).astype(f32)
        gext[pl.ds(pl.multiple_of(i * tile + top, 8), tile)] = glu

    mail.send(gext.at[pl.ds(length, top)], gext.at[pl.ds(0, top)], rh.at[1], me.up, me.has_up)
    for p in parts:
        ol.relay(1, p)
    strips = length // 64

    def filter_strip(n):
        i = strips - 1 - n

        @pl.when(jnp.logical_and(i == 0, me.has_down))
        def _():
            mail.arrived(gext.at[pl.ds(0, top)], rh.at[1], me.partner)

        base = pl.multiple_of(i * 64, 8)
        window = gext[pl.ds(base, 64 + top)]
        total = jnp.zeros((64, cw), f32) + cpar[pl.ds(c_lags + 1, 1), :]
        for k in range(c_lags + 1):
            begin = top - c_lags + k
            total = total + cpar[pl.ds(k, 1), :] * window[begin : begin + 64]
        filt[pl.ds(base, 64)] = total
        part_sum = jnp.sum(total, axis=1, keepdims=True)
        off = total - part_sum * (1.0 / cw)
        lane = lax.broadcasted_iota(jnp.int32, (64, 128), 1)
        spread = jnp.sum(off * off, axis=1, keepdims=True)
        stat[pl.ds(base, 64)] = jnp.where(lane == 0, part_sum, spread)

    pl.loop(0, strips // 4)(filter_strip)
    vg.first(0)
    pl.loop(strips // 4, strips)(filter_strip)

    packed = stat[...].T
    st_all[mine] = packed[0:2]
    for device in mates:
        mail.send(st_all.at[mine], st_all.at[mine], rs.at[mine], device)
    for i in range(1, vg.half):
        vg.first(i)

    for k in range(1, 8):
        d = (mine + k) % 8
        mail.arrived(st_all.at[d], rs.at[d], me.partner)
    total = sum(st_all[d, 0:1, :] for d in range(8))
    mean = total * (1.0 / (8 * cw))
    spread = jnp.zeros_like(mean)
    for d in range(8):
        shift = st_all[d, 0:1, :] * (1.0 / cw) - mean
        spread = spread + st_all[d, 1:2, :] + cw * shift * shift
    scale = lax.rsqrt(spread * (1.0 / (8 * cw)) + 1e-05)
    row = lax.broadcasted_iota(jnp.int32, (128, length), 0)
    stat[...] = jnp.where(row == 0, mean, scale).T

    @pl.loop(0, SEGMENTS)
    def _(i):
        here = pl.ds(pl.multiple_of(i * seg, 16), seg)
        pair = stat[here]
        v = (filt[here] - pair[:, 0:1]) * pair[:, 1:2] * cpar[pl.ds(c_lags + 2, 1), :]
        yall[here, pl.ds(own_at, cw)] = (v * jax.nn.sigmoid(v)).astype(bf16)

    yg = gather(0, cw, ry, rp)
    yg.start()
    vg.second()
    for i in range(yg.half):
        yg.first(i)
    for k in range(2, last):
        for p in parts:
            ol.relay(k, p)
    for k in range(1, last):
        for p in parts:
            ol.settle(k, p)
    vg.third()
    yg.second()
    yg.third()
    vg.last(pieces)
    yg.last(pieces)

    used, cols = cw + rwid, wz.shape[2]
    tile_rows = length // 8
    upward = me.z < part

    def multiply(d, k):
        here = pl.ds(pl.multiple_of(d * tile_rows, 16), tile_rows)
        total = jnp.zeros((tile_rows, cols), f32)
        for q in range(4):
            for c, block in ((me.c, wz.at[me.c * part + k]), (1 - me.c, wp.at[k])):
                left = yall[here, pl.ds(pl.multiple_of((q * 2 + c) * width, 128), width)]
                total = total + jnp.dot(
                    left[:, :used], block[pl.ds(q * used, used)], preferred_element_type=f32
                )
        cbuf[d, k] = total.astype(bf16)

    def place(q, c, k):
        return out.at[:, pl.ds(pl.multiple_of(((c * part + k) * 4 + q) * cols, 128), cols)]

    def target(i):
        flip = 3 - i // 2
        q = (me.q // 2 + flip // 2) % 2 * 2 + (me.q % 2 + flip % 2) % 2
        return q, (me.c + 1 + i) % 2

    def parcel(i, k):
        q, c = target(i)
        return pltpu.make_async_remote_copy(
            src_ref=cbuf.at[q * 2 + c, k], dst_ref=place(me.q, me.c, k), send_sem=ls.at[i, k],
            recv_sem=lr.at[mine, k], device_id=me.at(me.z * 4 + q, c), device_id_type=MESH,
        )

    def kept(k):
        return pltpu.make_async_copy(cbuf.at[mine, k], place(me.q, me.c, k), ls.at[7, k])

    def round_of(n):
        k = jnp.where(upward, n, part - 1 - n)

        @pl.loop(0, 7)
        def _(i):
            q, c = target(i)
            multiply(q * 2 + c, k)
            parcel(i, k).start()

        multiply(mine, k)
        kept(k).start()

    for n in range(part):
        k = jnp.where(upward, n, part - 1 - n)
        if n == part - 1:
            for p in parts:
                ol.settle(last, p)
        for p in parts:
            mail.arrived(wp.at[k, pl.ds(p * tall, tall)], rw.at[k, p], me.partner)
        round_of(n)

    @pl.loop(0, 7)
    def _(i):
        q, c = target(i)
        for k in range(part):
            mail.arrived(place(q, c, k), lr.at[q * 2 + c, k], me.partner)
            parcel(i, k).wait_send()

    for k in range(part):
        kept(k).wait()
    mail.finish()


def layer(planes, lags, tokens, norm_gain, val_w, gate_w, rgate_w, rin_w, taps, bias, cgain, staps, dmap, imap, rbase, jump, ocw, orw):
    rows, width_in = tokens.shape
    length = 8 * rows
    depth = rin_w.shape[0]
    cw, rwid = val_w.shape[1] // 4, rin_w.shape[1] // 4
    used, cols = cw + rwid, ocw.shape[1]
    width = used + -used % 128
    fold = (rwid + 127) // 128
    f32, bf16 = jnp.float32, jnp.bfloat16
    dma = pltpu.SemaphoreType.DMA
    top = lags[0] + -lags[0] % 16
    rtop = lags[1] + -lags[1] % 16
    part = planes // 2
    deep = planes * 4 * depth

    def vmem(*shape, dtype=bf16):
        return pltpu.VMEM(shape, dtype)

    def wide(*shape):
        return pltpu.VMEM(shape, f32)

    return pl.pallas_call(
        functools.partial(layer_kernel, planes, lags),
        out_shape=jax.ShapeDtypeStruct((rows, planes * 4 * cols), bf16),
        in_specs=[ANY] * 16,
        out_specs=ANY,
        scratch_shapes=[
            vmem(rows, width_in), wide(1, width_in), vmem(*rin_w.shape), vmem(*rgate_w.shape),
            vmem(4, depth, 2 * rwid), vmem(4, depth, 2 * cw),
            vmem(*taps.shape), wide(1, 4 * cw), wide(1, 4 * cw), vmem(*staps.shape),
            vmem(*dmap.shape), vmem(*imap.shape), wide(1, 4 * rwid), wide(*jump.shape),
            vmem(4, jump.shape[0] // 2, 2 * rwid), wide(lags[0] + 3 + -(lags[0] + 3) % 8, cw), wide(8, rwid),
            dma((32,)),
            vmem(length, width_in),
            vmem(deep, 2 * rwid),
            vmem(deep, 2 * cw),
            vmem(length, 2 * rwid),
            vmem(4, jump.shape[0] // 2, 2 * rwid),
            vmem(planes, 4 * used, cols),
            vmem(part, 4 * used, cols),
            vmem(length, 8 * width),
            vmem(8, part, rows, cols),
            wide(top + length, cw),
            wide(rtop + length, rwid),
            wide(length, cw),
            wide(fold, length, 128),
            wide(fold, length, 128),
            vmem(rwid, 2 * fold * 128),
            wide(length, 128),
            wide(8, 2, length),
            wide(8, 128),
            wide(planes, 8, 128),
            dma((160 + 20 * planes,)), dma((4, 4)), dma((4, 4)), dma((4,)), dma((4,)),
            dma((planes, 4)), dma((planes, 4)), dma((planes, OUT_PARTS)), dma((4,)),
            dma((4, 4)), dma((4, 4)), dma((4, 4)), dma((4, 4)), dma((part, OUT_PARTS)),
            dma((2,)), dma((8,)), dma((planes,)), dma((8, part)), dma((8, part)),
        ],
        compiler_params=pltpu.CompilerParams(
            collective_id=0, has_side_effects=True, vmem_limit_bytes=60 * 1024 * 1024
        ),
    )(
        tokens, norm_gain[None], val_w, gate_w, rgate_w, rin_w, taps, bias[None], cgain[None], staps,
        dmap, imap, rbase[None], jump, ocw, orw,
    )


def plane_shards(
    planes,
    tokens,
    norm_gain,
    conv_val_w,
    conv_gate_w,
    rec_gate_w,
    rec_in_w,
    conv_taps,
    conv_bias,
    conv_gain,
    short_taps,
    decay_map,
    input_map,
    decay_base,
    decay_jump,
    out_conv_w,
    out_rec_w,
):
    lags = (conv_taps.shape[0] - 1, short_taps.shape[0] - 1)
    return layer(
        planes, lags, tokens, norm_gain, conv_val_w, conv_gate_w, rec_gate_w, rec_in_w, conv_taps, conv_bias,
        conv_gain, short_taps, decay_map, input_map, decay_base, decay_jump, out_conv_w, out_rec_w,
    )


def solution(mesh):
    in_specs = (
        P(("sp", "tp"), None),
        P(),
        P("sp", "tp"),
        P("sp", "tp"),
        P("sp", "tp"),
        P("sp", "tp"),
        P(None, "tp"),
        P("tp"),
        P("tp"),
        P(None, "tp"),
        P("tp", None, None),
        P("tp", None, None),
        P("tp"),
        P("sp", "tp"),
        P("tp", "sp"),
        P("tp", "sp"),
    )
    out_specs = P(("sp", "tp"), None)
    count = mesh.shape["sp"]
    planar = mesh.shape["tp"] == 2 and count % 8 == 0 and count >= 16
    body = functools.partial(plane_shards, count // 4) if planar else shards
    return jax.shard_map(body, mesh=mesh, in_specs=in_specs, out_specs=out_specs, check_vma=False)
```

```python
import functools

import jax
import jax.numpy as jnp
from jax import lax
from jax.experimental import pallas as pl
from jax.experimental.pallas import tpu as pltpu
from jax.sharding import PartitionSpec as P

CONV_WIDTH = 1024


RATE_SCALE = 8.0


def passed_along(value, axis, by):
    count = lax.axis_size(axis)
    pairs = [(i, i + by) for i in range(count) if 0 <= i + by < count]
    return lax.ppermute(value, axis, pairs)


def prefix(part, axis, combine, identity):
    place = lax.axis_index(axis)
    gathered = jax.tree.map(lambda a: lax.all_gather(a, axis), part)
    state = jax.tree.map(lambda a, e: jnp.zeros_like(a) + jnp.asarray(e, a.dtype), part, identity)

    def one(step, state):
        return combine(
            state, jax.tree.map(lambda a: lax.dynamic_index_in_dim(a, step, 0, False), gathered)
        )

    return lax.fori_loop(0, place, one, state)


def norm_rows(values, gain):
    widened = values.astype(jnp.float32)
    inverse = lax.rsqrt(jnp.mean(widened * widened, axis=-1, keepdims=True) + 1e-06)
    return (widened * inverse * gain).astype(jnp.bfloat16)


def causal_window(edge, current, weights):
    extended = jnp.concatenate([edge, current], axis=0).astype(jnp.float32)
    taps_wide = weights.astype(jnp.float32)
    length = current.shape[0]
    result = jnp.zeros((length, current.shape[1]), jnp.float32)
    for lag_index in range(weights.shape[0]):
        result = result + taps_wide[lag_index][None, :] * extended[lag_index : lag_index + length]
    return result


def chain_step(earlier, latter):
    return (earlier[0] * latter[0], latter[0] * earlier[1] + latter[1])


def glu_of(conv_val, conv_gate):
    return (conv_val.astype(jnp.float32) * jax.nn.sigmoid(conv_gate.astype(jnp.float32))).astype(
        jnp.bfloat16
    )


def shards(
    tokens,
    norm_gain,
    conv_val_w,
    conv_gate_w,
    rec_gate_w,
    rec_in_w,
    conv_taps,
    conv_bias,
    conv_gain,
    short_taps,
    decay_map,
    input_map,
    decay_base,
    decay_jump,
    out_conv_w,
    out_rec_w,
):
    rec_cols = rec_in_w.shape[1]
    conv_lags = conv_taps.shape[0] - 1
    short_lags = short_taps.shape[0] - 1
    normed = norm_rows(tokens, norm_gain)
    val_full, gate_full = (
        lax.all_gather(conv_val_w, "sp", axis=0, tiled=True),
        lax.all_gather(conv_gate_w, "sp", axis=0, tiled=True),
    )
    all_rows = lax.all_gather(normed, "tp", axis=0, tiled=True)
    conv_val = jnp.dot(all_rows, val_full, preferred_element_type=jnp.float32).astype(jnp.bfloat16)
    conv_gate = jnp.dot(all_rows, gate_full, preferred_element_type=jnp.float32).astype(
        jnp.bfloat16
    )
    glu = glu_of(conv_val, conv_gate)
    conv_edge = passed_along(glu[-conv_lags:], "sp", 1)
    rgate_full, rin_full = (
        lax.all_gather(rec_gate_w, "sp", axis=0, tiled=True),
        lax.all_gather(rec_in_w, "sp", axis=0, tiled=True),
    )
    rec_gate = jnp.dot(all_rows, rgate_full, preferred_element_type=jnp.float32).astype(
        jnp.bfloat16
    )
    rec_in = jnp.dot(all_rows, rin_full, preferred_element_type=jnp.float32).astype(jnp.bfloat16)
    rec_edge = passed_along(rec_in[-short_lags:], "sp", 1)
    filtered = causal_window(conv_edge, glu, conv_taps) + conv_bias[None, :]
    row_total = lax.psum(jnp.sum(filtered, axis=1), "tp")
    centered = filtered - (row_total / CONV_WIDTH)[:, None]
    spread = lax.psum(jnp.sum(centered * centered, axis=1), "tp") / CONV_WIDTH
    conv_out = jax.nn.silu(centered * lax.rsqrt(spread + 1e-05)[:, None] * conv_gain).astype(
        jnp.bfloat16
    )
    smoothed = causal_window(rec_edge, rec_in, short_taps).astype(jnp.bfloat16)
    length = smoothed.shape[0]
    grouped = smoothed.reshape(length, decay_map.shape[0], decay_map.shape[1])
    retain = jax.nn.sigmoid(
        jnp.einsum("thi,hio->tho", grouped, decay_map, preferred_element_type=jnp.float32).reshape(
            length, rec_cols
        )
    )
    admit = jax.nn.sigmoid(
        jnp.einsum("thi,hio->tho", grouped, input_map, preferred_element_type=jnp.float32).reshape(
            length, rec_cols
        )
    )
    log_decay = -RATE_SCALE * retain * jax.nn.softplus(-decay_base)[None, :] + decay_jump
    decay = jnp.exp(log_decay)
    inflow = jnp.sqrt(-jnp.expm1(2.0 * log_decay)) * admit * smoothed.astype(jnp.float32)
    products, local_state = lax.associative_scan(chain_step, (decay, inflow), axis=0)
    entering = prefix(
        (products[-1], local_state[-1]),
        "sp",
        chain_step,
        (jnp.ones((rec_cols,), jnp.float32), jnp.zeros((rec_cols,), jnp.float32)),
    )
    state = local_state + products * entering[1][None, :]
    rec_out = (jax.nn.gelu(rec_gate.astype(jnp.float32)) * state).astype(jnp.bfloat16)
    conv_full, rec_full = (
        lax.all_gather(out_conv_w, "sp", axis=1, tiled=True),
        lax.all_gather(out_rec_w, "sp", axis=1, tiled=True),
    )
    return lax.psum_scatter(
        (
            jnp.dot(conv_out, conv_full, preferred_element_type=jnp.float32)
            + jnp.dot(rec_out, rec_full, preferred_element_type=jnp.float32)
        ).astype(jnp.bfloat16),
        "tp",
        scatter_dimension=0,
        tiled=True,
    )


MESH = pl.DeviceIdType.MESH
ANY = pl.BlockSpec(memory_space=pl.ANY)
VMEM = pl.BlockSpec(memory_space=pltpu.VMEM)
SEGMENTS = 8


class Spot:
    def __init__(self, planes):
        self.s, self.c = lax.axis_index("sp"), lax.axis_index("tp")
        self.z, self.q = self.s // 4, self.s % 4
        self.qx = self.q + 1 - 2 * (self.q % 2)
        self.qy = (self.q + 2) % 4
        self.qd = 3 - self.q
        self.has_up, self.has_down = self.z < planes - 1, self.z > 0
        self.up, self.down = self.at(self.s + 4, self.c), self.at(self.s - 4, self.c)
        self.partner = self.at(self.s, 1 - self.c)

    def at(self, s, c):
        return {"sp": s, "tp": c}

    def mate(self, q):
        return self.at(self.z * 4 + q, self.c)


class Mail:
    def __init__(self, send_sem):
        self.send_sem, self.count, self.open = send_sem, 0, []

    def send(self, src, dst, recv, device, when=None):
        copy = pltpu.make_async_remote_copy(
            src_ref=src, dst_ref=dst, send_sem=self.send_sem.at[self.count],
            recv_sem=recv, device_id=device, device_id_type=MESH,
        )
        self.count += 1
        self.open.append((copy.wait_send, when))
        if when is None:
            copy.start()
        else:
            pl.when(when)(copy.start)

    def local(self, src, dst):
        copy = pltpu.make_async_copy(src, dst, self.send_sem.at[self.count])
        self.count += 1
        copy.start()
        self.open.append((copy.wait, None))
        return self.open[-1]

    def arrived(self, dst, recv, device):
        pltpu.make_async_remote_copy(
            src_ref=dst, dst_ref=dst, send_sem=self.send_sem.at[0],
            recv_sem=recv, device_id=device, device_id_type=MESH,
        ).wait_recv()

    def finish(self):
        for wait, when in self.open:
            if when is None:
                wait()
            else:
                pl.when(when)(wait)


def greet(me, devices, line):
    barrier = pltpu.get_barrier_semaphore()
    for device in devices:
        pl.semaphore_signal(barrier, inc=1, device_id=device, device_id_type=MESH)
    amount = len(devices)
    if line:
        for has, device in ((me.has_up, me.up), (me.has_down, me.down)):
            @pl.when(has)
            def _():
                pl.semaphore_signal(barrier, inc=1, device_id=device, device_id_type=MESH)
        amount = amount + me.has_up.astype(jnp.int32) + me.has_down.astype(jnp.int32)
    pl.semaphore_wait(barrier, amount)


class PlaneGather:
    def __init__(self, me, mail, slot, recv, recv_pair):
        self.me, self.mail, self.slot = me, mail, slot
        self.recv, self.recv_pair = recv, recv_pair
        self.parts = recv.shape[1]
        self.half = self.parts // 2

    def start(self):
        me, mail = self.me, self.mail
        for h in range(self.parts):
            for q, part in ((me.qx, h), (me.qy, (h + self.half) % self.parts)):
                own = self.slot(me.q, me.c, part)
                mail.send(own, own, self.recv.at[me.q, part], me.mate(q))
        for part in range(self.parts):
            self.share(me.q, part, self.slot(me.q, me.c, part))

    def took(self, q, part):
        here = self.slot(q, self.me.c, part)
        self.mail.arrived(here, self.recv.at[q, part], self.me.partner)
        return here

    def share(self, q, part, here):
        self.mail.send(here, here, self.recv_pair.at[q, part], self.me.partner)

    def first(self, i):
        me = self.me
        for q, part, to in ((me.qx, i, me.qy), (me.qy, self.half + i, me.qx)):
            here = self.took(q, part)
            self.mail.send(here, here, self.recv.at[q, part], me.mate(to))
            self.share(q, part, here)

    def second(self):
        for i in range(self.half):
            for q, part in ((self.me.qx, self.half + i), (self.me.qy, i)):
                self.share(q, part, self.took(q, part))

    def third(self):
        for i in range(self.half):
            for part in (i, self.half + i):
                self.share(self.me.qd, part, self.took(self.me.qd, part))

    def last(self, origins):
        me = self.me
        for q in origins:
            for part in range(self.parts):
                self.mail.arrived(self.slot(q, 1 - me.c, part), self.recv_pair.at[q, part], me.partner)


def minus_expm1(y):
    series = 1.0 + y * (1.0 / 8.0)
    for n in (7.0, 6.0, 5.0, 4.0, 3.0, 2.0):
        series = 1.0 + y * (1.0 / n) * series
    return jnp.where(y > -0.35, -y * series, 1.0 - jnp.exp(y))


def gelu(v):
    return 0.5 * v * (1.0 + jnp.tanh(0.7978845608028654 * (v + 0.044715 * v * v * v)))


class Line:
    def __init__(self, me, mail, planes, slot, recv, seen=None):
        self.me, self.mail, self.planes = me, mail, planes
        self.slot, self.recv, self.seen = slot, recv, seen

    def own(self, piece, src, up=True, down=True):
        me = self.me
        for wanted, has, device in ((up, me.has_up, me.up), (down, me.has_down, me.down)):
            if wanted:
                self.mail.send(src, self.slot(me.z, piece), self.recv.at[me.z, piece], device, has)

    def ways(self, k):
        me = self.me
        return (
            (me.z - k, me.z >= k, me.up, me.has_up),
            (me.z + k, me.z + k < self.planes, me.down, me.has_down),
        )

    def take(self, origin, piece, when):
        here, sem = self.slot(origin, piece), self.recv.at[origin, piece]
        pl.when(when)(functools.partial(self.mail.arrived, here, sem, self.me.partner))
        if self.seen is not None:
            self.seen(origin, piece, when)
        return here, sem

    def relay(self, k, piece, up=True, down=True):
        for wanted, (origin, there, on, more) in zip((up, down), self.ways(k)):
            if wanted:
                when = jnp.logical_and(there, more)
                here, sem = self.take(origin, piece, when)
                self.mail.send(here, here, sem, on, when)

    def settle(self, k, piece, when=True):
        for origin, there, _, more in self.ways(k):
            self.take(origin, piece, there & jnp.logical_not(more) & when)


def small_softplus(v):
    u = jnp.exp(-jnp.abs(v))
    series = jnp.zeros_like(u)
    for n in (8.0, 7.0, 6.0, 5.0, 4.0, 3.0, 2.0, 1.0):
        series = 1.0 / n - u * series
    return jnp.maximum(v, 0.0) + jnp.where(u < 0.1, u * series, jnp.log(1.0 + u))


OUT_PARTS = 4


def layer_kernel(
    planes, lags, tokens, gain_in, val_w, gate_w, rgate_w, rin_w, taps_in, bias_in, cgain_in, staps_in,
    dmap_in, imap_in, base_in, jump_in, ocw, orw,
    out, x_ref, gain, rin_s, rgate_s, wr, wc, taps, bias, cgain, staps, dmap, imap, rbase, jump, jb, cpar, rpar,
    ld, xall, rwall, cwall, projr, jall, wz, wp, yall, yrest, cacc, cbuf, gext, rext, filt, dec, inf, maps, stat,
    st_all, carry, cr_all,
    send, rx, rpx, rwr, rwc, zr, zc, zo, rj, ry, rp, rv, rq, re, rf, rw, rh, rs, rc, ls, lr,
):
    me = Spot(planes)
    mail = Mail(send)
    c_lags, s_lags = lags
    f32, bf16 = jnp.float32, jnp.bfloat16
    rows, depth = x_ref.shape[0], wr.shape[1]
    length = xall.shape[0]
    cw, rwid = gext.shape[1], rpar.shape[1]
    seg = length // SEGMENTS
    lane_seg = dec.shape[1] // SEGMENTS
    top = gext.shape[0] - length
    rtop = rext.shape[0] - length
    fold = dec.shape[0]
    part = planes // 2
    major = rwid // 128 * 128
    minor = rwid - major
    mine = me.q * 2 + me.c
    others = (me.qx, me.qy, me.qd)
    pieces = (me.q,) + others
    parts = tuple(range(OUT_PARTS))
    tall = wz.shape[1] // OUT_PARTS
    last = planes - 1
    mates = [me.at(me.z * 4 + (me.q + dq) % 4, c) for dq in range(4) for c in (me.c, 1 - me.c)][1:]
    lined = [me.at((me.s + 4 * k) % (4 * planes), me.c) for k in range(1, planes)]
    loads = []

    def load(src, dst):
        copy = pltpu.make_async_copy(src, dst, ld.at[len(loads)])
        loads.append(copy)
        copy.start()
        return copy

    got_rec = [load(rin_w, rin_s), load(rgate_w, rgate_s)]
    got_x = [load(tokens, x_ref), load(gain_in, gain)]
    got_conv = []
    for q in range(4):
        got_conv.append(load(val_w.at[:, pl.ds(q * cw, cw)], wc.at[q, :, pl.ds(0, cw)]))
        got_conv.append(load(gate_w.at[:, pl.ds(q * cw, cw)], wc.at[q, :, pl.ds(cw, cw)]))
    got_out = []
    got_out.append(load(ocw, wz.at[me.z, pl.ds(0, 4 * cw)]))
    for q in range(4):
        at = 4 * cw + q * major
        got_out.append(load(orw.at[pl.ds(q * rwid, major)], wz.at[me.z, pl.ds(at, major)]))
        at = 4 * (cw + major) + q * minor
        got_out.append(load(orw.at[pl.ds(q * rwid + major, minor)], wz.at[me.z, pl.ds(at, minor)]))
    got_jump = [load(jump_in, jump)]
    got_small = [
        load(src, dst)
        for src, dst in (
            (taps_in, taps), (bias_in, bias), (cgain_in, cgain), (staps_in, staps),
            (dmap_in, dmap), (imap_in, imap), (base_in, rbase),
        )
    ]
    greet(me, mates + lined, False)
    for copy in got_rec:
        copy.wait()
    for q in range(4):
        lanes = slice(q * rwid, (q + 1) * rwid)
        wr[q] = jnp.concatenate([rin_s[:, lanes], rgate_s[:, lanes]], axis=1)

    def of_rows(ref):
        def slot(origin, piece):
            return ref.at[pl.ds(pl.multiple_of((origin * 4 + piece) * depth, depth), depth)]

        return slot

    def theirs_too(origin, piece, when):
        theirs = jnp.logical_and(origin // part != me.c, when)
        place = origin - (1 - me.c) * part
        rest = pl.ds(piece * tall, tall)
        mail.send(wz.at[origin, rest], wp.at[place, rest], rw.at[place, piece], me.partner, theirs)

    rl = Line(me, mail, planes, of_rows(rwall), zr)
    cl = Line(me, mail, planes, of_rows(cwall), zc)
    ol = Line(me, mail, planes, lambda origin, p: wz.at[origin, pl.ds(p * tall, tall)], zo, theirs_too)

    def out_own(p):
        ol.own(p, wz.at[me.z, pl.ds(p * tall, tall)])

    for q in others:
        mail.send(wr.at[q], rl.slot(me.z, me.q), rwr.at[me.q], me.mate(q))
    rl.own(me.q, wr.at[me.q])

    for copy in got_x:
        copy.wait()
    first_row = mine * rows

    @pl.loop(0, rows // 16)
    def _(i):
        values = x_ref[pl.ds(pl.multiple_of(i * 16, 16), 16)].astype(f32)
        inverse = lax.rsqrt(jnp.mean(values * values, axis=1, keepdims=True) + 1e-06)
        place = pl.ds(pl.multiple_of(first_row + i * 16, 16), 16)
        xall[place] = (values * inverse * gain[...]).astype(bf16)

    part_rows = rows // rx.shape[1]

    def xslot(q, c, h):
        return xall.at[pl.ds(pl.multiple_of((q * 2 + c) * rows + h * part_rows, 16), part_rows)]

    xg = PlaneGather(me, mail, xslot, rx, rpx)
    xg.start()
    for copy in got_conv + got_out:
        copy.wait()
    for q in others:
        mail.send(wc.at[q], cl.slot(me.z, me.q), rwc.at[me.q], me.mate(q))
    out_own(0)
    out_own(1)
    kept_here = [mail.local(wr.at[me.q], rl.slot(me.z, me.q)), mail.local(wc.at[me.q], cl.slot(me.z, me.q))]
    for entry in kept_here:
        mail.open.remove(entry)
        entry[0]()
    for p in parts:
        theirs_too(me.z, p, True)
    for copy in got_jump + got_small:
        copy.wait()
    half = jump.shape[0] // 2
    for q in range(4):
        lanes = slice(q * rwid, (q + 1) * rwid)
        jb[q] = jnp.concatenate([jump[:half, lanes], jump[half:, lanes]], axis=1).astype(bf16)
    jall[me.q] = jb[me.q]
    own_lanes = pl.ds(pl.multiple_of(me.q * cw, 128), cw)
    cpar[pl.ds(0, c_lags + 1)] = taps[:, own_lanes].astype(f32)
    cpar[pl.ds(c_lags + 1, 1)] = bias[:, own_lanes]
    cpar[pl.ds(c_lags + 2, 1)] = cgain[:, own_lanes]
    window = -(-rwid // 128) * 128
    wide_lanes = pl.ds(pl.multiple_of(me.q * rwid // 128 * 128, 128), window)

    def own_rec(values):
        moved = values[:, :rwid]
        for lead in sorted({q * rwid % 128 for q in range(4)} - {0}):
            moved = jnp.where(me.q * rwid % 128 == lead, values[:, lead : lead + rwid], moved)
        return moved

    rpar[pl.ds(0, s_lags + 1)] = own_rec(staps[:, wide_lanes].astype(f32))
    rpar[pl.ds(s_lags + 1, 1)] = own_rec(RATE_SCALE * small_softplus(-rbase[:, wide_lanes]))

    maps[...] = jnp.zeros_like(maps)
    size = dmap.shape[1]
    heads = rwid // size
    for h in range(heads):
        spot = pl.ds(h * size, size)
        maps[spot, pl.ds(h * size, size)] = dmap[me.q * heads + h]
        maps[spot, pl.ds(fold * 128 + h * size, size)] = imap[me.q * heads + h]

    for q in others:
        here = rl.slot(me.z, q)
        mail.arrived(here, rwr.at[q], me.partner)
        rl.own(q, here)
    for p in pieces:
        rl.relay(1, p)
    cl.own(me.q, wc.at[me.q])
    for i in range(xg.half):
        xg.first(i)
    for q in others:
        mail.send(jb.at[q], jall.at[me.q], rj.at[me.q], me.mate(q))
    for k in range(2, last):
        for p in pieces:
            rl.relay(k, p)
    xg.second()
    for q in others:
        here = cl.slot(me.z, q)
        mail.arrived(here, rwc.at[q], me.partner)
        cl.own(q, here)
    for k in range(1, planes):
        for p in pieces:
            rl.settle(k, p)
    xg.last(pieces[:3])

    tile = length // 4

    def project_rec(q):
        at = pl.ds(pl.multiple_of(q * tile, tile), tile)
        product = jnp.dot(xall[at], rwall[...], preferred_element_type=f32).astype(bf16)
        projr[at] = product
        rext[pl.ds(pl.multiple_of(q * tile + rtop, 16), tile)] = product[:, :rwid].astype(f32)

    @pl.loop(0, 3)
    def _(i):
        project_rec((me.q // 2 + i // 2) % 2 * 2 + (me.q % 2 + i % 2) % 2)

    for n, p in enumerate(pieces):
        cl.relay(1, p, n < 2, True)
    xg.third()
    xg.last(pieces[3:])
    project_rec(me.qd)

    mail.send(rext.at[pl.ds(length, rtop)], rext.at[pl.ds(0, rtop)], rh.at[0], me.up, me.has_up)
    for p in pieces[2:]:
        cl.relay(1, p, True, False)
    for k in range(2, last):
        for n, p in enumerate(pieces):
            cl.relay(k, p, n < 1, True)

    @pl.when(jnp.logical_not(me.has_down))
    def _():
        rext[pl.ds(0, rtop)] = jnp.zeros((rtop, rwid), f32)
        gext[pl.ds(0, top)] = jnp.zeros((top, cw), f32)

    softened = rpar[pl.ds(s_lags + 1, 1), :]

    @pl.loop(0, SEGMENTS)
    def _(n):
        step = (n + 1) // 2
        ring = (me.q // 2 + step % 4 // 2) % 2 * 2 + (me.q % 2 + step % 2) % 2
        i = jnp.where(n == SEGMENTS - 1, 2 * me.q, 2 * ring + n % 2)
        i = jnp.where(n == 0, 2 * me.q + 1, i)

        @pl.when(jnp.logical_and(i == 0, me.has_down))
        def _():
            mail.arrived(rext.at[pl.ds(0, rtop)], rh.at[0], me.partner)

        @pl.when(jnp.logical_and(n % 2 == 1, n < SEGMENTS - 1))
        def _():
            mail.arrived(jall.at[i // 2], rj.at[i // 2], me.partner)

        base = pl.multiple_of(i * seg, 8)
        window = rext[pl.ds(pl.multiple_of(base + rtop - 8, 8), seg + 8)]
        smooth = jnp.zeros((seg, rwid), f32)
        for k in range(s_lags + 1):
            smooth = smooth + rpar[pl.ds(k, 1), :] * window[8 - s_lags + k : 8 - s_lags + k + seg]
        smooth = smooth.astype(bf16)
        gates = jax.nn.sigmoid(jnp.dot(smooth, maps[...], preferred_element_type=f32))
        retain, admit = gates[:, :rwid], gates[:, fold * 128 : fold * 128 + rwid]
        wide = jall[i // 2].astype(f32)
        moved = jnp.where(i % 2 == 0, wide[:, :rwid], wide[:, rwid:])
        log_decay = moved - retain * softened
        decay = jnp.exp(log_decay)
        inflow = jnp.sqrt(minus_expm1(2.0 * log_decay)) * admit * smooth.astype(f32)
        for f in range(fold):
            w = min(128, rwid - f * 128)
            spot = pl.ds(pl.multiple_of(i * lane_seg, 8), seg)
            dec[f, spot, pl.ds(0, w)] = decay[:, f * 128 : f * 128 + w]
            inf[f, spot, pl.ds(0, w)] = inflow[:, f * 128 : f * 128 + w]

    def one(i, held):
        after = []
        for f in range(fold):
            at = pl.ds(i, SEGMENTS, stride=lane_seg)
            d = dec.at[f][at, :]
            product, state = held[2 * f] * d, held[2 * f + 1] * d + inf.at[f][at, :]
            dec.at[f][at, :] = product
            inf.at[f][at, :] = state
            after += [product, state]
        return tuple(after)

    flat = (SEGMENTS, 128)
    ends = lax.fori_loop(0, seg, one, (jnp.ones(flat, f32), jnp.zeros(flat, f32)) * fold, unroll=8)
    for f in range(fold):
        product, state = jnp.ones((1, 128), f32), jnp.zeros((1, 128), f32)
        for i in range(SEGMENTS):
            p, s = ends[2 * f][i : i + 1], ends[2 * f + 1][i : i + 1]
            product, state = product * p, p * state + s
        carry[pl.ds(2 * f, 1)] = product
        carry[pl.ds(2 * f + 1, 1)] = state
    for k in range(1, planes):
        mail.send(carry, cr_all.at[me.z], rc.at[me.z], lined[k - 1], me.z + k < planes)
    for k in range(2, last):
        for p in pieces[1:]:
            cl.relay(k, p, True, False)
    for p in parts[2:]:
        out_own(p)

    for k in range(1, planes):
        z = me.z - k
        pl.when(z >= 0)(functools.partial(mail.arrived, cr_all.at[z], rc.at[z], me.partner))
    entering = []
    for f in range(fold):
        held = jnp.zeros((1, 128), f32)
        for j in range(planes - 1):
            after = cr_all[j, pl.ds(2 * f, 1)] * held + cr_all[j, pl.ds(2 * f + 1, 1)]
            held = jnp.where(j < me.z, after, held)
        for i in range(SEGMENTS):
            entering.append(held)
            held = ends[2 * f][i : i + 1] * held + ends[2 * f + 1][i : i + 1]
    placed = me.c * 4 + me.q

    def rec_result(i):
        here, there = pl.ds(i * seg, seg), pl.ds(i * lane_seg, seg)
        state = [dec[f, there] * entering[f * SEGMENTS + i] + inf[f, there] for f in range(fold)]
        state = jnp.concatenate(state, axis=1)[:, :rwid]
        result = (gelu(projr[here, pl.ds(rwid, rwid)].astype(f32)) * state).astype(bf16)
        yall[here, pl.ds(pl.multiple_of(8 * cw + placed * major, 128), major)] = result[:, :major]
        return result[:, major:]

    for i in range(SEGMENTS // 2):
        pair = jnp.concatenate([rec_result(i), rec_result(i + SEGMENTS // 2)], axis=1)
        yrest[pl.ds(i * seg, seg), pl.ds(pl.multiple_of(placed * 2 * minor, 128), 2 * minor)] = pair

    def gather(buffer, lane, lanes, recv, recv_pair):
        tall_part = buffer.shape[0] // recv.shape[1]

        def slot(q, c, h):
            spot = pl.ds(pl.multiple_of(lane + (c * 4 + q) * lanes, 128), lanes)
            return buffer.at[pl.ds(h * tall_part, tall_part), spot]

        return PlaneGather(me, mail, slot, recv, recv_pair)

    mg = gather(yall, 8 * cw, major, rv, rq)
    eg = gather(yrest, 0, 2 * minor, re, rf)
    yg = gather(yall, 0, cw, ry, rp)
    mg.start()
    eg.start()
    for k in range(1, last):
        for p in pieces:
            cl.settle(k, p)
    plane_depth = 4 * depth
    is_last = (me.z == last).astype(jnp.int32)

    def conv_product(at, begin, size):
        deep = pl.ds(pl.multiple_of(begin, plane_depth), size)
        return jnp.dot(xall[at, deep], cwall[deep], preferred_element_type=f32)

    @pl.loop(0, 4)
    def _(i):
        at = pl.ds(pl.multiple_of(i * tile, tile), tile)
        cacc[at] = conv_product(at, is_last * plane_depth, last * plane_depth)

    for i in range(mg.half):
        mg.first(i)
    for p in parts:
        ol.relay(1, p)
    for p in pieces:
        cl.settle(last, p)

    @pl.loop(0, 4)
    def _(i):
        at = pl.ds(pl.multiple_of(i * tile, tile), tile)
        product = cacc[at] + conv_product(at, (1 - is_last) * last * plane_depth, plane_depth)
        product = product.astype(bf16).astype(f32)
        glu = (product[:, :cw] * jax.nn.sigmoid(product[:, cw:])).astype(bf16).astype(f32)
        gext[pl.ds(pl.multiple_of(i * tile + top, 8), tile)] = glu

    mail.send(gext.at[pl.ds(length, top)], gext.at[pl.ds(0, top)], rh.at[1], me.up, me.has_up)
    strips = length // 64

    def filter_strip(n):
        i = strips - 1 - n

        @pl.when(jnp.logical_and(i == 0, me.has_down))
        def _():
            mail.arrived(gext.at[pl.ds(0, top)], rh.at[1], me.partner)

        base = pl.multiple_of(i * 64, 8)
        window = gext[pl.ds(base, 64 + top)]
        total = jnp.zeros((64, cw), f32) + cpar[pl.ds(c_lags + 1, 1), :]
        for r in range(8):
            ks = [k for k in range(c_lags + 1) if (top - c_lags + k) % 8 == r]
            span = 64 + (8 if r else 0)
            shifted = jnp.zeros((span, cw), f32)
            for k in ks:
                begin = (top - c_lags + k) // 8 * 8
                shifted = shifted + cpar[pl.ds(k, 1), :] * window[begin : begin + span]
            total = total + shifted[r : r + 64]
        filt[pl.ds(base, 64)] = total
        part_sum = jnp.sum(total, axis=1, keepdims=True)
        off = total - part_sum * (1.0 / cw)
        lane = lax.broadcasted_iota(jnp.int32, (64, 128), 1)
        spread = jnp.sum(off * off, axis=1, keepdims=True)
        stat[pl.ds(base, 64)] = jnp.where(lane == 0, part_sum, spread)

    pl.loop(0, strips)(filter_strip)

    packed = stat[...].T
    st_all[mine] = packed[0:2]
    for device in mates:
        mail.send(st_all.at[mine], st_all.at[mine], rs.at[mine], device)
    for i in range(eg.half):
        eg.first(i)

    for k in range(1, 8):
        d = (mine + k) % 8
        mail.arrived(st_all.at[d], rs.at[d], me.partner)
    total = sum(st_all[d, 0:1, :] for d in range(8))
    mean = total * (1.0 / (8 * cw))
    spread = jnp.zeros_like(mean)
    for d in range(8):
        shift = st_all[d, 0:1, :] * (1.0 / cw) - mean
        spread = spread + st_all[d, 1:2, :] + cw * shift * shift
    scale = lax.rsqrt(spread * (1.0 / (8 * cw)) + 1e-05)
    row = lax.broadcasted_iota(jnp.int32, (128, length), 0)
    stat[...] = jnp.where(row == 0, mean, scale).T

    @pl.loop(0, SEGMENTS)
    def _(i):
        here = pl.ds(pl.multiple_of(i * seg, 16), seg)
        pair = stat[here]
        v = (filt[here] - pair[:, 0:1]) * pair[:, 1:2] * cpar[pl.ds(c_lags + 2, 1), :]
        yall[here, pl.ds(pl.multiple_of(placed * cw, 128), cw)] = (v * jax.nn.sigmoid(v)).astype(bf16)

    yg.start()
    for k in range(2, last):
        for p in parts:
            ol.relay(k, p)
    mg.second()
    eg.second()
    for i in range(yg.half):
        yg.first(i)
    mg.third()
    eg.third()
    mg.last(pieces)
    eg.last(pieces)
    rest_at = 8 * (cw + major)

    @pl.loop(0, SEGMENTS // 2)
    def _(i):
        values = yrest[pl.ds(pl.multiple_of(i * seg, 16), seg)]
        low = [values[:, j * 2 * minor : j * 2 * minor + minor] for j in range(8)]
        high = [values[:, j * 2 * minor + minor : (j + 1) * 2 * minor] for j in range(8)]
        for begin, chosen in ((0, low), (length // 2, high)):
            here = pl.ds(pl.multiple_of(begin + i * seg, 16), seg)
            yall[here, pl.ds(rest_at, 8 * minor)] = jnp.concatenate(chosen, axis=1)

    for k in range(1, last):
        for p in parts:
            ol.settle(k, p)
    yg.second()
    yg.third()
    yg.last(pieces)

    cols = wz.shape[2]
    upward = me.z < part
    far = last - me.z
    far_mine = far // part == me.c

    def multiply(q, k):
        here = pl.ds(pl.multiple_of(q * 2 * rows, 16), 2 * rows)
        total = jnp.zeros((2 * rows, cols), f32)
        for c, block in ((me.c, wz.at[me.c * part + k]), (1 - me.c, wp.at[k])):
            begin = 0
            for at, lanes in ((0, 4 * cw), (8 * cw, 4 * major), (rest_at, 4 * minor)):
                left = yall[here, pl.ds(pl.multiple_of(at + c * lanes, 128), lanes)]
                total = total + jnp.dot(left, block[pl.ds(begin, lanes)], preferred_element_type=f32)
                begin = begin + lanes
        total = total.astype(bf16)
        for c in range(2):
            cbuf[q * 2 + c, k] = total[c * rows : (c + 1) * rows]

    def place(q, c, k):
        return out.at[:, pl.ds(pl.multiple_of(((c * part + k) * 4 + q) * cols, 128), cols)]

    def mate_of(i):
        flip = 3 - i
        return (me.q // 2 + flip // 2) % 2 * 2 + (me.q % 2 + flip % 2) % 2

    def parcel(q, c, k):
        return pltpu.make_async_remote_copy(
            src_ref=cbuf.at[q * 2 + c, k], dst_ref=place(me.q, me.c, k), send_sem=ls.at[q * 2 + c, k],
            recv_sem=lr.at[mine, k], device_id=me.at(me.z * 4 + q, c), device_id_type=MESH,
        )

    def kept(k):
        return pltpu.make_async_copy(cbuf.at[mine, k], place(me.q, me.c, k), ls.at[mine, k])

    for n in range(part):
        k = jnp.where(upward, n, part - 1 - n)
        if n == part - 1:
            for p in parts:
                ol.settle(last, p, far_mine)
        for p in parts:
            mail.arrived(wp.at[k, pl.ds(p * tall, tall)], rw.at[k, p], me.partner)

        @pl.loop(0, 3)
        def _(i):
            q = mate_of(i)
            multiply(q, k)
            for c in (me.c, 1 - me.c):
                parcel(q, c, k).start()

        multiply(me.q, k)
        parcel(me.q, 1 - me.c, k).start()
        kept(k).start()

    for p in parts:
        ol.settle(last, p, jnp.logical_not(far_mine))

    @pl.loop(0, 4)
    def _(i):
        q = mate_of(i)
        for k in range(part):
            mail.arrived(place(q, 1 - me.c, k), lr.at[q * 2 + 1 - me.c, k], me.partner)
            parcel(q, 1 - me.c, k).wait_send()

    @pl.loop(0, 3)
    def _(i):
        q = mate_of(i)
        for k in range(part):
            mail.arrived(place(q, me.c, k), lr.at[q * 2 + me.c, k], me.partner)
            parcel(q, me.c, k).wait_send()

    for k in range(part):
        kept(k).wait()
    mail.finish()


def layer(planes, lags, tokens, norm_gain, val_w, gate_w, rgate_w, rin_w, taps, bias, cgain, staps, dmap, imap, rbase, jump, ocw, orw):
    rows, width_in = tokens.shape
    length = 8 * rows
    depth = rin_w.shape[0]
    cw, rwid = val_w.shape[1] // 4, rin_w.shape[1] // 4
    used, cols = cw + rwid, ocw.shape[1]
    minor = rwid % 128
    fold = (rwid + 127) // 128
    f32, bf16 = jnp.float32, jnp.bfloat16
    dma = pltpu.SemaphoreType.DMA
    top = lags[0] + -lags[0] % 16
    rtop = lags[1] + -lags[1] % 16
    part = planes // 2
    deep = planes * 4 * depth

    def vmem(*shape, dtype=bf16):
        return pltpu.VMEM(shape, dtype)

    def wide(*shape):
        return pltpu.VMEM(shape, f32)

    return pl.pallas_call(
        functools.partial(layer_kernel, planes, lags),
        out_shape=jax.ShapeDtypeStruct((rows, planes * 4 * cols), bf16),
        in_specs=[ANY] * 16,
        out_specs=ANY,
        scratch_shapes=[
            vmem(rows, width_in), wide(1, width_in), vmem(*rin_w.shape), vmem(*rgate_w.shape),
            vmem(4, depth, 2 * rwid), vmem(4, depth, 2 * cw),
            vmem(*taps.shape), wide(1, 4 * cw), wide(1, 4 * cw), vmem(*staps.shape),
            vmem(*dmap.shape), vmem(*imap.shape), wide(1, 4 * rwid), wide(*jump.shape),
            vmem(4, jump.shape[0] // 2, 2 * rwid), wide(lags[0] + 3 + -(lags[0] + 3) % 8, cw), wide(8, rwid),
            dma((32,)),
            vmem(length, width_in),
            vmem(deep, 2 * rwid),
            vmem(deep, 2 * cw),
            vmem(length, 2 * rwid),
            vmem(4, jump.shape[0] // 2, 2 * rwid),
            vmem(planes, 4 * used, cols),
            vmem(part, 4 * used, cols),
            vmem(length, 8 * used),
            vmem(length // 2, 16 * minor),
            wide(length, 2 * cw),
            vmem(8, part, rows, cols),
            wide(top + length, cw),
            wide(rtop + length, rwid),
            wide(length, cw),
            wide(fold, length + 8 * SEGMENTS, 128),
            wide(fold, length + 8 * SEGMENTS, 128),
            vmem(rwid, 2 * fold * 128),
            wide(length, 128),
            wide(8, 2, length),
            wide(8, 128),
            wide(planes, 8, 128),
            dma((180 + 20 * planes,)), dma((4, 4)), dma((4, 4)), dma((4,)), dma((4,)),
            dma((planes, 4)), dma((planes, 4)), dma((planes, OUT_PARTS)), dma((4,)),
            dma((4, 4)), dma((4, 4)), dma((4, 4)), dma((4, 4)), dma((4, 2)), dma((4, 2)), dma((part, OUT_PARTS)),
            dma((2,)), dma((8,)), dma((planes,)), dma((8, part)), dma((8, part)),
        ],
        compiler_params=pltpu.CompilerParams(
            collective_id=0, has_side_effects=True, vmem_limit_bytes=60 * 1024 * 1024
        ),
    )(
        tokens, norm_gain[None], val_w, gate_w, rgate_w, rin_w, taps, bias[None], cgain[None], staps,
        dmap, imap, rbase[None], jump, ocw, orw,
    )


def plane_shards(
    planes,
    tokens,
    norm_gain,
    conv_val_w,
    conv_gate_w,
    rec_gate_w,
    rec_in_w,
    conv_taps,
    conv_bias,
    conv_gain,
    short_taps,
    decay_map,
    input_map,
    decay_base,
    decay_jump,
    out_conv_w,
    out_rec_w,
):
    lags = (conv_taps.shape[0] - 1, short_taps.shape[0] - 1)
    return layer(
        planes, lags, tokens, norm_gain, conv_val_w, conv_gate_w, rec_gate_w, rec_in_w, conv_taps, conv_bias,
        conv_gain, short_taps, decay_map, input_map, decay_base, decay_jump, out_conv_w, out_rec_w,
    )


def solution(mesh):
    in_specs = (
        P(("sp", "tp"), None),
        P(),
        P("sp", "tp"),
        P("sp", "tp"),
        P("sp", "tp"),
        P("sp", "tp"),
        P(None, "tp"),
        P("tp"),
        P("tp"),
        P(None, "tp"),
        P("tp", None, None),
        P("tp", None, None),
        P("tp"),
        P("sp", "tp"),
        P("tp", "sp"),
        P("tp", "sp"),
    )
    out_specs = P(("sp", "tp"), None)
    count = mesh.shape["sp"]
    planar = mesh.shape["tp"] == 2 and count % 8 == 0 and count >= 16
    body = functools.partial(plane_shards, count // 4) if planar else shards
    return jax.shard_map(body, mesh=mesh, in_specs=in_specs, out_specs=out_specs, check_vma=False)
```

```python
import functools

import jax
import jax.numpy as jnp
from jax import lax
from jax.experimental import pallas as pl
from jax.experimental.pallas import tpu as pltpu
from jax.sharding import PartitionSpec as P

CONV_WIDTH = 1024


RATE_SCALE = 8.0


def passed_along(value, axis, by):
    count = lax.axis_size(axis)
    pairs = [(i, i + by) for i in range(count) if 0 <= i + by < count]
    return lax.ppermute(value, axis, pairs)


def prefix(part, axis, combine, identity):
    place = lax.axis_index(axis)
    gathered = jax.tree.map(lambda a: lax.all_gather(a, axis), part)
    state = jax.tree.map(lambda a, e: jnp.zeros_like(a) + jnp.asarray(e, a.dtype), part, identity)

    def one(step, state):
        return combine(
            state, jax.tree.map(lambda a: lax.dynamic_index_in_dim(a, step, 0, False), gathered)
        )

    return lax.fori_loop(0, place, one, state)


def norm_rows(values, gain):
    widened = values.astype(jnp.float32)
    inverse = lax.rsqrt(jnp.mean(widened * widened, axis=-1, keepdims=True) + 1e-06)
    return (widened * inverse * gain).astype(jnp.bfloat16)


def causal_window(edge, current, weights):
    extended = jnp.concatenate([edge, current], axis=0).astype(jnp.float32)
    taps_wide = weights.astype(jnp.float32)
    length = current.shape[0]
    result = jnp.zeros((length, current.shape[1]), jnp.float32)
    for lag_index in range(weights.shape[0]):
        result = result + taps_wide[lag_index][None, :] * extended[lag_index : lag_index + length]
    return result


def chain_step(earlier, latter):
    return (earlier[0] * latter[0], latter[0] * earlier[1] + latter[1])


def glu_of(conv_val, conv_gate):
    return (conv_val.astype(jnp.float32) * jax.nn.sigmoid(conv_gate.astype(jnp.float32))).astype(
        jnp.bfloat16
    )


def shards(
    tokens,
    norm_gain,
    conv_val_w,
    conv_gate_w,
    rec_gate_w,
    rec_in_w,
    conv_taps,
    conv_bias,
    conv_gain,
    short_taps,
    decay_map,
    input_map,
    decay_base,
    decay_jump,
    out_conv_w,
    out_rec_w,
):
    rec_cols = rec_in_w.shape[1]
    conv_lags = conv_taps.shape[0] - 1
    short_lags = short_taps.shape[0] - 1
    normed = norm_rows(tokens, norm_gain)
    val_full, gate_full = (
        lax.all_gather(conv_val_w, "sp", axis=0, tiled=True),
        lax.all_gather(conv_gate_w, "sp", axis=0, tiled=True),
    )
    all_rows = lax.all_gather(normed, "tp", axis=0, tiled=True)
    conv_val = jnp.dot(all_rows, val_full, preferred_element_type=jnp.float32).astype(jnp.bfloat16)
    conv_gate = jnp.dot(all_rows, gate_full, preferred_element_type=jnp.float32).astype(
        jnp.bfloat16
    )
    glu = glu_of(conv_val, conv_gate)
    conv_edge = passed_along(glu[-conv_lags:], "sp", 1)
    rgate_full, rin_full = (
        lax.all_gather(rec_gate_w, "sp", axis=0, tiled=True),
        lax.all_gather(rec_in_w, "sp", axis=0, tiled=True),
    )
    rec_gate = jnp.dot(all_rows, rgate_full, preferred_element_type=jnp.float32).astype(
        jnp.bfloat16
    )
    rec_in = jnp.dot(all_rows, rin_full, preferred_element_type=jnp.float32).astype(jnp.bfloat16)
    rec_edge = passed_along(rec_in[-short_lags:], "sp", 1)
    filtered = causal_window(conv_edge, glu, conv_taps) + conv_bias[None, :]
    row_total = lax.psum(jnp.sum(filtered, axis=1), "tp")
    centered = filtered - (row_total / CONV_WIDTH)[:, None]
    spread = lax.psum(jnp.sum(centered * centered, axis=1), "tp") / CONV_WIDTH
    conv_out = jax.nn.silu(centered * lax.rsqrt(spread + 1e-05)[:, None] * conv_gain).astype(
        jnp.bfloat16
    )
    smoothed = causal_window(rec_edge, rec_in, short_taps).astype(jnp.bfloat16)
    length = smoothed.shape[0]
    grouped = smoothed.reshape(length, decay_map.shape[0], decay_map.shape[1])
    retain = jax.nn.sigmoid(
        jnp.einsum("thi,hio->tho", grouped, decay_map, preferred_element_type=jnp.float32).reshape(
            length, rec_cols
        )
    )
    admit = jax.nn.sigmoid(
        jnp.einsum("thi,hio->tho", grouped, input_map, preferred_element_type=jnp.float32).reshape(
            length, rec_cols
        )
    )
    log_decay = -RATE_SCALE * retain * jax.nn.softplus(-decay_base)[None, :] + decay_jump
    decay = jnp.exp(log_decay)
    inflow = jnp.sqrt(-jnp.expm1(2.0 * log_decay)) * admit * smoothed.astype(jnp.float32)
    products, local_state = lax.associative_scan(chain_step, (decay, inflow), axis=0)
    entering = prefix(
        (products[-1], local_state[-1]),
        "sp",
        chain_step,
        (jnp.ones((rec_cols,), jnp.float32), jnp.zeros((rec_cols,), jnp.float32)),
    )
    state = local_state + products * entering[1][None, :]
    rec_out = (jax.nn.gelu(rec_gate.astype(jnp.float32)) * state).astype(jnp.bfloat16)
    conv_full, rec_full = (
        lax.all_gather(out_conv_w, "sp", axis=1, tiled=True),
        lax.all_gather(out_rec_w, "sp", axis=1, tiled=True),
    )
    return lax.psum_scatter(
        (
            jnp.dot(conv_out, conv_full, preferred_element_type=jnp.float32)
            + jnp.dot(rec_out, rec_full, preferred_element_type=jnp.float32)
        ).astype(jnp.bfloat16),
        "tp",
        scatter_dimension=0,
        tiled=True,
    )


MESH = pl.DeviceIdType.MESH
ANY = pl.BlockSpec(memory_space=pl.ANY)
VMEM = pl.BlockSpec(memory_space=pltpu.VMEM)
SEGMENTS = 8


class Spot:
    def __init__(self, planes):
        self.s, self.c = lax.axis_index("sp"), lax.axis_index("tp")
        self.z, self.q = self.s // 4, self.s % 4
        self.qx = self.q + 1 - 2 * (self.q % 2)
        self.qy = (self.q + 2) % 4
        self.qd = 3 - self.q
        self.has_up, self.has_down = self.z < planes - 1, self.z > 0
        self.up, self.down = self.at(self.s + 4, self.c), self.at(self.s - 4, self.c)
        self.partner = self.at(self.s, 1 - self.c)

    def at(self, s, c):
        return {"sp": s, "tp": c}

    def mate(self, q):
        return self.at(self.z * 4 + q, self.c)


class Mail:
    def __init__(self, send_sem):
        self.send_sem, self.count, self.open = send_sem, 0, []

    def send(self, src, dst, recv, device, when=None):
        copy = pltpu.make_async_remote_copy(
            src_ref=src, dst_ref=dst, send_sem=self.send_sem.at[self.count],
            recv_sem=recv, device_id=device, device_id_type=MESH,
        )
        self.count += 1
        self.open.append((copy.wait_send, when))
        if when is None:
            copy.start()
        else:
            pl.when(when)(copy.start)

    def local(self, src, dst):
        copy = pltpu.make_async_copy(src, dst, self.send_sem.at[self.count])
        self.count += 1
        copy.start()
        self.open.append((copy.wait, None))
        return self.open[-1]

    def arrived(self, dst, recv, device):
        pltpu.make_async_remote_copy(
            src_ref=dst, dst_ref=dst, send_sem=self.send_sem.at[0],
            recv_sem=recv, device_id=device, device_id_type=MESH,
        ).wait_recv()

    def finish(self):
        for wait, when in self.open:
            if when is None:
                wait()
            else:
                pl.when(when)(wait)


def greet(me, devices, line):
    barrier = pltpu.get_barrier_semaphore()
    for device in devices:
        pl.semaphore_signal(barrier, inc=1, device_id=device, device_id_type=MESH)
    amount = len(devices)
    if line:
        for has, device in ((me.has_up, me.up), (me.has_down, me.down)):
            @pl.when(has)
            def _():
                pl.semaphore_signal(barrier, inc=1, device_id=device, device_id_type=MESH)
        amount = amount + me.has_up.astype(jnp.int32) + me.has_down.astype(jnp.int32)
    pl.semaphore_wait(barrier, amount)


class PlaneGather:
    def __init__(self, me, mail, slot, recv, recv_pair):
        self.me, self.mail, self.slot = me, mail, slot
        self.recv, self.recv_pair = recv, recv_pair
        self.parts = recv.shape[1]
        self.half = self.parts // 2

    def start(self):
        me, mail = self.me, self.mail
        for h in range(self.parts):
            for q, part in ((me.qx, h), (me.qy, (h + self.half) % self.parts)):
                own = self.slot(me.q, me.c, part)
                mail.send(own, own, self.recv.at[me.q, part], me.mate(q))
        for part in range(self.parts):
            self.share(me.q, part, self.slot(me.q, me.c, part))

    def took(self, q, part):
        here = self.slot(q, self.me.c, part)
        self.mail.arrived(here, self.recv.at[q, part], self.me.partner)
        return here

    def share(self, q, part, here):
        self.mail.send(here, here, self.recv_pair.at[q, part], self.me.partner)

    def first(self, i):
        me = self.me
        for q, part, to in ((me.qx, i, me.qy), (me.qy, self.half + i, me.qx)):
            here = self.took(q, part)
            self.mail.send(here, here, self.recv.at[q, part], me.mate(to))
            self.share(q, part, here)

    def second(self):
        for i in range(self.half):
            for q, part in ((self.me.qx, self.half + i), (self.me.qy, i)):
                self.share(q, part, self.took(q, part))

    def third(self):
        for i in range(self.half):
            for part in (i, self.half + i):
                self.share(self.me.qd, part, self.took(self.me.qd, part))

    def last(self, origins):
        me = self.me
        for q in origins:
            for part in range(self.parts):
                self.mail.arrived(self.slot(q, 1 - me.c, part), self.recv_pair.at[q, part], me.partner)


def minus_expm1(y):
    series = 1.0 + y * (1.0 / 8.0)
    for n in (7.0, 6.0, 5.0, 4.0, 3.0, 2.0):
        series = 1.0 + y * (1.0 / n) * series
    return jnp.where(y > -0.35, -y * series, 1.0 - jnp.exp(y))


def gelu(v):
    return 0.5 * v * (1.0 + jnp.tanh(0.7978845608028654 * (v + 0.044715 * v * v * v)))


class Line:
    def __init__(self, me, mail, planes, slot, recv, seen=None):
        self.me, self.mail, self.planes = me, mail, planes
        self.slot, self.recv, self.seen = slot, recv, seen

    def own(self, piece, src, up=True, down=True):
        me = self.me
        for wanted, has, device in ((up, me.has_up, me.up), (down, me.has_down, me.down)):
            if wanted is not False:
                self.mail.send(src, self.slot(me.z, piece), self.recv.at[me.z, piece], device, has & wanted)

    def ways(self, k):
        me = self.me
        return (
            (me.z - k, me.z >= k, me.up, me.has_up),
            (me.z + k, me.z + k < self.planes, me.down, me.has_down),
        )

    def take(self, origin, piece, when):
        here, sem = self.slot(origin, piece), self.recv.at[origin, piece]
        pl.when(when)(functools.partial(self.mail.arrived, here, sem, self.me.partner))
        if self.seen is not None:
            self.seen(origin, piece, when)
        return here, sem

    def relay(self, k, piece, up=True, down=True):
        for wanted, (origin, there, on, more) in zip((up, down), self.ways(k)):
            if wanted:
                when = jnp.logical_and(there, more)
                here, sem = self.take(origin, piece, when)
                self.mail.send(here, here, sem, on, when)

    def await_up(self, k, piece):
        origin, there, _, more = self.ways(k)[0]
        return self.take(origin, piece, there & more)

    def forward_up(self, k, piece):
        origin, there, on, more = self.ways(k)[0]
        here, sem = self.slot(origin, piece), self.recv.at[origin, piece]
        self.mail.send(here, here, sem, on, there & more)

    def settle(self, k, piece, when=True):
        for origin, there, _, more in self.ways(k):
            self.take(origin, piece, there & jnp.logical_not(more) & when)


def small_softplus(v):
    u = jnp.exp(-jnp.abs(v))
    series = jnp.zeros_like(u)
    for n in (8.0, 7.0, 6.0, 5.0, 4.0, 3.0, 2.0, 1.0):
        series = 1.0 / n - u * series
    return jnp.maximum(v, 0.0) + jnp.where(u < 0.1, u * series, jnp.log(1.0 + u))


OUT_PARTS = 4


def layer_kernel(
    planes, lags, tokens, gain_in, val_w, gate_w, rgate_w, rin_w, taps_in, bias_in, cgain_in, staps_in,
    dmap_in, imap_in, base_in, jump_in, ocw, orw,
    out, x_ref, gain, rin_s, rgate_s, wr, wc, taps, bias, cgain, staps, dmap, imap, rbase, jump, jb, cpar, rpar,
    ld, xall, rwall, cwall, projr, jall, wz, wp, yall, yrest, cacc, cbuf, gext, rext, filt, dec, inf, maps, ft,
    st_all, carry, cr_all,
    send, rx, rpx, rwr, rwc, zr, zc, zo, rj, ry, rp, rv, rq, re, rf, rw, rh, rs, rc, ls, lr,
):
    me = Spot(planes)
    mail = Mail(send)
    c_lags, s_lags = lags
    f32, bf16 = jnp.float32, jnp.bfloat16
    rows, depth = x_ref.shape[0], wr.shape[1]
    length = xall.shape[0]
    cw, rwid = gext.shape[1], rpar.shape[1]
    seg = length // SEGMENTS
    lane_seg = dec.shape[1] // SEGMENTS
    top = gext.shape[0] - length
    rtop = rext.shape[0] - length
    fold = dec.shape[0]
    part = planes // 2
    major = rwid // 128 * 128
    minor = rwid - major
    mine = me.q * 2 + me.c
    others = (me.qx, me.qy, me.qd)
    pieces = (me.q,) + others
    parts = tuple(range(OUT_PARTS))
    tall = wz.shape[1] // OUT_PARTS
    last = planes - 1
    mates = [me.at(me.z * 4 + (me.q + dq) % 4, c) for dq in range(4) for c in (me.c, 1 - me.c)][1:]
    lined = [me.at((me.s + 4 * k) % (4 * planes), me.c) for k in range(1, planes)]
    loads = []

    def load(src, dst):
        copy = pltpu.make_async_copy(src, dst, ld.at[len(loads)])
        loads.append(copy)
        copy.start()
        return copy

    got_rec = [load(rin_w, rin_s), load(rgate_w, rgate_s)]
    got_x = [load(tokens, x_ref), load(gain_in, gain)]
    got_conv = []
    for q in range(4):
        got_conv.append(load(val_w.at[:, pl.ds(q * cw, cw)], wc.at[q, :, pl.ds(0, cw)]))
        got_conv.append(load(gate_w.at[:, pl.ds(q * cw, cw)], wc.at[q, :, pl.ds(cw, cw)]))
    got_out = []
    got_out.append(load(ocw, wz.at[me.z, pl.ds(0, 4 * cw)]))
    for q in range(4):
        at = 4 * cw + q * major
        got_out.append(load(orw.at[pl.ds(q * rwid, major)], wz.at[me.z, pl.ds(at, major)]))
        at = 4 * (cw + major) + q * minor
        got_out.append(load(orw.at[pl.ds(q * rwid + major, minor)], wz.at[me.z, pl.ds(at, minor)]))
    got_jump = [load(jump_in, jump)]
    got_small = [
        load(src, dst)
        for src, dst in (
            (taps_in, taps), (bias_in, bias), (cgain_in, cgain), (staps_in, staps),
            (dmap_in, dmap), (imap_in, imap), (base_in, rbase),
        )
    ]
    greet(me, mates + lined, False)
    for copy in got_rec:
        copy.wait()
    for q in range(4):
        lanes = slice(q * rwid, (q + 1) * rwid)
        wr[q] = jnp.concatenate([rin_s[:, lanes], rgate_s[:, lanes]], axis=1)

    def of_rows(ref):
        def slot(origin, piece):
            return ref.at[pl.ds(pl.multiple_of((origin * 4 + piece) * depth, depth), depth)]

        return slot

    def theirs_too(origin, piece, when):
        theirs = jnp.logical_and(origin // part != me.c, when)
        place = origin - (1 - me.c) * part
        rest = pl.ds(piece * tall, tall)
        mail.send(wz.at[origin, rest], wp.at[place, rest], rw.at[place, piece], me.partner, theirs)

    rl = Line(me, mail, planes, of_rows(rwall), zr)
    cl = Line(me, mail, planes, of_rows(cwall), zc)
    ol = Line(me, mail, planes, lambda origin, p: wz.at[origin, pl.ds(p * tall, tall)], zo, theirs_too)

    def out_own(p, up=True, down=True):
        ol.own(p, wz.at[me.z, pl.ds(p * tall, tall)], up, down)

    for q in others:
        mail.send(wr.at[q], rl.slot(me.z, me.q), rwr.at[me.q], me.mate(q))
    rl.own(me.q, wr.at[me.q])

    for copy in got_x:
        copy.wait()
    first_row = mine * rows

    @pl.loop(0, rows // 16)
    def _(i):
        values = x_ref[pl.ds(pl.multiple_of(i * 16, 16), 16)].astype(f32)
        inverse = lax.rsqrt(jnp.mean(values * values, axis=1, keepdims=True) + 1e-06)
        place = pl.ds(pl.multiple_of(first_row + i * 16, 16), 16)
        xall[place] = (values * inverse * gain[...]).astype(bf16)

    part_rows = rows // rx.shape[1]

    def xslot(q, c, h):
        return xall.at[pl.ds(pl.multiple_of((q * 2 + c) * rows + h * part_rows, 16), part_rows)]

    xg = PlaneGather(me, mail, xslot, rx, rpx)
    xg.start()
    for copy in got_conv + got_out:
        copy.wait()
    for q in others:
        mail.send(wc.at[q], cl.slot(me.z, me.q), rwc.at[me.q], me.mate(q))
    out_own(0)
    out_own(1)
    kept_here = [mail.local(wr.at[me.q], rl.slot(me.z, me.q)), mail.local(wc.at[me.q], cl.slot(me.z, me.q))]
    for entry in kept_here:
        mail.open.remove(entry)
        entry[0]()
    for p in parts:
        theirs_too(me.z, p, True)
    for copy in got_jump + got_small:
        copy.wait()
    half = jump.shape[0] // 2
    for q in range(4):
        lanes = slice(q * rwid, (q + 1) * rwid)
        jb[q] = jnp.concatenate([jump[:half, lanes], jump[half:, lanes]], axis=1).astype(bf16)
    jall[me.q] = jb[me.q]
    own_lanes = pl.ds(pl.multiple_of(me.q * cw, 128), cw)
    cpar[pl.ds(0, c_lags + 1)] = taps[:, own_lanes].astype(f32)
    cpar[pl.ds(c_lags + 1, 1)] = bias[:, own_lanes]
    cpar[pl.ds(c_lags + 2, 1)] = cgain[:, own_lanes]
    window = -(-rwid // 128) * 128
    wide_lanes = pl.ds(pl.multiple_of(me.q * rwid // 128 * 128, 128), window)

    def own_rec(values):
        moved = values[:, :rwid]
        for lead in sorted({q * rwid % 128 for q in range(4)} - {0}):
            moved = jnp.where(me.q * rwid % 128 == lead, values[:, lead : lead + rwid], moved)
        return moved

    rpar[pl.ds(0, s_lags + 1)] = own_rec(staps[:, wide_lanes].astype(f32))
    rpar[pl.ds(s_lags + 1, 1)] = own_rec(RATE_SCALE * small_softplus(-rbase[wide_lanes][None]))

    maps[...] = jnp.zeros_like(maps)
    size = dmap.shape[1]
    heads = rwid // size
    for h in range(heads):
        spot = pl.ds(h * size, size)
        maps[spot, pl.ds(h * size, size)] = dmap[me.q * heads + h]
        maps[spot, pl.ds(fold * 128 + h * size, size)] = imap[me.q * heads + h]

    for q in others:
        here = rl.slot(me.z, q)
        mail.arrived(here, rwr.at[q], me.partner)
        rl.own(q, here)
    for p in pieces:
        rl.relay(1, p)
    cl.own(me.q, wc.at[me.q])
    for i in range(xg.half):
        xg.first(i)
    for q in others:
        mail.send(jb.at[q], jall.at[me.q], rj.at[me.q], me.mate(q))
    for k in range(2, last):
        for p in pieces:
            rl.relay(k, p)
    xg.second()
    for q in others:
        here = cl.slot(me.z, q)
        mail.arrived(here, rwc.at[q], me.partner)
        cl.own(q, here)
    for k in range(1, planes):
        for p in pieces:
            rl.settle(k, p)
    xg.last(pieces[:3])

    tile = length // 4

    def project_rec(q):
        at = pl.ds(pl.multiple_of(q * tile, tile), tile)
        product = jnp.dot(xall[at], rwall[...], preferred_element_type=f32).astype(bf16)
        projr[at] = product
        rext[pl.ds(pl.multiple_of(q * tile + rtop, 16), tile)] = product[:, :rwid].astype(f32)

    @pl.loop(0, 3)
    def _(i):
        project_rec((me.q // 2 + i // 2) % 2 * 2 + (me.q % 2 + i % 2) % 2)

    for n, p in enumerate(pieces):
        cl.relay(1, p, n < 1, True)
    xg.third()
    xg.last(pieces[3:])
    project_rec(me.qd)

    mail.send(rext.at[pl.ds(length, rtop)], rext.at[pl.ds(0, rtop)], rh.at[0], me.up, me.has_up)
    for p in pieces[1:3]:
        cl.relay(1, p, True, False)
    for k in range(2, last):
        for p in pieces:
            cl.relay(k, p, False, True)

    @pl.when(jnp.logical_not(me.has_down))
    def _():
        rext[pl.ds(0, rtop)] = jnp.zeros((rtop, rwid), f32)
        gext[pl.ds(0, top)] = jnp.zeros((top, cw), f32)

    softened = rpar[pl.ds(s_lags + 1, 1), :]

    @pl.loop(0, SEGMENTS)
    def _(n):
        step = (n + 1) // 2
        ring = (me.q // 2 + step % 4 // 2) % 2 * 2 + (me.q % 2 + step % 2) % 2
        i = jnp.where(n == SEGMENTS - 1, 2 * me.q, 2 * ring + n % 2)
        i = jnp.where(n == 0, 2 * me.q + 1, i)

        @pl.when(jnp.logical_and(i == 0, me.has_down))
        def _():
            mail.arrived(rext.at[pl.ds(0, rtop)], rh.at[0], me.partner)

        @pl.when(jnp.logical_and(n % 2 == 1, n < SEGMENTS - 1))
        def _():
            mail.arrived(jall.at[i // 2], rj.at[i // 2], me.partner)

        base = pl.multiple_of(i * seg, 8)
        window = rext[pl.ds(pl.multiple_of(base + rtop - 8, 8), seg + 8)]
        smooth = jnp.zeros((seg, rwid), f32)
        for k in range(s_lags + 1):
            smooth = smooth + rpar[pl.ds(k, 1), :] * window[8 - s_lags + k : 8 - s_lags + k + seg]
        smooth = smooth.astype(bf16)
        gates = jax.nn.sigmoid(jnp.dot(smooth, maps[...], preferred_element_type=f32))
        retain, admit = gates[:, :rwid], gates[:, fold * 128 : fold * 128 + rwid]
        wide = jall[i // 2].astype(f32)
        moved = jnp.where(i % 2 == 0, wide[:, :rwid], wide[:, rwid:])
        log_decay = moved - retain * softened
        decay = jnp.exp(log_decay)
        inflow = jnp.sqrt(minus_expm1(2.0 * log_decay)) * admit * smooth.astype(f32)
        for f in range(fold):
            w = min(128, rwid - f * 128)
            spot = pl.ds(pl.multiple_of(i * lane_seg, 8), seg)
            dec[f, spot, pl.ds(0, w)] = decay[:, f * 128 : f * 128 + w]
            inf[f, spot, pl.ds(0, w)] = inflow[:, f * 128 : f * 128 + w]

    def one(i, held):
        after = []
        for f in range(fold):
            at = pl.ds(i, SEGMENTS, stride=lane_seg)
            d = dec.at[f][at, :]
            product, state = held[2 * f] * d, held[2 * f + 1] * d + inf.at[f][at, :]
            dec.at[f][at, :] = product
            inf.at[f][at, :] = state
            after += [product, state]
        return tuple(after)

    flat = (SEGMENTS, 128)
    ends = lax.fori_loop(0, seg, one, (jnp.ones(flat, f32), jnp.zeros(flat, f32)) * fold, unroll=8)
    for f in range(fold):
        product, state = jnp.ones((1, 128), f32), jnp.zeros((1, 128), f32)
        for i in range(SEGMENTS):
            p, s = ends[2 * f][i : i + 1], ends[2 * f + 1][i : i + 1]
            product, state = product * p, p * state + s
        carry[pl.ds(2 * f, 1)] = product
        carry[pl.ds(2 * f + 1, 1)] = state
    for k in range(1, planes):
        mail.send(carry, cr_all.at[me.z], rc.at[me.z], lined[k - 1], me.z + k < planes)
    early = me.z < planes - 2
    cl.relay(1, pieces[3], True, False)
    for k in range(2, last):
        for p in pieces[:2]:
            cl.relay(k, p, True, False)
    for p in parts[2:]:
        out_own(p, early, True)

    for k in range(1, planes):
        z = me.z - k
        pl.when(z >= 0)(functools.partial(mail.arrived, cr_all.at[z], rc.at[z], me.partner))
    entering = []
    for f in range(fold):
        held = jnp.zeros((1, 128), f32)
        for j in range(planes - 1):
            after = cr_all[j, pl.ds(2 * f, 1)] * held + cr_all[j, pl.ds(2 * f + 1, 1)]
            held = jnp.where(j < me.z, after, held)
        for i in range(SEGMENTS):
            entering.append(held)
            held = ends[2 * f][i : i + 1] * held + ends[2 * f + 1][i : i + 1]
    placed = me.c * 4 + me.q

    def rec_result(i):
        here, there = pl.ds(i * seg, seg), pl.ds(i * lane_seg, seg)
        state = [dec[f, there] * entering[f * SEGMENTS + i] + inf[f, there] for f in range(fold)]
        state = jnp.concatenate(state, axis=1)[:, :rwid]
        result = (gelu(projr[here, pl.ds(rwid, rwid)].astype(f32)) * state).astype(bf16)
        yall[here, pl.ds(pl.multiple_of(8 * cw + placed * major, 128), major)] = result[:, :major]
        return result[:, major:]

    for i in range(SEGMENTS // 2):
        pair = jnp.concatenate([rec_result(i), rec_result(i + SEGMENTS // 2)], axis=1)
        yrest[pl.ds(i * seg, seg), pl.ds(pl.multiple_of(placed * 2 * minor, 128), 2 * minor)] = pair

    def gather(buffer, lane, lanes, recv, recv_pair):
        tall_part = buffer.shape[0] // recv.shape[1]

        def slot(q, c, h):
            spot = pl.ds(pl.multiple_of(lane + (c * 4 + q) * lanes, 128), lanes)
            return buffer.at[pl.ds(h * tall_part, tall_part), spot]

        return PlaneGather(me, mail, slot, recv, recv_pair)

    mg = gather(yall, 8 * cw, major, rv, rq)
    eg = gather(yrest, 0, 2 * minor, re, rf)
    yg = gather(yall, 0, cw, ry, rp)
    mg.start()
    eg.start()
    for k in range(1, last):
        for p in pieces:
            cl.settle(k, p)
        for p in pieces[2:] if k > 1 else ():
            cl.await_up(k, p)
    plane_depth = 4 * depth
    is_last = (me.z == last).astype(jnp.int32)

    def conv_product(at, begin, size):
        deep = pl.ds(pl.multiple_of(begin, plane_depth), size)
        return jnp.dot(xall[at, deep], cwall[deep], preferred_element_type=f32)

    @pl.loop(0, 4)
    def _(i):
        at = pl.ds(pl.multiple_of(i * tile, tile), tile)
        cacc[at] = conv_product(at, is_last * plane_depth, last * plane_depth)

    middle = me.has_up & me.has_down

    def finish_conv(when):
        @pl.when(when)
        def _():
            @pl.loop(0, 4)
            def _(i):
                at = pl.ds(pl.multiple_of(i * tile, tile), tile)
                product = cacc[at] + conv_product(at, (1 - is_last) * last * plane_depth, plane_depth)
                product = product.astype(bf16).astype(f32)
                glu = (product[:, :cw] * jax.nn.sigmoid(product[:, cw:])).astype(bf16).astype(f32)
                gext[pl.ds(pl.multiple_of(i * tile + top, 8), tile)] = glu

        tail_rows = gext.at[pl.ds(length, top)]
        mail.send(tail_rows, gext.at[pl.ds(0, top)], rh.at[1], me.up, me.has_up & when)

    finish_conv(middle)
    for k in range(2, last):
        for p in pieces[2:]:
            cl.forward_up(k, p)
    for p in parts[2:]:
        out_own(p, jnp.logical_not(early), False)
    for i in range(mg.half):
        mg.first(i)
    for p in pieces:
        cl.settle(last, p)
    finish_conv(jnp.logical_not(middle))
    strips = length // 64

    def filter_strip(n):
        i = strips - 1 - n

        @pl.when(jnp.logical_and(i == 0, me.has_down))
        def _():
            mail.arrived(gext.at[pl.ds(0, top)], rh.at[1], me.partner)

        base = pl.multiple_of(i * 64, 8)
        window = gext[pl.ds(base, 64 + top)]
        total = jnp.zeros((64, cw), f32) + cpar[pl.ds(c_lags + 1, 1), :]
        for r in range(8):
            ks = [k for k in range(c_lags + 1) if (top - c_lags + k) % 8 == r]
            span = 64 + (8 if r else 0)
            shifted = jnp.zeros((span, cw), f32)
            for k in ks:
                begin = (top - c_lags + k) // 8 * 8
                shifted = shifted + cpar[pl.ds(k, 1), :] * window[begin : begin + span]
            total = total + shifted[r : r + 64]
        filt[pl.ds(base, 64)] = total

    pl.loop(0, strips)(filter_strip)

    turned = filt[...].T
    ft[...] = turned
    part_sum = jnp.sum(turned, axis=0, keepdims=True)
    off = turned - part_sum * (1.0 / cw)
    st_all[mine, pl.ds(0, 1)] = part_sum
    st_all[mine, pl.ds(1, 1)] = jnp.sum(off * off, axis=0, keepdims=True)
    for device in mates:
        mail.send(st_all.at[mine], st_all.at[mine], rs.at[mine], device)
    for i in range(eg.half):
        eg.first(i)
    for p in parts:
        ol.relay(1, p)

    for k in range(1, 8):
        d = (mine + k) % 8
        mail.arrived(st_all.at[d], rs.at[d], me.partner)
    total = sum(st_all[d, 0:1, :] for d in range(8))
    mean = total * (1.0 / (8 * cw))
    spread = jnp.zeros_like(mean)
    for d in range(8):
        shift = st_all[d, 0:1, :] * (1.0 / cw) - mean
        spread = spread + st_all[d, 1:2, :] + cw * shift * shift
    scale = lax.rsqrt(spread * (1.0 / (8 * cw)) + 1e-05)
    gain_col = jnp.broadcast_to(cpar[pl.ds(c_lags + 2, 1), :], (8, cw)).T[:, 0:1]
    v = (ft[...] - mean) * scale * gain_col
    yall[:, pl.ds(pl.multiple_of(placed * cw, 128), cw)] = (v * jax.nn.sigmoid(v)).T.astype(bf16)
    yg.start()
    mg.second()
    eg.second()
    mg.third()
    eg.third()
    for i in range(yg.half):
        yg.first(i)
    for k in range(2, last):
        for p in parts:
            ol.relay(k, p)
    mg.last(pieces)
    eg.last(pieces)
    rest_at = 8 * (cw + major)

    @pl.loop(0, SEGMENTS // 2)
    def _(i):
        values = yrest[pl.ds(pl.multiple_of(i * seg, 16), seg)]
        low = [values[:, j * 2 * minor : j * 2 * minor + minor] for j in range(8)]
        high = [values[:, j * 2 * minor + minor : (j + 1) * 2 * minor] for j in range(8)]
        for begin, chosen in ((0, low), (length // 2, high)):
            here = pl.ds(pl.multiple_of(begin + i * seg, 16), seg)
            yall[here, pl.ds(rest_at, 8 * minor)] = jnp.concatenate(chosen, axis=1)

    for k in range(1, last):
        for p in parts:
            ol.settle(k, p)
    yg.second()
    yg.third()
    yg.last(pieces)

    cols = wz.shape[2]
    upward = me.z < part
    far = last - me.z
    far_mine = far // part == me.c

    def multiply(q, k):
        here = pl.ds(pl.multiple_of(q * 2 * rows, 16), 2 * rows)
        total = jnp.zeros((2 * rows, cols), f32)
        for c, block in ((me.c, wz.at[me.c * part + k]), (1 - me.c, wp.at[k])):
            begin = 0
            for at, lanes in ((0, 4 * cw), (8 * cw, 4 * major), (rest_at, 4 * minor)):
                left = yall[here, pl.ds(pl.multiple_of(at + c * lanes, 128), lanes)]
                total = total + jnp.dot(left, block[pl.ds(begin, lanes)], preferred_element_type=f32)
                begin = begin + lanes
        total = total.astype(bf16)
        for c in range(2):
            cbuf[q * 2 + c, k] = total[c * rows : (c + 1) * rows]

    def place(q, c, k):
        return out.at[:, pl.ds(pl.multiple_of(((c * part + k) * 4 + q) * cols, 128), cols)]

    def mate_of(i):
        flip = 3 - i
        return (me.q // 2 + flip // 2) % 2 * 2 + (me.q % 2 + flip % 2) % 2

    def parcel(q, c, k):
        return pltpu.make_async_remote_copy(
            src_ref=cbuf.at[q * 2 + c, k], dst_ref=place(me.q, me.c, k), send_sem=ls.at[q * 2 + c, k],
            recv_sem=lr.at[mine, k], device_id=me.at(me.z * 4 + q, c), device_id_type=MESH,
        )

    def kept(k):
        return pltpu.make_async_copy(cbuf.at[mine, k], place(me.q, me.c, k), ls.at[mine, k])

    for n in range(part):
        k = jnp.where(upward, n, part - 1 - n)
        if n == part - 1:
            for p in parts:
                ol.settle(last, p, far_mine)
        for p in parts:
            mail.arrived(wp.at[k, pl.ds(p * tall, tall)], rw.at[k, p], me.partner)

        @pl.loop(0, 3)
        def _(i):
            q = mate_of(i)
            multiply(q, k)
            for c in (me.c, 1 - me.c):
                parcel(q, c, k).start()

        multiply(me.q, k)
        parcel(me.q, 1 - me.c, k).start()
        kept(k).start()

    for p in parts:
        ol.settle(last, p, jnp.logical_not(far_mine))

    @pl.loop(0, 4)
    def _(i):
        q = mate_of(i)
        for k in range(part):
            mail.arrived(place(q, 1 - me.c, k), lr.at[q * 2 + 1 - me.c, k], me.partner)
            parcel(q, 1 - me.c, k).wait_send()

    @pl.loop(0, 3)
    def _(i):
        q = mate_of(i)
        for k in range(part):
            mail.arrived(place(q, me.c, k), lr.at[q * 2 + me.c, k], me.partner)
            parcel(q, me.c, k).wait_send()

    for k in range(part):
        kept(k).wait()
    mail.finish()


def layer(planes, lags, tokens, norm_gain, val_w, gate_w, rgate_w, rin_w, taps, bias, cgain, staps, dmap, imap, rbase, jump, ocw, orw):
    rows, width_in = tokens.shape
    length = 8 * rows
    depth = rin_w.shape[0]
    cw, rwid = val_w.shape[1] // 4, rin_w.shape[1] // 4
    used, cols = cw + rwid, ocw.shape[1]
    minor = rwid % 128
    fold = (rwid + 127) // 128
    f32, bf16 = jnp.float32, jnp.bfloat16
    dma = pltpu.SemaphoreType.DMA
    top = lags[0] + -lags[0] % 16
    rtop = lags[1] + -lags[1] % 16
    part = planes // 2
    deep = planes * 4 * depth

    def vmem(*shape, dtype=bf16):
        return pltpu.VMEM(shape, dtype)

    def wide(*shape):
        return pltpu.VMEM(shape, f32)

    return pl.pallas_call(
        functools.partial(layer_kernel, planes, lags),
        out_shape=jax.ShapeDtypeStruct((rows, planes * 4 * cols), bf16),
        in_specs=[ANY] * 16,
        out_specs=ANY,
        scratch_shapes=[
            vmem(rows, width_in), wide(1, width_in), vmem(*rin_w.shape), vmem(*rgate_w.shape),
            vmem(4, depth, 2 * rwid), vmem(4, depth, 2 * cw),
            vmem(*taps.shape), wide(1, 4 * cw), wide(1, 4 * cw), vmem(*staps.shape),
            vmem(*dmap.shape), vmem(*imap.shape), wide(4 * rwid), wide(*jump.shape),
            vmem(4, jump.shape[0] // 2, 2 * rwid), wide(lags[0] + 3 + -(lags[0] + 3) % 8, cw), wide(8, rwid),
            dma((32,)),
            vmem(length, width_in),
            vmem(deep, 2 * rwid),
            vmem(deep, 2 * cw),
            vmem(length, 2 * rwid),
            vmem(4, jump.shape[0] // 2, 2 * rwid),
            vmem(planes, 4 * used, cols),
            vmem(part, 4 * used, cols),
            vmem(length, 8 * used),
            vmem(length // 2, 16 * minor),
            wide(length, 2 * cw),
            vmem(8, part, rows, cols),
            wide(top + length, cw),
            wide(rtop + length, rwid),
            wide(length, cw),
            wide(fold, length + 8 * SEGMENTS, 128),
            wide(fold, length + 8 * SEGMENTS, 128),
            vmem(rwid, 2 * fold * 128),
            wide(cw, length),
            wide(8, 2, length),
            wide(8, 128),
            wide(planes, 8, 128),
            dma((180 + 20 * planes,)), dma((4, 4)), dma((4, 4)), dma((4,)), dma((4,)),
            dma((planes, 4)), dma((planes, 4)), dma((planes, OUT_PARTS)), dma((4,)),
            dma((4, 4)), dma((4, 4)), dma((4, 4)), dma((4, 4)), dma((4, 2)), dma((4, 2)), dma((part, OUT_PARTS)),
            dma((2,)), dma((8,)), dma((planes,)), dma((8, part)), dma((8, part)),
        ],
        compiler_params=pltpu.CompilerParams(
            collective_id=0, has_side_effects=True, vmem_limit_bytes=60 * 1024 * 1024
        ),
    )(
        tokens, norm_gain[None], val_w, gate_w, rgate_w, rin_w, taps, bias[None], cgain[None], staps,
        dmap, imap, rbase, jump, ocw, orw,
    )


def plane_shards(
    planes,
    tokens,
    norm_gain,
    conv_val_w,
    conv_gate_w,
    rec_gate_w,
    rec_in_w,
    conv_taps,
    conv_bias,
    conv_gain,
    short_taps,
    decay_map,
    input_map,
    decay_base,
    decay_jump,
    out_conv_w,
    out_rec_w,
):
    lags = (conv_taps.shape[0] - 1, short_taps.shape[0] - 1)
    return layer(
        planes, lags, tokens, norm_gain, conv_val_w, conv_gate_w, rec_gate_w, rec_in_w, conv_taps, conv_bias,
        conv_gain, short_taps, decay_map, input_map, decay_base, decay_jump, out_conv_w, out_rec_w,
    )


def solution(mesh):
    in_specs = (
        P(("sp", "tp"), None),
        P(),
        P("sp", "tp"),
        P("sp", "tp"),
        P("sp", "tp"),
        P("sp", "tp"),
        P(None, "tp"),
        P("tp"),
        P("tp"),
        P(None, "tp"),
        P("tp", None, None),
        P("tp", None, None),
        P("tp"),
        P("sp", "tp"),
        P("tp", "sp"),
        P("tp", "sp"),
    )
    out_specs = P(("sp", "tp"), None)
    count = mesh.shape["sp"]
    planar = mesh.shape["tp"] == 2 and count % 8 == 0 and count >= 16
    body = functools.partial(plane_shards, count // 4) if planar else shards
    return jax.shard_map(body, mesh=mesh, in_specs=in_specs, out_specs=out_specs, check_vma=False)
```

```python
import functools

import jax
import jax.numpy as jnp
from jax import lax
from jax.experimental import pallas as pl
from jax.experimental.pallas import tpu as pltpu
from jax.sharding import PartitionSpec as P

CONV_WIDTH = 1024


RATE_SCALE = 8.0


def passed_along(value, axis, by):
    count = lax.axis_size(axis)
    pairs = [(i, i + by) for i in range(count) if 0 <= i + by < count]
    return lax.ppermute(value, axis, pairs)


def prefix(part, axis, combine, identity):
    place = lax.axis_index(axis)
    gathered = jax.tree.map(lambda a: lax.all_gather(a, axis), part)
    state = jax.tree.map(lambda a, e: jnp.zeros_like(a) + jnp.asarray(e, a.dtype), part, identity)

    def one(step, state):
        return combine(
            state, jax.tree.map(lambda a: lax.dynamic_index_in_dim(a, step, 0, False), gathered)
        )

    return lax.fori_loop(0, place, one, state)


def norm_rows(values, gain):
    widened = values.astype(jnp.float32)
    inverse = lax.rsqrt(jnp.mean(widened * widened, axis=-1, keepdims=True) + 1e-06)
    return (widened * inverse * gain).astype(jnp.bfloat16)


def causal_window(edge, current, weights):
    extended = jnp.concatenate([edge, current], axis=0).astype(jnp.float32)
    taps_wide = weights.astype(jnp.float32)
    length = current.shape[0]
    result = jnp.zeros((length, current.shape[1]), jnp.float32)
    for lag_index in range(weights.shape[0]):
        result = result + taps_wide[lag_index][None, :] * extended[lag_index : lag_index + length]
    return result


def chain_step(earlier, latter):
    return (earlier[0] * latter[0], latter[0] * earlier[1] + latter[1])


def glu_of(conv_val, conv_gate):
    return (conv_val.astype(jnp.float32) * jax.nn.sigmoid(conv_gate.astype(jnp.float32))).astype(
        jnp.bfloat16
    )


def shards(
    tokens,
    norm_gain,
    conv_val_w,
    conv_gate_w,
    rec_gate_w,
    rec_in_w,
    conv_taps,
    conv_bias,
    conv_gain,
    short_taps,
    decay_map,
    input_map,
    decay_base,
    decay_jump,
    out_conv_w,
    out_rec_w,
):
    rec_cols = rec_in_w.shape[1]
    conv_lags = conv_taps.shape[0] - 1
    short_lags = short_taps.shape[0] - 1
    normed = norm_rows(tokens, norm_gain)
    val_full, gate_full = (
        lax.all_gather(conv_val_w, "sp", axis=0, tiled=True),
        lax.all_gather(conv_gate_w, "sp", axis=0, tiled=True),
    )
    all_rows = lax.all_gather(normed, "tp", axis=0, tiled=True)
    conv_val = jnp.dot(all_rows, val_full, preferred_element_type=jnp.float32).astype(jnp.bfloat16)
    conv_gate = jnp.dot(all_rows, gate_full, preferred_element_type=jnp.float32).astype(
        jnp.bfloat16
    )
    glu = glu_of(conv_val, conv_gate)
    conv_edge = passed_along(glu[-conv_lags:], "sp", 1)
    rgate_full, rin_full = (
        lax.all_gather(rec_gate_w, "sp", axis=0, tiled=True),
        lax.all_gather(rec_in_w, "sp", axis=0, tiled=True),
    )
    rec_gate = jnp.dot(all_rows, rgate_full, preferred_element_type=jnp.float32).astype(
        jnp.bfloat16
    )
    rec_in = jnp.dot(all_rows, rin_full, preferred_element_type=jnp.float32).astype(jnp.bfloat16)
    rec_edge = passed_along(rec_in[-short_lags:], "sp", 1)
    filtered = causal_window(conv_edge, glu, conv_taps) + conv_bias[None, :]
    row_total = lax.psum(jnp.sum(filtered, axis=1), "tp")
    centered = filtered - (row_total / CONV_WIDTH)[:, None]
    spread = lax.psum(jnp.sum(centered * centered, axis=1), "tp") / CONV_WIDTH
    conv_out = jax.nn.silu(centered * lax.rsqrt(spread + 1e-05)[:, None] * conv_gain).astype(
        jnp.bfloat16
    )
    smoothed = causal_window(rec_edge, rec_in, short_taps).astype(jnp.bfloat16)
    length = smoothed.shape[0]
    grouped = smoothed.reshape(length, decay_map.shape[0], decay_map.shape[1])
    retain = jax.nn.sigmoid(
        jnp.einsum("thi,hio->tho", grouped, decay_map, preferred_element_type=jnp.float32).reshape(
            length, rec_cols
        )
    )
    admit = jax.nn.sigmoid(
        jnp.einsum("thi,hio->tho", grouped, input_map, preferred_element_type=jnp.float32).reshape(
            length, rec_cols
        )
    )
    log_decay = -RATE_SCALE * retain * jax.nn.softplus(-decay_base)[None, :] + decay_jump
    decay = jnp.exp(log_decay)
    inflow = jnp.sqrt(-jnp.expm1(2.0 * log_decay)) * admit * smoothed.astype(jnp.float32)
    products, local_state = lax.associative_scan(chain_step, (decay, inflow), axis=0)
    entering = prefix(
        (products[-1], local_state[-1]),
        "sp",
        chain_step,
        (jnp.ones((rec_cols,), jnp.float32), jnp.zeros((rec_cols,), jnp.float32)),
    )
    state = local_state + products * entering[1][None, :]
    rec_out = (jax.nn.gelu(rec_gate.astype(jnp.float32)) * state).astype(jnp.bfloat16)
    conv_full, rec_full = (
        lax.all_gather(out_conv_w, "sp", axis=1, tiled=True),
        lax.all_gather(out_rec_w, "sp", axis=1, tiled=True),
    )
    return lax.psum_scatter(
        (
            jnp.dot(conv_out, conv_full, preferred_element_type=jnp.float32)
            + jnp.dot(rec_out, rec_full, preferred_element_type=jnp.float32)
        ).astype(jnp.bfloat16),
        "tp",
        scatter_dimension=0,
        tiled=True,
    )


MESH = pl.DeviceIdType.MESH
ANY = pl.BlockSpec(memory_space=pl.ANY)
VMEM = pl.BlockSpec(memory_space=pltpu.VMEM)
SEGMENTS = 8


class Spot:
    def __init__(self, planes):
        self.s, self.c = lax.axis_index("sp"), lax.axis_index("tp")
        self.z, self.q = self.s // 4, self.s % 4
        self.qx = self.q + 1 - 2 * (self.q % 2)
        self.qy = (self.q + 2) % 4
        self.qd = 3 - self.q
        self.has_up, self.has_down = self.z < planes - 1, self.z > 0
        self.up, self.down = self.at(self.s + 4, self.c), self.at(self.s - 4, self.c)
        self.partner = self.at(self.s, 1 - self.c)

    def at(self, s, c):
        return {"sp": s, "tp": c}

    def mate(self, q):
        return self.at(self.z * 4 + q, self.c)


class Mail:
    def __init__(self, send_sem):
        self.send_sem, self.count, self.open = send_sem, 0, []

    def send(self, src, dst, recv, device, when=None):
        copy = pltpu.make_async_remote_copy(
            src_ref=src, dst_ref=dst, send_sem=self.send_sem.at[self.count],
            recv_sem=recv, device_id=device, device_id_type=MESH,
        )
        self.count += 1
        self.open.append((copy.wait_send, when))
        if when is None:
            copy.start()
        else:
            pl.when(when)(copy.start)

    def local(self, src, dst):
        copy = pltpu.make_async_copy(src, dst, self.send_sem.at[self.count])
        self.count += 1
        copy.start()
        self.open.append((copy.wait, None))
        return self.open[-1]

    def arrived(self, dst, recv, device):
        pltpu.make_async_remote_copy(
            src_ref=dst, dst_ref=dst, send_sem=self.send_sem.at[0],
            recv_sem=recv, device_id=device, device_id_type=MESH,
        ).wait_recv()

    def finish(self):
        for wait, when in self.open:
            if when is None:
                wait()
            else:
                pl.when(when)(wait)


def greet(me, devices, line):
    barrier = pltpu.get_barrier_semaphore()
    for device in devices:
        pl.semaphore_signal(barrier, inc=1, device_id=device, device_id_type=MESH)
    amount = len(devices)
    if line:
        for has, device in ((me.has_up, me.up), (me.has_down, me.down)):
            @pl.when(has)
            def _():
                pl.semaphore_signal(barrier, inc=1, device_id=device, device_id_type=MESH)
        amount = amount + me.has_up.astype(jnp.int32) + me.has_down.astype(jnp.int32)
    pl.semaphore_wait(barrier, amount)


class PlaneGather:
    def __init__(self, me, mail, slot, recv, recv_pair):
        self.me, self.mail, self.slot = me, mail, slot
        self.recv, self.recv_pair = recv, recv_pair
        self.parts = recv.shape[1]
        self.half = self.parts // 2

    def start(self):
        me, mail = self.me, self.mail
        for h in range(self.parts):
            for q, part in ((me.qx, h), (me.qy, (h + self.half) % self.parts)):
                own = self.slot(me.q, me.c, part)
                mail.send(own, own, self.recv.at[me.q, part], me.mate(q))
        for part in range(self.parts):
            self.share(me.q, part, self.slot(me.q, me.c, part))

    def took(self, q, part):
        here = self.slot(q, self.me.c, part)
        self.mail.arrived(here, self.recv.at[q, part], self.me.partner)
        return here

    def share(self, q, part, here):
        self.mail.send(here, here, self.recv_pair.at[q, part], self.me.partner)

    def first(self, i):
        me = self.me
        for q, part, to in ((me.qx, i, me.qy), (me.qy, self.half + i, me.qx)):
            here = self.took(q, part)
            self.mail.send(here, here, self.recv.at[q, part], me.mate(to))
            self.share(q, part, here)

    def second(self):
        for i in range(self.half):
            for q, part in ((self.me.qx, self.half + i), (self.me.qy, i)):
                self.share(q, part, self.took(q, part))

    def third(self, i):
        for part in (i, self.half + i):
            self.share(self.me.qd, part, self.took(self.me.qd, part))

    def paired(self, q, part):
        me = self.me
        self.mail.arrived(self.slot(q, 1 - me.c, part), self.recv_pair.at[q, part], me.partner)

    def last(self, origins):
        for q in origins:
            for part in range(self.parts):
                self.paired(q, part)


def minus_expm1(y):
    series = 1.0 + y * (1.0 / 8.0)
    for n in (7.0, 6.0, 5.0, 4.0, 3.0, 2.0):
        series = 1.0 + y * (1.0 / n) * series
    return jnp.where(y > -0.35, -y * series, 1.0 - jnp.exp(y))


def gelu(v):
    return 0.5 * v * (1.0 + jnp.tanh(0.7978845608028654 * (v + 0.044715 * v * v * v)))


class Line:
    def __init__(self, me, mail, planes, slot, recv, seen=None):
        self.me, self.mail, self.planes = me, mail, planes
        self.slot, self.recv, self.seen = slot, recv, seen

    def own(self, piece, src, up=True, down=True):
        me = self.me
        for wanted, has, device in ((up, me.has_up, me.up), (down, me.has_down, me.down)):
            if wanted is not False:
                self.mail.send(src, self.slot(me.z, piece), self.recv.at[me.z, piece], device, has & wanted)

    def ways(self, k):
        me = self.me
        return (
            (me.z - k, me.z >= k, me.up, me.has_up),
            (me.z + k, me.z + k < self.planes, me.down, me.has_down),
        )

    def take(self, origin, piece, when):
        here, sem = self.slot(origin, piece), self.recv.at[origin, piece]
        pl.when(when)(functools.partial(self.mail.arrived, here, sem, self.me.partner))
        if self.seen is not None:
            self.seen(origin, piece, when)
        return here, sem

    def relay(self, k, piece, up=True, down=True):
        for wanted, (origin, there, on, more) in zip((up, down), self.ways(k)):
            if wanted:
                when = jnp.logical_and(there, more)
                here, sem = self.take(origin, piece, when)
                self.mail.send(here, here, sem, on, when)

    def await_up(self, k, piece):
        origin, there, _, more = self.ways(k)[0]
        return self.take(origin, piece, there & more)

    def forward_up(self, k, piece):
        origin, there, on, more = self.ways(k)[0]
        here, sem = self.slot(origin, piece), self.recv.at[origin, piece]
        self.mail.send(here, here, sem, on, there & more)

    def settle(self, k, piece, when=True):
        for origin, there, _, more in self.ways(k):
            self.take(origin, piece, there & jnp.logical_not(more) & when)


def small_softplus(v):
    u = jnp.exp(-jnp.abs(v))
    series = jnp.zeros_like(u)
    for n in (8.0, 7.0, 6.0, 5.0, 4.0, 3.0, 2.0, 1.0):
        series = 1.0 / n - u * series
    return jnp.maximum(v, 0.0) + jnp.where(u < 0.1, u * series, jnp.log(1.0 + u))


OUT_PARTS = 4


def layer_kernel(
    planes, lags, tokens, gain_in, val_w, gate_w, rgate_w, rin_w, taps_in, bias_in, cgain_in, staps_in,
    dmap_in, imap_in, base_in, jump_in, ocw, orw,
    out, x_ref, gain, rin_s, rgate_s, wr, wc, taps, bias, cgain, staps, dmap, imap, rbase, jump, jb, cpar, rpar,
    ld, xall, rwall, cwall, projr, jall, wz, wp, yall, yrest, cacc, cbuf, gext, rext, filt, dec, inf, maps, ft,
    st_all, carry, cr_all,
    send, rx, rpx, rwr, rwc, zr, zc, zo, rj, ry, rp, rv, rq, re, rf, rw, rh, rs, rc, ls, lr,
):
    me = Spot(planes)
    mail = Mail(send)
    c_lags, s_lags = lags
    f32, bf16 = jnp.float32, jnp.bfloat16
    rows, depth = x_ref.shape[0], wr.shape[1]
    length = xall.shape[0]
    cw, rwid = gext.shape[1], rpar.shape[1]
    seg = length // SEGMENTS
    lane_seg = dec.shape[1] // SEGMENTS
    top = gext.shape[0] - length
    rtop = rext.shape[0] - length
    fold = dec.shape[0]
    part = planes // 2
    major = rwid // 128 * 128
    minor = rwid - major
    mine = me.q * 2 + me.c
    others = (me.qx, me.qy, me.qd)
    pieces = (me.q,) + others
    parts = tuple(range(OUT_PARTS))
    tall, half_cols = wz.shape[1] // 2, wz.shape[2] // 2

    def cut(p):
        return pl.ds(p % 2 * tall, tall), pl.ds(p // 2 * half_cols, half_cols)

    last = planes - 1
    mates = [me.at(me.z * 4 + (me.q + dq) % 4, c) for dq in range(4) for c in (me.c, 1 - me.c)][1:]
    lined = [me.at((me.s + 4 * k) % (4 * planes), me.c) for k in range(1, planes)]
    loads = []

    def load(src, dst):
        copy = pltpu.make_async_copy(src, dst, ld.at[len(loads)])
        loads.append(copy)
        copy.start()
        return copy

    got_rec = [load(rin_w, rin_s), load(rgate_w, rgate_s)]
    got_x = [load(tokens, x_ref), load(gain_in, gain)]
    got_conv = []
    for q in range(4):
        got_conv.append(load(val_w.at[:, pl.ds(q * cw, cw)], wc.at[q, :, pl.ds(0, cw)]))
        got_conv.append(load(gate_w.at[:, pl.ds(q * cw, cw)], wc.at[q, :, pl.ds(cw, cw)]))
    got_out = []
    got_out.append(load(ocw, wz.at[me.z, pl.ds(0, 4 * cw)]))
    for q in range(4):
        at = 4 * cw + q * major
        got_out.append(load(orw.at[pl.ds(q * rwid, major)], wz.at[me.z, pl.ds(at, major)]))
        at = 4 * (cw + major) + q * minor
        got_out.append(load(orw.at[pl.ds(q * rwid + major, minor)], wz.at[me.z, pl.ds(at, minor)]))
    got_jump = [load(jump_in, jump)]
    got_small = [
        load(src, dst)
        for src, dst in (
            (taps_in, taps), (bias_in, bias), (cgain_in, cgain), (staps_in, staps),
            (dmap_in, dmap), (imap_in, imap), (base_in, rbase),
        )
    ]
    greet(me, mates + lined, False)
    for copy in got_rec:
        copy.wait()
    for q in range(4):
        lanes = slice(q * rwid, (q + 1) * rwid)
        wr[q] = jnp.concatenate([rin_s[:, lanes], rgate_s[:, lanes]], axis=1)

    def of_rows(ref):
        def slot(origin, piece):
            return ref.at[pl.ds(pl.multiple_of((origin * 4 + piece) * depth, depth), depth)]

        return slot

    def theirs_too(origin, piece, when):
        theirs = jnp.logical_and(origin // part != me.c, when)
        place = origin - (1 - me.c) * part
        mail.send(wz.at[(origin, *cut(piece))], wp.at[(place, *cut(piece))], rw.at[place, piece], me.partner, theirs)

    rl = Line(me, mail, planes, of_rows(rwall), zr)
    cl = Line(me, mail, planes, of_rows(cwall), zc)
    ol = Line(me, mail, planes, lambda origin, p: wz.at[(origin, *cut(p))], zo, theirs_too)

    def out_own(p, up=True, down=True):
        ol.own(p, wz.at[(me.z, *cut(p))], up, down)

    for q in others:
        mail.send(wr.at[q], rl.slot(me.z, me.q), rwr.at[me.q], me.mate(q))
    rl.own(me.q, wr.at[me.q])

    for copy in got_x:
        copy.wait()
    first_row = mine * rows

    @pl.loop(0, rows // 16)
    def _(i):
        values = x_ref[pl.ds(pl.multiple_of(i * 16, 16), 16)].astype(f32)
        inverse = lax.rsqrt(jnp.mean(values * values, axis=1, keepdims=True) + 1e-06)
        place = pl.ds(pl.multiple_of(first_row + i * 16, 16), 16)
        xall[place] = (values * inverse * gain[...]).astype(bf16)

    part_rows = rows // rx.shape[1]

    def xslot(q, c, h):
        return xall.at[pl.ds(pl.multiple_of((q * 2 + c) * rows + h * part_rows, 16), part_rows)]

    xg = PlaneGather(me, mail, xslot, rx, rpx)
    xg.start()
    for copy in got_conv + got_out:
        copy.wait()
    for q in others:
        mail.send(wc.at[q], cl.slot(me.z, me.q), rwc.at[me.q], me.mate(q))
    cl.own(me.q, wc.at[me.q])
    out_own(0)
    kept_here = [mail.local(wr.at[me.q], rl.slot(me.z, me.q)), mail.local(wc.at[me.q], cl.slot(me.z, me.q))]
    for entry in kept_here:
        mail.open.remove(entry)
        entry[0]()
    for p in parts:
        theirs_too(me.z, p, True)
    for copy in got_jump + got_small:
        copy.wait()
    half = jump.shape[0] // 2
    for q in range(4):
        lanes = slice(q * rwid, (q + 1) * rwid)
        jb[q] = jnp.concatenate([jump[:half, lanes], jump[half:, lanes]], axis=1).astype(bf16)
    jall[me.q] = jb[me.q]
    own_lanes = pl.ds(pl.multiple_of(me.q * cw, 128), cw)
    cpar[pl.ds(0, c_lags + 1)] = taps[:, own_lanes].astype(f32)
    cpar[pl.ds(c_lags + 1, 1)] = bias[:, own_lanes]
    cpar[pl.ds(c_lags + 2, 1)] = cgain[:, own_lanes]
    window = -(-rwid // 128) * 128
    wide_lanes = pl.ds(pl.multiple_of(me.q * rwid // 128 * 128, 128), window)

    def own_rec(values):
        moved = values[:, :rwid]
        for lead in sorted({q * rwid % 128 for q in range(4)} - {0}):
            moved = jnp.where(me.q * rwid % 128 == lead, values[:, lead : lead + rwid], moved)
        return moved

    rpar[pl.ds(0, s_lags + 1)] = own_rec(staps[:, wide_lanes].astype(f32))
    rpar[pl.ds(s_lags + 1, 1)] = own_rec(RATE_SCALE * small_softplus(-rbase[wide_lanes][None]))

    maps[...] = jnp.zeros_like(maps)
    size = dmap.shape[1]
    heads = rwid // size
    for h in range(heads):
        spot = pl.ds(h * size, size)
        maps[spot, pl.ds(h * size, size)] = dmap[me.q * heads + h]
        maps[spot, pl.ds(fold * 128 + h * size, size)] = imap[me.q * heads + h]

    for q in others:
        here = rl.slot(me.z, q)
        mail.arrived(here, rwr.at[q], me.partner)
        rl.own(q, here)
    for p in pieces:
        rl.relay(1, p)
    for i in range(xg.half):
        xg.first(i)
    for q in others:
        mail.send(jb.at[q], jall.at[me.q], rj.at[me.q], me.mate(q))
    for k in range(2, last):
        for p in pieces:
            rl.relay(k, p)
    xg.second()
    for q in others:
        here = cl.slot(me.z, q)
        mail.arrived(here, rwc.at[q], me.partner)
        cl.own(q, here)
    for k in range(1, planes):
        for p in pieces:
            rl.settle(k, p)
    xg.last(pieces[:3])

    tile = length // 4

    def project_rec(q):
        at = pl.ds(pl.multiple_of(q * tile, tile), tile)
        product = jnp.dot(xall[at], rwall[...], preferred_element_type=f32).astype(bf16)
        projr[at] = product
        rext[pl.ds(pl.multiple_of(q * tile + rtop, 16), tile)] = product[:, :rwid].astype(f32)

    @pl.loop(0, 3)
    def _(i):
        project_rec((me.q // 2 + i // 2) % 2 * 2 + (me.q % 2 + i % 2) % 2)

    for n, p in enumerate(pieces):
        cl.relay(1, p, n < 1, True)
    for i in range(xg.half):
        xg.third(i)
    xg.last(pieces[3:])
    project_rec(me.qd)

    mail.send(rext.at[pl.ds(length, rtop)], rext.at[pl.ds(0, rtop)], rh.at[0], me.up, me.has_up)
    for p in pieces[1:3]:
        cl.relay(1, p, True, False)
    for k in range(2, last):
        for p in pieces:
            cl.relay(k, p, False, True)

    @pl.when(jnp.logical_not(me.has_down))
    def _():
        rext[pl.ds(0, rtop)] = jnp.zeros((rtop, rwid), f32)
        gext[pl.ds(0, top)] = jnp.zeros((top, cw), f32)

    softened = rpar[pl.ds(s_lags + 1, 1), :]

    @pl.loop(0, SEGMENTS)
    def _(n):
        step = (n + 1) // 2
        ring = (me.q // 2 + step % 4 // 2) % 2 * 2 + (me.q % 2 + step % 2) % 2
        i = jnp.where(n == SEGMENTS - 1, 2 * me.q, 2 * ring + n % 2)
        i = jnp.where(n == 0, 2 * me.q + 1, i)

        @pl.when(jnp.logical_and(i == 0, me.has_down))
        def _():
            mail.arrived(rext.at[pl.ds(0, rtop)], rh.at[0], me.partner)

        @pl.when(jnp.logical_and(n % 2 == 1, n < SEGMENTS - 1))
        def _():
            mail.arrived(jall.at[i // 2], rj.at[i // 2], me.partner)

        base = pl.multiple_of(i * seg, 8)
        window = rext[pl.ds(pl.multiple_of(base + rtop - 8, 8), seg + 8)]
        smooth = jnp.zeros((seg, rwid), f32)
        for k in range(s_lags + 1):
            smooth = smooth + rpar[pl.ds(k, 1), :] * window[8 - s_lags + k : 8 - s_lags + k + seg]
        smooth = smooth.astype(bf16)
        gates = jax.nn.sigmoid(jnp.dot(smooth, maps[...], preferred_element_type=f32))
        retain, admit = gates[:, :rwid], gates[:, fold * 128 : fold * 128 + rwid]
        wide = jall[i // 2].astype(f32)
        moved = jnp.where(i % 2 == 0, wide[:, :rwid], wide[:, rwid:])
        log_decay = moved - retain * softened
        decay = jnp.exp(log_decay)
        inflow = jnp.sqrt(minus_expm1(2.0 * log_decay)) * admit * smooth.astype(f32)
        for f in range(fold):
            w = min(128, rwid - f * 128)
            spot = pl.ds(pl.multiple_of(i * lane_seg, 8), seg)
            dec[f, spot, pl.ds(0, w)] = decay[:, f * 128 : f * 128 + w]
            inf[f, spot, pl.ds(0, w)] = inflow[:, f * 128 : f * 128 + w]

    def one(i, held):
        after = []
        for f in range(fold):
            at = pl.ds(i, SEGMENTS, stride=lane_seg)
            d = dec.at[f][at, :]
            product, state = held[2 * f] * d, held[2 * f + 1] * d + inf.at[f][at, :]
            dec.at[f][at, :] = product
            inf.at[f][at, :] = state
            after += [product, state]
        return tuple(after)

    flat = (SEGMENTS, 128)
    ends = lax.fori_loop(0, seg, one, (jnp.ones(flat, f32), jnp.zeros(flat, f32)) * fold, unroll=8)
    for f in range(fold):
        product, state = jnp.ones((1, 128), f32), jnp.zeros((1, 128), f32)
        for i in range(SEGMENTS):
            p, s = ends[2 * f][i : i + 1], ends[2 * f + 1][i : i + 1]
            product, state = product * p, p * state + s
        carry[pl.ds(2 * f, 1)] = product
        carry[pl.ds(2 * f + 1, 1)] = state
    for k in range(1, planes):
        mail.send(carry, cr_all.at[me.z], rc.at[me.z], lined[k - 1], me.z + k < planes)
    early = me.z < planes - 2
    cl.relay(1, pieces[3], True, False)
    for k in range(2, last):
        for p in pieces[:2]:
            cl.relay(k, p, True, False)
    for p in parts[1:]:
        out_own(p, early, True)

    for k in range(1, planes):
        z = me.z - k
        pl.when(z >= 0)(functools.partial(mail.arrived, cr_all.at[z], rc.at[z], me.partner))
    entering = []
    for f in range(fold):
        held = jnp.zeros((1, 128), f32)
        for j in range(planes - 1):
            after = cr_all[j, pl.ds(2 * f, 1)] * held + cr_all[j, pl.ds(2 * f + 1, 1)]
            held = jnp.where(j < me.z, after, held)
        for i in range(SEGMENTS):
            entering.append(held)
            held = ends[2 * f][i : i + 1] * held + ends[2 * f + 1][i : i + 1]
    placed = me.c * 4 + me.q

    def rec_result(i):
        here, there = pl.ds(i * seg, seg), pl.ds(i * lane_seg, seg)
        state = [dec[f, there] * entering[f * SEGMENTS + i] + inf[f, there] for f in range(fold)]
        state = jnp.concatenate(state, axis=1)[:, :rwid]
        result = (gelu(projr[here, pl.ds(rwid, rwid)].astype(f32)) * state).astype(bf16)
        yall[here, pl.ds(pl.multiple_of(8 * cw + placed * major, 128), major)] = result[:, :major]
        return result[:, major:]

    for i in range(SEGMENTS // 2):
        pair = jnp.concatenate([rec_result(i), rec_result(i + SEGMENTS // 2)], axis=1)
        yrest[pl.ds(i * seg, seg), pl.ds(pl.multiple_of(placed * 2 * minor, 128), 2 * minor)] = pair

    def gather(buffer, lane, lanes, recv, recv_pair):
        tall_part = buffer.shape[0] // recv.shape[1]

        def slot(q, c, h):
            spot = pl.ds(pl.multiple_of(lane + (c * 4 + q) * lanes, 128), lanes)
            return buffer.at[pl.ds(h * tall_part, tall_part), spot]

        return PlaneGather(me, mail, slot, recv, recv_pair)

    mg = gather(yall, 8 * cw, major, rv, rq)
    eg = gather(yrest, 0, 2 * minor, re, rf)
    yg = gather(yall, 0, cw, ry, rp)
    mg.start()
    eg.start()
    for k in range(1, last):
        for p in pieces:
            cl.settle(k, p)
        for p in pieces[2:] if k > 1 else ():
            cl.await_up(k, p)
    plane_depth = 4 * depth
    is_last = (me.z == last).astype(jnp.int32)

    def conv_product(at, begin, size):
        deep = pl.ds(pl.multiple_of(begin, plane_depth), size)
        return jnp.dot(xall[at, deep], cwall[deep], preferred_element_type=f32)

    @pl.loop(0, 4)
    def _(i):
        at = pl.ds(pl.multiple_of(i * tile, tile), tile)
        cacc[at] = conv_product(at, is_last * plane_depth, last * plane_depth)

    middle = me.has_up & me.has_down

    def finish_conv(when):
        @pl.when(when)
        def _():
            @pl.loop(0, 4)
            def _(i):
                at = pl.ds(pl.multiple_of(i * tile, tile), tile)
                product = cacc[at] + conv_product(at, (1 - is_last) * last * plane_depth, plane_depth)
                product = product.astype(bf16).astype(f32)
                glu = (product[:, :cw] * jax.nn.sigmoid(product[:, cw:])).astype(bf16).astype(f32)
                gext[pl.ds(pl.multiple_of(i * tile + top, 8), tile)] = glu

        tail_rows = gext.at[pl.ds(length, top)]
        mail.send(tail_rows, gext.at[pl.ds(0, top)], rh.at[1], me.up, me.has_up & when)

    finish_conv(middle)
    for k in range(2, last):
        for p in pieces[2:]:
            cl.forward_up(k, p)
    for p in parts[1:]:
        out_own(p, jnp.logical_not(early), False)
    mg.first(0)
    for p in pieces:
        cl.settle(last, p)
    finish_conv(jnp.logical_not(middle))
    strips = length // 64

    def filter_strip(n):
        i = strips - 1 - n

        @pl.when(jnp.logical_and(i == 0, me.has_down))
        def _():
            mail.arrived(gext.at[pl.ds(0, top)], rh.at[1], me.partner)

        base = pl.multiple_of(i * 64, 8)
        window = gext[pl.ds(base, 64 + top)]
        total = jnp.zeros((64, cw), f32) + cpar[pl.ds(c_lags + 1, 1), :]
        for r in range(8):
            ks = [k for k in range(c_lags + 1) if (top - c_lags + k) % 8 == r]
            span = 64 + (8 if r else 0)
            shifted = jnp.zeros((span, cw), f32)
            for k in ks:
                begin = (top - c_lags + k) // 8 * 8
                shifted = shifted + cpar[pl.ds(k, 1), :] * window[begin : begin + span]
            total = total + shifted[r : r + 64]
        filt[pl.ds(base, 64)] = total

    pl.loop(0, strips)(filter_strip)

    turned = filt[...].T
    ft[...] = turned
    part_sum = jnp.sum(turned, axis=0, keepdims=True)
    off = turned - part_sum * (1.0 / cw)
    st_all[mine, pl.ds(0, 1)] = part_sum
    st_all[mine, pl.ds(1, 1)] = jnp.sum(off * off, axis=0, keepdims=True)
    for device in mates:
        mail.send(st_all.at[mine], st_all.at[mine], rs.at[mine], device)
    for i in range(1, mg.half):
        mg.first(i)
    for i in range(eg.half):
        eg.first(i)
    for p in parts:
        ol.relay(1, p)

    for k in range(1, 8):
        d = (mine + k) % 8
        mail.arrived(st_all.at[d], rs.at[d], me.partner)
    total = sum(st_all[d, 0:1, :] for d in range(8))
    mean = total * (1.0 / (8 * cw))
    spread = jnp.zeros_like(mean)
    for d in range(8):
        shift = st_all[d, 0:1, :] * (1.0 / cw) - mean
        spread = spread + st_all[d, 1:2, :] + cw * shift * shift
    scale = lax.rsqrt(spread * (1.0 / (8 * cw)) + 1e-05)
    gain_col = jnp.broadcast_to(cpar[pl.ds(c_lags + 2, 1), :], (8, cw)).T[:, 0:1]
    v = (ft[...] - mean) * scale * gain_col
    yall[:, pl.ds(pl.multiple_of(placed * cw, 128), cw)] = (v * jax.nn.sigmoid(v)).T.astype(bf16)
    yg.start()
    mg.second()
    eg.second()
    for g in (mg, eg):
        for i in range(g.half):
            g.third(i)
    for i in range(yg.half):
        yg.first(i)
    for k in range(2, last):
        for p in parts:
            ol.relay(k, p)
    mg.last(pieces)
    eg.last(pieces)
    rest_at = 8 * (cw + major)

    @pl.loop(0, SEGMENTS // 2)
    def _(i):
        values = yrest[pl.ds(pl.multiple_of(i * seg, 16), seg)]
        low = [values[:, j * 2 * minor : j * 2 * minor + minor] for j in range(8)]
        high = [values[:, j * 2 * minor + minor : (j + 1) * 2 * minor] for j in range(8)]
        for begin, chosen in ((0, low), (length // 2, high)):
            here = pl.ds(pl.multiple_of(begin + i * seg, 16), seg)
            yall[here, pl.ds(rest_at, 8 * minor)] = jnp.concatenate(chosen, axis=1)

    yg.second()
    yg.third(0)
    for k in range(1, last):
        for p in parts:
            ol.settle(k, p)

    cols = wz.shape[2]
    upward = me.z < part
    far = last - me.z
    far_mine = far // part == me.c

    def lanes_of(h):
        return pl.ds(0, cols) if h is None else pl.ds(h * half_cols, half_cols)

    def multiply(q, k, h):
        here = pl.ds(pl.multiple_of(q * 2 * rows, 16), 2 * rows)
        total = jnp.zeros((2 * rows, cols if h is None else half_cols), f32)
        for c, block in ((me.c, wz.at[me.c * part + k]), (1 - me.c, wp.at[k])):
            begin = 0
            for at, lanes in ((0, 4 * cw), (8 * cw, 4 * major), (rest_at, 4 * minor)):
                left = yall[here, pl.ds(pl.multiple_of(at + c * lanes, 128), lanes)]
                right = block[pl.ds(begin, lanes), lanes_of(h)]
                total = total + jnp.dot(left, right, preferred_element_type=f32)
                begin = begin + lanes
        total = total.astype(bf16)
        for c in range(2):
            cbuf[q * 2 + c, k, :, lanes_of(h)] = total[c * rows : (c + 1) * rows]

    def place(q, c, k, h):
        at = ((c * part + k) * 4 + q) * cols + (0 if h is None else h * half_cols)
        return out.at[:, pl.ds(pl.multiple_of(at, 128), cols if h is None else half_cols)]

    def mate_of(i):
        flip = 3 - i
        return (me.q // 2 + flip // 2) % 2 * 2 + (me.q % 2 + flip % 2) % 2

    def parcel(q, c, k, h):
        return pltpu.make_async_remote_copy(
            src_ref=cbuf.at[q * 2 + c, k, :, lanes_of(h)], dst_ref=place(me.q, me.c, k, h),
            send_sem=ls.at[q * 2 + c, k, h or 0], recv_sem=lr.at[mine, k, h or 0],
            device_id=me.at(me.z * 4 + q, c), device_id_type=MESH,
        )

    def kept(k, h):
        src = cbuf.at[mine, k, :, lanes_of(h)]
        return pltpu.make_async_copy(src, place(me.q, me.c, k, h), ls.at[mine, k, h or 0])

    def serve(q, k, h):
        multiply(q, k, h)
        pl.when(q != me.q)(lambda: parcel(q, me.c, k, h).start())
        parcel(q, 1 - me.c, k, h).start()
        pl.when(q == me.q)(lambda: kept(k, h).start())

    def ready(k, ps):
        for p in ps:
            mail.arrived(wp.at[(k, *cut(p))], rw.at[k, p], me.partner)

    order = [jnp.where(upward, n, part - 1 - n) for n in range(part)]
    ready(order[0], parts)
    for i in range(yg.half):
        if i:
            yg.third(i)
        for q in pieces:
            yg.paired(q, i)
            yg.paired(q, yg.half + i)

        @pl.loop(0, 2)
        def _(n):
            serve(n * yg.half + i, order[0], None)

    for n in range(1, part - 1):
        ready(order[n], parts)
        pl.loop(0, 4)(lambda i: serve(mate_of(i), order[n], None))
    for h in range(2):
        halves = parts[2 * h : 2 * h + 2]
        for p in halves:
            ol.settle(last, p, far_mine)
        ready(order[-1], halves)
        pl.loop(0, 4)(lambda i: serve(mate_of(i), order[-1], h))
    for p in parts:
        ol.settle(last, p, jnp.logical_not(far_mine))
    rounds = [(k, None) for k in order[:-1]] + [(order[-1], 0), (order[-1], 1)]

    @pl.loop(0, 4)
    def _(i):
        q = mate_of(i)
        for k, h in rounds:
            mail.arrived(place(q, 1 - me.c, k, h), lr.at[q * 2 + 1 - me.c, k, h or 0], me.partner)
            parcel(q, 1 - me.c, k, h).wait_send()

    @pl.loop(0, 3)
    def _(i):
        q = mate_of(i)
        for k, h in rounds:
            mail.arrived(place(q, me.c, k, h), lr.at[q * 2 + me.c, k, h or 0], me.partner)
            parcel(q, me.c, k, h).wait_send()

    for k, h in rounds:
        kept(k, h).wait()
    mail.finish()


def handed_out_kernel(src, dst, held, got, sent):
    count = got.shape[0]
    tall = src.shape[0] // count
    spots = [pl.ds(i * tall, tall) for i in range(count)]
    taken = [pltpu.make_async_copy(src.at[s], held.at[s], got.at[i]) for i, s in enumerate(spots)]
    given = [pltpu.make_async_copy(held.at[s], dst.at[s], sent.at[i]) for i, s in enumerate(spots)]
    for copy in taken:
        copy.start()
    for came, goes in zip(taken, given):
        came.wait()
        goes.start()
    for copy in given:
        copy.wait()


def handed_out(result):
    dma = pltpu.SemaphoreType.DMA
    return pl.pallas_call(
        handed_out_kernel,
        out_shape=jax.ShapeDtypeStruct(result.shape, result.dtype),
        in_specs=[ANY],
        out_specs=ANY,
        scratch_shapes=[pltpu.VMEM(result.shape, result.dtype), dma((6,)), dma((6,))],
    )(result)


def layer(planes, lags, tokens, norm_gain, val_w, gate_w, rgate_w, rin_w, taps, bias, cgain, staps, dmap, imap, rbase, jump, ocw, orw):
    rows, width_in = tokens.shape
    length = 8 * rows
    depth = rin_w.shape[0]
    cw, rwid = val_w.shape[1] // 4, rin_w.shape[1] // 4
    used, cols = cw + rwid, ocw.shape[1]
    minor = rwid % 128
    fold = (rwid + 127) // 128
    f32, bf16 = jnp.float32, jnp.bfloat16
    dma = pltpu.SemaphoreType.DMA
    top = lags[0] + -lags[0] % 16
    rtop = lags[1] + -lags[1] % 16
    part = planes // 2
    deep = planes * 4 * depth

    def vmem(*shape, dtype=bf16):
        return pltpu.VMEM(shape, dtype)

    def wide(*shape):
        return pltpu.VMEM(shape, f32)

    return pl.pallas_call(
        functools.partial(layer_kernel, planes, lags),
        out_shape=jax.ShapeDtypeStruct((rows, planes * 4 * cols), bf16),
        in_specs=[ANY] * 16,
        out_specs=ANY,
        scratch_shapes=[
            vmem(rows, width_in), wide(1, width_in), vmem(*rin_w.shape), vmem(*rgate_w.shape),
            vmem(4, depth, 2 * rwid), vmem(4, depth, 2 * cw),
            vmem(*taps.shape), wide(1, 4 * cw), wide(1, 4 * cw), vmem(*staps.shape),
            vmem(*dmap.shape), vmem(*imap.shape), wide(4 * rwid), wide(*jump.shape),
            vmem(4, jump.shape[0] // 2, 2 * rwid), wide(lags[0] + 3 + -(lags[0] + 3) % 8, cw), wide(8, rwid),
            dma((32,)),
            vmem(length, width_in),
            vmem(deep, 2 * rwid),
            vmem(deep, 2 * cw),
            vmem(length, 2 * rwid),
            vmem(4, jump.shape[0] // 2, 2 * rwid),
            vmem(planes, 4 * used, cols),
            vmem(part, 4 * used, cols),
            vmem(length, 8 * used),
            vmem(length // 2, 16 * minor),
            wide(length, 2 * cw),
            vmem(8, part, rows, cols),
            wide(top + length, cw),
            wide(rtop + length, rwid),
            wide(length, cw),
            wide(fold, length + 8 * SEGMENTS, 128),
            wide(fold, length + 8 * SEGMENTS, 128),
            vmem(rwid, 2 * fold * 128),
            wide(cw, length),
            wide(8, 2, length),
            wide(8, 128),
            wide(planes, 8, 128),
            dma((180 + 20 * planes,)), dma((4, 4)), dma((4, 4)), dma((4,)), dma((4,)),
            dma((planes, 4)), dma((planes, 4)), dma((planes, OUT_PARTS)), dma((4,)),
            dma((4, 4)), dma((4, 4)), dma((4, 4)), dma((4, 4)), dma((4, 2)), dma((4, 2)), dma((part, OUT_PARTS)),
            dma((2,)), dma((8,)), dma((planes,)), dma((8, part, 2)), dma((8, part, 2)),
        ],
        compiler_params=pltpu.CompilerParams(
            collective_id=0, has_side_effects=True, vmem_limit_bytes=60 * 1024 * 1024
        ),
    )(
        tokens, norm_gain[None], val_w, gate_w, rgate_w, rin_w, taps, bias[None], cgain[None], staps,
        dmap, imap, rbase, jump, ocw, orw,
    )


def plane_shards(
    planes,
    tokens,
    norm_gain,
    conv_val_w,
    conv_gate_w,
    rec_gate_w,
    rec_in_w,
    conv_taps,
    conv_bias,
    conv_gain,
    short_taps,
    decay_map,
    input_map,
    decay_base,
    decay_jump,
    out_conv_w,
    out_rec_w,
):
    lags = (conv_taps.shape[0] - 1, short_taps.shape[0] - 1)
    return handed_out(layer(
        planes, lags, tokens, norm_gain, conv_val_w, conv_gate_w, rec_gate_w, rec_in_w, conv_taps, conv_bias,
        conv_gain, short_taps, decay_map, input_map, decay_base, decay_jump, out_conv_w, out_rec_w,
    ))


def solution(mesh):
    in_specs = (
        P(("sp", "tp"), None),
        P(),
        P("sp", "tp"),
        P("sp", "tp"),
        P("sp", "tp"),
        P("sp", "tp"),
        P(None, "tp"),
        P("tp"),
        P("tp"),
        P(None, "tp"),
        P("tp", None, None),
        P("tp", None, None),
        P("tp"),
        P("sp", "tp"),
        P("tp", "sp"),
        P("tp", "sp"),
    )
    out_specs = P(("sp", "tp"), None)
    count = mesh.shape["sp"]
    planar = mesh.shape["tp"] == 2 and count % 8 == 0 and count >= 16
    body = functools.partial(plane_shards, count // 4) if planar else shards
    return jax.shard_map(body, mesh=mesh, in_specs=in_specs, out_specs=out_specs, check_vma=False)
```

```python
import functools

import jax
import jax.numpy as jnp
from jax import lax
from jax.experimental import pallas as pl
from jax.experimental.pallas import tpu as pltpu
from jax.sharding import PartitionSpec as P

CONV_WIDTH = 1024


RATE_SCALE = 8.0


def passed_along(value, axis, by):
    count = lax.axis_size(axis)
    pairs = [(i, i + by) for i in range(count) if 0 <= i + by < count]
    return lax.ppermute(value, axis, pairs)


def prefix(part, axis, combine, identity):
    place = lax.axis_index(axis)
    gathered = jax.tree.map(lambda a: lax.all_gather(a, axis), part)
    state = jax.tree.map(lambda a, e: jnp.zeros_like(a) + jnp.asarray(e, a.dtype), part, identity)

    def one(step, state):
        return combine(
            state, jax.tree.map(lambda a: lax.dynamic_index_in_dim(a, step, 0, False), gathered)
        )

    return lax.fori_loop(0, place, one, state)


def norm_rows(values, gain):
    widened = values.astype(jnp.float32)
    inverse = lax.rsqrt(jnp.mean(widened * widened, axis=-1, keepdims=True) + 1e-06)
    return (widened * inverse * gain).astype(jnp.bfloat16)


def causal_window(edge, current, weights):
    extended = jnp.concatenate([edge, current], axis=0).astype(jnp.float32)
    taps_wide = weights.astype(jnp.float32)
    length = current.shape[0]
    result = jnp.zeros((length, current.shape[1]), jnp.float32)
    for lag_index in range(weights.shape[0]):
        result = result + taps_wide[lag_index][None, :] * extended[lag_index : lag_index + length]
    return result


def chain_step(earlier, latter):
    return (earlier[0] * latter[0], latter[0] * earlier[1] + latter[1])


def glu_of(conv_val, conv_gate):
    return (conv_val.astype(jnp.float32) * jax.nn.sigmoid(conv_gate.astype(jnp.float32))).astype(
        jnp.bfloat16
    )


def shards(
    tokens,
    norm_gain,
    conv_val_w,
    conv_gate_w,
    rec_gate_w,
    rec_in_w,
    conv_taps,
    conv_bias,
    conv_gain,
    short_taps,
    decay_map,
    input_map,
    decay_base,
    decay_jump,
    out_conv_w,
    out_rec_w,
):
    rec_cols = rec_in_w.shape[1]
    conv_lags = conv_taps.shape[0] - 1
    short_lags = short_taps.shape[0] - 1
    normed = norm_rows(tokens, norm_gain)
    val_full, gate_full = (
        lax.all_gather(conv_val_w, "sp", axis=0, tiled=True),
        lax.all_gather(conv_gate_w, "sp", axis=0, tiled=True),
    )
    all_rows = lax.all_gather(normed, "tp", axis=0, tiled=True)
    conv_val = jnp.dot(all_rows, val_full, preferred_element_type=jnp.float32).astype(jnp.bfloat16)
    conv_gate = jnp.dot(all_rows, gate_full, preferred_element_type=jnp.float32).astype(
        jnp.bfloat16
    )
    glu = glu_of(conv_val, conv_gate)
    conv_edge = passed_along(glu[-conv_lags:], "sp", 1)
    rgate_full, rin_full = (
        lax.all_gather(rec_gate_w, "sp", axis=0, tiled=True),
        lax.all_gather(rec_in_w, "sp", axis=0, tiled=True),
    )
    rec_gate = jnp.dot(all_rows, rgate_full, preferred_element_type=jnp.float32).astype(
        jnp.bfloat16
    )
    rec_in = jnp.dot(all_rows, rin_full, preferred_element_type=jnp.float32).astype(jnp.bfloat16)
    rec_edge = passed_along(rec_in[-short_lags:], "sp", 1)
    filtered = causal_window(conv_edge, glu, conv_taps) + conv_bias[None, :]
    row_total = lax.psum(jnp.sum(filtered, axis=1), "tp")
    centered = filtered - (row_total / CONV_WIDTH)[:, None]
    spread = lax.psum(jnp.sum(centered * centered, axis=1), "tp") / CONV_WIDTH
    conv_out = jax.nn.silu(centered * lax.rsqrt(spread + 1e-05)[:, None] * conv_gain).astype(
        jnp.bfloat16
    )
    smoothed = causal_window(rec_edge, rec_in, short_taps).astype(jnp.bfloat16)
    length = smoothed.shape[0]
    grouped = smoothed.reshape(length, decay_map.shape[0], decay_map.shape[1])
    retain = jax.nn.sigmoid(
        jnp.einsum("thi,hio->tho", grouped, decay_map, preferred_element_type=jnp.float32).reshape(
            length, rec_cols
        )
    )
    admit = jax.nn.sigmoid(
        jnp.einsum("thi,hio->tho", grouped, input_map, preferred_element_type=jnp.float32).reshape(
            length, rec_cols
        )
    )
    log_decay = -RATE_SCALE * retain * jax.nn.softplus(-decay_base)[None, :] + decay_jump
    decay = jnp.exp(log_decay)
    inflow = jnp.sqrt(-jnp.expm1(2.0 * log_decay)) * admit * smoothed.astype(jnp.float32)
    products, local_state = lax.associative_scan(chain_step, (decay, inflow), axis=0)
    entering = prefix(
        (products[-1], local_state[-1]),
        "sp",
        chain_step,
        (jnp.ones((rec_cols,), jnp.float32), jnp.zeros((rec_cols,), jnp.float32)),
    )
    state = local_state + products * entering[1][None, :]
    rec_out = (jax.nn.gelu(rec_gate.astype(jnp.float32)) * state).astype(jnp.bfloat16)
    conv_full, rec_full = (
        lax.all_gather(out_conv_w, "sp", axis=1, tiled=True),
        lax.all_gather(out_rec_w, "sp", axis=1, tiled=True),
    )
    return lax.psum_scatter(
        (
            jnp.dot(conv_out, conv_full, preferred_element_type=jnp.float32)
            + jnp.dot(rec_out, rec_full, preferred_element_type=jnp.float32)
        ).astype(jnp.bfloat16),
        "tp",
        scatter_dimension=0,
        tiled=True,
    )


MESH = pl.DeviceIdType.MESH
ANY = pl.BlockSpec(memory_space=pl.ANY)
VMEM = pl.BlockSpec(memory_space=pltpu.VMEM)
SEGMENTS = 8


class Spot:
    def __init__(self, planes):
        self.s, self.c = lax.axis_index("sp"), lax.axis_index("tp")
        self.z, self.q = self.s // 4, self.s % 4
        self.qx = self.q + 1 - 2 * (self.q % 2)
        self.qy = (self.q + 2) % 4
        self.qd = 3 - self.q
        self.has_up, self.has_down = self.z < planes - 1, self.z > 0
        self.up, self.down = self.at(self.s + 4, self.c), self.at(self.s - 4, self.c)
        self.partner = self.at(self.s, 1 - self.c)

    def at(self, s, c):
        return {"sp": s, "tp": c}

    def mate(self, q):
        return self.at(self.z * 4 + q, self.c)


class Mail:
    def __init__(self, send_sem):
        self.send_sem, self.count, self.open = send_sem, 0, []

    def send(self, src, dst, recv, device, when=None):
        copy = pltpu.make_async_remote_copy(
            src_ref=src, dst_ref=dst, send_sem=self.send_sem.at[self.count],
            recv_sem=recv, device_id=device, device_id_type=MESH,
        )
        self.count += 1
        self.open.append((copy.wait_send, when))
        if when is None:
            copy.start()
        else:
            pl.when(when)(copy.start)

    def local(self, src, dst):
        copy = pltpu.make_async_copy(src, dst, self.send_sem.at[self.count])
        self.count += 1
        copy.start()
        self.open.append((copy.wait, None))
        return self.open[-1]

    def arrived(self, dst, recv, device):
        pltpu.make_async_remote_copy(
            src_ref=dst, dst_ref=dst, send_sem=self.send_sem.at[0],
            recv_sem=recv, device_id=device, device_id_type=MESH,
        ).wait_recv()

    def finish(self):
        for wait, when in self.open:
            if when is None:
                wait()
            else:
                pl.when(when)(wait)


def greet(me, devices, line):
    barrier = pltpu.get_barrier_semaphore()
    for device in devices:
        pl.semaphore_signal(barrier, inc=1, device_id=device, device_id_type=MESH)
    amount = len(devices)
    if line:
        for has, device in ((me.has_up, me.up), (me.has_down, me.down)):
            @pl.when(has)
            def _():
                pl.semaphore_signal(barrier, inc=1, device_id=device, device_id_type=MESH)
        amount = amount + me.has_up.astype(jnp.int32) + me.has_down.astype(jnp.int32)
    pl.semaphore_wait(barrier, amount)


class PlaneGather:
    def __init__(self, me, mail, slot, recv, recv_pair):
        self.me, self.mail, self.slot = me, mail, slot
        self.recv, self.recv_pair = recv, recv_pair
        self.parts = recv.shape[1]
        self.half = self.parts // 2

    def start(self):
        me, mail = self.me, self.mail
        for h in range(self.parts):
            for q, part in ((me.qx, h), (me.qy, (h + self.half) % self.parts)):
                own = self.slot(me.q, me.c, part)
                mail.send(own, own, self.recv.at[me.q, part], me.mate(q))
        for part in range(self.parts):
            self.share(me.q, part, self.slot(me.q, me.c, part))

    def took(self, q, part):
        here = self.slot(q, self.me.c, part)
        self.mail.arrived(here, self.recv.at[q, part], self.me.partner)
        return here

    def share(self, q, part, here):
        self.mail.send(here, here, self.recv_pair.at[q, part], self.me.partner)

    def first(self, i):
        me = self.me
        for q, part, to in ((me.qx, i, me.qy), (me.qy, self.half + i, me.qx)):
            here = self.took(q, part)
            self.mail.send(here, here, self.recv.at[q, part], me.mate(to))
            self.share(q, part, here)

    def second(self):
        for i in range(self.half):
            for q, part in ((self.me.qx, self.half + i), (self.me.qy, i)):
                self.share(q, part, self.took(q, part))

    def third(self, i):
        for part in (i, self.half + i):
            self.share(self.me.qd, part, self.took(self.me.qd, part))

    def paired(self, q, part):
        me = self.me
        self.mail.arrived(self.slot(q, 1 - me.c, part), self.recv_pair.at[q, part], me.partner)

    def last(self, origins):
        for q in origins:
            for part in range(self.parts):
                self.paired(q, part)


def one_minus_exp(y, grown):
    series = 1.0 + y * (1.0 / 5.0)
    for n in (4.0, 3.0, 2.0):
        series = 1.0 + y * (1.0 / n) * series
    return jnp.where(y > -0.25, -y * series, 1.0 - grown)


def gelu(v):
    return 0.5 * v * (1.0 + jnp.tanh(0.7978845608028654 * (v + 0.044715 * v * v * v)))


class Line:
    def __init__(self, me, mail, planes, slot, recv, seen=None):
        self.me, self.mail, self.planes = me, mail, planes
        self.slot, self.recv, self.seen = slot, recv, seen

    def own(self, piece, src, up=True, down=True):
        me = self.me
        for wanted, has, device in ((up, me.has_up, me.up), (down, me.has_down, me.down)):
            if wanted is not False:
                self.mail.send(src, self.slot(me.z, piece), self.recv.at[me.z, piece], device, has & wanted)

    def ways(self, k):
        me = self.me
        return (
            (me.z - k, me.z >= k, me.up, me.has_up),
            (me.z + k, me.z + k < self.planes, me.down, me.has_down),
        )

    def take(self, origin, piece, when):
        here, sem = self.slot(origin, piece), self.recv.at[origin, piece]
        pl.when(when)(functools.partial(self.mail.arrived, here, sem, self.me.partner))
        if self.seen is not None:
            self.seen(origin, piece, when)
        return here, sem

    def relay(self, k, piece, up=True, down=True):
        for wanted, (origin, there, on, more) in zip((up, down), self.ways(k)):
            if wanted:
                when = jnp.logical_and(there, more)
                here, sem = self.take(origin, piece, when)
                self.mail.send(here, here, sem, on, when)

    def await_up(self, k, piece):
        origin, there, _, more = self.ways(k)[0]
        return self.take(origin, piece, there & more)

    def forward_up(self, k, piece):
        origin, there, on, more = self.ways(k)[0]
        here, sem = self.slot(origin, piece), self.recv.at[origin, piece]
        self.mail.send(here, here, sem, on, there & more)

    def settle(self, k, piece, when=True):
        for origin, there, _, more in self.ways(k):
            self.take(origin, piece, there & jnp.logical_not(more) & when)


def small_softplus(v):
    u = jnp.exp(-jnp.abs(v))
    series = jnp.zeros_like(u)
    for n in (8.0, 7.0, 6.0, 5.0, 4.0, 3.0, 2.0, 1.0):
        series = 1.0 / n - u * series
    return jnp.maximum(v, 0.0) + jnp.where(u < 0.1, u * series, jnp.log(1.0 + u))


OUT_PARTS = 4


def layer_kernel(
    planes, lags, tokens, gain_in, val_w, gate_w, rgate_w, rin_w, taps_in, bias_in, cgain_in, staps_in,
    dmap_in, imap_in, base_in, jump_in, ocw, orw,
    out, x_ref, gain, rin_s, rgate_s, wr, wc, taps, bias, cgain, staps, dmap, imap, rbase, jump, jb, cpar, rpar,
    ld, xall, rwall, cwall, projr, jall, wz, wp, yall, yrest, cacc, cbuf, gext, rext, filt, dec, inf, maps, ft,
    st_all, carry, cr_all,
    send, rx, rpx, rwr, rwc, zr, zc, zo, rj, ry, rp, rv, rq, re, rf, rw, rh, rs, rc, ls, lr,
):
    me = Spot(planes)
    mail = Mail(send)
    c_lags, s_lags = lags
    f32, bf16 = jnp.float32, jnp.bfloat16
    rows, depth = x_ref.shape[0], wr.shape[1]
    length = xall.shape[0]
    cw, rwid = gext.shape[1], rpar.shape[1]
    seg = length // SEGMENTS
    lane_seg = dec.shape[1] // SEGMENTS
    top = gext.shape[0] - length
    rtop = rext.shape[0] - length
    fold = dec.shape[0]
    part = planes // 2
    major = rwid // 128 * 128
    minor = rwid - major
    mine = me.q * 2 + me.c
    others = (me.qx, me.qy, me.qd)
    pieces = (me.q,) + others
    parts = tuple(range(OUT_PARTS))
    tall, half_cols = wz.shape[1] // 2, wz.shape[2] // 2

    def cut(p):
        return pl.ds(p % 2 * tall, tall), pl.ds(p // 2 * half_cols, half_cols)

    last = planes - 1
    mates = [me.at(me.z * 4 + (me.q + dq) % 4, c) for dq in range(4) for c in (me.c, 1 - me.c)][1:]
    lined = [me.at((me.s + 4 * k) % (4 * planes), me.c) for k in range(1, planes)]
    loads = []

    def load(src, dst):
        copy = pltpu.make_async_copy(src, dst, ld.at[len(loads)])
        loads.append(copy)
        copy.start()
        return copy

    got_rec = [load(rin_w, rin_s), load(rgate_w, rgate_s)]
    got_x = [load(tokens, x_ref), load(gain_in, gain)]
    got_conv = []
    for q in range(4):
        got_conv.append(load(val_w.at[:, pl.ds(q * cw, cw)], wc.at[q, :, pl.ds(0, cw)]))
        got_conv.append(load(gate_w.at[:, pl.ds(q * cw, cw)], wc.at[q, :, pl.ds(cw, cw)]))
    got_out = []
    got_out.append(load(ocw, wz.at[me.z, pl.ds(0, 4 * cw)]))
    for q in range(4):
        at = 4 * cw + q * major
        got_out.append(load(orw.at[pl.ds(q * rwid, major)], wz.at[me.z, pl.ds(at, major)]))
        at = 4 * (cw + major) + q * minor
        got_out.append(load(orw.at[pl.ds(q * rwid + major, minor)], wz.at[me.z, pl.ds(at, minor)]))
    got_jump = [load(jump_in, jump)]
    got_small = [
        load(src, dst)
        for src, dst in (
            (taps_in, taps), (bias_in, bias), (cgain_in, cgain), (staps_in, staps),
            (dmap_in, dmap), (imap_in, imap), (base_in, rbase),
        )
    ]
    greet(me, mates + lined, False)
    for copy in got_rec:
        copy.wait()
    for q in range(4):
        lanes = slice(q * rwid, (q + 1) * rwid)
        wr[q] = jnp.concatenate([rin_s[:, lanes], rgate_s[:, lanes]], axis=1)

    def of_rows(ref):
        def slot(origin, piece):
            return ref.at[pl.ds(pl.multiple_of((origin * 4 + piece) * depth, depth), depth)]

        return slot

    def theirs_too(origin, piece, when):
        theirs = jnp.logical_and(origin // part != me.c, when)
        place = origin - (1 - me.c) * part
        mail.send(wz.at[(origin, *cut(piece))], wp.at[(place, *cut(piece))], rw.at[place, piece], me.partner, theirs)

    rl = Line(me, mail, planes, of_rows(rwall), zr)
    cl = Line(me, mail, planes, of_rows(cwall), zc)
    ol = Line(me, mail, planes, lambda origin, p: wz.at[(origin, *cut(p))], zo, theirs_too)

    def out_own(p, up=True, down=True):
        ol.own(p, wz.at[(me.z, *cut(p))], up, down)

    for q in others:
        mail.send(wr.at[q], rl.slot(me.z, me.q), rwr.at[me.q], me.mate(q))
    rl.own(me.q, wr.at[me.q])

    for copy in got_x:
        copy.wait()
    first_row = mine * rows

    @pl.loop(0, rows // 16)
    def _(i):
        values = x_ref[pl.ds(pl.multiple_of(i * 16, 16), 16)].astype(f32)
        inverse = lax.rsqrt(jnp.mean(values * values, axis=1, keepdims=True) + 1e-06)
        place = pl.ds(pl.multiple_of(first_row + i * 16, 16), 16)
        xall[place] = (values * inverse * gain[...]).astype(bf16)

    part_rows = rows // rx.shape[1]

    def xslot(q, c, h):
        return xall.at[pl.ds(pl.multiple_of((q * 2 + c) * rows + h * part_rows, 16), part_rows)]

    xg = PlaneGather(me, mail, xslot, rx, rpx)
    xg.start()
    for copy in got_conv + got_out:
        copy.wait()
    for q in others:
        mail.send(wc.at[q], cl.slot(me.z, me.q), rwc.at[me.q], me.mate(q))
    cl.own(me.q, wc.at[me.q])
    out_own(0)
    kept_here = [mail.local(wr.at[me.q], rl.slot(me.z, me.q)), mail.local(wc.at[me.q], cl.slot(me.z, me.q))]
    for entry in kept_here:
        mail.open.remove(entry)
        entry[0]()
    for p in parts:
        theirs_too(me.z, p, True)
    for copy in got_jump + got_small:
        copy.wait()
    half = jump.shape[0] // 2
    for q in range(4):
        lanes = slice(q * rwid, (q + 1) * rwid)
        jb[q] = jnp.concatenate([jump[:half, lanes], jump[half:, lanes]], axis=1).astype(bf16)
    jall[me.q] = jb[me.q]
    own_lanes = pl.ds(pl.multiple_of(me.q * cw, 128), cw)
    cpar[pl.ds(0, c_lags + 1)] = taps[:, own_lanes].astype(f32)
    cpar[pl.ds(c_lags + 1, 1)] = bias[:, own_lanes]
    cpar[pl.ds(c_lags + 2, 1)] = cgain[:, own_lanes]
    window = -(-rwid // 128) * 128
    wide_lanes = pl.ds(pl.multiple_of(me.q * rwid // 128 * 128, 128), window)

    def own_rec(values):
        moved = values[:, :rwid]
        for lead in sorted({q * rwid % 128 for q in range(4)} - {0}):
            moved = jnp.where(me.q * rwid % 128 == lead, values[:, lead : lead + rwid], moved)
        return moved

    rpar[pl.ds(0, s_lags + 1)] = own_rec(staps[:, wide_lanes].astype(f32))
    rpar[pl.ds(s_lags + 1, 1)] = own_rec(RATE_SCALE * small_softplus(-rbase[wide_lanes][None]))

    maps[...] = jnp.zeros_like(maps)
    size = dmap.shape[1]
    heads = rwid // size
    for h in range(heads):
        spot = pl.ds(h * size, size)
        maps[spot, pl.ds(h * size, size)] = dmap[me.q * heads + h]
        maps[spot, pl.ds(fold * 128 + h * size, size)] = imap[me.q * heads + h]

    for q in others:
        here = rl.slot(me.z, q)
        mail.arrived(here, rwr.at[q], me.partner)
        rl.own(q, here)
    for p in pieces:
        rl.relay(1, p)
    for i in range(xg.half):
        xg.first(i)
    for q in others:
        mail.send(jb.at[q], jall.at[me.q], rj.at[me.q], me.mate(q))
    for k in range(2, last):
        for p in pieces:
            rl.relay(k, p)
    xg.second()
    for q in others:
        here = cl.slot(me.z, q)
        mail.arrived(here, rwc.at[q], me.partner)
        cl.own(q, here)
    for k in range(1, planes):
        for p in pieces:
            rl.settle(k, p)
    xg.last(pieces[:3])

    tile = length // 4

    def project_rec(begin, size):
        at = pl.ds(pl.multiple_of(begin, 64), size)
        product = jnp.dot(xall[at], rwall[...], preferred_element_type=f32).astype(bf16)
        projr[at] = product
        rext[pl.ds(pl.multiple_of(begin + rtop, 16), size)] = product[:, :rwid].astype(f32)

    @pl.loop(0, 3)
    def _(i):
        project_rec(((me.q // 2 + i // 2) % 2 * 2 + (me.q % 2 + i % 2) % 2) * tile, tile)

    for n, p in enumerate(pieces):
        cl.relay(1, p, n < 2, True)
    for i in range(xg.half):
        xg.third(i)
    project_rec((me.qd * 2 + me.c) * rows, rows)
    xg.last(pieces[3:])
    project_rec((me.qd * 2 + 1 - me.c) * rows, rows)

    mail.send(rext.at[pl.ds(length, rtop)], rext.at[pl.ds(0, rtop)], rh.at[0], me.up, me.has_up)
    for p in pieces[2:]:
        cl.relay(1, p, True, False)
    for k in range(2, last):
        for p in pieces:
            cl.relay(k, p, False, True)

    @pl.when(jnp.logical_not(me.has_down))
    def _():
        rext[pl.ds(0, rtop)] = jnp.zeros((rtop, rwid), f32)
        gext[pl.ds(0, top)] = jnp.zeros((top, cw), f32)

    softened = rpar[pl.ds(s_lags + 1, 1), :]

    @pl.loop(0, SEGMENTS)
    def _(n):
        step = (n + 1) // 2
        ring = (me.q // 2 + step % 4 // 2) % 2 * 2 + (me.q % 2 + step % 2) % 2
        i = jnp.where(n == SEGMENTS - 1, 2 * me.q, 2 * ring + n % 2)
        i = jnp.where(n == 0, 2 * me.q + 1, i)

        @pl.when(jnp.logical_and(i == 0, me.has_down))
        def _():
            mail.arrived(rext.at[pl.ds(0, rtop)], rh.at[0], me.partner)

        @pl.when(jnp.logical_and(n % 2 == 1, n < SEGMENTS - 1))
        def _():
            mail.arrived(jall.at[i // 2], rj.at[i // 2], me.partner)

        base = pl.multiple_of(i * seg, 8)
        window = rext[pl.ds(pl.multiple_of(base + rtop - 8, 8), seg + 8)]
        smooth = jnp.zeros((seg, rwid), f32)
        for k in range(s_lags + 1):
            smooth = smooth + rpar[pl.ds(k, 1), :] * window[8 - s_lags + k : 8 - s_lags + k + seg]
        smooth = smooth.astype(bf16)
        gates = jax.nn.sigmoid(jnp.dot(smooth, maps[...], preferred_element_type=f32))
        retain, admit = gates[:, :rwid], gates[:, fold * 128 : fold * 128 + rwid]
        wide = jall[i // 2].astype(f32)
        moved = jnp.where(i % 2 == 0, wide[:, :rwid], wide[:, rwid:])
        log_decay = moved - retain * softened
        decay = jnp.exp(log_decay)
        inflow = jnp.sqrt(one_minus_exp(log_decay, decay) * (1.0 + decay)) * admit * smooth.astype(f32)
        for f in range(fold):
            w = min(128, rwid - f * 128)
            spot = pl.ds(pl.multiple_of(i * lane_seg, 8), seg)
            dec[f, spot, pl.ds(0, w)] = decay[:, f * 128 : f * 128 + w]
            inf[f, spot, pl.ds(0, w)] = inflow[:, f * 128 : f * 128 + w]

    def one(i, held):
        after = []
        for f in range(fold):
            at = pl.ds(i, SEGMENTS, stride=lane_seg)
            d = dec.at[f][at, :]
            product, state = held[2 * f] * d, held[2 * f + 1] * d + inf.at[f][at, :]
            dec.at[f][at, :] = product
            inf.at[f][at, :] = state
            after += [product, state]
        return tuple(after)

    flat = (SEGMENTS, 128)
    ends = lax.fori_loop(0, seg, one, (jnp.ones(flat, f32), jnp.zeros(flat, f32)) * fold, unroll=8)
    for f in range(fold):
        product, state = jnp.ones((1, 128), f32), jnp.zeros((1, 128), f32)
        for i in range(SEGMENTS):
            p, s = ends[2 * f][i : i + 1], ends[2 * f + 1][i : i + 1]
            product, state = product * p, p * state + s
        carry[pl.ds(2 * f, 1)] = product
        carry[pl.ds(2 * f + 1, 1)] = state
    for k in range(1, planes):
        mail.send(carry, cr_all.at[me.z], rc.at[me.z], lined[k - 1], me.z + k < planes)
    early = me.z < planes - 2
    for k in range(2, last):
        for p in pieces[:3]:
            cl.relay(k, p, True, False)
    for p in parts[1:]:
        out_own(p, early, True)

    for i in range(SEGMENTS):
        there = pl.ds(i * lane_seg, seg)
        factor = gelu(projr[pl.ds(i * seg, seg), pl.ds(rwid, rwid)].astype(f32))
        for f in range(fold):
            w = min(128, rwid - f * 128)
            lanes = pl.ds(0, w)
            dec[f, there, lanes] = dec[f, there, lanes] * factor[:, f * 128 : f * 128 + w]
            inf[f, there, lanes] = inf[f, there, lanes] * factor[:, f * 128 : f * 128 + w]

    for k in range(1, planes):
        z = me.z - k
        pl.when(z >= 0)(functools.partial(mail.arrived, cr_all.at[z], rc.at[z], me.partner))
    entering = []
    for f in range(fold):
        held = jnp.zeros((1, 128), f32)
        for j in range(planes - 1):
            after = cr_all[j, pl.ds(2 * f, 1)] * held + cr_all[j, pl.ds(2 * f + 1, 1)]
            held = jnp.where(j < me.z, after, held)
        for i in range(SEGMENTS):
            entering.append(held)
            held = ends[2 * f][i : i + 1] * held + ends[2 * f + 1][i : i + 1]
    placed = me.c * 4 + me.q

    def rec_result(i):
        here, there = pl.ds(i * seg, seg), pl.ds(i * lane_seg, seg)
        state = [dec[f, there] * entering[f * SEGMENTS + i] + inf[f, there] for f in range(fold)]
        result = jnp.concatenate(state, axis=1)[:, :rwid].astype(bf16)
        yall[here, pl.ds(pl.multiple_of(8 * cw + placed * major, 128), major)] = result[:, :major]
        return result[:, major:]

    for i in range(SEGMENTS // 2):
        pair = jnp.concatenate([rec_result(i), rec_result(i + SEGMENTS // 2)], axis=1)
        yrest[pl.ds(i * seg, seg), pl.ds(pl.multiple_of(placed * 2 * minor, 128), 2 * minor)] = pair

    def gather(buffer, lane, lanes, recv, recv_pair):
        tall_part = buffer.shape[0] // recv.shape[1]

        def slot(q, c, h):
            spot = pl.ds(pl.multiple_of(lane + (c * 4 + q) * lanes, 128), lanes)
            return buffer.at[pl.ds(h * tall_part, tall_part), spot]

        return PlaneGather(me, mail, slot, recv, recv_pair)

    mg = gather(yall, 8 * cw, major, rv, rq)
    eg = gather(yrest, 0, 2 * minor, re, rf)
    yg = gather(yall, 0, cw, ry, rp)
    mg.start()
    eg.start()
    for k in range(1, last):
        for p in pieces:
            cl.settle(k, p)
        for p in pieces[3:] if k > 1 else ():
            cl.await_up(k, p)
    plane_depth = 4 * depth
    is_last = (me.z == last).astype(jnp.int32)

    def conv_product(at, begin, size):
        deep = pl.ds(pl.multiple_of(begin, plane_depth), size)
        return jnp.dot(xall[at, deep], cwall[deep], preferred_element_type=f32)

    @pl.loop(0, 4)
    def _(i):
        at = pl.ds(pl.multiple_of(i * tile, tile), tile)
        cacc[at] = conv_product(at, is_last * plane_depth, last * plane_depth)

    middle = me.has_up & me.has_down

    def finish_conv(when):
        @pl.when(when)
        def _():
            @pl.loop(0, 4)
            def _(i):
                at = pl.ds(pl.multiple_of(i * tile, tile), tile)
                product = cacc[at] + conv_product(at, (1 - is_last) * last * plane_depth, plane_depth)
                product = product.astype(bf16).astype(f32)
                glu = (product[:, :cw] * jax.nn.sigmoid(product[:, cw:])).astype(bf16).astype(f32)
                gext[pl.ds(pl.multiple_of(i * tile + top, 8), tile)] = glu

        tail_rows = gext.at[pl.ds(length, top)]
        mail.send(tail_rows, gext.at[pl.ds(0, top)], rh.at[1], me.up, me.has_up & when)

    finish_conv(middle)
    for k in range(2, last):
        for p in pieces[3:]:
            cl.forward_up(k, p)
    for p in parts[1:]:
        out_own(p, jnp.logical_not(early), False)
    mg.first(0)
    for p in pieces:
        cl.settle(last, p)
    finish_conv(jnp.logical_not(middle))
    strips = length // 64

    def filter_strip(n):
        i = strips - 1 - n

        @pl.when(jnp.logical_and(i == 0, me.has_down))
        def _():
            mail.arrived(gext.at[pl.ds(0, top)], rh.at[1], me.partner)

        base = pl.multiple_of(i * 64, 8)
        window = gext[pl.ds(base, 64 + top)]
        total = jnp.zeros((64, cw), f32) + cpar[pl.ds(c_lags + 1, 1), :]
        for r in range(8):
            ks = [k for k in range(c_lags + 1) if (top - c_lags + k) % 8 == r]
            span = 64 + (8 if r else 0)
            shifted = jnp.zeros((span, cw), f32)
            for k in ks:
                begin = (top - c_lags + k) // 8 * 8
                shifted = shifted + cpar[pl.ds(k, 1), :] * window[begin : begin + span]
            total = total + shifted[r : r + 64]
        filt[pl.ds(base, 64)] = total

    pl.loop(0, strips)(filter_strip)

    turned = filt[...].T
    ft[...] = turned
    part_sum = jnp.sum(turned, axis=0, keepdims=True)
    off = turned - part_sum * (1.0 / cw)
    st_all[mine, pl.ds(0, 1)] = part_sum
    st_all[mine, pl.ds(1, 1)] = jnp.sum(off * off, axis=0, keepdims=True)
    for device in mates:
        mail.send(st_all.at[mine], st_all.at[mine], rs.at[mine], device)
    for i in range(1, mg.half):
        mg.first(i)
    for i in range(eg.half):
        eg.first(i)
    for p in parts:
        ol.relay(1, p)

    for k in range(1, 8):
        d = (mine + k) % 8
        mail.arrived(st_all.at[d], rs.at[d], me.partner)
    total = sum(st_all[d, 0:1, :] for d in range(8))
    mean = total * (1.0 / (8 * cw))
    spread = jnp.zeros_like(mean)
    for d in range(8):
        shift = st_all[d, 0:1, :] * (1.0 / cw) - mean
        spread = spread + st_all[d, 1:2, :] + cw * shift * shift
    scale = lax.rsqrt(spread * (1.0 / (8 * cw)) + 1e-05)
    gain_col = jnp.broadcast_to(cpar[pl.ds(c_lags + 2, 1), :], (8, cw)).T[:, 0:1]
    v = (ft[...] - mean) * scale * gain_col
    yall[:, pl.ds(pl.multiple_of(placed * cw, 128), cw)] = (v * jax.nn.sigmoid(v)).T.astype(bf16)
    yg.start()
    mg.second()
    eg.second()
    for g in (mg, eg):
        for i in range(g.half):
            g.third(i)
    for i in range(yg.half):
        yg.first(i)
    for k in range(2, last):
        for p in parts:
            ol.relay(k, p)
    mg.last(pieces)
    eg.last(pieces)
    rest_at = 8 * (cw + major)

    @pl.loop(0, SEGMENTS // 2)
    def _(i):
        values = yrest[pl.ds(pl.multiple_of(i * seg, 16), seg)]
        low = [values[:, j * 2 * minor : j * 2 * minor + minor] for j in range(8)]
        high = [values[:, j * 2 * minor + minor : (j + 1) * 2 * minor] for j in range(8)]
        for begin, chosen in ((0, low), (length // 2, high)):
            here = pl.ds(pl.multiple_of(begin + i * seg, 16), seg)
            yall[here, pl.ds(rest_at, 8 * minor)] = jnp.concatenate(chosen, axis=1)

    yg.second()
    yg.third(0)
    for k in range(1, last):
        for p in parts:
            ol.settle(k, p)

    cols = wz.shape[2]
    upward = me.z < part
    far = last - me.z
    far_mine = far // part == me.c

    def lanes_of(h):
        return pl.ds(0, cols) if h is None else pl.ds(h * half_cols, half_cols)

    def multiply(q, k, h):
        here = pl.ds(pl.multiple_of(q * 2 * rows, 16), 2 * rows)
        total = jnp.zeros((2 * rows, cols if h is None else half_cols), f32)
        for c, block in ((me.c, wz.at[me.c * part + k]), (1 - me.c, wp.at[k])):
            begin = 0
            for at, lanes in ((0, 4 * cw), (8 * cw, 4 * major), (rest_at, 4 * minor)):
                left = yall[here, pl.ds(pl.multiple_of(at + c * lanes, 128), lanes)]
                right = block[pl.ds(begin, lanes), lanes_of(h)]
                total = total + jnp.dot(left, right, preferred_element_type=f32)
                begin = begin + lanes
        total = total.astype(bf16)
        for c in range(2):
            cbuf[q * 2 + c, k, :, lanes_of(h)] = total[c * rows : (c + 1) * rows]

    def place(q, c, k, h):
        at = ((c * part + k) * 4 + q) * cols + (0 if h is None else h * half_cols)
        return out.at[:, pl.ds(pl.multiple_of(at, 128), cols if h is None else half_cols)]

    def mate_of(i):
        flip = 3 - i
        return (me.q // 2 + flip // 2) % 2 * 2 + (me.q % 2 + flip % 2) % 2

    def parcel(q, c, k, h):
        return pltpu.make_async_remote_copy(
            src_ref=cbuf.at[q * 2 + c, k, :, lanes_of(h)], dst_ref=place(me.q, me.c, k, h),
            send_sem=ls.at[q * 2 + c, k, h or 0], recv_sem=lr.at[mine, k, h or 0],
            device_id=me.at(me.z * 4 + q, c), device_id_type=MESH,
        )

    def kept(k, h):
        src = cbuf.at[mine, k, :, lanes_of(h)]
        return pltpu.make_async_copy(src, place(me.q, me.c, k, h), ls.at[mine, k, h or 0])

    def serve(q, k, h):
        multiply(q, k, h)
        pl.when(q != me.q)(lambda: parcel(q, me.c, k, h).start())
        parcel(q, 1 - me.c, k, h).start()
        pl.when(q == me.q)(lambda: kept(k, h).start())

    def ready(k, ps):
        for p in ps:
            mail.arrived(wp.at[(k, *cut(p))], rw.at[k, p], me.partner)

    order = [jnp.where(upward, n, part - 1 - n) for n in range(part)]
    ready(order[0], parts)
    for i in range(yg.half):
        if i:
            yg.third(i)
        for q in pieces:
            yg.paired(q, i)
            yg.paired(q, yg.half + i)

        @pl.loop(0, 2)
        def _(n):
            serve(n * yg.half + i, order[0], None)

    for n in range(1, part - 1):
        ready(order[n], parts)
        pl.loop(0, 4)(lambda i: serve(mate_of(i), order[n], None))
    for h in range(2):
        halves = parts[2 * h : 2 * h + 2]
        for p in halves:
            ol.settle(last, p, far_mine)
        ready(order[-1], halves)
        pl.loop(0, 4)(lambda i: serve(mate_of(i), order[-1], h))
    for p in parts:
        ol.settle(last, p, jnp.logical_not(far_mine))
    rounds = [(k, None) for k in order[:-1]] + [(order[-1], 0), (order[-1], 1)]

    @pl.loop(0, 4)
    def _(i):
        q = mate_of(i)
        for k, h in rounds:
            mail.arrived(place(q, 1 - me.c, k, h), lr.at[q * 2 + 1 - me.c, k, h or 0], me.partner)
            parcel(q, 1 - me.c, k, h).wait_send()

    @pl.loop(0, 3)
    def _(i):
        q = mate_of(i)
        for k, h in rounds:
            mail.arrived(place(q, me.c, k, h), lr.at[q * 2 + me.c, k, h or 0], me.partner)
            parcel(q, me.c, k, h).wait_send()

    for k, h in rounds:
        kept(k, h).wait()
    mail.finish()


def handed_out_kernel(src, dst, held, got, sent):
    count = got.shape[0]
    tall = src.shape[0] // count
    spots = [pl.ds(i * tall, tall) for i in range(count)]
    taken = [pltpu.make_async_copy(src.at[s], held.at[s], got.at[i]) for i, s in enumerate(spots)]
    given = [pltpu.make_async_copy(held.at[s], dst.at[s], sent.at[i]) for i, s in enumerate(spots)]
    for copy in taken:
        copy.start()
    for came, goes in zip(taken, given):
        came.wait()
        goes.start()
    for copy in given:
        copy.wait()


def handed_out(result):
    dma = pltpu.SemaphoreType.DMA
    return pl.pallas_call(
        handed_out_kernel,
        out_shape=jax.ShapeDtypeStruct(result.shape, result.dtype),
        in_specs=[ANY],
        out_specs=ANY,
        scratch_shapes=[pltpu.VMEM(result.shape, result.dtype), dma((6,)), dma((6,))],
    )(result)


def layer(planes, lags, tokens, norm_gain, val_w, gate_w, rgate_w, rin_w, taps, bias, cgain, staps, dmap, imap, rbase, jump, ocw, orw):
    rows, width_in = tokens.shape
    length = 8 * rows
    depth = rin_w.shape[0]
    cw, rwid = val_w.shape[1] // 4, rin_w.shape[1] // 4
    used, cols = cw + rwid, ocw.shape[1]
    minor = rwid % 128
    fold = (rwid + 127) // 128
    f32, bf16 = jnp.float32, jnp.bfloat16
    dma = pltpu.SemaphoreType.DMA
    top = lags[0] + -lags[0] % 16
    rtop = lags[1] + -lags[1] % 16
    part = planes // 2
    deep = planes * 4 * depth

    def vmem(*shape, dtype=bf16):
        return pltpu.VMEM(shape, dtype)

    def wide(*shape):
        return pltpu.VMEM(shape, f32)

    return pl.pallas_call(
        functools.partial(layer_kernel, planes, lags),
        out_shape=jax.ShapeDtypeStruct((rows, planes * 4 * cols), bf16),
        in_specs=[ANY] * 16,
        out_specs=ANY,
        scratch_shapes=[
            vmem(rows, width_in), wide(1, width_in), vmem(*rin_w.shape), vmem(*rgate_w.shape),
            vmem(4, depth, 2 * rwid), vmem(4, depth, 2 * cw),
            vmem(*taps.shape), wide(1, 4 * cw), wide(1, 4 * cw), vmem(*staps.shape),
            vmem(*dmap.shape), vmem(*imap.shape), wide(4 * rwid), wide(*jump.shape),
            vmem(4, jump.shape[0] // 2, 2 * rwid), wide(lags[0] + 3 + -(lags[0] + 3) % 8, cw), wide(8, rwid),
            dma((32,)),
            vmem(length, width_in),
            vmem(deep, 2 * rwid),
            vmem(deep, 2 * cw),
            vmem(length, 2 * rwid),
            vmem(4, jump.shape[0] // 2, 2 * rwid),
            vmem(planes, 4 * used, cols),
            vmem(part, 4 * used, cols),
            vmem(length, 8 * used),
            vmem(length // 2, 16 * minor),
            wide(length, 2 * cw),
            vmem(8, part, rows, cols),
            wide(top + length, cw),
            wide(rtop + length, rwid),
            wide(length, cw),
            wide(fold, length + 8 * SEGMENTS, 128),
            wide(fold, length + 8 * SEGMENTS, 128),
            vmem(rwid, 2 * fold * 128),
            wide(cw, length),
            wide(8, 2, length),
            wide(8, 128),
            wide(planes, 8, 128),
            dma((180 + 20 * planes,)), dma((4, 4)), dma((4, 4)), dma((4,)), dma((4,)),
            dma((planes, 4)), dma((planes, 4)), dma((planes, OUT_PARTS)), dma((4,)),
            dma((4, 4)), dma((4, 4)), dma((4, 4)), dma((4, 4)), dma((4, 2)), dma((4, 2)), dma((part, OUT_PARTS)),
            dma((2,)), dma((8,)), dma((planes,)), dma((8, part, 2)), dma((8, part, 2)),
        ],
        compiler_params=pltpu.CompilerParams(
            collective_id=0, has_side_effects=True, vmem_limit_bytes=60 * 1024 * 1024
        ),
    )(
        tokens, norm_gain[None], val_w, gate_w, rgate_w, rin_w, taps, bias[None], cgain[None], staps,
        dmap, imap, rbase, jump, ocw, orw,
    )


def plane_shards(
    planes,
    tokens,
    norm_gain,
    conv_val_w,
    conv_gate_w,
    rec_gate_w,
    rec_in_w,
    conv_taps,
    conv_bias,
    conv_gain,
    short_taps,
    decay_map,
    input_map,
    decay_base,
    decay_jump,
    out_conv_w,
    out_rec_w,
):
    lags = (conv_taps.shape[0] - 1, short_taps.shape[0] - 1)
    return handed_out(layer(
        planes, lags, tokens, norm_gain, conv_val_w, conv_gate_w, rec_gate_w, rec_in_w, conv_taps, conv_bias,
        conv_gain, short_taps, decay_map, input_map, decay_base, decay_jump, out_conv_w, out_rec_w,
    ))


def solution(mesh):
    in_specs = (
        P(("sp", "tp"), None),
        P(),
        P("sp", "tp"),
        P("sp", "tp"),
        P("sp", "tp"),
        P("sp", "tp"),
        P(None, "tp"),
        P("tp"),
        P("tp"),
        P(None, "tp"),
        P("tp", None, None),
        P("tp", None, None),
        P("tp"),
        P("sp", "tp"),
        P("tp", "sp"),
        P("tp", "sp"),
    )
    out_specs = P(("sp", "tp"), None)
    count = mesh.shape["sp"]
    planar = mesh.shape["tp"] == 2 and count % 8 == 0 and count >= 16
    body = functools.partial(plane_shards, count // 4) if planar else shards
    return jax.shard_map(body, mesh=mesh, in_specs=in_specs, out_specs=out_specs, check_vma=False)
```

```python
import functools

import jax
import jax.numpy as jnp
from jax import lax
from jax.experimental import pallas as pl
from jax.experimental.pallas import tpu as pltpu
from jax.sharding import PartitionSpec as P

CONV_WIDTH = 1024


RATE_SCALE = 8.0


def passed_along(value, axis, by):
    count = lax.axis_size(axis)
    pairs = [(i, i + by) for i in range(count) if 0 <= i + by < count]
    return lax.ppermute(value, axis, pairs)


def prefix(part, axis, combine, identity):
    place = lax.axis_index(axis)
    gathered = jax.tree.map(lambda a: lax.all_gather(a, axis), part)
    state = jax.tree.map(lambda a, e: jnp.zeros_like(a) + jnp.asarray(e, a.dtype), part, identity)

    def one(step, state):
        return combine(
            state, jax.tree.map(lambda a: lax.dynamic_index_in_dim(a, step, 0, False), gathered)
        )

    return lax.fori_loop(0, place, one, state)


def norm_rows(values, gain):
    widened = values.astype(jnp.float32)
    inverse = lax.rsqrt(jnp.mean(widened * widened, axis=-1, keepdims=True) + 1e-06)
    return (widened * inverse * gain).astype(jnp.bfloat16)


def causal_window(edge, current, weights):
    extended = jnp.concatenate([edge, current], axis=0).astype(jnp.float32)
    taps_wide = weights.astype(jnp.float32)
    length = current.shape[0]
    result = jnp.zeros((length, current.shape[1]), jnp.float32)
    for lag_index in range(weights.shape[0]):
        result = result + taps_wide[lag_index][None, :] * extended[lag_index : lag_index + length]
    return result


def chain_step(earlier, latter):
    return (earlier[0] * latter[0], latter[0] * earlier[1] + latter[1])


def glu_of(conv_val, conv_gate):
    return (conv_val.astype(jnp.float32) * jax.nn.sigmoid(conv_gate.astype(jnp.float32))).astype(
        jnp.bfloat16
    )


def shards(
    tokens,
    norm_gain,
    conv_val_w,
    conv_gate_w,
    rec_gate_w,
    rec_in_w,
    conv_taps,
    conv_bias,
    conv_gain,
    short_taps,
    decay_map,
    input_map,
    decay_base,
    decay_jump,
    out_conv_w,
    out_rec_w,
):
    rec_cols = rec_in_w.shape[1]
    conv_lags = conv_taps.shape[0] - 1
    short_lags = short_taps.shape[0] - 1
    normed = norm_rows(tokens, norm_gain)
    val_full, gate_full = (
        lax.all_gather(conv_val_w, "sp", axis=0, tiled=True),
        lax.all_gather(conv_gate_w, "sp", axis=0, tiled=True),
    )
    all_rows = lax.all_gather(normed, "tp", axis=0, tiled=True)
    conv_val = jnp.dot(all_rows, val_full, preferred_element_type=jnp.float32).astype(jnp.bfloat16)
    conv_gate = jnp.dot(all_rows, gate_full, preferred_element_type=jnp.float32).astype(
        jnp.bfloat16
    )
    glu = glu_of(conv_val, conv_gate)
    conv_edge = passed_along(glu[-conv_lags:], "sp", 1)
    rgate_full, rin_full = (
        lax.all_gather(rec_gate_w, "sp", axis=0, tiled=True),
        lax.all_gather(rec_in_w, "sp", axis=0, tiled=True),
    )
    rec_gate = jnp.dot(all_rows, rgate_full, preferred_element_type=jnp.float32).astype(
        jnp.bfloat16
    )
    rec_in = jnp.dot(all_rows, rin_full, preferred_element_type=jnp.float32).astype(jnp.bfloat16)
    rec_edge = passed_along(rec_in[-short_lags:], "sp", 1)
    filtered = causal_window(conv_edge, glu, conv_taps) + conv_bias[None, :]
    row_total = lax.psum(jnp.sum(filtered, axis=1), "tp")
    centered = filtered - (row_total / CONV_WIDTH)[:, None]
    spread = lax.psum(jnp.sum(centered * centered, axis=1), "tp") / CONV_WIDTH
    conv_out = jax.nn.silu(centered * lax.rsqrt(spread + 1e-05)[:, None] * conv_gain).astype(
        jnp.bfloat16
    )
    smoothed = causal_window(rec_edge, rec_in, short_taps).astype(jnp.bfloat16)
    length = smoothed.shape[0]
    grouped = smoothed.reshape(length, decay_map.shape[0], decay_map.shape[1])
    retain = jax.nn.sigmoid(
        jnp.einsum("thi,hio->tho", grouped, decay_map, preferred_element_type=jnp.float32).reshape(
            length, rec_cols
        )
    )
    admit = jax.nn.sigmoid(
        jnp.einsum("thi,hio->tho", grouped, input_map, preferred_element_type=jnp.float32).reshape(
            length, rec_cols
        )
    )
    log_decay = -RATE_SCALE * retain * jax.nn.softplus(-decay_base)[None, :] + decay_jump
    decay = jnp.exp(log_decay)
    inflow = jnp.sqrt(-jnp.expm1(2.0 * log_decay)) * admit * smoothed.astype(jnp.float32)
    products, local_state = lax.associative_scan(chain_step, (decay, inflow), axis=0)
    entering = prefix(
        (products[-1], local_state[-1]),
        "sp",
        chain_step,
        (jnp.ones((rec_cols,), jnp.float32), jnp.zeros((rec_cols,), jnp.float32)),
    )
    state = local_state + products * entering[1][None, :]
    rec_out = (jax.nn.gelu(rec_gate.astype(jnp.float32)) * state).astype(jnp.bfloat16)
    conv_full, rec_full = (
        lax.all_gather(out_conv_w, "sp", axis=1, tiled=True),
        lax.all_gather(out_rec_w, "sp", axis=1, tiled=True),
    )
    return lax.psum_scatter(
        (
            jnp.dot(conv_out, conv_full, preferred_element_type=jnp.float32)
            + jnp.dot(rec_out, rec_full, preferred_element_type=jnp.float32)
        ).astype(jnp.bfloat16),
        "tp",
        scatter_dimension=0,
        tiled=True,
    )


MESH = pl.DeviceIdType.MESH
ANY = pl.BlockSpec(memory_space=pl.ANY)
VMEM = pl.BlockSpec(memory_space=pltpu.VMEM)
SEGMENTS = 8


class Spot:
    def __init__(self, planes):
        self.s, self.c = lax.axis_index("sp"), lax.axis_index("tp")
        self.z, self.q = self.s // 4, self.s % 4
        self.qx = self.q + 1 - 2 * (self.q % 2)
        self.qy = (self.q + 2) % 4
        self.qd = 3 - self.q
        self.has_up, self.has_down = self.z < planes - 1, self.z > 0
        self.up, self.down = self.at(self.s + 4, self.c), self.at(self.s - 4, self.c)
        self.partner = self.at(self.s, 1 - self.c)

    def at(self, s, c):
        return {"sp": s, "tp": c}

    def mate(self, q):
        return self.at(self.z * 4 + q, self.c)


class Mail:
    def __init__(self, send_sem):
        self.send_sem, self.tag, self.open = send_sem, "early", []
        self.free = list(range(send_sem.shape[0]))

    def claim(self):
        self.free.sort()
        return self.free.pop(0)

    def send(self, src, dst, recv, device, when=None, index=None):
        index = self.claim() if index is None else index
        copy = pltpu.make_async_remote_copy(
            src_ref=src, dst_ref=dst, send_sem=self.send_sem.at[index],
            recv_sem=recv, device_id=device, device_id_type=MESH,
        )
        self.open.append((self.tag, index, copy.wait_send, when))
        if when is None:
            copy.start()
        else:
            pl.when(when)(copy.start)
        return index

    def load(self, src, dst):
        index = self.claim()
        copy = pltpu.make_async_copy(src, dst, self.send_sem.at[index])
        copy.start()
        return index, copy

    def loaded(self, copies):
        for index, copy in copies:
            copy.wait()
            self.free.append(index)

    def arrived(self, dst, recv, device):
        pltpu.make_async_remote_copy(
            src_ref=dst, dst_ref=dst, send_sem=self.send_sem.at[0],
            recv_sem=recv, device_id=device, device_id_type=MESH,
        ).wait_recv()

    def finish(self, *tags):
        done = [entry for entry in self.open if not tags or entry[0] in tags]
        self.open = [entry for entry in self.open if entry not in done]
        for _, index, wait, when in done:
            if when is None:
                wait()
            else:
                pl.when(when)(wait)
        self.free.extend({entry[1] for entry in done})


def greet(me, devices, line):
    barrier = pltpu.get_barrier_semaphore()
    for device in devices:
        pl.semaphore_signal(barrier, inc=1, device_id=device, device_id_type=MESH)
    amount = len(devices)
    if line:
        for has, device in ((me.has_up, me.up), (me.has_down, me.down)):
            @pl.when(has)
            def _():
                pl.semaphore_signal(barrier, inc=1, device_id=device, device_id_type=MESH)
        amount = amount + me.has_up.astype(jnp.int32) + me.has_down.astype(jnp.int32)
    pl.semaphore_wait(barrier, amount)


class PlaneGather:
    def __init__(self, me, mail, slot, recv, recv_pair):
        self.me, self.mail, self.slot = me, mail, slot
        self.recv, self.recv_pair = recv, recv_pair
        self.parts = recv.shape[1]
        self.half = self.parts // 2

    def start(self):
        me, mail = self.me, self.mail
        for h in range(self.parts):
            for q, part in ((me.qx, h), (me.qy, (h + self.half) % self.parts)):
                own = self.slot(me.q, me.c, part)
                mail.send(own, own, self.recv.at[me.q, part], me.mate(q))
        for part in range(self.parts):
            self.share(me.q, part, self.slot(me.q, me.c, part))

    def took(self, q, part):
        here = self.slot(q, self.me.c, part)
        self.mail.arrived(here, self.recv.at[q, part], self.me.partner)
        return here

    def share(self, q, part, here):
        self.mail.send(here, here, self.recv_pair.at[q, part], self.me.partner)

    def first(self, i):
        me = self.me
        for q, part, to in ((me.qx, i, me.qy), (me.qy, self.half + i, me.qx)):
            here = self.took(q, part)
            self.mail.send(here, here, self.recv.at[q, part], me.mate(to))
            self.share(q, part, here)

    def second(self):
        for i in range(self.half):
            for q, part in ((self.me.qx, self.half + i), (self.me.qy, i)):
                self.share(q, part, self.took(q, part))

    def third(self, i):
        for part in (i, self.half + i):
            self.share(self.me.qd, part, self.took(self.me.qd, part))

    def paired(self, q, part):
        me = self.me
        self.mail.arrived(self.slot(q, 1 - me.c, part), self.recv_pair.at[q, part], me.partner)

    def last(self, origins):
        for q in origins:
            for part in range(self.parts):
                self.paired(q, part)


def one_minus_exp(y, grown):
    series = 1.0 + y * (1.0 / 5.0)
    for n in (4.0, 3.0, 2.0):
        series = 1.0 + y * (1.0 / n) * series
    return jnp.where(y > -0.25, -y * series, 1.0 - grown)


def gelu(v):
    return 0.5 * v * (1.0 + jnp.tanh(0.7978845608028654 * (v + 0.044715 * v * v * v)))


class Line:
    def __init__(self, me, mail, planes, slot, recv, seen=None):
        self.me, self.mail, self.planes = me, mail, planes
        self.slot, self.recv, self.seen = slot, recv, seen

    def own(self, piece, src, up=True, down=True):
        me = self.me
        for wanted, has, device in ((up, me.has_up, me.up), (down, me.has_down, me.down)):
            if wanted is not False:
                self.post(src, me.z, piece, device, has & wanted)

    def post(self, src, origin, piece, device, when):
        self.mail.send(src, self.slot(origin, piece), self.recv.at[origin, piece], device, when)

    def mine(self, origin):
        return True

    def ways(self, k):
        me = self.me
        return (
            (me.z - k, me.z >= k, me.up, me.has_up),
            (me.z + k, me.z + k < self.planes, me.down, me.has_down),
        )

    def take(self, origin, piece, when, index=None):
        here, sem = self.slot(origin, piece), self.recv.at[origin, piece]
        pl.when(when)(functools.partial(self.mail.arrived, here, sem, self.me.partner))
        return None if self.seen is None else self.seen(origin, piece, when, index)

    def relay(self, k, piece, up=True, down=True):
        for wanted, (origin, there, on, more) in zip((up, down), self.ways(k)):
            if wanted:
                when = jnp.logical_and(there, more)
                here = self.slot(origin, piece)
                self.take(origin, piece, when)
                self.post(here, origin, piece, on, when)

    def await_up(self, k, piece):
        origin, there, _, more = self.ways(k)[0]
        return self.take(origin, piece, there & more)

    def forward_up(self, k, piece):
        origin, there, on, more = self.ways(k)[0]
        here, sem = self.slot(origin, piece), self.recv.at[origin, piece]
        self.mail.send(here, here, sem, on, there & more)

    def settle(self, k, piece):
        me = self.me
        lowest, highest = jnp.logical_not(me.has_down), jnp.logical_not(me.has_up)
        origin = jnp.where(lowest, me.z + k, me.z - k)
        here, sem = self.slot(origin, piece), self.recv.at[origin, piece]
        pl.when((lowest | highest) & self.mine(origin))(functools.partial(self.mail.arrived, here, sem, me.partner))


class OutLine(Line):
    def __init__(self, me, mail, planes, slot, recv, seen, other, other_recv):
        super().__init__(me, mail, planes, slot, recv, seen)
        self.other, self.other_recv = other, other_recv

    def mine(self, origin):
        return origin // (self.planes // 2) == self.me.c

    def post(self, src, origin, piece, device, when):
        me = self.me
        z = device["sp"] // 4
        ends = (z == 0) | (z == self.planes - 1)
        cross = ends & jnp.logical_not(self.mine(origin))
        here, sem = self.slot(origin, piece), self.recv.at[origin, piece]
        index = self.mail.send(src, here, sem, device, when & jnp.logical_not(cross))
        place = origin - (1 - me.c) * (self.planes // 2)
        sem = self.other_recv.at[place, piece]
        device = me.at(device["sp"], 1 - me.c)
        self.mail.send(src, self.other(place, piece), sem, device, when & cross, index)


def small_softplus(v):
    u = jnp.exp(-jnp.abs(v))
    series = jnp.zeros_like(u)
    for n in (8.0, 7.0, 6.0, 5.0, 4.0, 3.0, 2.0, 1.0):
        series = 1.0 / n - u * series
    return jnp.maximum(v, 0.0) + jnp.where(u < 0.1, u * series, jnp.log(1.0 + u))


OUT_PARTS = 4
POOL = 84


def layer_kernel(
    planes, lags, tokens, gain_in, val_w, gate_w, rgate_w, rin_w, taps_in, bias_in, cgain_in, staps_in,
    dmap_in, imap_in, base_in, jump_in, ocw, orw,
    out, x_ref, gain, rin_s, rgate_s, wr, wc, taps, bias, cgain, staps, dmap, imap, rbase, jump, jb, cpar, rpar,
    xall, rwall, cwall, projr, jall, wz, wp, yall, yrest, cacc, cbuf, gext, rext, filt, dec, inf, maps, ft,
    st_all, carry, cr_all,
    send, rx, rpx, rwr, rwc, zrc, zo, rj, rvq, re, rf, rw, rh, rs, rc,
):
    me = Spot(planes)
    mail = Mail(send)
    c_lags, s_lags = lags
    f32, bf16 = jnp.float32, jnp.bfloat16
    rows, depth = x_ref.shape[0], wr.shape[1]
    length = xall.shape[0]
    cw, rwid = gext.shape[1], rpar.shape[1]
    seg = length // SEGMENTS
    lane_seg = dec.shape[1] // SEGMENTS
    top = gext.shape[0] - length
    rtop = rext.shape[0] - length
    fold = dec.shape[0]
    part = planes // 2
    major = rwid // 128 * 128
    minor = rwid - major
    mine = me.q * 2 + me.c
    others = (me.qx, me.qy, me.qd)
    pieces = (me.q,) + others
    parts = tuple(range(OUT_PARTS))
    tall, half_cols = wz.shape[1] // 2, wz.shape[2] // 2

    def cut(p):
        return pl.ds(p % 2 * tall, tall), pl.ds(p // 2 * half_cols, half_cols)

    last = planes - 1
    mates = [me.at(me.z * 4 + (me.q + dq) % 4, c) for dq in range(4) for c in (me.c, 1 - me.c)][1:]
    lined = [me.at((me.s + 4 * k) % (4 * planes), me.c) for k in range(1, planes)]
    crossed = [me.at((me.s + 4 * k) % (4 * planes), 1 - me.c) for k in range(1, planes)]
    load = mail.load
    got_rec = [load(rin_w, rin_s), load(rgate_w, rgate_s)]
    got_x = [load(tokens, x_ref), load(gain_in, gain)]
    got_conv = []
    for q in range(4):
        got_conv.append(load(val_w.at[:, pl.ds(q * cw, cw)], wc.at[q, :, pl.ds(0, cw)]))
        got_conv.append(load(gate_w.at[:, pl.ds(q * cw, cw)], wc.at[q, :, pl.ds(cw, cw)]))
    got_out = []
    got_out.append(load(ocw, wz.at[me.z, pl.ds(0, 4 * cw)]))
    for q in range(4):
        at = 4 * cw + q * major
        got_out.append(load(orw.at[pl.ds(q * rwid, major)], wz.at[me.z, pl.ds(at, major)]))
        at = 4 * (cw + major) + q * minor
        got_out.append(load(orw.at[pl.ds(q * rwid + major, minor)], wz.at[me.z, pl.ds(at, minor)]))
    got_jump = [load(jump_in, jump)]
    got_small = [
        load(src, dst)
        for src, dst in (
            (taps_in, taps), (bias_in, bias), (cgain_in, cgain), (staps_in, staps),
            (dmap_in, dmap), (imap_in, imap), (base_in, rbase),
        )
    ]
    greet(me, mates + lined + crossed, False)
    mail.loaded(got_rec)
    for q in range(4):
        lanes = slice(q * rwid, (q + 1) * rwid)
        wr[q] = jnp.concatenate([rin_s[:, lanes], rgate_s[:, lanes]], axis=1)

    def of_rows(ref):
        def slot(origin, piece):
            return ref.at[pl.ds(pl.multiple_of((origin * 4 + piece) * depth, depth), depth)]

        return slot

    def theirs_too(origin, piece, when, index=None):
        theirs = jnp.logical_and(origin // part != me.c, when)
        place = origin - (1 - me.c) * part
        here, there = wz.at[(origin, *cut(piece))], wp.at[(place, *cut(piece))]
        return mail.send(here, there, rw.at[place, piece], me.partner, theirs, index)

    rl = Line(me, mail, planes, of_rows(rwall), zrc.at[0])
    cl = Line(me, mail, planes, of_rows(cwall), zrc.at[1])
    ol = OutLine(
        me, mail, planes, lambda origin, p: wz.at[(origin, *cut(p))], zo, theirs_too,
        lambda place, p: wp.at[(place, *cut(p))], rw,
    )

    def out_own(p, up=True, down=True):
        ol.own(p, wz.at[(me.z, *cut(p))], up, down)

    mail.tag = "first"
    for q in others:
        mail.send(wr.at[q], rl.slot(me.z, me.q), rwr.at[me.q], me.mate(q))
    rl.own(me.q, wr.at[me.q])

    mail.loaded(got_x)
    first_row = mine * rows

    @pl.loop(0, rows // 16)
    def _(i):
        values = x_ref[pl.ds(pl.multiple_of(i * 16, 16), 16)].astype(f32)
        inverse = lax.rsqrt(jnp.mean(values * values, axis=1, keepdims=True) + 1e-06)
        place = pl.ds(pl.multiple_of(first_row + i * 16, 16), 16)
        xall[place] = (values * inverse * gain[...]).astype(bf16)

    part_rows = rows // rx.shape[1]

    def xslot(q, c, h):
        return xall.at[pl.ds(pl.multiple_of((q * 2 + c) * rows + h * part_rows, 16), part_rows)]

    xg = PlaneGather(me, mail, xslot, rx, rpx)
    xg.start()
    mail.loaded(got_conv + got_out)
    for q in others:
        mail.send(wc.at[q], cl.slot(me.z, me.q), rwc.at[me.q], me.mate(q))
    cl.own(me.q, wc.at[me.q])
    out_own(0)
    mail.loaded([load(wr.at[me.q], rl.slot(me.z, me.q)), load(wc.at[me.q], cl.slot(me.z, me.q))])
    for p in parts:
        theirs_too(me.z, p, True)
    mail.loaded(got_jump + got_small)
    half = jump.shape[0] // 2
    for q in range(4):
        lanes = slice(q * rwid, (q + 1) * rwid)
        jb[q] = jnp.concatenate([jump[:half, lanes], jump[half:, lanes]], axis=1).astype(bf16)
    jall[me.q] = jb[me.q]
    own_lanes = pl.ds(pl.multiple_of(me.q * cw, 128), cw)
    cpar[pl.ds(0, c_lags + 1)] = taps[:, own_lanes].astype(f32)
    cpar[pl.ds(c_lags + 1, 1)] = bias[:, own_lanes]
    cpar[pl.ds(c_lags + 2, 1)] = cgain[:, own_lanes]
    window = -(-rwid // 128) * 128
    wide_lanes = pl.ds(pl.multiple_of(me.q * rwid // 128 * 128, 128), window)

    def own_rec(values):
        moved = values[:, :rwid]
        for lead in sorted({q * rwid % 128 for q in range(4)} - {0}):
            moved = jnp.where(me.q * rwid % 128 == lead, values[:, lead : lead + rwid], moved)
        return moved

    rpar[pl.ds(0, s_lags + 1)] = own_rec(staps[:, wide_lanes].astype(f32))
    rpar[pl.ds(s_lags + 1, 1)] = own_rec(RATE_SCALE * small_softplus(-rbase[wide_lanes][None]))

    maps[...] = jnp.zeros_like(maps)
    size = dmap.shape[1]
    heads = rwid // size
    for h in range(heads):
        spot = pl.ds(h * size, size)
        maps[spot, pl.ds(h * size, size)] = dmap[me.q * heads + h]
        maps[spot, pl.ds(fold * 128 + h * size, size)] = imap[me.q * heads + h]

    for q in others:
        here = rl.slot(me.z, q)
        mail.arrived(here, rwr.at[q], me.partner)
        rl.own(q, here)
    for p in pieces:
        rl.relay(1, p)
    mail.tag = "early"
    for i in range(xg.half):
        xg.first(i)
    for q in others:
        mail.send(jb.at[q], jall.at[me.q], rj.at[me.q], me.mate(q))
    for k in range(2, last):
        for p in pieces:
            rl.relay(k, p)
    xg.second()
    for q in others:
        here = cl.slot(me.z, q)
        mail.arrived(here, rwc.at[q], me.partner)
        cl.own(q, here)
    for k in range(1, planes):
        for p in pieces:
            rl.settle(k, p)
    xg.last(pieces[:3])

    tile = length // 4

    def project_rec(begin, size):
        at = pl.ds(pl.multiple_of(begin, 64), size)
        product = jnp.dot(xall[at], rwall[...], preferred_element_type=f32).astype(bf16)
        projr[at] = product
        rext[pl.ds(pl.multiple_of(begin + rtop, 16), size)] = product[:, :rwid].astype(f32)

    @pl.loop(0, 3)
    def _(i):
        project_rec(((me.q // 2 + i // 2) % 2 * 2 + (me.q % 2 + i % 2) % 2) * tile, tile)

    mail.tag = "conv"
    for n, p in enumerate(pieces):
        cl.relay(1, p, n < 2, True)
    mail.tag = "early"
    for i in range(xg.half):
        xg.third(i)
    mail.finish("first")
    project_rec((me.qd * 2 + me.c) * rows, rows)
    xg.last(pieces[3:])
    project_rec((me.qd * 2 + 1 - me.c) * rows, rows)

    mail.tag = "conv"
    mail.send(rext.at[pl.ds(length, rtop)], rext.at[pl.ds(0, rtop)], rh.at[0], me.up, me.has_up)
    for p in pieces[2:]:
        cl.relay(1, p, True, False)
    for k in range(2, last):
        for p in pieces:
            cl.relay(k, p, False, True)

    @pl.when(jnp.logical_not(me.has_down))
    def _():
        rext[pl.ds(0, rtop)] = jnp.zeros((rtop, rwid), f32)
        gext[pl.ds(0, top)] = jnp.zeros((top, cw), f32)

    softened = rpar[pl.ds(s_lags + 1, 1), :]

    @pl.loop(0, SEGMENTS)
    def _(n):
        step = (n + 1) // 2
        ring = (me.q // 2 + step % 4 // 2) % 2 * 2 + (me.q % 2 + step % 2) % 2
        i = jnp.where(n == SEGMENTS - 1, 2 * me.q, 2 * ring + n % 2)
        i = jnp.where(n == 0, 2 * me.q + 1, i)

        @pl.when(jnp.logical_and(i == 0, me.has_down))
        def _():
            mail.arrived(rext.at[pl.ds(0, rtop)], rh.at[0], me.partner)

        @pl.when(jnp.logical_and(n % 2 == 1, n < SEGMENTS - 1))
        def _():
            mail.arrived(jall.at[i // 2], rj.at[i // 2], me.partner)

        base = pl.multiple_of(i * seg, 8)
        window = rext[pl.ds(pl.multiple_of(base + rtop - 8, 8), seg + 8)]
        smooth = jnp.zeros((seg, rwid), f32)
        for k in range(s_lags + 1):
            smooth = smooth + rpar[pl.ds(k, 1), :] * window[8 - s_lags + k : 8 - s_lags + k + seg]
        smooth = smooth.astype(bf16)
        gates = jax.nn.sigmoid(jnp.dot(smooth, maps[...], preferred_element_type=f32))
        retain, admit = gates[:, :rwid], gates[:, fold * 128 : fold * 128 + rwid]
        wide = jall[i // 2].astype(f32)
        moved = jnp.where(i % 2 == 0, wide[:, :rwid], wide[:, rwid:])
        log_decay = moved - retain * softened
        decay = jnp.exp(log_decay)
        inflow = jnp.sqrt(one_minus_exp(log_decay, decay) * (1.0 + decay)) * admit * smooth.astype(f32)
        for f in range(fold):
            w = min(128, rwid - f * 128)
            spot = pl.ds(pl.multiple_of(i * lane_seg, 8), seg)
            dec[f, spot, pl.ds(0, w)] = decay[:, f * 128 : f * 128 + w]
            inf[f, spot, pl.ds(0, w)] = inflow[:, f * 128 : f * 128 + w]

    def one(i, held):
        after = []
        for f in range(fold):
            at = pl.ds(i, SEGMENTS, stride=lane_seg)
            d = dec.at[f][at, :]
            product, state = held[2 * f] * d, held[2 * f + 1] * d + inf.at[f][at, :]
            dec.at[f][at, :] = product
            inf.at[f][at, :] = state
            after += [product, state]
        return tuple(after)

    flat = (SEGMENTS, 128)
    ends = lax.fori_loop(0, seg, one, (jnp.ones(flat, f32), jnp.zeros(flat, f32)) * fold, unroll=8)
    for f in range(fold):
        product, state = jnp.ones((1, 128), f32), jnp.zeros((1, 128), f32)
        for i in range(SEGMENTS):
            p, s = ends[2 * f][i : i + 1], ends[2 * f + 1][i : i + 1]
            product, state = product * p, p * state + s
        carry[pl.ds(2 * f, 1)] = product
        carry[pl.ds(2 * f + 1, 1)] = state
    for k in range(1, planes):
        mail.send(carry, cr_all.at[me.z], rc.at[me.z], lined[k - 1], me.z + k < planes)
    early = me.z < planes - 2
    for k in range(2, last):
        for p in pieces[:3]:
            cl.relay(k, p, True, False)
    mail.tag = "gather"
    for p in parts[1:]:
        out_own(p, early, True)
    mail.finish("early")

    for i in range(SEGMENTS):
        there = pl.ds(i * lane_seg, seg)
        factor = gelu(projr[pl.ds(i * seg, seg), pl.ds(rwid, rwid)].astype(f32))
        for f in range(fold):
            w = min(128, rwid - f * 128)
            lanes = pl.ds(0, w)
            dec[f, there, lanes] = dec[f, there, lanes] * factor[:, f * 128 : f * 128 + w]
            inf[f, there, lanes] = inf[f, there, lanes] * factor[:, f * 128 : f * 128 + w]

    for k in range(1, planes):
        z = me.z - k
        pl.when(z >= 0)(functools.partial(mail.arrived, cr_all.at[z], rc.at[z], me.partner))
    entering = []
    for f in range(fold):
        held = jnp.zeros((1, 128), f32)
        for j in range(planes - 1):
            after = cr_all[j, pl.ds(2 * f, 1)] * held + cr_all[j, pl.ds(2 * f + 1, 1)]
            held = jnp.where(j < me.z, after, held)
        for i in range(SEGMENTS):
            entering.append(held)
            held = ends[2 * f][i : i + 1] * held + ends[2 * f + 1][i : i + 1]
    placed = me.c * 4 + me.q

    def rec_result(i):
        here, there = pl.ds(i * seg, seg), pl.ds(i * lane_seg, seg)
        state = [dec[f, there] * entering[f * SEGMENTS + i] + inf[f, there] for f in range(fold)]
        result = jnp.concatenate(state, axis=1)[:, :rwid].astype(bf16)
        yall[here, pl.ds(pl.multiple_of(8 * cw + placed * major, 128), major)] = result[:, :major]
        return result[:, major:]

    for i in range(SEGMENTS // 2):
        pair = jnp.concatenate([rec_result(i), rec_result(i + SEGMENTS // 2)], axis=1)
        yrest[pl.ds(i * seg, seg), pl.ds(pl.multiple_of(placed * 2 * minor, 128), 2 * minor)] = pair

    def gather(buffer, lane, lanes, recv, recv_pair):
        tall_part = buffer.shape[0] // recv.shape[1]

        def slot(q, c, h):
            spot = pl.ds(pl.multiple_of(lane + (c * 4 + q) * lanes, 128), lanes)
            return buffer.at[pl.ds(h * tall_part, tall_part), spot]

        return PlaneGather(me, mail, slot, recv, recv_pair)

    mg = gather(yall, 8 * cw, major, rvq.at[0], rvq.at[1])
    eg = gather(yrest, 0, 2 * minor, re, rf)
    yg = gather(yall, 0, cw, rx, rpx)
    mail.tag = "conv"
    mg.start()
    eg.start()
    mail.tag = "gather"
    for k in range(1, last):
        for p in pieces:
            cl.settle(k, p)
        for p in pieces[3:] if k > 1 else ():
            cl.await_up(k, p)
    plane_depth = 4 * depth
    is_last = (me.z == last).astype(jnp.int32)

    def conv_product(at, begin, size):
        deep = pl.ds(pl.multiple_of(begin, plane_depth), size)
        return jnp.dot(xall[at, deep], cwall[deep], preferred_element_type=f32)

    @pl.loop(0, 4)
    def _(i):
        at = pl.ds(pl.multiple_of(i * tile, tile), tile)
        cacc[at] = conv_product(at, is_last * plane_depth, last * plane_depth)

    middle = me.has_up & me.has_down

    def finish_conv(when):
        @pl.when(when)
        def _():
            @pl.loop(0, 4)
            def _(i):
                at = pl.ds(pl.multiple_of(i * tile, tile), tile)
                product = cacc[at] + conv_product(at, (1 - is_last) * last * plane_depth, plane_depth)
                product = product.astype(bf16).astype(f32)
                glu = (product[:, :cw] * jax.nn.sigmoid(product[:, cw:])).astype(bf16).astype(f32)
                gext[pl.ds(pl.multiple_of(i * tile + top, 8), tile)] = glu

        tail_rows = gext.at[pl.ds(length, top)]
        mail.send(tail_rows, gext.at[pl.ds(0, top)], rh.at[1], me.up, me.has_up & when)

    finish_conv(middle)
    for k in range(2, last):
        for p in pieces[3:]:
            cl.forward_up(k, p)
    for p in parts[1:]:
        out_own(p, jnp.logical_not(early), False)
    mg.first(0)
    for p in pieces:
        cl.settle(last, p)
    finish_conv(jnp.logical_not(middle))
    strips = length // 64

    def filter_strip(n):
        i = strips - 1 - n

        @pl.when(jnp.logical_and(i == 0, me.has_down))
        def _():
            mail.arrived(gext.at[pl.ds(0, top)], rh.at[1], me.partner)

        base = pl.multiple_of(i * 64, 8)
        window = gext[pl.ds(base, 64 + top)]
        total = jnp.zeros((64, cw), f32) + cpar[pl.ds(c_lags + 1, 1), :]
        for r in range(8):
            ks = [k for k in range(c_lags + 1) if (top - c_lags + k) % 8 == r]
            span = 64 + (8 if r else 0)
            shifted = jnp.zeros((span, cw), f32)
            for k in ks:
                begin = (top - c_lags + k) // 8 * 8
                shifted = shifted + cpar[pl.ds(k, 1), :] * window[begin : begin + span]
            total = total + shifted[r : r + 64]
        filt[pl.ds(base, 64)] = total

    pl.loop(0, strips)(filter_strip)

    turned = filt[...].T
    ft[...] = turned
    part_sum = jnp.sum(turned, axis=0, keepdims=True)
    off = turned - part_sum * (1.0 / cw)
    st_all[mine, pl.ds(0, 1)] = part_sum
    st_all[mine, pl.ds(1, 1)] = jnp.sum(off * off, axis=0, keepdims=True)
    for device in mates:
        mail.send(st_all.at[mine], st_all.at[mine], rs.at[mine], device)
    for i in range(1, mg.half):
        mg.first(i)
    for i in range(eg.half):
        eg.first(i)
    mail.tag = "out"
    for p in parts:
        ol.relay(1, p)
    mail.tag = "gather"
    mail.finish("conv")

    for k in range(1, 8):
        d = (mine + k) % 8
        mail.arrived(st_all.at[d], rs.at[d], me.partner)
    total = sum(st_all[d, 0:1, :] for d in range(8))
    mean = total * (1.0 / (8 * cw))
    spread = jnp.zeros_like(mean)
    for d in range(8):
        shift = st_all[d, 0:1, :] * (1.0 / cw) - mean
        spread = spread + st_all[d, 1:2, :] + cw * shift * shift
    scale = lax.rsqrt(spread * (1.0 / (8 * cw)) + 1e-05)
    gain_col = jnp.broadcast_to(cpar[pl.ds(c_lags + 2, 1), :], (8, cw)).T[:, 0:1]
    v = (ft[...] - mean) * scale * gain_col
    yall[:, pl.ds(pl.multiple_of(placed * cw, 128), cw)] = (v * jax.nn.sigmoid(v)).T.astype(bf16)
    mail.tag = "begun"
    yg.start()
    mail.tag = "share"
    mg.second()
    eg.second()
    for g in (mg, eg):
        for i in range(g.half):
            g.third(i)
    mail.tag = "last"
    mail.finish("gather")
    for i in range(yg.half):
        yg.first(i)
    for k in range(2, last):
        for p in parts:
            ol.relay(k, p)
    mg.last(pieces)
    eg.last(pieces)
    mail.finish("share")
    rest_at = 8 * (cw + major)

    @pl.loop(0, SEGMENTS // 2)
    def _(i):
        values = yrest[pl.ds(pl.multiple_of(i * seg, 16), seg)]
        low = [values[:, j * 2 * minor : j * 2 * minor + minor] for j in range(8)]
        high = [values[:, j * 2 * minor + minor : (j + 1) * 2 * minor] for j in range(8)]
        for begin, chosen in ((0, low), (length // 2, high)):
            here = pl.ds(pl.multiple_of(begin + i * seg, 16), seg)
            yall[here, pl.ds(rest_at, 8 * minor)] = jnp.concatenate(chosen, axis=1)

    yg.second()
    yg.third(0)
    for k in range(1, last):
        for p in parts:
            ol.settle(k, p)

    cols = wz.shape[2]
    upward = me.z < part

    def lanes_of(h):
        return pl.ds(0, cols) if h is None else pl.ds(h * half_cols, half_cols)

    def summed(q, k, h, low, high):
        here = pl.ds(pl.multiple_of(q * 2 * rows, 16), 2 * rows)
        total = jnp.zeros((2 * rows, cols if h is None else half_cols), f32)
        for c, block in ((me.c, wz.at[me.c * part + k]), (1 - me.c, wp.at[k])):
            begin = 0
            for at, lanes in ((0, 4 * cw), (8 * cw, 4 * major), (rest_at, 4 * minor)):
                first, end = max(begin, low), min(begin + lanes, high)
                if first < end:
                    spot = pl.multiple_of(at + c * lanes + first - begin, 128)
                    right = block[pl.ds(first, end - first), lanes_of(h)]
                    left_part = yall[here, pl.ds(spot, end - first)]
                    total = total + jnp.dot(left_part, right, preferred_element_type=f32)
                begin = begin + lanes
        return here, total

    def multiply(q, k, h):
        here, total = summed(q, k, h, tall if h == 1 else 0, 2 * tall)
        if h == 1:
            total = total + cacc[here, pl.ds(0, half_cols)]
        total = total.astype(bf16)
        for c in range(2):
            cbuf[q * 2 + c, k, :, lanes_of(h)] = total[c * rows : (c + 1) * rows]

    def place(q, c, k, h):
        at = ((c * part + k) * 4 + q) * cols + (0 if h is None else h * half_cols)
        return out.at[:, pl.ds(pl.multiple_of(at, 128), cols if h is None else half_cols)]

    def mate_of(i):
        flip = 3 - i
        return (me.q // 2 + flip // 2) % 2 * 2 + (me.q % 2 + flip % 2) % 2

    mail.finish("begun")

    def left(d, k, h):
        return rvq.at[k, d // 2, d % 2 * 2 + (h or 0)]

    def landed(d, k, h):
        return zrc.at[k, d // 2, d % 2 * 2 + (h or 0)]

    def parcel(q, c, k, h):
        return pltpu.make_async_remote_copy(
            src_ref=cbuf.at[q * 2 + c, k, :, lanes_of(h)], dst_ref=place(me.q, me.c, k, h),
            send_sem=left(q * 2 + c, k, h), recv_sem=landed(mine, k, h),
            device_id=me.at(me.z * 4 + q, c), device_id_type=MESH,
        )

    def kept(k, h):
        src = cbuf.at[mine, k, :, lanes_of(h)]
        return pltpu.make_async_copy(src, place(me.q, me.c, k, h), left(mine, k, h))

    def serve(q, k, h):
        multiply(q, k, h)
        pl.when(q != me.q)(lambda: parcel(q, me.c, k, h).start())
        parcel(q, 1 - me.c, k, h).start()
        pl.when(q == me.q)(lambda: kept(k, h).start())

    def ready(k, ps):
        for p in ps:
            mail.arrived(wp.at[(k, *cut(p))], rw.at[k, p], me.partner)

    order = [jnp.where(upward, n, part - 1 - n) for n in range(part)]
    ready(order[0], parts)
    for i in range(yg.half):
        if i:
            yg.third(i)
        for q in pieces:
            yg.paired(q, i)
            yg.paired(q, yg.half + i)

        @pl.loop(0, 2)
        def _(n):
            serve(n * yg.half + i, order[0], None)

    for n in range(1, part - 1):
        ready(order[n], parts)
        pl.loop(0, 4)(lambda i: serve(mate_of(i), order[n], None))
    k_far = order[-1]
    for p in parts[:2]:
        ol.settle(last, p)
    ready(k_far, parts[:2])
    pl.loop(0, 4)(lambda i: serve(mate_of(i), k_far, 0))
    ol.settle(last, 2)
    ready(k_far, parts[2:3])

    @pl.loop(0, 4)
    def _(q):
        here, total = summed(q, k_far, 1, 0, tall)
        cacc[here, pl.ds(0, half_cols)] = total

    ol.settle(last, 3)
    ready(k_far, parts[3:])
    pl.loop(0, 4)(lambda i: serve(mate_of(i), k_far, 1))
    rounds = [(k, None) for k in order[:-1]] + [(order[-1], 0), (order[-1], 1)]

    @pl.loop(0, 4)
    def _(i):
        q = mate_of(i)
        for k, h in rounds:
            mail.arrived(place(q, 1 - me.c, k, h), landed(q * 2 + 1 - me.c, k, h), me.partner)
            parcel(q, 1 - me.c, k, h).wait_send()

    @pl.loop(0, 3)
    def _(i):
        q = mate_of(i)
        for k, h in rounds:
            mail.arrived(place(q, me.c, k, h), landed(q * 2 + me.c, k, h), me.partner)
            parcel(q, me.c, k, h).wait_send()

    for k, h in rounds:
        kept(k, h).wait()
    mail.finish()


def handed_out_kernel(src, dst, held, got, sent):
    count = got.shape[0]
    tall = src.shape[0] // count
    spots = [pl.ds(i * tall, tall) for i in range(count)]
    taken = [pltpu.make_async_copy(src.at[s], held.at[s], got.at[i]) for i, s in enumerate(spots)]
    given = [pltpu.make_async_copy(held.at[s], dst.at[s], sent.at[i]) for i, s in enumerate(spots)]
    for copy in taken:
        copy.start()
    for came, goes in zip(taken, given):
        came.wait()
        goes.start()
    for copy in given:
        copy.wait()


def handed_out(result):
    dma = pltpu.SemaphoreType.DMA
    return pl.pallas_call(
        handed_out_kernel,
        out_shape=jax.ShapeDtypeStruct(result.shape, result.dtype),
        in_specs=[ANY],
        out_specs=ANY,
        scratch_shapes=[pltpu.VMEM(result.shape, result.dtype), dma((6,)), dma((6,))],
    )(result)


def layer(planes, lags, tokens, norm_gain, val_w, gate_w, rgate_w, rin_w, taps, bias, cgain, staps, dmap, imap, rbase, jump, ocw, orw):
    rows, width_in = tokens.shape
    length = 8 * rows
    depth = rin_w.shape[0]
    cw, rwid = val_w.shape[1] // 4, rin_w.shape[1] // 4
    used, cols = cw + rwid, ocw.shape[1]
    minor = rwid % 128
    fold = (rwid + 127) // 128
    f32, bf16 = jnp.float32, jnp.bfloat16
    dma = pltpu.SemaphoreType.DMA
    top = lags[0] + -lags[0] % 16
    rtop = lags[1] + -lags[1] % 16
    part = planes // 2
    deep = planes * 4 * depth

    def vmem(*shape, dtype=bf16):
        return pltpu.VMEM(shape, dtype)

    def wide(*shape):
        return pltpu.VMEM(shape, f32)

    return pl.pallas_call(
        functools.partial(layer_kernel, planes, lags),
        out_shape=jax.ShapeDtypeStruct((rows, planes * 4 * cols), bf16),
        in_specs=[ANY] * 16,
        out_specs=ANY,
        scratch_shapes=[
            vmem(rows, width_in), wide(1, width_in), vmem(*rin_w.shape), vmem(*rgate_w.shape),
            vmem(4, depth, 2 * rwid), vmem(4, depth, 2 * cw),
            vmem(*taps.shape), wide(1, 4 * cw), wide(1, 4 * cw), vmem(*staps.shape),
            vmem(*dmap.shape), vmem(*imap.shape), wide(4 * rwid), wide(*jump.shape),
            vmem(4, jump.shape[0] // 2, 2 * rwid), wide(lags[0] + 3 + -(lags[0] + 3) % 8, cw), wide(8, rwid),
            vmem(length, width_in),
            vmem(deep, 2 * rwid),
            vmem(deep, 2 * cw),
            vmem(length, 2 * rwid),
            vmem(4, jump.shape[0] // 2, 2 * rwid),
            vmem(planes, 4 * used, cols),
            vmem(part, 4 * used, cols),
            vmem(length, 8 * used),
            vmem(length // 2, 16 * minor),
            wide(length, 2 * cw),
            vmem(8, part, rows, cols),
            wide(top + length, cw),
            wide(rtop + length, rwid),
            wide(length, cw),
            wide(fold, length + 8 * SEGMENTS, 128),
            wide(fold, length + 8 * SEGMENTS, 128),
            vmem(rwid, 2 * fold * 128),
            wide(cw, length),
            wide(8, 2, length),
            wide(8, 128),
            wide(planes, 8, 128),
            dma((POOL,)), dma((4, 4)), dma((4, 4)), dma((4,)), dma((4,)),
            dma((part, planes, 4)), dma((planes, OUT_PARTS)), dma((4,)),
            dma((part, 4, 4)), dma((4, 2)), dma((4, 2)), dma((part, OUT_PARTS)),
            dma((2,)), dma((8,)), dma((planes,)),
        ],
        compiler_params=pltpu.CompilerParams(
            collective_id=0, has_side_effects=True, vmem_limit_bytes=60 * 1024 * 1024
        ),
    )(
        tokens, norm_gain[None], val_w, gate_w, rgate_w, rin_w, taps, bias[None], cgain[None], staps,
        dmap, imap, rbase, jump, ocw, orw,
    )


def plane_shards(
    planes,
    tokens,
    norm_gain,
    conv_val_w,
    conv_gate_w,
    rec_gate_w,
    rec_in_w,
    conv_taps,
    conv_bias,
    conv_gain,
    short_taps,
    decay_map,
    input_map,
    decay_base,
    decay_jump,
    out_conv_w,
    out_rec_w,
):
    lags = (conv_taps.shape[0] - 1, short_taps.shape[0] - 1)
    return handed_out(layer(
        planes, lags, tokens, norm_gain, conv_val_w, conv_gate_w, rec_gate_w, rec_in_w, conv_taps, conv_bias,
        conv_gain, short_taps, decay_map, input_map, decay_base, decay_jump, out_conv_w, out_rec_w,
    ))


def solution(mesh):
    in_specs = (
        P(("sp", "tp"), None),
        P(),
        P("sp", "tp"),
        P("sp", "tp"),
        P("sp", "tp"),
        P("sp", "tp"),
        P(None, "tp"),
        P("tp"),
        P("tp"),
        P(None, "tp"),
        P("tp", None, None),
        P("tp", None, None),
        P("tp"),
        P("sp", "tp"),
        P("tp", "sp"),
        P("tp", "sp"),
    )
    out_specs = P(("sp", "tp"), None)
    count = mesh.shape["sp"]
    planar = mesh.shape["tp"] == 2 and count % 8 == 0 and count >= 16
    body = functools.partial(plane_shards, count // 4) if planar else shards
    return jax.shard_map(body, mesh=mesh, in_specs=in_specs, out_specs=out_specs, check_vma=False)
```

```python
import functools

import jax
import jax.numpy as jnp
from jax import lax
from jax.experimental import pallas as pl
from jax.experimental.pallas import tpu as pltpu
from jax.sharding import PartitionSpec as P

CONV_WIDTH = 1024


RATE_SCALE = 8.0


def passed_along(value, axis, by):
    count = lax.axis_size(axis)
    pairs = [(i, i + by) for i in range(count) if 0 <= i + by < count]
    return lax.ppermute(value, axis, pairs)


def prefix(part, axis, combine, identity):
    place = lax.axis_index(axis)
    gathered = jax.tree.map(lambda a: lax.all_gather(a, axis), part)
    state = jax.tree.map(lambda a, e: jnp.zeros_like(a) + jnp.asarray(e, a.dtype), part, identity)

    def one(step, state):
        return combine(
            state, jax.tree.map(lambda a: lax.dynamic_index_in_dim(a, step, 0, False), gathered)
        )

    return lax.fori_loop(0, place, one, state)


def norm_rows(values, gain):
    widened = values.astype(jnp.float32)
    inverse = lax.rsqrt(jnp.mean(widened * widened, axis=-1, keepdims=True) + 1e-06)
    return (widened * inverse * gain).astype(jnp.bfloat16)


def causal_window(edge, current, weights):
    extended = jnp.concatenate([edge, current], axis=0).astype(jnp.float32)
    taps_wide = weights.astype(jnp.float32)
    length = current.shape[0]
    result = jnp.zeros((length, current.shape[1]), jnp.float32)
    for lag_index in range(weights.shape[0]):
        result = result + taps_wide[lag_index][None, :] * extended[lag_index : lag_index + length]
    return result


def chain_step(earlier, latter):
    return (earlier[0] * latter[0], latter[0] * earlier[1] + latter[1])


def glu_of(conv_val, conv_gate):
    return (conv_val.astype(jnp.float32) * jax.nn.sigmoid(conv_gate.astype(jnp.float32))).astype(
        jnp.bfloat16
    )


def shards(
    tokens,
    norm_gain,
    conv_val_w,
    conv_gate_w,
    rec_gate_w,
    rec_in_w,
    conv_taps,
    conv_bias,
    conv_gain,
    short_taps,
    decay_map,
    input_map,
    decay_base,
    decay_jump,
    out_conv_w,
    out_rec_w,
):
    rec_cols = rec_in_w.shape[1]
    conv_lags = conv_taps.shape[0] - 1
    short_lags = short_taps.shape[0] - 1
    normed = norm_rows(tokens, norm_gain)
    val_full, gate_full = (
        lax.all_gather(conv_val_w, "sp", axis=0, tiled=True),
        lax.all_gather(conv_gate_w, "sp", axis=0, tiled=True),
    )
    all_rows = lax.all_gather(normed, "tp", axis=0, tiled=True)
    conv_val = jnp.dot(all_rows, val_full, preferred_element_type=jnp.float32).astype(jnp.bfloat16)
    conv_gate = jnp.dot(all_rows, gate_full, preferred_element_type=jnp.float32).astype(
        jnp.bfloat16
    )
    glu = glu_of(conv_val, conv_gate)
    conv_edge = passed_along(glu[-conv_lags:], "sp", 1)
    rgate_full, rin_full = (
        lax.all_gather(rec_gate_w, "sp", axis=0, tiled=True),
        lax.all_gather(rec_in_w, "sp", axis=0, tiled=True),
    )
    rec_gate = jnp.dot(all_rows, rgate_full, preferred_element_type=jnp.float32).astype(
        jnp.bfloat16
    )
    rec_in = jnp.dot(all_rows, rin_full, preferred_element_type=jnp.float32).astype(jnp.bfloat16)
    rec_edge = passed_along(rec_in[-short_lags:], "sp", 1)
    filtered = causal_window(conv_edge, glu, conv_taps) + conv_bias[None, :]
    row_total = lax.psum(jnp.sum(filtered, axis=1), "tp")
    centered = filtered - (row_total / CONV_WIDTH)[:, None]
    spread = lax.psum(jnp.sum(centered * centered, axis=1), "tp") / CONV_WIDTH
    conv_out = jax.nn.silu(centered * lax.rsqrt(spread + 1e-05)[:, None] * conv_gain).astype(
        jnp.bfloat16
    )
    smoothed = causal_window(rec_edge, rec_in, short_taps).astype(jnp.bfloat16)
    length = smoothed.shape[0]
    grouped = smoothed.reshape(length, decay_map.shape[0], decay_map.shape[1])
    retain = jax.nn.sigmoid(
        jnp.einsum("thi,hio->tho", grouped, decay_map, preferred_element_type=jnp.float32).reshape(
            length, rec_cols
        )
    )
    admit = jax.nn.sigmoid(
        jnp.einsum("thi,hio->tho", grouped, input_map, preferred_element_type=jnp.float32).reshape(
            length, rec_cols
        )
    )
    log_decay = -RATE_SCALE * retain * jax.nn.softplus(-decay_base)[None, :] + decay_jump
    decay = jnp.exp(log_decay)
    inflow = jnp.sqrt(-jnp.expm1(2.0 * log_decay)) * admit * smoothed.astype(jnp.float32)
    products, local_state = lax.associative_scan(chain_step, (decay, inflow), axis=0)
    entering = prefix(
        (products[-1], local_state[-1]),
        "sp",
        chain_step,
        (jnp.ones((rec_cols,), jnp.float32), jnp.zeros((rec_cols,), jnp.float32)),
    )
    state = local_state + products * entering[1][None, :]
    rec_out = (jax.nn.gelu(rec_gate.astype(jnp.float32)) * state).astype(jnp.bfloat16)
    conv_full, rec_full = (
        lax.all_gather(out_conv_w, "sp", axis=1, tiled=True),
        lax.all_gather(out_rec_w, "sp", axis=1, tiled=True),
    )
    return lax.psum_scatter(
        (
            jnp.dot(conv_out, conv_full, preferred_element_type=jnp.float32)
            + jnp.dot(rec_out, rec_full, preferred_element_type=jnp.float32)
        ).astype(jnp.bfloat16),
        "tp",
        scatter_dimension=0,
        tiled=True,
    )


MESH = pl.DeviceIdType.MESH
ANY = pl.BlockSpec(memory_space=pl.ANY)
VMEM = pl.BlockSpec(memory_space=pltpu.VMEM)
SEGMENTS = 8


class Spot:
    def __init__(self, planes):
        self.s, self.c = lax.axis_index("sp"), lax.axis_index("tp")
        self.z, self.q = self.s // 4, self.s % 4
        self.qx = self.q + 1 - 2 * (self.q % 2)
        self.qy = (self.q + 2) % 4
        self.qd = 3 - self.q
        self.has_up, self.has_down = self.z < planes - 1, self.z > 0
        self.up, self.down = self.at(self.s + 4, self.c), self.at(self.s - 4, self.c)
        self.partner = self.at(self.s, 1 - self.c)

    def at(self, s, c):
        return {"sp": s, "tp": c}

    def mate(self, q):
        return self.at(self.z * 4 + q, self.c)


class Mail:
    def __init__(self, send_sem):
        self.send_sem, self.tag, self.open = send_sem, "early", []
        self.free = list(range(send_sem.shape[0]))

    def claim(self):
        self.free.sort()
        return self.free.pop(0)

    def send(self, src, dst, recv, device, when=None, index=None):
        index = self.claim() if index is None else index
        copy = pltpu.make_async_remote_copy(
            src_ref=src, dst_ref=dst, send_sem=self.send_sem.at[index],
            recv_sem=recv, device_id=device, device_id_type=MESH,
        )
        self.open.append((self.tag, index, copy.wait_send, when))
        if when is None:
            copy.start()
        else:
            pl.when(when)(copy.start)
        return index

    def load(self, src, dst):
        index = self.claim()
        copy = pltpu.make_async_copy(src, dst, self.send_sem.at[index])
        copy.start()
        return index, copy

    def loaded(self, copies):
        for index, copy in copies:
            copy.wait()
            self.free.append(index)

    def arrived(self, dst, recv, device):
        pltpu.make_async_remote_copy(
            src_ref=dst, dst_ref=dst, send_sem=self.send_sem.at[0],
            recv_sem=recv, device_id=device, device_id_type=MESH,
        ).wait_recv()

    def finish(self, *tags):
        done = [entry for entry in self.open if not tags or entry[0] in tags]
        self.open = [entry for entry in self.open if entry not in done]
        for _, index, wait, when in done:
            if when is None:
                wait()
            else:
                pl.when(when)(wait)
        self.free.extend({entry[1] for entry in done})


def greet(me, devices, line):
    barrier = pltpu.get_barrier_semaphore()
    for device in devices:
        pl.semaphore_signal(barrier, inc=1, device_id=device, device_id_type=MESH)
    amount = len(devices)
    if line:
        for has, device in ((me.has_up, me.up), (me.has_down, me.down)):
            @pl.when(has)
            def _():
                pl.semaphore_signal(barrier, inc=1, device_id=device, device_id_type=MESH)
        amount = amount + me.has_up.astype(jnp.int32) + me.has_down.astype(jnp.int32)
    pl.semaphore_wait(barrier, amount)


class PlaneGather:
    def __init__(self, me, mail, slot, recv, recv_pair):
        self.me, self.mail, self.slot = me, mail, slot
        self.recv, self.recv_pair = recv, recv_pair
        self.parts = recv.shape[1]
        self.half = self.parts // 2

    def start(self):
        me, mail = self.me, self.mail
        for h in range(self.parts):
            for q, part in ((me.qx, h), (me.qy, (h + self.half) % self.parts)):
                own = self.slot(me.q, me.c, part)
                mail.send(own, own, self.recv.at[me.q, part], me.mate(q))
        for part in range(self.parts):
            self.share(me.q, part, self.slot(me.q, me.c, part))

    def took(self, q, part):
        here = self.slot(q, self.me.c, part)
        self.mail.arrived(here, self.recv.at[q, part], self.me.partner)
        return here

    def share(self, q, part, here):
        self.mail.send(here, here, self.recv_pair.at[q, part], self.me.partner)

    def first(self, i):
        me = self.me
        for q, part, to in ((me.qx, i, me.qy), (me.qy, self.half + i, me.qx)):
            here = self.took(q, part)
            self.mail.send(here, here, self.recv.at[q, part], me.mate(to))
            self.share(q, part, here)

    def second(self):
        for i in range(self.half):
            for q, part in ((self.me.qx, self.half + i), (self.me.qy, i)):
                self.share(q, part, self.took(q, part))

    def third(self, i):
        for part in (i, self.half + i):
            self.share(self.me.qd, part, self.took(self.me.qd, part))

    def paired(self, q, part):
        me = self.me
        self.mail.arrived(self.slot(q, 1 - me.c, part), self.recv_pair.at[q, part], me.partner)

    def last(self, origins):
        for q in origins:
            for part in range(self.parts):
                self.paired(q, part)


class RowGather(PlaneGather):
    def start(self):
        me, mail = self.me, self.mail
        for to_x, to_y in ((me.qx, me.qy), (me.q, me.qd), (me.qd, me.q), (me.qy, me.qx)):
            for q, part in ((me.qx, to_x), (me.qy, to_y)):
                own = self.slot(me.q, me.c, part)
                mail.send(own, own, self.recv.at[me.q, part], me.mate(q))
        for part in range(self.parts):
            self.share(me.q, part, self.slot(me.q, me.c, part))

    def first(self, i):
        me = self.me
        part = (me.q, me.qx)[i]
        for q, to in ((me.qx, me.qy), (me.qy, me.qx)):
            here = self.took(q, part)
            self.mail.send(here, here, self.recv.at[q, part], me.mate(to))
            self.share(q, part, here)

    def second(self):
        me = self.me
        for part in (me.qd, me.qy):
            for q in (me.qx, me.qy):
                self.share(q, part, self.took(q, part))

    def third(self, i):
        me = self.me
        for part in ((me.qx, me.qy), (me.q, me.qd))[i]:
            self.share(me.qd, part, self.took(me.qd, part))


def one_minus_exp(y, grown):
    series = 1.0 + y * (1.0 / 5.0)
    for n in (4.0, 3.0, 2.0):
        series = 1.0 + y * (1.0 / n) * series
    return jnp.where(y > -0.25, -y * series, 1.0 - grown)


def gelu(v):
    return 0.5 * v * (1.0 + jnp.tanh(0.7978845608028654 * (v + 0.044715 * v * v * v)))


class Line:
    def __init__(self, me, mail, planes, slot, recv, seen=None):
        self.me, self.mail, self.planes = me, mail, planes
        self.slot, self.recv, self.seen = slot, recv, seen

    def own(self, piece, src, up=True, down=True):
        me = self.me
        for wanted, has, device in ((up, me.has_up, me.up), (down, me.has_down, me.down)):
            if wanted is not False:
                self.post(src, me.z, piece, device, has & wanted)

    def post(self, src, origin, piece, device, when):
        self.mail.send(src, self.slot(origin, piece), self.recv.at[origin, piece], device, when)

    def mine(self, origin):
        return True

    def ways(self, k):
        me = self.me
        return (
            (me.z - k, me.z >= k, me.up, me.has_up),
            (me.z + k, me.z + k < self.planes, me.down, me.has_down),
        )

    def take(self, origin, piece, when, index=None):
        here, sem = self.slot(origin, piece), self.recv.at[origin, piece]
        pl.when(when)(functools.partial(self.mail.arrived, here, sem, self.me.partner))
        return None if self.seen is None else self.seen(origin, piece, when, index)

    def relay(self, k, piece, up=True, down=True):
        for wanted, (origin, there, on, more) in zip((up, down), self.ways(k)):
            if wanted:
                when = jnp.logical_and(there, more)
                here = self.slot(origin, piece)
                self.take(origin, piece, when)
                self.post(here, origin, piece, on, when)

    def await_up(self, k, piece):
        origin, there, _, more = self.ways(k)[0]
        return self.take(origin, piece, there & more)

    def forward_up(self, k, piece):
        origin, there, on, more = self.ways(k)[0]
        here, sem = self.slot(origin, piece), self.recv.at[origin, piece]
        self.mail.send(here, here, sem, on, there & more)

    def settle(self, k, piece):
        me = self.me
        lowest, highest = jnp.logical_not(me.has_down), jnp.logical_not(me.has_up)
        origin = jnp.where(lowest, me.z + k, me.z - k)
        here, sem = self.slot(origin, piece), self.recv.at[origin, piece]
        pl.when((lowest | highest) & self.mine(origin))(functools.partial(self.mail.arrived, here, sem, me.partner))


class OutLine(Line):
    def __init__(self, me, mail, planes, slot, recv, seen, other, other_recv):
        super().__init__(me, mail, planes, slot, recv, seen)
        self.other, self.other_recv = other, other_recv

    def mine(self, origin):
        return origin // (self.planes // 2) == self.me.c

    def post(self, src, origin, piece, device, when):
        me = self.me
        z = device["sp"] // 4
        ends = (z == 0) | (z == self.planes - 1)
        cross = ends & jnp.logical_not(self.mine(origin))
        here, sem = self.slot(origin, piece), self.recv.at[origin, piece]
        index = self.mail.send(src, here, sem, device, when & jnp.logical_not(cross))
        place = origin - (1 - me.c) * (self.planes // 2)
        sem = self.other_recv.at[place, piece]
        device = me.at(device["sp"], 1 - me.c)
        self.mail.send(src, self.other(place, piece), sem, device, when & cross, index)


def small_softplus(v):
    u = jnp.exp(-jnp.abs(v))
    series = jnp.zeros_like(u)
    for n in (8.0, 7.0, 6.0, 5.0, 4.0, 3.0, 2.0, 1.0):
        series = 1.0 / n - u * series
    return jnp.maximum(v, 0.0) + jnp.where(u < 0.1, u * series, jnp.log(1.0 + u))


OUT_PARTS = 4
POOL = 84


def layer_kernel(
    planes, lags, tokens, gain_in, val_w, gate_w, rgate_w, rin_w, taps_in, bias_in, cgain_in, staps_in,
    dmap_in, imap_in, base_in, jump_in, ocw, orw,
    out, x_ref, gain, rin_s, rgate_s, wr, wc, taps, bias, cgain, staps, dmap, imap, rbase, jump, jb, cpar, rpar,
    xall, rwall, cwall, projr, jall, wz, wp, yall, yrest, cacc, cbuf, gext, rext, filt, dec, inf, maps, ft,
    st_all, carry, cr_all,
    send, rx, rpx, rwr, rwc, zrc, zo, rj, rvq, re, rf, rw, rh, rs, rc,
):
    me = Spot(planes)
    mail = Mail(send)
    c_lags, s_lags = lags
    f32, bf16 = jnp.float32, jnp.bfloat16
    rows, depth = x_ref.shape[0], wr.shape[1]
    length = xall.shape[0]
    cw, rwid = gext.shape[1], rpar.shape[1]
    seg = length // SEGMENTS
    lane_seg = dec.shape[1] // SEGMENTS
    top = gext.shape[0] - length
    rtop = rext.shape[0] - length
    fold = dec.shape[0]
    part = planes // 2
    major = rwid // 128 * 128
    minor = rwid - major
    mine = me.q * 2 + me.c
    others = (me.qx, me.qy, me.qd)
    pieces = (me.q,) + others
    parts = tuple(range(OUT_PARTS))
    tall, half_cols = wz.shape[1] // 2, wz.shape[2] // 2

    def cut(p):
        return pl.ds(p % 2 * tall, tall), pl.ds(p // 2 * half_cols, half_cols)

    last = planes - 1
    mates = [me.at(me.z * 4 + (me.q + dq) % 4, c) for dq in range(4) for c in (me.c, 1 - me.c)][1:]
    lined = [me.at((me.s + 4 * k) % (4 * planes), me.c) for k in range(1, planes)]
    crossed = [me.at((me.s + 4 * k) % (4 * planes), 1 - me.c) for k in range(1, planes)]
    load = mail.load
    got_rec = [load(rin_w, rin_s), load(rgate_w, rgate_s)]
    got_x = [load(tokens, x_ref), load(gain_in, gain)]
    got_conv = []
    for q in range(4):
        got_conv.append(load(val_w.at[:, pl.ds(q * cw, cw)], wc.at[q, :, pl.ds(0, cw)]))
        got_conv.append(load(gate_w.at[:, pl.ds(q * cw, cw)], wc.at[q, :, pl.ds(cw, cw)]))
    got_out = []
    got_out.append(load(ocw, wz.at[me.z, pl.ds(0, 4 * cw)]))
    for q in range(4):
        at = 4 * cw + q * major
        got_out.append(load(orw.at[pl.ds(q * rwid, major)], wz.at[me.z, pl.ds(at, major)]))
        at = 4 * (cw + major) + q * minor
        got_out.append(load(orw.at[pl.ds(q * rwid + major, minor)], wz.at[me.z, pl.ds(at, minor)]))
    got_jump = [load(jump_in, jump)]
    got_small = [
        load(src, dst)
        for src, dst in (
            (taps_in, taps), (bias_in, bias), (cgain_in, cgain), (staps_in, staps),
            (dmap_in, dmap), (imap_in, imap), (base_in, rbase),
        )
    ]
    greet(me, mates + lined + crossed, False)
    mail.loaded(got_rec)
    for q in range(4):
        lanes = slice(q * rwid, (q + 1) * rwid)
        wr[q] = jnp.concatenate([rin_s[:, lanes], rgate_s[:, lanes]], axis=1)

    def of_rows(ref):
        def slot(origin, piece):
            return ref.at[pl.ds(pl.multiple_of((origin * 4 + piece) * depth, depth), depth)]

        return slot

    def theirs_too(origin, piece, when, index=None):
        theirs = jnp.logical_and(origin // part != me.c, when)
        place = origin - (1 - me.c) * part
        here, there = wz.at[(origin, *cut(piece))], wp.at[(place, *cut(piece))]
        return mail.send(here, there, rw.at[place, piece], me.partner, theirs, index)

    rl = Line(me, mail, planes, of_rows(rwall), zrc.at[0])
    cl = Line(me, mail, planes, of_rows(cwall), zrc.at[1])
    ol = OutLine(
        me, mail, planes, lambda origin, p: wz.at[(origin, *cut(p))], zo, theirs_too,
        lambda place, p: wp.at[(place, *cut(p))], rw,
    )

    def out_own(p, up=True, down=True):
        ol.own(p, wz.at[(me.z, *cut(p))], up, down)

    mail.tag = "first"
    for q in others:
        mail.send(wr.at[q], rl.slot(me.z, me.q), rwr.at[me.q], me.mate(q))
    rl.own(me.q, wr.at[me.q])

    mail.loaded(got_x)
    first_row = mine * rows

    @pl.loop(0, rows // 16)
    def _(i):
        values = x_ref[pl.ds(pl.multiple_of(i * 16, 16), 16)].astype(f32)
        inverse = lax.rsqrt(jnp.mean(values * values, axis=1, keepdims=True) + 1e-06)
        place = pl.ds(pl.multiple_of(first_row + i * 16, 16), 16)
        xall[place] = (values * inverse * gain[...]).astype(bf16)

    part_rows = rows // rx.shape[1]

    def xslot(q, c, h):
        return xall.at[pl.ds(pl.multiple_of((q * 2 + c) * rows + h * part_rows, 16), part_rows)]

    xg = PlaneGather(me, mail, xslot, rx, rpx)
    xg.start()
    mail.loaded(got_conv + got_out)
    for q in others:
        mail.send(wc.at[q], cl.slot(me.z, me.q), rwc.at[me.q], me.mate(q))
    cl.own(me.q, wc.at[me.q])
    out_own(0)
    mail.loaded([load(wr.at[me.q], rl.slot(me.z, me.q)), load(wc.at[me.q], cl.slot(me.z, me.q))])
    for p in parts:
        theirs_too(me.z, p, True)
    mail.loaded(got_jump + got_small)
    half = jump.shape[0] // 2
    for q in range(4):
        lanes = slice(q * rwid, (q + 1) * rwid)
        jb[q] = jnp.concatenate([jump[:half, lanes], jump[half:, lanes]], axis=1).astype(bf16)
    jall[me.q] = jb[me.q]
    own_lanes = pl.ds(pl.multiple_of(me.q * cw, 128), cw)
    cpar[pl.ds(0, c_lags + 1)] = taps[:, own_lanes].astype(f32)
    cpar[pl.ds(c_lags + 1, 1)] = bias[:, own_lanes]
    cpar[pl.ds(c_lags + 2, 1)] = cgain[:, own_lanes]
    window = -(-rwid // 128) * 128
    wide_lanes = pl.ds(pl.multiple_of(me.q * rwid // 128 * 128, 128), window)

    def own_rec(values):
        moved = values[:, :rwid]
        for lead in sorted({q * rwid % 128 for q in range(4)} - {0}):
            moved = jnp.where(me.q * rwid % 128 == lead, values[:, lead : lead + rwid], moved)
        return moved

    rpar[pl.ds(0, s_lags + 1)] = own_rec(staps[:, wide_lanes].astype(f32))
    rpar[pl.ds(s_lags + 1, 1)] = own_rec(RATE_SCALE * small_softplus(-rbase[wide_lanes][None]))

    maps[...] = jnp.zeros_like(maps)
    size = dmap.shape[1]
    heads = rwid // size
    for h in range(heads):
        spot = pl.ds(h * size, size)
        maps[spot, pl.ds(h * size, size)] = dmap[me.q * heads + h]
        maps[spot, pl.ds(fold * 128 + h * size, size)] = imap[me.q * heads + h]

    for q in others:
        here = rl.slot(me.z, q)
        mail.arrived(here, rwr.at[q], me.partner)
        rl.own(q, here)
    for p in pieces:
        rl.relay(1, p)
    mail.tag = "early"
    for i in range(xg.half):
        xg.first(i)
    for q in others:
        mail.send(jb.at[q], jall.at[me.q], rj.at[me.q], me.mate(q))
    for k in range(2, last):
        for p in pieces:
            rl.relay(k, p)
    xg.second()
    for q in others:
        here = cl.slot(me.z, q)
        mail.arrived(here, rwc.at[q], me.partner)
        cl.own(q, here)
    for k in range(1, planes):
        for p in pieces:
            rl.settle(k, p)
    xg.last(pieces[:3])

    tile = length // 4

    def project_rec(begin, size):
        at = pl.ds(pl.multiple_of(begin, 64), size)
        product = jnp.dot(xall[at], rwall[...], preferred_element_type=f32).astype(bf16)
        projr[at] = product
        rext[pl.ds(pl.multiple_of(begin + rtop, 16), size)] = product[:, :rwid].astype(f32)

    @pl.loop(0, 3)
    def _(i):
        project_rec(((me.q // 2 + i // 2) % 2 * 2 + (me.q % 2 + i % 2) % 2) * tile, tile)

    mail.tag = "conv"
    for n, p in enumerate(pieces):
        cl.relay(1, p, n < 2, True)
    mail.tag = "early"
    for i in range(xg.half):
        xg.third(i)
    softened = rpar[pl.ds(s_lags + 1, 1), :]

    def gate_segment(n):
        step = (n + 1) // 2
        ring = (me.q // 2 + step % 4 // 2) % 2 * 2 + (me.q % 2 + step % 2) % 2
        i = jnp.where(n == SEGMENTS - 1, 2 * me.q, 2 * ring + n % 2)
        i = jnp.where(n == 0, 2 * me.q + 1, i)

        @pl.when(jnp.logical_and(i == 0, me.has_down))
        def _():
            mail.arrived(rext.at[pl.ds(0, rtop)], rh.at[0], me.partner)

        @pl.when(jnp.logical_and(n % 2 == 1, n < SEGMENTS - 1))
        def _():
            mail.arrived(jall.at[i // 2], rj.at[i // 2], me.partner)

        base = pl.multiple_of(i * seg, 8)
        window = rext[pl.ds(pl.multiple_of(base + rtop - 8, 8), seg + 8)]
        smooth = jnp.zeros((seg, rwid), f32)
        for k in range(s_lags + 1):
            smooth = smooth + rpar[pl.ds(k, 1), :] * window[8 - s_lags + k : 8 - s_lags + k + seg]
        smooth = smooth.astype(bf16)
        gates = jax.nn.sigmoid(jnp.dot(smooth, maps[...], preferred_element_type=f32))
        retain, admit = gates[:, :rwid], gates[:, fold * 128 : fold * 128 + rwid]
        wide = jall[i // 2].astype(f32)
        moved = jnp.where(i % 2 == 0, wide[:, :rwid], wide[:, rwid:])
        log_decay = moved - retain * softened
        decay = jnp.exp(log_decay)
        inflow = jnp.sqrt(one_minus_exp(log_decay, decay) * (1.0 + decay)) * admit * smooth.astype(f32)
        for f in range(fold):
            w = min(128, rwid - f * 128)
            spot = pl.ds(pl.multiple_of(i * lane_seg, 8), seg)
            dec[f, spot, pl.ds(0, w)] = decay[:, f * 128 : f * 128 + w]
            inf[f, spot, pl.ds(0, w)] = inflow[:, f * 128 : f * 128 + w]

    mail.finish("first")
    project_rec((me.qd * 2 + me.c) * rows, rows)
    pl.loop(0, 1)(gate_segment)
    xg.last(pieces[3:])
    project_rec((me.qd * 2 + 1 - me.c) * rows, rows)

    mail.tag = "conv"
    mail.send(rext.at[pl.ds(length, rtop)], rext.at[pl.ds(0, rtop)], rh.at[0], me.up, me.has_up)
    for p in pieces[2:]:
        cl.relay(1, p, True, False)
    for k in range(2, last):
        for p in pieces:
            cl.relay(k, p, False, True)

    @pl.when(jnp.logical_not(me.has_down))
    def _():
        rext[pl.ds(0, rtop)] = jnp.zeros((rtop, rwid), f32)
        gext[pl.ds(0, top)] = jnp.zeros((top, cw), f32)

    pl.loop(1, SEGMENTS)(gate_segment)

    def one(i, held):
        after = []
        for f in range(fold):
            at = pl.ds(i, SEGMENTS, stride=lane_seg)
            d = dec.at[f][at, :]
            product, state = held[2 * f] * d, held[2 * f + 1] * d + inf.at[f][at, :]
            dec.at[f][at, :] = product
            inf.at[f][at, :] = state
            after += [product, state]
        return tuple(after)

    flat = (SEGMENTS, 128)
    ends = lax.fori_loop(0, seg, one, (jnp.ones(flat, f32), jnp.zeros(flat, f32)) * fold, unroll=8)
    for f in range(fold):
        product, state = jnp.ones((1, 128), f32), jnp.zeros((1, 128), f32)
        for i in range(SEGMENTS):
            p, s = ends[2 * f][i : i + 1], ends[2 * f + 1][i : i + 1]
            product, state = product * p, p * state + s
        carry[pl.ds(2 * f, 1)] = product
        carry[pl.ds(2 * f + 1, 1)] = state
    for k in range(1, planes):
        mail.send(carry, cr_all.at[me.z], rc.at[me.z], lined[k - 1], me.z + k < planes)
    early = me.z < planes - 2
    for k in range(2, last):
        for p in pieces[:3]:
            cl.relay(k, p, True, False)
    mail.tag = "gather"
    for p in parts[1:]:
        out_own(p, early, True)
    mail.finish("early")

    for i in range(SEGMENTS):
        there = pl.ds(i * lane_seg, seg)
        factor = gelu(projr[pl.ds(i * seg, seg), pl.ds(rwid, rwid)].astype(f32))
        for f in range(fold):
            w = min(128, rwid - f * 128)
            lanes = pl.ds(0, w)
            dec[f, there, lanes] = dec[f, there, lanes] * factor[:, f * 128 : f * 128 + w]
            inf[f, there, lanes] = inf[f, there, lanes] * factor[:, f * 128 : f * 128 + w]

    for k in range(1, planes):
        z = me.z - k
        pl.when(z >= 0)(functools.partial(mail.arrived, cr_all.at[z], rc.at[z], me.partner))
    entering = []
    for f in range(fold):
        held = jnp.zeros((1, 128), f32)
        for j in range(planes - 1):
            after = cr_all[j, pl.ds(2 * f, 1)] * held + cr_all[j, pl.ds(2 * f + 1, 1)]
            held = jnp.where(j < me.z, after, held)
        for i in range(SEGMENTS):
            entering.append(held)
            held = ends[2 * f][i : i + 1] * held + ends[2 * f + 1][i : i + 1]
    placed = me.c * 4 + me.q

    def rec_result(i):
        here, there = pl.ds(i * seg, seg), pl.ds(i * lane_seg, seg)
        state = [dec[f, there] * entering[f * SEGMENTS + i] + inf[f, there] for f in range(fold)]
        result = jnp.concatenate(state, axis=1)[:, :rwid].astype(bf16)
        yall[here, pl.ds(pl.multiple_of(8 * cw + placed * major, 128), major)] = result[:, :major]
        return result[:, major:]

    for i in range(SEGMENTS // 2):
        pair = jnp.concatenate([rec_result(i), rec_result(i + SEGMENTS // 2)], axis=1)
        yrest[pl.ds(i * seg, seg), pl.ds(pl.multiple_of(placed * 2 * minor, 128), 2 * minor)] = pair

    def gather(buffer, lane, lanes, recv, recv_pair, kind=PlaneGather):
        tall_part = buffer.shape[0] // recv.shape[1]

        def slot(q, c, h):
            spot = pl.ds(pl.multiple_of(lane + (c * 4 + q) * lanes, 128), lanes)
            return buffer.at[pl.ds(pl.multiple_of(h * tall_part, 16), tall_part), spot]

        return kind(me, mail, slot, recv, recv_pair)

    mg = gather(yall, 8 * cw, major, rvq.at[0], rvq.at[1])
    eg = gather(yrest, 0, 2 * minor, re, rf)
    yg = gather(yall, 0, cw, rx, rpx, RowGather)
    mail.tag = "conv"
    mg.start()
    eg.start()
    mail.tag = "gather"
    for k in range(1, last):
        for p in pieces:
            cl.settle(k, p)
        for p in pieces[3:] if k > 1 else ():
            cl.await_up(k, p)
    plane_depth = 4 * depth
    is_last = (me.z == last).astype(jnp.int32)

    def conv_product(at, begin, size):
        deep = pl.ds(pl.multiple_of(begin, plane_depth), size)
        return jnp.dot(xall[at, deep], cwall[deep], preferred_element_type=f32)

    @pl.loop(0, 4)
    def _(i):
        at = pl.ds(pl.multiple_of(i * tile, tile), tile)
        cacc[at] = conv_product(at, is_last * plane_depth, last * plane_depth)

    middle = me.has_up & me.has_down

    def finish_conv(when):
        @pl.when(when)
        def _():
            @pl.loop(0, 4)
            def _(i):
                at = pl.ds(pl.multiple_of(i * tile, tile), tile)
                product = cacc[at] + conv_product(at, (1 - is_last) * last * plane_depth, plane_depth)
                product = product.astype(bf16).astype(f32)
                glu = (product[:, :cw] * jax.nn.sigmoid(product[:, cw:])).astype(bf16).astype(f32)
                gext[pl.ds(pl.multiple_of(i * tile + top, 8), tile)] = glu

        tail_rows = gext.at[pl.ds(length, top)]
        mail.send(tail_rows, gext.at[pl.ds(0, top)], rh.at[1], me.up, me.has_up & when)

    finish_conv(middle)
    for k in range(2, last):
        for p in pieces[3:]:
            cl.forward_up(k, p)
    for p in parts[1:]:
        out_own(p, jnp.logical_not(early), False)
    mg.first(0)
    for p in pieces:
        cl.settle(last, p)
    finish_conv(jnp.logical_not(middle))
    strips = length // 64

    def filter_strip(n):
        i = strips - 1 - n

        @pl.when(jnp.logical_and(i == 0, me.has_down))
        def _():
            mail.arrived(gext.at[pl.ds(0, top)], rh.at[1], me.partner)

        base = pl.multiple_of(i * 64, 8)
        window = gext[pl.ds(base, 64 + top)]
        total = jnp.zeros((64, cw), f32) + cpar[pl.ds(c_lags + 1, 1), :]
        for r in range(8):
            ks = [k for k in range(c_lags + 1) if (top - c_lags + k) % 8 == r]
            span = 64 + (8 if r else 0)
            shifted = jnp.zeros((span, cw), f32)
            for k in ks:
                begin = (top - c_lags + k) // 8 * 8
                shifted = shifted + cpar[pl.ds(k, 1), :] * window[begin : begin + span]
            total = total + shifted[r : r + 64]
        filt[pl.ds(base, 64)] = total

    pl.loop(0, strips)(filter_strip)

    turned = filt[...].T
    ft[...] = turned
    part_sum = jnp.sum(turned, axis=0, keepdims=True)
    off = turned - part_sum * (1.0 / cw)
    st_all[mine, pl.ds(0, 1)] = part_sum
    st_all[mine, pl.ds(1, 1)] = jnp.sum(off * off, axis=0, keepdims=True)
    for device in mates:
        mail.send(st_all.at[mine], st_all.at[mine], rs.at[mine], device)
    for i in range(1, mg.half):
        mg.first(i)
    for i in range(eg.half):
        eg.first(i)
    mail.tag = "out"
    for p in parts:
        ol.relay(1, p)
    mail.tag = "gather"
    mail.finish("conv")

    for k in range(1, 8):
        d = (mine + k) % 8
        mail.arrived(st_all.at[d], rs.at[d], me.partner)
    total = sum(st_all[d, 0:1, :] for d in range(8))
    mean = total * (1.0 / (8 * cw))
    spread = jnp.zeros_like(mean)
    for d in range(8):
        shift = st_all[d, 0:1, :] * (1.0 / cw) - mean
        spread = spread + st_all[d, 1:2, :] + cw * shift * shift
    scale = lax.rsqrt(spread * (1.0 / (8 * cw)) + 1e-05)
    gain_col = jnp.broadcast_to(cpar[pl.ds(c_lags + 2, 1), :], (8, cw)).T[:, 0:1]
    v = (ft[...] - mean) * scale * gain_col
    yall[:, pl.ds(pl.multiple_of(placed * cw, 128), cw)] = (v * jax.nn.sigmoid(v)).T.astype(bf16)
    mail.tag = "begun"
    yg.start()
    mail.tag = "share"
    mg.second()
    eg.second()
    for g in (mg, eg):
        for i in range(g.half):
            g.third(i)
    mail.tag = "last"
    mail.finish("gather")
    for i in range(yg.half):
        yg.first(i)
    for k in range(2, last):
        for p in parts:
            ol.relay(k, p)
    mg.last(pieces)
    eg.last(pieces)
    mail.finish("share")
    rest_at = 8 * (cw + major)

    @pl.loop(0, SEGMENTS // 2)
    def _(i):
        values = yrest[pl.ds(pl.multiple_of(i * seg, 16), seg)]
        low = [values[:, j * 2 * minor : j * 2 * minor + minor] for j in range(8)]
        high = [values[:, j * 2 * minor + minor : (j + 1) * 2 * minor] for j in range(8)]
        for begin, chosen in ((0, low), (length // 2, high)):
            here = pl.ds(pl.multiple_of(begin + i * seg, 16), seg)
            yall[here, pl.ds(rest_at, 8 * minor)] = jnp.concatenate(chosen, axis=1)

    yg.second()
    yg.third(0)
    for k in range(1, last):
        for p in parts:
            ol.settle(k, p)

    cols = wz.shape[2]
    upward = me.z < part

    def lanes_of(h):
        return pl.ds(0, cols) if h is None else pl.ds(h * half_cols, half_cols)

    def summed(q, k, h, low, high):
        here = pl.ds(pl.multiple_of(q * 2 * rows, 16), 2 * rows)
        total = jnp.zeros((2 * rows, cols if h is None else half_cols), f32)
        for c, block in ((me.c, wz.at[me.c * part + k]), (1 - me.c, wp.at[k])):
            begin = 0
            for at, lanes in ((0, 4 * cw), (8 * cw, 4 * major), (rest_at, 4 * minor)):
                first, end = max(begin, low), min(begin + lanes, high)
                if first < end:
                    spot = pl.multiple_of(at + c * lanes + first - begin, 128)
                    right = block[pl.ds(first, end - first), lanes_of(h)]
                    left_part = yall[here, pl.ds(spot, end - first)]
                    total = total + jnp.dot(left_part, right, preferred_element_type=f32)
                begin = begin + lanes
        return here, total

    def multiply(q, k, h):
        here, total = summed(q, k, h, tall if h == 1 else 0, 2 * tall)
        if h == 1:
            total = total + cacc[here, pl.ds(0, half_cols)]
        total = total.astype(bf16)
        for c in range(2):
            cbuf[q * 2 + c, k, :, lanes_of(h)] = total[c * rows : (c + 1) * rows]

    def place(q, c, k, h):
        at = ((c * part + k) * 4 + q) * cols + (0 if h is None else h * half_cols)
        return out.at[:, pl.ds(pl.multiple_of(at, 128), cols if h is None else half_cols)]

    def mate_of(i):
        flip = 3 - i
        return (me.q // 2 + flip // 2) % 2 * 2 + (me.q % 2 + flip % 2) % 2

    mail.finish("begun")

    def left(d, k, h):
        return rvq.at[k, d // 2, d % 2 * 2 + (h or 0)]

    def landed(d, k, h):
        return zrc.at[k, d // 2, d % 2 * 2 + (h or 0)]

    def parcel(q, c, k, h):
        return pltpu.make_async_remote_copy(
            src_ref=cbuf.at[q * 2 + c, k, :, lanes_of(h)], dst_ref=place(me.q, me.c, k, h),
            send_sem=left(q * 2 + c, k, h), recv_sem=landed(mine, k, h),
            device_id=me.at(me.z * 4 + q, c), device_id_type=MESH,
        )

    def kept(k, h):
        src = cbuf.at[mine, k, :, lanes_of(h)]
        return pltpu.make_async_copy(src, place(me.q, me.c, k, h), left(mine, k, h))

    def serve(q, k, h):
        multiply(q, k, h)
        pl.when(q != me.q)(lambda: parcel(q, me.c, k, h).start())
        parcel(q, 1 - me.c, k, h).start()
        pl.when(q == me.q)(lambda: kept(k, h).start())

    def ready(k, ps):
        for p in ps:
            mail.arrived(wp.at[(k, *cut(p))], rw.at[k, p], me.partner)

    order = [jnp.where(upward, n, part - 1 - n) for n in range(part)]
    ready(order[0], parts)
    for i in range(yg.half):
        if i:
            yg.third(i)
        for q in pieces:
            for row_part in ((me.qx, me.qy), (me.q, me.qd))[i]:
                yg.paired(q, row_part)

        @pl.loop(0, 2)
        def _(n):
            serve(mate_of(3 - 3 * (1 - n) if i else 2 - n), order[0], None)

    for n in range(1, part - 1):
        ready(order[n], parts)
        pl.loop(0, 4)(lambda i: serve(mate_of(i), order[n], None))
    k_far = order[-1]
    for p in parts[:2]:
        ol.settle(last, p)
    ready(k_far, parts[:2])
    pl.loop(0, 4)(lambda i: serve(mate_of(i), k_far, 0))
    ol.settle(last, 2)
    ready(k_far, parts[2:3])

    @pl.loop(0, 4)
    def _(q):
        here, total = summed(q, k_far, 1, 0, tall)
        cacc[here, pl.ds(0, half_cols)] = total

    ol.settle(last, 3)
    ready(k_far, parts[3:])
    pl.loop(0, 4)(lambda i: serve(mate_of(i), k_far, 1))
    rounds = [(k, None) for k in order[:-1]] + [(order[-1], 0), (order[-1], 1)]

    @pl.loop(0, 4)
    def _(i):
        q = mate_of(i)
        for k, h in rounds:
            mail.arrived(place(q, 1 - me.c, k, h), landed(q * 2 + 1 - me.c, k, h), me.partner)
            parcel(q, 1 - me.c, k, h).wait_send()

    @pl.loop(0, 3)
    def _(i):
        q = mate_of(i)
        for k, h in rounds:
            mail.arrived(place(q, me.c, k, h), landed(q * 2 + me.c, k, h), me.partner)
            parcel(q, me.c, k, h).wait_send()

    for k, h in rounds:
        kept(k, h).wait()
    mail.finish()


def handed_out_kernel(src, dst, held, got, sent):
    count = got.shape[0]
    tall = src.shape[0] // count
    spots = [pl.ds(i * tall, tall) for i in range(count)]
    taken = [pltpu.make_async_copy(src.at[s], held.at[s], got.at[i]) for i, s in enumerate(spots)]
    given = [pltpu.make_async_copy(held.at[s], dst.at[s], sent.at[i]) for i, s in enumerate(spots)]
    for copy in taken:
        copy.start()
    for came, goes in zip(taken, given):
        came.wait()
        goes.start()
    for copy in given:
        copy.wait()


def handed_out(result):
    dma = pltpu.SemaphoreType.DMA
    return pl.pallas_call(
        handed_out_kernel,
        out_shape=jax.ShapeDtypeStruct(result.shape, result.dtype),
        in_specs=[ANY],
        out_specs=ANY,
        scratch_shapes=[pltpu.VMEM(result.shape, result.dtype), dma((6,)), dma((6,))],
    )(result)


def layer(planes, lags, tokens, norm_gain, val_w, gate_w, rgate_w, rin_w, taps, bias, cgain, staps, dmap, imap, rbase, jump, ocw, orw):
    rows, width_in = tokens.shape
    length = 8 * rows
    depth = rin_w.shape[0]
    cw, rwid = val_w.shape[1] // 4, rin_w.shape[1] // 4
    used, cols = cw + rwid, ocw.shape[1]
    minor = rwid % 128
    fold = (rwid + 127) // 128
    f32, bf16 = jnp.float32, jnp.bfloat16
    dma = pltpu.SemaphoreType.DMA
    top = lags[0] + -lags[0] % 16
    rtop = lags[1] + -lags[1] % 16
    part = planes // 2
    deep = planes * 4 * depth

    def vmem(*shape, dtype=bf16):
        return pltpu.VMEM(shape, dtype)

    def wide(*shape):
        return pltpu.VMEM(shape, f32)

    return pl.pallas_call(
        functools.partial(layer_kernel, planes, lags),
        out_shape=jax.ShapeDtypeStruct((rows, planes * 4 * cols), bf16),
        in_specs=[ANY] * 16,
        out_specs=ANY,
        scratch_shapes=[
            vmem(rows, width_in), wide(1, width_in), vmem(*rin_w.shape), vmem(*rgate_w.shape),
            vmem(4, depth, 2 * rwid), vmem(4, depth, 2 * cw),
            vmem(*taps.shape), wide(1, 4 * cw), wide(1, 4 * cw), vmem(*staps.shape),
            vmem(*dmap.shape), vmem(*imap.shape), wide(4 * rwid), wide(*jump.shape),
            vmem(4, jump.shape[0] // 2, 2 * rwid), wide(lags[0] + 3 + -(lags[0] + 3) % 8, cw), wide(8, rwid),
            vmem(length, width_in),
            vmem(deep, 2 * rwid),
            vmem(deep, 2 * cw),
            vmem(length, 2 * rwid),
            vmem(4, jump.shape[0] // 2, 2 * rwid),
            vmem(planes, 4 * used, cols),
            vmem(part, 4 * used, cols),
            vmem(length, 8 * used),
            vmem(length // 2, 16 * minor),
            wide(length, 2 * cw),
            vmem(8, part, rows, cols),
            wide(top + length, cw),
            wide(rtop + length, rwid),
            wide(length, cw),
            wide(fold, length + 8 * SEGMENTS, 128),
            wide(fold, length + 8 * SEGMENTS, 128),
            vmem(rwid, 2 * fold * 128),
            wide(cw, length),
            wide(8, 2, length),
            wide(8, 128),
            wide(planes, 8, 128),
            dma((POOL,)), dma((4, 4)), dma((4, 4)), dma((4,)), dma((4,)),
            dma((part, planes, 4)), dma((planes, OUT_PARTS)), dma((4,)),
            dma((part, 4, 4)), dma((4, 2)), dma((4, 2)), dma((part, OUT_PARTS)),
            dma((2,)), dma((8,)), dma((planes,)),
        ],
        compiler_params=pltpu.CompilerParams(
            collective_id=0, has_side_effects=True, vmem_limit_bytes=60 * 1024 * 1024
        ),
    )(
        tokens, norm_gain[None], val_w, gate_w, rgate_w, rin_w, taps, bias[None], cgain[None], staps,
        dmap, imap, rbase, jump, ocw, orw,
    )


def plane_shards(
    planes,
    tokens,
    norm_gain,
    conv_val_w,
    conv_gate_w,
    rec_gate_w,
    rec_in_w,
    conv_taps,
    conv_bias,
    conv_gain,
    short_taps,
    decay_map,
    input_map,
    decay_base,
    decay_jump,
    out_conv_w,
    out_rec_w,
):
    lags = (conv_taps.shape[0] - 1, short_taps.shape[0] - 1)
    return handed_out(layer(
        planes, lags, tokens, norm_gain, conv_val_w, conv_gate_w, rec_gate_w, rec_in_w, conv_taps, conv_bias,
        conv_gain, short_taps, decay_map, input_map, decay_base, decay_jump, out_conv_w, out_rec_w,
    ))


def solution(mesh):
    in_specs = (
        P(("sp", "tp"), None),
        P(),
        P("sp", "tp"),
        P("sp", "tp"),
        P("sp", "tp"),
        P("sp", "tp"),
        P(None, "tp"),
        P("tp"),
        P("tp"),
        P(None, "tp"),
        P("tp", None, None),
        P("tp", None, None),
        P("tp"),
        P("sp", "tp"),
        P("tp", "sp"),
        P("tp", "sp"),
    )
    out_specs = P(("sp", "tp"), None)
    count = mesh.shape["sp"]
    planar = mesh.shape["tp"] == 2 and count % 8 == 0 and count >= 16
    body = functools.partial(plane_shards, count // 4) if planar else shards
    return jax.shard_map(body, mesh=mesh, in_specs=in_specs, out_specs=out_specs, check_vma=False)
```

```python
import functools

import jax
import jax.numpy as jnp
from jax import lax
from jax.experimental import pallas as pl
from jax.experimental.pallas import tpu as pltpu
from jax.sharding import PartitionSpec as P

CONV_WIDTH = 1024


RATE_SCALE = 8.0


def passed_along(value, axis, by):
    count = lax.axis_size(axis)
    pairs = [(i, i + by) for i in range(count) if 0 <= i + by < count]
    return lax.ppermute(value, axis, pairs)


def prefix(part, axis, combine, identity):
    place = lax.axis_index(axis)
    gathered = jax.tree.map(lambda a: lax.all_gather(a, axis), part)
    state = jax.tree.map(lambda a, e: jnp.zeros_like(a) + jnp.asarray(e, a.dtype), part, identity)

    def one(step, state):
        return combine(
            state, jax.tree.map(lambda a: lax.dynamic_index_in_dim(a, step, 0, False), gathered)
        )

    return lax.fori_loop(0, place, one, state)


def norm_rows(values, gain):
    widened = values.astype(jnp.float32)
    inverse = lax.rsqrt(jnp.mean(widened * widened, axis=-1, keepdims=True) + 1e-06)
    return (widened * inverse * gain).astype(jnp.bfloat16)


def causal_window(edge, current, weights):
    extended = jnp.concatenate([edge, current], axis=0).astype(jnp.float32)
    taps_wide = weights.astype(jnp.float32)
    length = current.shape[0]
    result = jnp.zeros((length, current.shape[1]), jnp.float32)
    for lag_index in range(weights.shape[0]):
        result = result + taps_wide[lag_index][None, :] * extended[lag_index : lag_index + length]
    return result


def chain_step(earlier, latter):
    return (earlier[0] * latter[0], latter[0] * earlier[1] + latter[1])


def glu_of(conv_val, conv_gate):
    return (conv_val.astype(jnp.float32) * jax.nn.sigmoid(conv_gate.astype(jnp.float32))).astype(
        jnp.bfloat16
    )


def shards(
    tokens,
    norm_gain,
    conv_val_w,
    conv_gate_w,
    rec_gate_w,
    rec_in_w,
    conv_taps,
    conv_bias,
    conv_gain,
    short_taps,
    decay_map,
    input_map,
    decay_base,
    decay_jump,
    out_conv_w,
    out_rec_w,
):
    rec_cols = rec_in_w.shape[1]
    conv_lags = conv_taps.shape[0] - 1
    short_lags = short_taps.shape[0] - 1
    normed = norm_rows(tokens, norm_gain)
    val_full, gate_full = (
        lax.all_gather(conv_val_w, "sp", axis=0, tiled=True),
        lax.all_gather(conv_gate_w, "sp", axis=0, tiled=True),
    )
    all_rows = lax.all_gather(normed, "tp", axis=0, tiled=True)
    conv_val = jnp.dot(all_rows, val_full, preferred_element_type=jnp.float32).astype(jnp.bfloat16)
    conv_gate = jnp.dot(all_rows, gate_full, preferred_element_type=jnp.float32).astype(
        jnp.bfloat16
    )
    glu = glu_of(conv_val, conv_gate)
    conv_edge = passed_along(glu[-conv_lags:], "sp", 1)
    rgate_full, rin_full = (
        lax.all_gather(rec_gate_w, "sp", axis=0, tiled=True),
        lax.all_gather(rec_in_w, "sp", axis=0, tiled=True),
    )
    rec_gate = jnp.dot(all_rows, rgate_full, preferred_element_type=jnp.float32).astype(
        jnp.bfloat16
    )
    rec_in = jnp.dot(all_rows, rin_full, preferred_element_type=jnp.float32).astype(jnp.bfloat16)
    rec_edge = passed_along(rec_in[-short_lags:], "sp", 1)
    filtered = causal_window(conv_edge, glu, conv_taps) + conv_bias[None, :]
    row_total = lax.psum(jnp.sum(filtered, axis=1), "tp")
    centered = filtered - (row_total / CONV_WIDTH)[:, None]
    spread = lax.psum(jnp.sum(centered * centered, axis=1), "tp") / CONV_WIDTH
    conv_out = jax.nn.silu(centered * lax.rsqrt(spread + 1e-05)[:, None] * conv_gain).astype(
        jnp.bfloat16
    )
    smoothed = causal_window(rec_edge, rec_in, short_taps).astype(jnp.bfloat16)
    length = smoothed.shape[0]
    grouped = smoothed.reshape(length, decay_map.shape[0], decay_map.shape[1])
    retain = jax.nn.sigmoid(
        jnp.einsum("thi,hio->tho", grouped, decay_map, preferred_element_type=jnp.float32).reshape(
            length, rec_cols
        )
    )
    admit = jax.nn.sigmoid(
        jnp.einsum("thi,hio->tho", grouped, input_map, preferred_element_type=jnp.float32).reshape(
            length, rec_cols
        )
    )
    log_decay = -RATE_SCALE * retain * jax.nn.softplus(-decay_base)[None, :] + decay_jump
    decay = jnp.exp(log_decay)
    inflow = jnp.sqrt(-jnp.expm1(2.0 * log_decay)) * admit * smoothed.astype(jnp.float32)
    products, local_state = lax.associative_scan(chain_step, (decay, inflow), axis=0)
    entering = prefix(
        (products[-1], local_state[-1]),
        "sp",
        chain_step,
        (jnp.ones((rec_cols,), jnp.float32), jnp.zeros((rec_cols,), jnp.float32)),
    )
    state = local_state + products * entering[1][None, :]
    rec_out = (jax.nn.gelu(rec_gate.astype(jnp.float32)) * state).astype(jnp.bfloat16)
    conv_full, rec_full = (
        lax.all_gather(out_conv_w, "sp", axis=1, tiled=True),
        lax.all_gather(out_rec_w, "sp", axis=1, tiled=True),
    )
    return lax.psum_scatter(
        (
            jnp.dot(conv_out, conv_full, preferred_element_type=jnp.float32)
            + jnp.dot(rec_out, rec_full, preferred_element_type=jnp.float32)
        ).astype(jnp.bfloat16),
        "tp",
        scatter_dimension=0,
        tiled=True,
    )


MESH = pl.DeviceIdType.MESH
ANY = pl.BlockSpec(memory_space=pl.ANY)
VMEM = pl.BlockSpec(memory_space=pltpu.VMEM)
SEGMENTS = 8


class Spot:
    def __init__(self, planes):
        self.s, self.c = lax.axis_index("sp"), lax.axis_index("tp")
        self.z, self.q = self.s // 4, self.s % 4
        self.qx = self.q + 1 - 2 * (self.q % 2)
        self.qy = (self.q + 2) % 4
        self.qd = 3 - self.q
        self.has_up, self.has_down = self.z < planes - 1, self.z > 0
        self.up, self.down = self.at(self.s + 4, self.c), self.at(self.s - 4, self.c)
        self.partner = self.at(self.s, 1 - self.c)

    def at(self, s, c):
        return {"sp": s, "tp": c}

    def mate(self, q):
        return self.at(self.z * 4 + q, self.c)


class Mail:
    def __init__(self, send_sem):
        self.send_sem, self.tag, self.open = send_sem, "early", []
        self.free = list(range(send_sem.shape[0]))

    def claim(self):
        self.free.sort()
        return self.free.pop(0)

    def send(self, src, dst, recv, device, when=None, index=None):
        index = self.claim() if index is None else index
        copy = pltpu.make_async_remote_copy(
            src_ref=src, dst_ref=dst, send_sem=self.send_sem.at[index],
            recv_sem=recv, device_id=device, device_id_type=MESH,
        )
        self.open.append((self.tag, index, copy.wait_send, when))
        if when is None:
            copy.start()
        else:
            pl.when(when)(copy.start)
        return index

    def load(self, src, dst):
        index = self.claim()
        copy = pltpu.make_async_copy(src, dst, self.send_sem.at[index])
        copy.start()
        return index, copy

    def loaded(self, copies):
        for index, copy in copies:
            copy.wait()
            self.free.append(index)

    def arrived(self, dst, recv, device):
        pltpu.make_async_remote_copy(
            src_ref=dst, dst_ref=dst, send_sem=self.send_sem.at[0],
            recv_sem=recv, device_id=device, device_id_type=MESH,
        ).wait_recv()

    def finish(self, *tags):
        done = [entry for entry in self.open if not tags or entry[0] in tags]
        self.open = [entry for entry in self.open if entry not in done]
        for _, index, wait, when in done:
            if when is None:
                wait()
            else:
                pl.when(when)(wait)
        self.free.extend({entry[1] for entry in done})


def greet(me, devices, line):
    barrier = pltpu.get_barrier_semaphore()
    for device in devices:
        pl.semaphore_signal(barrier, inc=1, device_id=device, device_id_type=MESH)
    amount = len(devices)
    for has, neighbours in line:
        @pl.when(has)
        def _():
            for device in neighbours:
                pl.semaphore_signal(barrier, inc=1, device_id=device, device_id_type=MESH)
        amount = amount + len(neighbours) * has.astype(jnp.int32)
    pl.semaphore_wait(barrier, amount)


class PlaneGather:
    def __init__(self, me, mail, slot, recv, recv_pair):
        self.me, self.mail, self.slot = me, mail, slot
        self.recv, self.recv_pair = recv, recv_pair
        self.parts = recv.shape[1]
        self.half = self.parts // 2

    def start(self):
        me, mail = self.me, self.mail
        for h in range(self.parts):
            for q, part in ((me.qx, h), (me.qy, (h + self.half) % self.parts)):
                own = self.slot(me.q, me.c, part)
                mail.send(own, own, self.recv.at[me.q, part], me.mate(q))
        for part in range(self.parts):
            self.share(me.q, part, self.slot(me.q, me.c, part))

    def took(self, q, part):
        here = self.slot(q, self.me.c, part)
        self.mail.arrived(here, self.recv.at[q, part], self.me.partner)
        return here

    def share(self, q, part, here):
        self.mail.send(here, here, self.recv_pair.at[q, part], self.me.partner)

    def first(self, i):
        me = self.me
        for q, part, to in ((me.qx, i, me.qy), (me.qy, self.half + i, me.qx)):
            here = self.took(q, part)
            self.mail.send(here, here, self.recv.at[q, part], me.mate(to))
            self.share(q, part, here)

    def second(self):
        for i in range(self.half):
            for q, part in ((self.me.qx, self.half + i), (self.me.qy, i)):
                self.share(q, part, self.took(q, part))

    def third(self, i):
        for part in (i, self.half + i):
            self.share(self.me.qd, part, self.took(self.me.qd, part))

    def paired(self, q, part):
        me = self.me
        self.mail.arrived(self.slot(q, 1 - me.c, part), self.recv_pair.at[q, part], me.partner)

    def last(self, origins):
        for q in origins:
            for part in range(self.parts):
                self.paired(q, part)


class RowGather(PlaneGather):
    def start(self):
        me, mail = self.me, self.mail
        for to_x, to_y in ((me.qx, me.qy), (me.q, me.qd), (me.qd, me.q), (me.qy, me.qx)):
            for q, part in ((me.qx, to_x), (me.qy, to_y)):
                own = self.slot(me.q, me.c, part)
                mail.send(own, own, self.recv.at[me.q, part], me.mate(q))
        for part in range(self.parts):
            self.share(me.q, part, self.slot(me.q, me.c, part))

    def first(self, i):
        me = self.me
        part = (me.q, me.qx)[i]
        for q, to in ((me.qx, me.qy), (me.qy, me.qx)):
            here = self.took(q, part)
            self.mail.send(here, here, self.recv.at[q, part], me.mate(to))
            self.share(q, part, here)

    def second(self):
        me = self.me
        for part in (me.qd, me.qy):
            for q in (me.qx, me.qy):
                self.share(q, part, self.took(q, part))

    def third(self, i):
        me = self.me
        for part in ((me.qx, me.qy), (me.q, me.qd))[i]:
            self.share(me.qd, part, self.took(me.qd, part))


def one_minus_exp(y, grown):
    series = 1.0 + y * (1.0 / 5.0)
    for n in (4.0, 3.0, 2.0):
        series = 1.0 + y * (1.0 / n) * series
    return jnp.where(y > -0.25, -y * series, 1.0 - grown)


def gelu(v):
    return 0.5 * v * (1.0 + jnp.tanh(0.7978845608028654 * (v + 0.044715 * v * v * v)))


class Line:
    def __init__(self, me, mail, planes, slot, recv, seen=None):
        self.me, self.mail, self.planes = me, mail, planes
        self.slot, self.recv, self.seen = slot, recv, seen

    def own(self, piece, src, up=True, down=True):
        me = self.me
        for wanted, has, device in ((up, me.has_up, me.up), (down, me.has_down, me.down)):
            if wanted is not False:
                self.post(src, me.z, piece, device, has & wanted)

    def post(self, src, origin, piece, device, when):
        self.mail.send(src, self.slot(origin, piece), self.recv.at[origin, piece], device, when)

    def mine(self, origin):
        return True

    def ways(self, k):
        me = self.me
        return (
            (me.z - k, me.z >= k, me.up, me.has_up),
            (me.z + k, me.z + k < self.planes, me.down, me.has_down),
        )

    def take(self, origin, piece, when, index=None):
        here, sem = self.slot(origin, piece), self.recv.at[origin, piece]
        pl.when(when)(functools.partial(self.mail.arrived, here, sem, self.me.partner))
        return None if self.seen is None else self.seen(origin, piece, when, index)

    def relay(self, k, piece, up=True, down=True):
        for wanted, (origin, there, on, more) in zip((up, down), self.ways(k)):
            if wanted:
                when = jnp.logical_and(there, more)
                here = self.slot(origin, piece)
                self.take(origin, piece, when)
                self.post(here, origin, piece, on, when)

    def await_up(self, k, piece):
        origin, there, _, more = self.ways(k)[0]
        return self.take(origin, piece, there & more)

    def forward_up(self, k, piece):
        origin, there, on, more = self.ways(k)[0]
        here, sem = self.slot(origin, piece), self.recv.at[origin, piece]
        self.mail.send(here, here, sem, on, there & more)

    def settle(self, k, piece):
        me = self.me
        lowest, highest = jnp.logical_not(me.has_down), jnp.logical_not(me.has_up)
        origin = jnp.where(lowest, me.z + k, me.z - k)
        here, sem = self.slot(origin, piece), self.recv.at[origin, piece]
        pl.when((lowest | highest) & self.mine(origin))(functools.partial(self.mail.arrived, here, sem, me.partner))


class OutLine(Line):
    def __init__(self, me, mail, planes, slot, recv, seen, other, other_recv):
        super().__init__(me, mail, planes, slot, recv, seen)
        self.other, self.other_recv = other, other_recv

    def mine(self, origin):
        return origin // (self.planes // 2) == self.me.c

    def post(self, src, origin, piece, device, when):
        me = self.me
        z = device["sp"] // 4
        ends = (z == 0) | (z == self.planes - 1)
        cross = ends & jnp.logical_not(self.mine(origin))
        here, sem = self.slot(origin, piece), self.recv.at[origin, piece]
        index = self.mail.send(src, here, sem, device, when & jnp.logical_not(cross))
        place = origin - (1 - me.c) * (self.planes // 2)
        sem = self.other_recv.at[place, piece]
        device = me.at(device["sp"], 1 - me.c)
        self.mail.send(src, self.other(place, piece), sem, device, when & cross, index)


def small_softplus(v):
    u = jnp.exp(-jnp.abs(v))
    series = jnp.zeros_like(u)
    for n in (8.0, 7.0, 6.0, 5.0, 4.0, 3.0, 2.0, 1.0):
        series = 1.0 / n - u * series
    return jnp.maximum(v, 0.0) + jnp.where(u < 0.1, u * series, jnp.log(1.0 + u))


OUT_PARTS = 4
POOL = 84


def layer_kernel(
    planes, lags, tokens, gain_in, val_w, gate_w, rgate_w, rin_w, taps_in, bias_in, cgain_in, staps_in,
    dmap_in, imap_in, base_in, jump_in, ocw, orw,
    out, x_ref, gain, rin_s, rgate_s, wr, wc, taps, bias, cgain, staps, dmap, imap, rbase, jump, jb, cpar, rpar,
    xall, rwall, cwall, projr, jall, wz, wp, yall, yrest, cacc, cbuf, gext, rext, filt, dec, inf, maps, ft,
    st_all, carry, cr_all,
    send, rx, rpx, rwr, rwc, zrc, zo, rj, rvq, re, rf, rw, rh, rs, rc,
):
    me = Spot(planes)
    mail = Mail(send)
    c_lags, s_lags = lags
    f32, bf16 = jnp.float32, jnp.bfloat16
    rows, depth = x_ref.shape[0], wr.shape[1]
    length = xall.shape[0]
    cw, rwid = gext.shape[1], rpar.shape[1]
    seg = length // SEGMENTS
    lane_seg = dec.shape[1] // SEGMENTS
    top = gext.shape[0] - length
    rtop = rext.shape[0] - length
    fold = dec.shape[0]
    part = planes // 2
    major = rwid // 128 * 128
    minor = rwid - major
    mine = me.q * 2 + me.c
    others = (me.qx, me.qy, me.qd)
    pieces = (me.q,) + others
    parts = tuple(range(OUT_PARTS))
    tall, half_cols = wz.shape[1] // 2, wz.shape[2] // 2

    def cut(p):
        return pl.ds(p % 2 * tall, tall), pl.ds(p // 2 * half_cols, half_cols)

    last = planes - 1
    mates = [me.at(me.z * 4 + (me.q + dq) % 4, c) for dq in range(4) for c in (me.c, 1 - me.c)][1:]
    lined = [me.at((me.s + 4 * k) % (4 * planes), me.c) for k in range(1, planes)]
    load = mail.load
    got_rec = [load(rin_w, rin_s), load(rgate_w, rgate_s)]
    got_x = [load(tokens, x_ref), load(gain_in, gain)]
    got_conv = []
    for q in range(4):
        got_conv.append(load(val_w.at[:, pl.ds(q * cw, cw)], wc.at[q, :, pl.ds(0, cw)]))
        got_conv.append(load(gate_w.at[:, pl.ds(q * cw, cw)], wc.at[q, :, pl.ds(cw, cw)]))
    got_out = []
    got_out.append(load(ocw, wz.at[me.z, pl.ds(0, 4 * cw)]))
    for q in range(4):
        at = 4 * cw + q * major
        got_out.append(load(orw.at[pl.ds(q * rwid, major)], wz.at[me.z, pl.ds(at, major)]))
        at = 4 * (cw + major) + q * minor
        got_out.append(load(orw.at[pl.ds(q * rwid + major, minor)], wz.at[me.z, pl.ds(at, minor)]))
    got_jump = [load(jump_in, jump)]
    got_small = [
        load(src, dst)
        for src, dst in (
            (taps_in, taps), (bias_in, bias), (cgain_in, cgain), (staps_in, staps),
            (dmap_in, dmap), (imap_in, imap), (base_in, rbase),
        )
    ]
    above, below = (me.up, me.at(me.s + 4, 1 - me.c)), (me.down, me.at(me.s - 4, 1 - me.c))
    greet(me, mates, ((me.has_up, above), (me.has_down, below)))
    mail.loaded(got_rec)
    for q in range(4):
        lanes = slice(q * rwid, (q + 1) * rwid)
        wr[q] = jnp.concatenate([rin_s[:, lanes], rgate_s[:, lanes]], axis=1)

    def of_rows(ref):
        def slot(origin, piece):
            return ref.at[pl.ds(pl.multiple_of((origin * 4 + piece) * depth, depth), depth)]

        return slot

    def theirs_too(origin, piece, when, index=None):
        theirs = jnp.logical_and(origin // part != me.c, when)
        place = origin - (1 - me.c) * part
        here, there = wz.at[(origin, *cut(piece))], wp.at[(place, *cut(piece))]
        return mail.send(here, there, rw.at[place, piece], me.partner, theirs, index)

    rl = Line(me, mail, planes, of_rows(rwall), zrc.at[0])
    cl = Line(me, mail, planes, of_rows(cwall), zrc.at[1])
    ol = OutLine(
        me, mail, planes, lambda origin, p: wz.at[(origin, *cut(p))], zo, theirs_too,
        lambda place, p: wp.at[(place, *cut(p))], rw,
    )

    def out_own(p, up=True, down=True):
        ol.own(p, wz.at[(me.z, *cut(p))], up, down)

    mail.tag = "first"
    for q in others:
        mail.send(wr.at[q], rl.slot(me.z, me.q), rwr.at[me.q], me.mate(q))
    rl.own(me.q, wr.at[me.q])

    mail.loaded(got_x)
    first_row = mine * rows

    @pl.loop(0, rows // 16)
    def _(i):
        values = x_ref[pl.ds(pl.multiple_of(i * 16, 16), 16)].astype(f32)
        inverse = lax.rsqrt(jnp.mean(values * values, axis=1, keepdims=True) + 1e-06)
        place = pl.ds(pl.multiple_of(first_row + i * 16, 16), 16)
        xall[place] = (values * inverse * gain[...]).astype(bf16)

    part_rows = rows // rx.shape[1]

    def xslot(q, c, h):
        return xall.at[pl.ds(pl.multiple_of((q * 2 + c) * rows + h * part_rows, 16), part_rows)]

    xg = PlaneGather(me, mail, xslot, rx, rpx)
    xg.start()
    mail.loaded(got_conv + got_out)
    for q in others:
        mail.send(wc.at[q], cl.slot(me.z, me.q), rwc.at[me.q], me.mate(q))
    cl.own(me.q, wc.at[me.q])
    out_own(0)
    mail.loaded([load(wr.at[me.q], rl.slot(me.z, me.q)), load(wc.at[me.q], cl.slot(me.z, me.q))])
    for p in parts:
        theirs_too(me.z, p, True)
    mail.loaded(got_jump + got_small)
    half = jump.shape[0] // 2
    for q in range(4):
        lanes = slice(q * rwid, (q + 1) * rwid)
        jb[q] = jnp.concatenate([jump[:half, lanes], jump[half:, lanes]], axis=1).astype(bf16)
    jall[me.q] = jb[me.q]
    own_lanes = pl.ds(pl.multiple_of(me.q * cw, 128), cw)
    cpar[pl.ds(0, c_lags + 1)] = taps[:, own_lanes].astype(f32)
    cpar[pl.ds(c_lags + 1, 1)] = bias[:, own_lanes]
    cpar[pl.ds(c_lags + 2, 1)] = cgain[:, own_lanes]
    window = -(-rwid // 128) * 128
    wide_lanes = pl.ds(pl.multiple_of(me.q * rwid // 128 * 128, 128), window)

    def own_rec(values):
        moved = values[:, :rwid]
        for lead in sorted({q * rwid % 128 for q in range(4)} - {0}):
            moved = jnp.where(me.q * rwid % 128 == lead, values[:, lead : lead + rwid], moved)
        return moved

    rpar[pl.ds(0, s_lags + 1)] = own_rec(staps[:, wide_lanes].astype(f32))
    rpar[pl.ds(s_lags + 1, 1)] = own_rec(RATE_SCALE * small_softplus(-rbase[wide_lanes][None]))

    maps[...] = jnp.zeros_like(maps)
    size = dmap.shape[1]
    heads = rwid // size
    for h in range(heads):
        spot = pl.ds(h * size, size)
        maps[spot, pl.ds(h * size, size)] = dmap[me.q * heads + h]
        maps[spot, pl.ds(fold * 128 + h * size, size)] = imap[me.q * heads + h]

    for q in others:
        here = rl.slot(me.z, q)
        mail.arrived(here, rwr.at[q], me.partner)
        rl.own(q, here)
    for p in pieces:
        rl.relay(1, p)
    mail.tag = "early"
    for i in range(xg.half):
        xg.first(i)
    for q in others:
        mail.send(jb.at[q], jall.at[me.q], rj.at[me.q], me.mate(q))
    for k in range(2, last):
        for p in pieces:
            rl.relay(k, p)
    xg.second()
    for q in others:
        here = cl.slot(me.z, q)
        mail.arrived(here, rwc.at[q], me.partner)
        cl.own(q, here)
    for k in range(1, planes):
        for p in pieces:
            rl.settle(k, p)
    xg.last(pieces[:3])

    tile = length // 4

    def project_rec(begin, size):
        at = pl.ds(pl.multiple_of(begin, 64), size)
        product = jnp.dot(xall[at], rwall[...], preferred_element_type=f32).astype(bf16)
        projr[at] = product
        rext[pl.ds(pl.multiple_of(begin + rtop, 16), size)] = product[:, :rwid].astype(f32)

    @pl.loop(0, 3)
    def _(i):
        project_rec(((me.q // 2 + i // 2) % 2 * 2 + (me.q % 2 + i % 2) % 2) * tile, tile)

    mail.tag = "conv"
    for n, p in enumerate(pieces):
        cl.relay(1, p, n < 2, True)
    mail.tag = "early"
    for i in range(xg.half):
        xg.third(i)
    softened = rpar[pl.ds(s_lags + 1, 1), :]

    def gate_segment(n):
        step = (n + 1) // 2
        ring = (me.q // 2 + step % 4 // 2) % 2 * 2 + (me.q % 2 + step % 2) % 2
        i = jnp.where(n == SEGMENTS - 1, 2 * me.q, 2 * ring + n % 2)
        i = jnp.where(n == 0, 2 * me.q + 1, i)

        @pl.when(jnp.logical_and(i == 0, me.has_down))
        def _():
            mail.arrived(rext.at[pl.ds(0, rtop)], rh.at[0], me.partner)

        @pl.when(jnp.logical_and(n % 2 == 1, n < SEGMENTS - 1))
        def _():
            mail.arrived(jall.at[i // 2], rj.at[i // 2], me.partner)

        base = pl.multiple_of(i * seg, 8)
        window = rext[pl.ds(pl.multiple_of(base + rtop - 8, 8), seg + 8)]
        smooth = jnp.zeros((seg, rwid), f32)
        for k in range(s_lags + 1):
            smooth = smooth + rpar[pl.ds(k, 1), :] * window[8 - s_lags + k : 8 - s_lags + k + seg]
        smooth = smooth.astype(bf16)
        gates = jax.nn.sigmoid(jnp.dot(smooth, maps[...], preferred_element_type=f32))
        retain, admit = gates[:, :rwid], gates[:, fold * 128 : fold * 128 + rwid]
        wide = jall[i // 2].astype(f32)
        moved = jnp.where(i % 2 == 0, wide[:, :rwid], wide[:, rwid:])
        log_decay = moved - retain * softened
        decay = jnp.exp(log_decay)
        inflow = jnp.sqrt(one_minus_exp(log_decay, decay) * (1.0 + decay)) * admit * smooth.astype(f32)
        for f in range(fold):
            w = min(128, rwid - f * 128)
            spot = pl.ds(pl.multiple_of(i * lane_seg, 8), seg)
            dec[f, spot, pl.ds(0, w)] = decay[:, f * 128 : f * 128 + w]
            inf[f, spot, pl.ds(0, w)] = inflow[:, f * 128 : f * 128 + w]

    mail.finish("first")
    project_rec((me.qd * 2 + me.c) * rows, rows)
    pl.loop(0, 1)(gate_segment)
    xg.last(pieces[3:])
    project_rec((me.qd * 2 + 1 - me.c) * rows, rows)

    mail.tag = "conv"
    mail.send(rext.at[pl.ds(length, rtop)], rext.at[pl.ds(0, rtop)], rh.at[0], me.up, me.has_up)
    for p in pieces[2:]:
        cl.relay(1, p, True, False)
    for k in range(2, last):
        for p in pieces:
            cl.relay(k, p, False, True)

    @pl.when(jnp.logical_not(me.has_down))
    def _():
        rext[pl.ds(0, rtop)] = jnp.zeros((rtop, rwid), f32)
        gext[pl.ds(0, top)] = jnp.zeros((top, cw), f32)

    pl.loop(1, SEGMENTS)(gate_segment)

    def one(i, held):
        after = []
        for f in range(fold):
            at = pl.ds(i, SEGMENTS, stride=lane_seg)
            d = dec.at[f][at, :]
            product, state = held[2 * f] * d, held[2 * f + 1] * d + inf.at[f][at, :]
            dec.at[f][at, :] = product
            inf.at[f][at, :] = state
            after += [product, state]
        return tuple(after)

    flat = (SEGMENTS, 128)
    ends = lax.fori_loop(0, seg, one, (jnp.ones(flat, f32), jnp.zeros(flat, f32)) * fold, unroll=8)
    for f in range(fold):
        product, state = jnp.ones((1, 128), f32), jnp.zeros((1, 128), f32)
        for i in range(SEGMENTS):
            p, s = ends[2 * f][i : i + 1], ends[2 * f + 1][i : i + 1]
            product, state = product * p, p * state + s
        carry[pl.ds(2 * f, 1)] = product
        carry[pl.ds(2 * f + 1, 1)] = state
    for k in range(1, planes):
        mail.send(carry, cr_all.at[me.z], rc.at[me.z], lined[k - 1], me.z + k < planes)
    early = me.z < planes - 2
    for k in range(2, last):
        for p in pieces[:3]:
            cl.relay(k, p, True, False)
    mail.tag = "gather"
    for p in parts[1:]:
        out_own(p, early, True)
    mail.finish("early")

    for i in range(SEGMENTS):
        there = pl.ds(i * lane_seg, seg)
        factor = gelu(projr[pl.ds(i * seg, seg), pl.ds(rwid, rwid)].astype(f32))
        for f in range(fold):
            w = min(128, rwid - f * 128)
            lanes = pl.ds(0, w)
            dec[f, there, lanes] = dec[f, there, lanes] * factor[:, f * 128 : f * 128 + w]
            inf[f, there, lanes] = inf[f, there, lanes] * factor[:, f * 128 : f * 128 + w]

    for k in range(1, planes):
        z = me.z - k
        pl.when(z >= 0)(functools.partial(mail.arrived, cr_all.at[z], rc.at[z], me.partner))
    entering = []
    for f in range(fold):
        held = jnp.zeros((1, 128), f32)
        for j in range(planes - 1):
            after = cr_all[j, pl.ds(2 * f, 1)] * held + cr_all[j, pl.ds(2 * f + 1, 1)]
            held = jnp.where(j < me.z, after, held)
        for i in range(SEGMENTS):
            entering.append(held)
            held = ends[2 * f][i : i + 1] * held + ends[2 * f + 1][i : i + 1]
    placed = me.c * 4 + me.q

    def rec_result(i):
        here, there = pl.ds(i * seg, seg), pl.ds(i * lane_seg, seg)
        state = [dec[f, there] * entering[f * SEGMENTS + i] + inf[f, there] for f in range(fold)]
        result = jnp.concatenate(state, axis=1)[:, :rwid].astype(bf16)
        yall[here, pl.ds(pl.multiple_of(8 * cw + placed * major, 128), major)] = result[:, :major]
        return result[:, major:]

    for i in range(SEGMENTS // 2):
        pair = jnp.concatenate([rec_result(i), rec_result(i + SEGMENTS // 2)], axis=1)
        yrest[pl.ds(i * seg, seg), pl.ds(pl.multiple_of(placed * 2 * minor, 128), 2 * minor)] = pair

    def gather(buffer, lane, lanes, recv, recv_pair, kind=PlaneGather):
        tall_part = buffer.shape[0] // recv.shape[1]

        def slot(q, c, h):
            spot = pl.ds(pl.multiple_of(lane + (c * 4 + q) * lanes, 128), lanes)
            return buffer.at[pl.ds(pl.multiple_of(h * tall_part, 16), tall_part), spot]

        return kind(me, mail, slot, recv, recv_pair)

    mg = gather(yall, 8 * cw, major, rvq.at[0], rvq.at[1])
    eg = gather(yrest, 0, 2 * minor, re, rf)
    yg = gather(yall, 0, cw, rx, rpx, RowGather)
    mail.tag = "conv"
    mg.start()
    eg.start()
    mail.tag = "gather"
    for k in range(1, last):
        for p in pieces:
            cl.settle(k, p)
        for p in pieces[3:] if k > 1 else ():
            cl.await_up(k, p)
    plane_depth = 4 * depth
    is_last = (me.z == last).astype(jnp.int32)

    def conv_product(at, begin, size):
        deep = pl.ds(pl.multiple_of(begin, plane_depth), size)
        return jnp.dot(xall[at, deep], cwall[deep], preferred_element_type=f32)

    @pl.loop(0, 4)
    def _(i):
        at = pl.ds(pl.multiple_of(i * tile, tile), tile)
        cacc[at] = conv_product(at, is_last * plane_depth, last * plane_depth)

    middle = me.has_up & me.has_down

    def finish_conv(when):
        @pl.when(when)
        def _():
            @pl.loop(0, 4)
            def _(i):
                at = pl.ds(pl.multiple_of(i * tile, tile), tile)
                product = cacc[at] + conv_product(at, (1 - is_last) * last * plane_depth, plane_depth)
                product = product.astype(bf16).astype(f32)
                glu = (product[:, :cw] * jax.nn.sigmoid(product[:, cw:])).astype(bf16).astype(f32)
                gext[pl.ds(pl.multiple_of(i * tile + top, 8), tile)] = glu

        tail_rows = gext.at[pl.ds(length, top)]
        mail.send(tail_rows, gext.at[pl.ds(0, top)], rh.at[1], me.up, me.has_up & when)

    finish_conv(middle)
    for k in range(2, last):
        for p in pieces[3:]:
            cl.forward_up(k, p)
    for p in parts[1:]:
        out_own(p, jnp.logical_not(early), False)
    mg.first(0)
    for p in pieces:
        cl.settle(last, p)
    finish_conv(jnp.logical_not(middle))
    strips = length // 64

    def filter_strip(n):
        i = strips - 1 - n

        @pl.when(jnp.logical_and(i == 0, me.has_down))
        def _():
            mail.arrived(gext.at[pl.ds(0, top)], rh.at[1], me.partner)

        base = pl.multiple_of(i * 64, 8)
        window = gext[pl.ds(base, 64 + top)]
        total = jnp.zeros((64, cw), f32) + cpar[pl.ds(c_lags + 1, 1), :]
        for r in range(8):
            ks = [k for k in range(c_lags + 1) if (top - c_lags + k) % 8 == r]
            span = 64 + (8 if r else 0)
            shifted = jnp.zeros((span, cw), f32)
            for k in ks:
                begin = (top - c_lags + k) // 8 * 8
                shifted = shifted + cpar[pl.ds(k, 1), :] * window[begin : begin + span]
            total = total + shifted[r : r + 64]
        filt[pl.ds(base, 64)] = total

    pl.loop(0, strips)(filter_strip)

    turned = filt[...].T
    ft[...] = turned
    part_sum = jnp.sum(turned, axis=0, keepdims=True)
    off = turned - part_sum * (1.0 / cw)
    st_all[mine, pl.ds(0, 1)] = part_sum
    st_all[mine, pl.ds(1, 1)] = jnp.sum(off * off, axis=0, keepdims=True)
    for device in mates:
        mail.send(st_all.at[mine], st_all.at[mine], rs.at[mine], device)
    for i in range(1, mg.half):
        mg.first(i)
    for i in range(eg.half):
        eg.first(i)
    mail.tag = "out"
    for p in parts:
        ol.relay(1, p)
    mail.tag = "gather"
    mail.finish("conv")

    for k in range(1, 8):
        d = (mine + k) % 8
        mail.arrived(st_all.at[d], rs.at[d], me.partner)
    total = sum(st_all[d, 0:1, :] for d in range(8))
    mean = total * (1.0 / (8 * cw))
    spread = jnp.zeros_like(mean)
    for d in range(8):
        shift = st_all[d, 0:1, :] * (1.0 / cw) - mean
        spread = spread + st_all[d, 1:2, :] + cw * shift * shift
    scale = lax.rsqrt(spread * (1.0 / (8 * cw)) + 1e-05)
    gain_col = jnp.broadcast_to(cpar[pl.ds(c_lags + 2, 1), :], (8, cw)).T[:, 0:1]
    v = (ft[...] - mean) * scale * gain_col
    yall[:, pl.ds(pl.multiple_of(placed * cw, 128), cw)] = (v * jax.nn.sigmoid(v)).T.astype(bf16)
    mail.tag = "begun"
    yg.start()
    mail.tag = "share"
    mg.second()
    eg.second()
    for g in (mg, eg):
        for i in range(g.half):
            g.third(i)
    mail.tag = "last"
    mail.finish("gather")
    for i in range(yg.half):
        yg.first(i)
    for k in range(2, last):
        for p in parts:
            ol.relay(k, p)
    mg.last(pieces)
    eg.last(pieces)
    mail.finish("share")
    rest_at = 8 * (cw + major)

    @pl.loop(0, SEGMENTS // 2)
    def _(i):
        values = yrest[pl.ds(pl.multiple_of(i * seg, 16), seg)]
        low = [values[:, j * 2 * minor : j * 2 * minor + minor] for j in range(8)]
        high = [values[:, j * 2 * minor + minor : (j + 1) * 2 * minor] for j in range(8)]
        for begin, chosen in ((0, low), (length // 2, high)):
            here = pl.ds(pl.multiple_of(begin + i * seg, 16), seg)
            yall[here, pl.ds(rest_at, 8 * minor)] = jnp.concatenate(chosen, axis=1)

    yg.second()
    yg.third(0)
    for k in range(1, last):
        for p in parts:
            ol.settle(k, p)

    cols = wz.shape[2]
    upward = me.z < part

    def lanes_of(h):
        return pl.ds(0, cols) if h is None else pl.ds(h * half_cols, half_cols)

    def summed(q, k, h, low, high):
        here = pl.ds(pl.multiple_of(q * 2 * rows, 16), 2 * rows)
        total = jnp.zeros((2 * rows, cols if h is None else half_cols), f32)
        for c, block in ((me.c, wz.at[me.c * part + k]), (1 - me.c, wp.at[k])):
            begin = 0
            for at, lanes in ((0, 4 * cw), (8 * cw, 4 * major), (rest_at, 4 * minor)):
                first, end = max(begin, low), min(begin + lanes, high)
                if first < end:
                    spot = pl.multiple_of(at + c * lanes + first - begin, 128)
                    right = block[pl.ds(first, end - first), lanes_of(h)]
                    left_part = yall[here, pl.ds(spot, end - first)]
                    total = total + jnp.dot(left_part, right, preferred_element_type=f32)
                begin = begin + lanes
        return here, total

    def multiply(q, k, h):
        here, total = summed(q, k, h, tall if h == 1 else 0, 2 * tall)
        if h == 1:
            total = total + cacc[here, pl.ds(0, half_cols)]
        total = total.astype(bf16)
        for c in range(2):
            cbuf[q * 2 + c, k, :, lanes_of(h)] = total[c * rows : (c + 1) * rows]

    def place(q, c, k, h):
        at = ((c * part + k) * 4 + q) * cols + (0 if h is None else h * half_cols)
        return out.at[:, pl.ds(pl.multiple_of(at, 128), cols if h is None else half_cols)]

    def mate_of(i):
        flip = 3 - i
        return (me.q // 2 + flip // 2) % 2 * 2 + (me.q % 2 + flip % 2) % 2

    mail.finish("begun")

    def left(d, k, h):
        return rvq.at[k, d // 2, d % 2 * 2 + (h or 0)]

    def landed(d, k, h):
        return zrc.at[k, d // 2, d % 2 * 2 + (h or 0)]

    def parcel(q, c, k, h):
        return pltpu.make_async_remote_copy(
            src_ref=cbuf.at[q * 2 + c, k, :, lanes_of(h)], dst_ref=place(me.q, me.c, k, h),
            send_sem=left(q * 2 + c, k, h), recv_sem=landed(mine, k, h),
            device_id=me.at(me.z * 4 + q, c), device_id_type=MESH,
        )

    def kept(k, h):
        src = cbuf.at[mine, k, :, lanes_of(h)]
        return pltpu.make_async_copy(src, place(me.q, me.c, k, h), left(mine, k, h))

    def serve(q, k, h):
        multiply(q, k, h)
        pl.when(q != me.q)(lambda: parcel(q, me.c, k, h).start())
        parcel(q, 1 - me.c, k, h).start()
        pl.when(q == me.q)(lambda: kept(k, h).start())

    def ready(k, ps):
        for p in ps:
            mail.arrived(wp.at[(k, *cut(p))], rw.at[k, p], me.partner)

    order = [jnp.where(upward, n, part - 1 - n) for n in range(part)]
    ready(order[0], parts)
    for i in range(yg.half):
        if i:
            yg.third(i)
        for q in pieces:
            for row_part in ((me.qx, me.qy), (me.q, me.qd))[i]:
                yg.paired(q, row_part)

        @pl.loop(0, 2)
        def _(n):
            serve(mate_of(3 - 3 * (1 - n) if i else 2 - n), order[0], None)

    for n in range(1, part - 1):
        ready(order[n], parts)
        pl.loop(0, 4)(lambda i: serve(mate_of(i), order[n], None))
    k_far = order[-1]
    for p in parts[:2]:
        ol.settle(last, p)
    ready(k_far, parts[:2])
    pl.loop(0, 4)(lambda i: serve(mate_of(i), k_far, 0))
    ol.settle(last, 2)
    ready(k_far, parts[2:3])

    @pl.loop(0, 4)
    def _(q):
        here, total = summed(q, k_far, 1, 0, tall)
        cacc[here, pl.ds(0, half_cols)] = total

    ol.settle(last, 3)
    ready(k_far, parts[3:])
    pl.loop(0, 4)(lambda i: serve(mate_of(i), k_far, 1))
    rounds = [(k, None) for k in order[:-1]] + [(order[-1], 0), (order[-1], 1)]

    @pl.loop(0, 4)
    def _(i):
        q = mate_of(i)
        for k, h in rounds:
            mail.arrived(place(q, 1 - me.c, k, h), landed(q * 2 + 1 - me.c, k, h), me.partner)
            parcel(q, 1 - me.c, k, h).wait_send()

    @pl.loop(0, 3)
    def _(i):
        q = mate_of(i)
        for k, h in rounds:
            mail.arrived(place(q, me.c, k, h), landed(q * 2 + me.c, k, h), me.partner)
            parcel(q, me.c, k, h).wait_send()

    for k, h in rounds:
        kept(k, h).wait()
    mail.finish()


def handed_out_kernel(src, dst, held, got, sent):
    count = got.shape[0]
    tall = src.shape[0] // count
    spots = [pl.ds(i * tall, tall) for i in range(count)]
    taken = [pltpu.make_async_copy(src.at[s], held.at[s], got.at[i]) for i, s in enumerate(spots)]
    given = [pltpu.make_async_copy(held.at[s], dst.at[s], sent.at[i]) for i, s in enumerate(spots)]
    for copy in taken:
        copy.start()
    for came, goes in zip(taken, given):
        came.wait()
        goes.start()
    for copy in given:
        copy.wait()


def handed_out(result):
    dma = pltpu.SemaphoreType.DMA
    return pl.pallas_call(
        handed_out_kernel,
        out_shape=jax.ShapeDtypeStruct(result.shape, result.dtype),
        in_specs=[ANY],
        out_specs=ANY,
        scratch_shapes=[pltpu.VMEM(result.shape, result.dtype), dma((6,)), dma((6,))],
    )(result)


def layer(planes, lags, tokens, norm_gain, val_w, gate_w, rgate_w, rin_w, taps, bias, cgain, staps, dmap, imap, rbase, jump, ocw, orw):
    rows, width_in = tokens.shape
    length = 8 * rows
    depth = rin_w.shape[0]
    cw, rwid = val_w.shape[1] // 4, rin_w.shape[1] // 4
    used, cols = cw + rwid, ocw.shape[1]
    minor = rwid % 128
    fold = (rwid + 127) // 128
    f32, bf16 = jnp.float32, jnp.bfloat16
    dma = pltpu.SemaphoreType.DMA
    top = lags[0] + -lags[0] % 16
    rtop = lags[1] + -lags[1] % 16
    part = planes // 2
    deep = planes * 4 * depth

    def vmem(*shape, dtype=bf16):
        return pltpu.VMEM(shape, dtype)

    def wide(*shape):
        return pltpu.VMEM(shape, f32)

    return pl.pallas_call(
        functools.partial(layer_kernel, planes, lags),
        out_shape=jax.ShapeDtypeStruct((rows, planes * 4 * cols), bf16),
        in_specs=[ANY] * 16,
        out_specs=ANY,
        scratch_shapes=[
            vmem(rows, width_in), wide(1, width_in), vmem(*rin_w.shape), vmem(*rgate_w.shape),
            vmem(4, depth, 2 * rwid), vmem(4, depth, 2 * cw),
            vmem(*taps.shape), wide(1, 4 * cw), wide(1, 4 * cw), vmem(*staps.shape),
            vmem(*dmap.shape), vmem(*imap.shape), wide(4 * rwid), wide(*jump.shape),
            vmem(4, jump.shape[0] // 2, 2 * rwid), wide(lags[0] + 3 + -(lags[0] + 3) % 8, cw), wide(8, rwid),
            vmem(length, width_in),
            vmem(deep, 2 * rwid),
            vmem(deep, 2 * cw),
            vmem(length, 2 * rwid),
            vmem(4, jump.shape[0] // 2, 2 * rwid),
            vmem(planes, 4 * used, cols),
            vmem(part, 4 * used, cols),
            vmem(length, 8 * used),
            vmem(length // 2, 16 * minor),
            wide(length, 2 * cw),
            vmem(8, part, rows, cols),
            wide(top + length, cw),
            wide(rtop + length, rwid),
            wide(length, cw),
            wide(fold, length + 8 * SEGMENTS, 128),
            wide(fold, length + 8 * SEGMENTS, 128),
            vmem(rwid, 2 * fold * 128),
            wide(cw, length),
            wide(8, 2, length),
            wide(8, 128),
            wide(planes, 8, 128),
            dma((POOL,)), dma((4, 4)), dma((4, 4)), dma((4,)), dma((4,)),
            dma((part, planes, 4)), dma((planes, OUT_PARTS)), dma((4,)),
            dma((part, 4, 4)), dma((4, 2)), dma((4, 2)), dma((part, OUT_PARTS)),
            dma((2,)), dma((8,)), dma((planes,)),
        ],
        compiler_params=pltpu.CompilerParams(
            collective_id=0, has_side_effects=True, vmem_limit_bytes=60 * 1024 * 1024
        ),
    )(
        tokens, norm_gain[None], val_w, gate_w, rgate_w, rin_w, taps, bias[None], cgain[None], staps,
        dmap, imap, rbase, jump, ocw, orw,
    )


def plane_shards(
    planes,
    tokens,
    norm_gain,
    conv_val_w,
    conv_gate_w,
    rec_gate_w,
    rec_in_w,
    conv_taps,
    conv_bias,
    conv_gain,
    short_taps,
    decay_map,
    input_map,
    decay_base,
    decay_jump,
    out_conv_w,
    out_rec_w,
):
    lags = (conv_taps.shape[0] - 1, short_taps.shape[0] - 1)
    return handed_out(layer(
        planes, lags, tokens, norm_gain, conv_val_w, conv_gate_w, rec_gate_w, rec_in_w, conv_taps, conv_bias,
        conv_gain, short_taps, decay_map, input_map, decay_base, decay_jump, out_conv_w, out_rec_w,
    ))


def solution(mesh):
    in_specs = (
        P(("sp", "tp"), None),
        P(),
        P("sp", "tp"),
        P("sp", "tp"),
        P("sp", "tp"),
        P("sp", "tp"),
        P(None, "tp"),
        P("tp"),
        P("tp"),
        P(None, "tp"),
        P("tp", None, None),
        P("tp", None, None),
        P("tp"),
        P("sp", "tp"),
        P("tp", "sp"),
        P("tp", "sp"),
    )
    out_specs = P(("sp", "tp"), None)
    count = mesh.shape["sp"]
    planar = mesh.shape["tp"] == 2 and count % 8 == 0 and count >= 16
    body = functools.partial(plane_shards, count // 4) if planar else shards
    return jax.shard_map(body, mesh=mesh, in_specs=in_specs, out_specs=out_specs, check_vma=False)
```

```python
import functools

import jax
import jax.numpy as jnp
from jax import lax
from jax.experimental import pallas as pl
from jax.experimental.pallas import tpu as pltpu
from jax.sharding import PartitionSpec as P

CONV_WIDTH = 1024


RATE_SCALE = 8.0


def passed_along(value, axis, by):
    count = lax.axis_size(axis)
    pairs = [(i, i + by) for i in range(count) if 0 <= i + by < count]
    return lax.ppermute(value, axis, pairs)


def prefix(part, axis, combine, identity):
    place = lax.axis_index(axis)
    gathered = jax.tree.map(lambda a: lax.all_gather(a, axis), part)
    state = jax.tree.map(lambda a, e: jnp.zeros_like(a) + jnp.asarray(e, a.dtype), part, identity)

    def one(step, state):
        return combine(
            state, jax.tree.map(lambda a: lax.dynamic_index_in_dim(a, step, 0, False), gathered)
        )

    return lax.fori_loop(0, place, one, state)


def norm_rows(values, gain):
    widened = values.astype(jnp.float32)
    inverse = lax.rsqrt(jnp.mean(widened * widened, axis=-1, keepdims=True) + 1e-06)
    return (widened * inverse * gain).astype(jnp.bfloat16)


def causal_window(edge, current, weights):
    extended = jnp.concatenate([edge, current], axis=0).astype(jnp.float32)
    taps_wide = weights.astype(jnp.float32)
    length = current.shape[0]
    result = jnp.zeros((length, current.shape[1]), jnp.float32)
    for lag_index in range(weights.shape[0]):
        result = result + taps_wide[lag_index][None, :] * extended[lag_index : lag_index + length]
    return result


def chain_step(earlier, latter):
    return (earlier[0] * latter[0], latter[0] * earlier[1] + latter[1])


def glu_of(conv_val, conv_gate):
    return (conv_val.astype(jnp.float32) * jax.nn.sigmoid(conv_gate.astype(jnp.float32))).astype(
        jnp.bfloat16
    )


def shards(
    tokens,
    norm_gain,
    conv_val_w,
    conv_gate_w,
    rec_gate_w,
    rec_in_w,
    conv_taps,
    conv_bias,
    conv_gain,
    short_taps,
    decay_map,
    input_map,
    decay_base,
    decay_jump,
    out_conv_w,
    out_rec_w,
):
    rec_cols = rec_in_w.shape[1]
    conv_lags = conv_taps.shape[0] - 1
    short_lags = short_taps.shape[0] - 1
    normed = norm_rows(tokens, norm_gain)
    val_full, gate_full = (
        lax.all_gather(conv_val_w, "sp", axis=0, tiled=True),
        lax.all_gather(conv_gate_w, "sp", axis=0, tiled=True),
    )
    all_rows = lax.all_gather(normed, "tp", axis=0, tiled=True)
    conv_val = jnp.dot(all_rows, val_full, preferred_element_type=jnp.float32).astype(jnp.bfloat16)
    conv_gate = jnp.dot(all_rows, gate_full, preferred_element_type=jnp.float32).astype(
        jnp.bfloat16
    )
    glu = glu_of(conv_val, conv_gate)
    conv_edge = passed_along(glu[-conv_lags:], "sp", 1)
    rgate_full, rin_full = (
        lax.all_gather(rec_gate_w, "sp", axis=0, tiled=True),
        lax.all_gather(rec_in_w, "sp", axis=0, tiled=True),
    )
    rec_gate = jnp.dot(all_rows, rgate_full, preferred_element_type=jnp.float32).astype(
        jnp.bfloat16
    )
    rec_in = jnp.dot(all_rows, rin_full, preferred_element_type=jnp.float32).astype(jnp.bfloat16)
    rec_edge = passed_along(rec_in[-short_lags:], "sp", 1)
    filtered = causal_window(conv_edge, glu, conv_taps) + conv_bias[None, :]
    row_total = lax.psum(jnp.sum(filtered, axis=1), "tp")
    centered = filtered - (row_total / CONV_WIDTH)[:, None]
    spread = lax.psum(jnp.sum(centered * centered, axis=1), "tp") / CONV_WIDTH
    conv_out = jax.nn.silu(centered * lax.rsqrt(spread + 1e-05)[:, None] * conv_gain).astype(
        jnp.bfloat16
    )
    smoothed = causal_window(rec_edge, rec_in, short_taps).astype(jnp.bfloat16)
    length = smoothed.shape[0]
    grouped = smoothed.reshape(length, decay_map.shape[0], decay_map.shape[1])
    retain = jax.nn.sigmoid(
        jnp.einsum("thi,hio->tho", grouped, decay_map, preferred_element_type=jnp.float32).reshape(
            length, rec_cols
        )
    )
    admit = jax.nn.sigmoid(
        jnp.einsum("thi,hio->tho", grouped, input_map, preferred_element_type=jnp.float32).reshape(
            length, rec_cols
        )
    )
    log_decay = -RATE_SCALE * retain * jax.nn.softplus(-decay_base)[None, :] + decay_jump
    decay = jnp.exp(log_decay)
    inflow = jnp.sqrt(-jnp.expm1(2.0 * log_decay)) * admit * smoothed.astype(jnp.float32)
    products, local_state = lax.associative_scan(chain_step, (decay, inflow), axis=0)
    entering = prefix(
        (products[-1], local_state[-1]),
        "sp",
        chain_step,
        (jnp.ones((rec_cols,), jnp.float32), jnp.zeros((rec_cols,), jnp.float32)),
    )
    state = local_state + products * entering[1][None, :]
    rec_out = (jax.nn.gelu(rec_gate.astype(jnp.float32)) * state).astype(jnp.bfloat16)
    conv_full, rec_full = (
        lax.all_gather(out_conv_w, "sp", axis=1, tiled=True),
        lax.all_gather(out_rec_w, "sp", axis=1, tiled=True),
    )
    return lax.psum_scatter(
        (
            jnp.dot(conv_out, conv_full, preferred_element_type=jnp.float32)
            + jnp.dot(rec_out, rec_full, preferred_element_type=jnp.float32)
        ).astype(jnp.bfloat16),
        "tp",
        scatter_dimension=0,
        tiled=True,
    )


MESH = pl.DeviceIdType.MESH
ANY = pl.BlockSpec(memory_space=pl.ANY)
VMEM = pl.BlockSpec(memory_space=pltpu.VMEM)
SEGMENTS = 8


class Spot:
    def __init__(self, planes):
        self.s, self.c = lax.axis_index("sp"), lax.axis_index("tp")
        self.z, self.q = self.s // 4, self.s % 4
        self.qx = self.q + 1 - 2 * (self.q % 2)
        self.qy = (self.q + 2) % 4
        self.qd = 3 - self.q
        self.has_up, self.has_down = self.z < planes - 1, self.z > 0
        self.up, self.down = self.at(self.s + 4, self.c), self.at(self.s - 4, self.c)
        self.partner = self.at(self.s, 1 - self.c)

    def at(self, s, c):
        return {"sp": s, "tp": c}

    def mate(self, q):
        return self.at(self.z * 4 + q, self.c)


class Mail:
    def __init__(self, send_sem):
        self.send_sem, self.tag, self.open = send_sem, "early", []
        self.free = list(range(send_sem.shape[0]))

    def claim(self):
        self.free.sort()
        return self.free.pop(0)

    def send(self, src, dst, recv, device, when=None, index=None):
        index = self.claim() if index is None else index
        copy = pltpu.make_async_remote_copy(
            src_ref=src, dst_ref=dst, send_sem=self.send_sem.at[index],
            recv_sem=recv, device_id=device, device_id_type=MESH,
        )
        self.open.append((self.tag, index, copy.wait_send, when))
        if when is None:
            copy.start()
        else:
            pl.when(when)(copy.start)
        return index

    def load(self, src, dst):
        index = self.claim()
        copy = pltpu.make_async_copy(src, dst, self.send_sem.at[index])
        copy.start()
        return index, copy

    def loaded(self, copies):
        for index, copy in copies:
            copy.wait()
            self.free.append(index)

    def arrived(self, dst, recv, device):
        pltpu.make_async_remote_copy(
            src_ref=dst, dst_ref=dst, send_sem=self.send_sem.at[0],
            recv_sem=recv, device_id=device, device_id_type=MESH,
        ).wait_recv()

    def finish(self, *tags):
        done = [entry for entry in self.open if not tags or entry[0] in tags]
        self.open = [entry for entry in self.open if entry not in done]
        for _, index, wait, when in done:
            if when is None:
                wait()
            else:
                pl.when(when)(wait)
        self.free.extend({entry[1] for entry in done})


def greet(me, devices, line):
    barrier = pltpu.get_barrier_semaphore()
    for device in devices:
        pl.semaphore_signal(barrier, inc=1, device_id=device, device_id_type=MESH)
    amount = len(devices)
    for has, neighbours in line:
        @pl.when(has)
        def _():
            for device in neighbours:
                pl.semaphore_signal(barrier, inc=1, device_id=device, device_id_type=MESH)
        amount = amount + len(neighbours) * has.astype(jnp.int32)
    pl.semaphore_wait(barrier, amount)


class PlaneGather:
    def __init__(self, me, mail, slot, recv, recv_pair):
        self.me, self.mail, self.slot = me, mail, slot
        self.recv, self.recv_pair = recv, recv_pair
        self.parts = recv.shape[1]
        self.half = self.parts // 2

    def start(self):
        me, mail = self.me, self.mail
        for h in range(self.parts):
            for q, part in ((me.qx, h), (me.qy, (h + self.half) % self.parts)):
                own = self.slot(me.q, me.c, part)
                mail.send(own, own, self.recv.at[me.q, part], me.mate(q))
        for part in range(self.parts):
            self.share(me.q, part, self.slot(me.q, me.c, part))

    def took(self, q, part):
        here = self.slot(q, self.me.c, part)
        self.mail.arrived(here, self.recv.at[q, part], self.me.partner)
        return here

    def share(self, q, part, here):
        self.mail.send(here, here, self.recv_pair.at[q, part], self.me.partner)

    def first(self, i):
        me = self.me
        for q, part, to in ((me.qx, i, me.qy), (me.qy, self.half + i, me.qx)):
            here = self.took(q, part)
            self.mail.send(here, here, self.recv.at[q, part], me.mate(to))
            self.share(q, part, here)

    def second(self):
        for i in range(self.half):
            for q, part in ((self.me.qx, self.half + i), (self.me.qy, i)):
                self.share(q, part, self.took(q, part))

    def third(self, i):
        for part in (i, self.half + i):
            self.share(self.me.qd, part, self.took(self.me.qd, part))

    def paired(self, q, part):
        me = self.me
        self.mail.arrived(self.slot(q, 1 - me.c, part), self.recv_pair.at[q, part], me.partner)

    def last(self, origins):
        for q in origins:
            for part in range(self.parts):
                self.paired(q, part)


class RowGather(PlaneGather):
    def start(self):
        me, mail = self.me, self.mail
        for to_x, to_y in ((me.qx, me.qy), (me.q, me.qd), (me.qd, me.q), (me.qy, me.qx)):
            for q, part in ((me.qx, to_x), (me.qy, to_y)):
                own = self.slot(me.q, me.c, part)
                mail.send(own, own, self.recv.at[me.q, part], me.mate(q))
        for part in range(self.parts):
            self.share(me.q, part, self.slot(me.q, me.c, part))

    def first(self, i):
        me = self.me
        part = (me.q, me.qx)[i]
        for q, to in ((me.qx, me.qy), (me.qy, me.qx)):
            here = self.took(q, part)
            self.mail.send(here, here, self.recv.at[q, part], me.mate(to))
            self.share(q, part, here)

    def second(self):
        me = self.me
        for part in (me.qd, me.qy):
            for q in (me.qx, me.qy):
                self.share(q, part, self.took(q, part))

    def third(self, i):
        me = self.me
        for part in ((me.qx, me.qy), (me.q, me.qd))[i]:
            self.share(me.qd, part, self.took(me.qd, part))


def one_minus_exp(y, grown):
    series = 1.0 + y * (1.0 / 5.0)
    for n in (4.0, 3.0, 2.0):
        series = 1.0 + y * (1.0 / n) * series
    return jnp.where(y > -0.25, -y * series, 1.0 - grown)


def gelu(v):
    return 0.5 * v * (1.0 + jnp.tanh(0.7978845608028654 * (v + 0.044715 * v * v * v)))


class Line:
    def __init__(self, me, mail, planes, slot, recv, seen=None):
        self.me, self.mail, self.planes = me, mail, planes
        self.slot, self.recv, self.seen = slot, recv, seen

    def own(self, piece, src, up=True, down=True):
        me = self.me
        for wanted, has, device in ((up, me.has_up, me.up), (down, me.has_down, me.down)):
            if wanted is not False:
                self.post(src, me.z, piece, device, has & wanted)

    def post(self, src, origin, piece, device, when):
        self.mail.send(src, self.slot(origin, piece), self.recv.at[origin, piece], device, when)

    def mine(self, origin):
        return True

    def ways(self, k):
        me = self.me
        return (
            (me.z - k, me.z >= k, me.up, me.has_up),
            (me.z + k, me.z + k < self.planes, me.down, me.has_down),
        )

    def take(self, origin, piece, when, index=None):
        here, sem = self.slot(origin, piece), self.recv.at[origin, piece]
        pl.when(when)(functools.partial(self.mail.arrived, here, sem, self.me.partner))
        return None if self.seen is None else self.seen(origin, piece, when, index)

    def relay(self, k, piece, up=True, down=True):
        for wanted, (origin, there, on, more) in zip((up, down), self.ways(k)):
            if wanted:
                when = jnp.logical_and(there, more)
                here = self.slot(origin, piece)
                self.take(origin, piece, when)
                self.post(here, origin, piece, on, when)

    def await_up(self, k, piece):
        origin, there, _, more = self.ways(k)[0]
        return self.take(origin, piece, there & more)

    def forward_up(self, k, piece):
        origin, there, on, more = self.ways(k)[0]
        here, sem = self.slot(origin, piece), self.recv.at[origin, piece]
        self.mail.send(here, here, sem, on, there & more)

    def settle(self, k, piece):
        me = self.me
        lowest, highest = jnp.logical_not(me.has_down), jnp.logical_not(me.has_up)
        origin = jnp.where(lowest, me.z + k, me.z - k)
        here, sem = self.slot(origin, piece), self.recv.at[origin, piece]
        pl.when((lowest | highest) & self.mine(origin))(functools.partial(self.mail.arrived, here, sem, me.partner))


class OutLine(Line):
    def __init__(self, me, mail, planes, slot, recv, seen, other, other_recv):
        super().__init__(me, mail, planes, slot, recv, seen)
        self.other, self.other_recv = other, other_recv

    def mine(self, origin):
        return origin // (self.planes // 2) == self.me.c

    def post(self, src, origin, piece, device, when):
        me = self.me
        z = device["sp"] // 4
        ends = (z == 0) | (z == self.planes - 1)
        cross = ends & jnp.logical_not(self.mine(origin))
        here, sem = self.slot(origin, piece), self.recv.at[origin, piece]
        index = self.mail.send(src, here, sem, device, when & jnp.logical_not(cross))
        place = origin - (1 - me.c) * (self.planes // 2)
        sem = self.other_recv.at[place, piece]
        device = me.at(device["sp"], 1 - me.c)
        self.mail.send(src, self.other(place, piece), sem, device, when & cross, index)


def small_softplus(v):
    u = jnp.exp(-jnp.abs(v))
    series = jnp.zeros_like(u)
    for n in (8.0, 7.0, 6.0, 5.0, 4.0, 3.0, 2.0, 1.0):
        series = 1.0 / n - u * series
    return jnp.maximum(v, 0.0) + jnp.where(u < 0.1, u * series, jnp.log(1.0 + u))


OUT_PARTS = 4
POOL = 84


def layer_kernel(
    planes, lags, tokens, gain_in, val_w, gate_w, rgate_w, rin_w, taps_in, bias_in, cgain_in, staps_in,
    dmap_in, imap_in, base_in, jump_in, ocw, orw,
    out, x_ref, gain, rin_s, rgate_s, wr, wc, taps, bias, cgain, staps, dmap, imap, rbase, jump, jb, cpar, rpar,
    xall, rwall, cwall, projr, jall, wz, wp, yall, yrest, cacc, cbuf, gext, rext, filt, dec, inf, maps, ft,
    st_all, carry, cr_all,
    send, rx, rpx, rwr, rwc, zrc, zo, rj, rvq, re, rf, rw, rh, rs, rc,
):
    me = Spot(planes)
    mail = Mail(send)
    c_lags, s_lags = lags
    f32, bf16 = jnp.float32, jnp.bfloat16
    rows, depth = x_ref.shape[0], wr.shape[1]
    length = xall.shape[0]
    cw, rwid = gext.shape[1], rpar.shape[1]
    seg = length // SEGMENTS
    lane_seg = dec.shape[1] // SEGMENTS
    top = gext.shape[0] - length
    rtop = rext.shape[0] - length
    fold = dec.shape[0]
    part = planes // 2
    major = rwid // 128 * 128
    minor = rwid - major
    mine = me.q * 2 + me.c
    others = (me.qx, me.qy, me.qd)
    pieces = (me.q,) + others
    parts = tuple(range(OUT_PARTS))
    tall, half_cols = wz.shape[1] // 2, wz.shape[2] // 2

    def cut(p):
        return pl.ds(p % 2 * tall, tall), pl.ds(p // 2 * half_cols, half_cols)

    last = planes - 1
    mates = [me.at(me.z * 4 + (me.q + dq) % 4, c) for dq in range(4) for c in (me.c, 1 - me.c)][1:]
    lined = [me.at((me.s + 4 * k) % (4 * planes), me.c) for k in range(1, planes)]
    load = mail.load
    got_rec = [load(rin_w, rin_s), load(rgate_w, rgate_s)]
    got_x = [load(tokens, x_ref), load(gain_in, gain)]
    got_conv = []
    for q in range(4):
        got_conv.append(load(val_w.at[:, pl.ds(q * cw, cw)], wc.at[q, :, pl.ds(0, cw)]))
        got_conv.append(load(gate_w.at[:, pl.ds(q * cw, cw)], wc.at[q, :, pl.ds(cw, cw)]))
    got_out = []
    got_out.append(load(ocw, wz.at[me.z, pl.ds(0, 4 * cw)]))
    for q in range(4):
        at = 4 * cw + q * major
        got_out.append(load(orw.at[pl.ds(q * rwid, major)], wz.at[me.z, pl.ds(at, major)]))
        at = 4 * (cw + major) + q * minor
        got_out.append(load(orw.at[pl.ds(q * rwid + major, minor)], wz.at[me.z, pl.ds(at, minor)]))
    got_jump = [load(jump_in, jump)]
    got_small = [
        load(src, dst)
        for src, dst in (
            (taps_in, taps), (bias_in, bias), (cgain_in, cgain), (staps_in, staps),
            (dmap_in, dmap), (imap_in, imap), (base_in, rbase),
        )
    ]
    above, below = (me.up, me.at(me.s + 4, 1 - me.c)), (me.down, me.at(me.s - 4, 1 - me.c))
    greet(me, mates, ((me.has_up, above), (me.has_down, below)))
    mail.loaded(got_rec)
    for q in range(4):
        lanes = slice(q * rwid, (q + 1) * rwid)
        wr[q] = jnp.concatenate([rin_s[:, lanes], rgate_s[:, lanes]], axis=1)

    def of_rows(ref):
        def slot(origin, piece):
            return ref.at[pl.ds(pl.multiple_of((origin * 4 + piece) * depth, depth), depth)]

        return slot

    def theirs_too(origin, piece, when, index=None):
        theirs = jnp.logical_and(origin // part != me.c, when)
        place = origin - (1 - me.c) * part
        here, there = wz.at[(origin, *cut(piece))], wp.at[(place, *cut(piece))]
        return mail.send(here, there, rw.at[place, piece], me.partner, theirs, index)

    rl = Line(me, mail, planes, of_rows(rwall), zrc.at[0])
    cl = Line(me, mail, planes, of_rows(cwall), zrc.at[1])
    ol = OutLine(
        me, mail, planes, lambda origin, p: wz.at[(origin, *cut(p))], zo, theirs_too,
        lambda place, p: wp.at[(place, *cut(p))], rw,
    )

    def out_own(p, up=True, down=True):
        ol.own(p, wz.at[(me.z, *cut(p))], up, down)

    mail.tag = "first"
    for q in others:
        mail.send(wr.at[q], rl.slot(me.z, me.q), rwr.at[me.q], me.mate(q))
    rl.own(me.q, wr.at[me.q])

    mail.loaded(got_x)
    first_row = mine * rows

    @pl.loop(0, rows // 16)
    def _(i):
        values = x_ref[pl.ds(pl.multiple_of(i * 16, 16), 16)].astype(f32)
        inverse = lax.rsqrt(jnp.mean(values * values, axis=1, keepdims=True) + 1e-06)
        place = pl.ds(pl.multiple_of(first_row + i * 16, 16), 16)
        xall[place] = (values * inverse * gain[...]).astype(bf16)

    part_rows = rows // rx.shape[1]

    def xslot(q, c, h):
        return xall.at[pl.ds(pl.multiple_of((q * 2 + c) * rows + h * part_rows, 16), part_rows)]

    xg = PlaneGather(me, mail, xslot, rx, rpx)
    xg.start()
    mail.loaded(got_conv + got_out)
    for q in others:
        mail.send(wc.at[q], cl.slot(me.z, me.q), rwc.at[me.q], me.mate(q))
    cl.own(me.q, wc.at[me.q])
    out_own(0)
    mail.loaded([load(wr.at[me.q], rl.slot(me.z, me.q)), load(wc.at[me.q], cl.slot(me.z, me.q))])
    for p in parts:
        theirs_too(me.z, p, True)
    mail.loaded(got_jump + got_small)
    half = jump.shape[0] // 2
    for q in range(4):
        lanes = slice(q * rwid, (q + 1) * rwid)
        jb[q] = jnp.concatenate([jump[:half, lanes], jump[half:, lanes]], axis=1).astype(bf16)
    jall[me.q] = jb[me.q]
    own_lanes = pl.ds(pl.multiple_of(me.q * cw, 128), cw)
    cpar[pl.ds(0, c_lags + 1)] = taps[:, own_lanes].astype(f32)
    cpar[pl.ds(c_lags + 1, 1)] = bias[:, own_lanes]
    cpar[pl.ds(c_lags + 2, 1)] = cgain[:, own_lanes]
    window = -(-rwid // 128) * 128
    wide_lanes = pl.ds(pl.multiple_of(me.q * rwid // 128 * 128, 128), window)

    def own_rec(values):
        moved = values[:, :rwid]
        for lead in sorted({q * rwid % 128 for q in range(4)} - {0}):
            moved = jnp.where(me.q * rwid % 128 == lead, values[:, lead : lead + rwid], moved)
        return moved

    rpar[pl.ds(0, s_lags + 1)] = own_rec(staps[:, wide_lanes].astype(f32))
    rpar[pl.ds(s_lags + 1, 1)] = own_rec(RATE_SCALE * small_softplus(-rbase[wide_lanes][None]))

    maps[...] = jnp.zeros_like(maps)
    size = dmap.shape[1]
    heads = rwid // size
    for h in range(heads):
        spot = pl.ds(h * size, size)
        maps[spot, pl.ds(h * size, size)] = dmap[me.q * heads + h]
        maps[spot, pl.ds(fold * 128 + h * size, size)] = imap[me.q * heads + h]

    for q in others:
        here = rl.slot(me.z, q)
        mail.arrived(here, rwr.at[q], me.partner)
        rl.own(q, here)
    for p in pieces:
        rl.relay(1, p)
    mail.tag = "early"
    for i in range(xg.half):
        xg.first(i)
    for q in others:
        mail.send(jb.at[q], jall.at[me.q], rj.at[me.q], me.mate(q))
    for k in range(2, last):
        for p in pieces:
            rl.relay(k, p)
    xg.second()
    for q in others:
        here = cl.slot(me.z, q)
        mail.arrived(here, rwc.at[q], me.partner)
        cl.own(q, here)
    for k in range(1, planes):
        for p in pieces:
            rl.settle(k, p)
    xg.last(pieces[:3])

    tile = length // 4

    def project_rec(begin, size):
        at = pl.ds(pl.multiple_of(begin, 64), size)
        product = jnp.dot(xall[at], rwall[...], preferred_element_type=f32).astype(bf16)
        projr[at] = product
        rext[pl.ds(pl.multiple_of(begin + rtop, 16), size)] = product[:, :rwid].astype(f32)

    @pl.loop(0, 3)
    def _(i):
        project_rec(((me.q // 2 + i // 2) % 2 * 2 + (me.q % 2 + i % 2) % 2) * tile, tile)

    mail.tag = "conv"
    for n, p in enumerate(pieces):
        cl.relay(1, p, n < 2, True)
    mail.tag = "early"
    for i in range(xg.half):
        xg.third(i)
    softened = rpar[pl.ds(s_lags + 1, 1), :]

    def gate_segment(n):
        step = (n + 1) // 2
        ring = (me.q // 2 + step % 4 // 2) % 2 * 2 + (me.q % 2 + step % 2) % 2
        i = jnp.where(n == SEGMENTS - 1, 2 * me.q, 2 * ring + n % 2)
        i = jnp.where(n == 0, 2 * me.q + 1, i)

        @pl.when(jnp.logical_and(i == 0, me.has_down))
        def _():
            mail.arrived(rext.at[pl.ds(0, rtop)], rh.at[0], me.partner)

        @pl.when(jnp.logical_and(n % 2 == 1, n < SEGMENTS - 1))
        def _():
            mail.arrived(jall.at[i // 2], rj.at[i // 2], me.partner)

        base = pl.multiple_of(i * seg, 8)
        window = rext[pl.ds(pl.multiple_of(base + rtop - 8, 8), seg + 8)]
        smooth = jnp.zeros((seg, rwid), f32)
        for k in range(s_lags + 1):
            smooth = smooth + rpar[pl.ds(k, 1), :] * window[8 - s_lags + k : 8 - s_lags + k + seg]
        smooth = smooth.astype(bf16)
        gates = jax.nn.sigmoid(jnp.dot(smooth, maps[...], preferred_element_type=f32))
        retain, admit = gates[:, :rwid], gates[:, fold * 128 : fold * 128 + rwid]
        wide = jall[i // 2].astype(f32)
        moved = jnp.where(i % 2 == 0, wide[:, :rwid], wide[:, rwid:])
        log_decay = moved - retain * softened
        decay = jnp.exp(log_decay)
        inflow = jnp.sqrt(one_minus_exp(log_decay, decay) * (1.0 + decay)) * admit * smooth.astype(f32)
        for f in range(fold):
            w = min(128, rwid - f * 128)
            spot = pl.ds(pl.multiple_of(i * lane_seg, 8), seg)
            dec[f, spot, pl.ds(0, w)] = decay[:, f * 128 : f * 128 + w]
            inf[f, spot, pl.ds(0, w)] = inflow[:, f * 128 : f * 128 + w]

    mail.finish("first")
    project_rec((me.qd * 2 + me.c) * rows, rows)
    pl.loop(0, 1)(gate_segment)
    xg.last(pieces[3:])
    project_rec((me.qd * 2 + 1 - me.c) * rows, rows)

    mail.tag = "conv"
    mail.send(rext.at[pl.ds(length, rtop)], rext.at[pl.ds(0, rtop)], rh.at[0], me.up, me.has_up)
    for p in pieces[2:]:
        cl.relay(1, p, True, False)
    for k in range(2, last):
        for p in pieces:
            cl.relay(k, p, False, True)

    @pl.when(jnp.logical_not(me.has_down))
    def _():
        rext[pl.ds(0, rtop)] = jnp.zeros((rtop, rwid), f32)
        gext[pl.ds(0, top)] = jnp.zeros((top, cw), f32)

    pl.loop(1, SEGMENTS)(gate_segment)

    def one(i, held):
        after = []
        for f in range(fold):
            at = pl.ds(i, SEGMENTS, stride=lane_seg)
            d = dec.at[f][at, :]
            product, state = held[2 * f] * d, held[2 * f + 1] * d + inf.at[f][at, :]
            dec.at[f][at, :] = product
            inf.at[f][at, :] = state
            after += [product, state]
        return tuple(after)

    flat = (SEGMENTS, 128)
    ends = lax.fori_loop(0, seg, one, (jnp.ones(flat, f32), jnp.zeros(flat, f32)) * fold, unroll=8)
    for f in range(fold):
        product, state = jnp.ones((1, 128), f32), jnp.zeros((1, 128), f32)
        for i in range(SEGMENTS):
            p, s = ends[2 * f][i : i + 1], ends[2 * f + 1][i : i + 1]
            product, state = product * p, p * state + s
        carry[pl.ds(2 * f, 1)] = product
        carry[pl.ds(2 * f + 1, 1)] = state
    for k in range(1, planes):
        mail.send(carry, cr_all.at[me.z], rc.at[me.z], lined[k - 1], me.z + k < planes)
    early = me.z < planes - 2
    for k in range(2, last):
        for p in pieces[:3]:
            cl.relay(k, p, True, False)
    mail.tag = "gather"
    for p in parts[1:]:
        out_own(p, early, True)
    mail.finish("early")

    for i in range(SEGMENTS):
        there = pl.ds(i * lane_seg, seg)
        factor = gelu(projr[pl.ds(i * seg, seg), pl.ds(rwid, rwid)].astype(f32))
        for f in range(fold):
            w = min(128, rwid - f * 128)
            lanes = pl.ds(0, w)
            dec[f, there, lanes] = dec[f, there, lanes] * factor[:, f * 128 : f * 128 + w]
            inf[f, there, lanes] = inf[f, there, lanes] * factor[:, f * 128 : f * 128 + w]

    for k in range(1, planes):
        z = me.z - k
        pl.when(z >= 0)(functools.partial(mail.arrived, cr_all.at[z], rc.at[z], me.partner))
    entering = []
    for f in range(fold):
        held = jnp.zeros((1, 128), f32)
        for j in range(planes - 1):
            after = cr_all[j, pl.ds(2 * f, 1)] * held + cr_all[j, pl.ds(2 * f + 1, 1)]
            held = jnp.where(j < me.z, after, held)
        for i in range(SEGMENTS):
            entering.append(held)
            held = ends[2 * f][i : i + 1] * held + ends[2 * f + 1][i : i + 1]
    placed = me.c * 4 + me.q

    def rec_result(i):
        here, there = pl.ds(i * seg, seg), pl.ds(i * lane_seg, seg)
        state = [dec[f, there] * entering[f * SEGMENTS + i] + inf[f, there] for f in range(fold)]
        result = jnp.concatenate(state, axis=1)[:, :rwid].astype(bf16)
        yall[here, pl.ds(pl.multiple_of(8 * cw + placed * major, 128), major)] = result[:, :major]
        return result[:, major:]

    for i in range(SEGMENTS // 2):
        pair = jnp.concatenate([rec_result(i), rec_result(i + SEGMENTS // 2)], axis=1)
        yrest[pl.ds(i * seg, seg), pl.ds(pl.multiple_of(placed * 2 * minor, 128), 2 * minor)] = pair

    def gather(buffer, lane, lanes, recv, recv_pair, kind=PlaneGather):
        tall_part = buffer.shape[0] // recv.shape[1]

        def slot(q, c, h):
            spot = pl.ds(pl.multiple_of(lane + (c * 4 + q) * lanes, 128), lanes)
            return buffer.at[pl.ds(pl.multiple_of(h * tall_part, 16), tall_part), spot]

        return kind(me, mail, slot, recv, recv_pair)

    mg = gather(yall, 8 * cw, major, rvq.at[0], rvq.at[1])
    eg = gather(yrest, 0, 2 * minor, re, rf)
    yg = gather(yall, 0, cw, rx, rpx, RowGather)
    mail.tag = "conv"
    mg.start()
    eg.start()
    mail.tag = "gather"
    for k in range(1, last):
        for p in pieces:
            cl.settle(k, p)
        for p in pieces[3:] if k > 1 else ():
            cl.await_up(k, p)
    plane_depth = 4 * depth
    is_last = (me.z == last).astype(jnp.int32)

    def conv_product(at, begin, size):
        deep = pl.ds(pl.multiple_of(begin, plane_depth), size)
        return jnp.dot(xall[at, deep], cwall[deep], preferred_element_type=f32)

    @pl.loop(0, 4)
    def _(i):
        at = pl.ds(pl.multiple_of(i * tile, tile), tile)
        cacc[at] = conv_product(at, is_last * plane_depth, last * plane_depth)

    middle = me.has_up & me.has_down

    def finish_conv(when):
        @pl.when(when)
        def _():
            @pl.loop(0, 4)
            def _(i):
                at = pl.ds(pl.multiple_of(i * tile, tile), tile)
                product = cacc[at] + conv_product(at, (1 - is_last) * last * plane_depth, plane_depth)
                product = product.astype(bf16).astype(f32)
                glu = (product[:, :cw] * jax.nn.sigmoid(product[:, cw:])).astype(bf16).astype(f32)
                gext[pl.ds(pl.multiple_of(i * tile + top, 8), tile)] = glu

        tail_rows = gext.at[pl.ds(length, top)]
        mail.send(tail_rows, gext.at[pl.ds(0, top)], rh.at[1], me.up, me.has_up & when)

    finish_conv(middle)
    for k in range(2, last):
        for p in pieces[3:]:
            cl.forward_up(k, p)
    for p in parts[1:]:
        out_own(p, jnp.logical_not(early), False)
    mg.first(0)
    for p in pieces:
        cl.settle(last, p)
    finish_conv(jnp.logical_not(middle))
    strips = length // 64

    def filter_strip(n):
        i = strips - 1 - n

        base = pl.multiple_of(i * 64, 8)
        window = gext[pl.ds(base, 64 + top)]
        total = jnp.zeros((64, cw), f32) + cpar[pl.ds(c_lags + 1, 1), :]
        for r in range(8):
            ks = [k for k in range(c_lags + 1) if (top - c_lags + k) % 8 == r]
            span = 64 + (8 if r else 0)
            shifted = jnp.zeros((span, cw), f32)
            for k in ks:
                begin = (top - c_lags + k) // 8 * 8
                shifted = shifted + cpar[pl.ds(k, 1), :] * window[begin : begin + span]
            total = total + shifted[r : r + 64]
        filt[pl.ds(base, 64)] = total

    pl.loop(0, strips - 2, unroll=2)(filter_strip)
    filter_strip(strips - 2)
    tail_halo = gext.at[pl.ds(0, top)]
    pl.when(me.has_down)(functools.partial(mail.arrived, tail_halo, rh.at[1], me.partner))
    filter_strip(strips - 1)

    turned = filt[...].T
    ft[...] = turned
    part_sum = jnp.sum(turned, axis=0, keepdims=True)
    off = turned - part_sum * (1.0 / cw)
    st_all[mine, pl.ds(0, 1)] = part_sum
    st_all[mine, pl.ds(1, 1)] = jnp.sum(off * off, axis=0, keepdims=True)
    for device in mates:
        mail.send(st_all.at[mine], st_all.at[mine], rs.at[mine], device)
    for i in range(1, mg.half):
        mg.first(i)
    for i in range(eg.half):
        eg.first(i)
    mail.tag = "out"
    for p in parts:
        ol.relay(1, p)
    mail.tag = "gather"
    mail.finish("conv")

    for k in range(1, 8):
        d = (mine + k) % 8
        mail.arrived(st_all.at[d], rs.at[d], me.partner)
    total = sum(st_all[d, 0:1, :] for d in range(8))
    mean = total * (1.0 / (8 * cw))
    spread = jnp.zeros_like(mean)
    for d in range(8):
        shift = st_all[d, 0:1, :] * (1.0 / cw) - mean
        spread = spread + st_all[d, 1:2, :] + cw * shift * shift
    scale = lax.rsqrt(spread * (1.0 / (8 * cw)) + 1e-05)
    gain_col = jnp.broadcast_to(cpar[pl.ds(c_lags + 2, 1), :], (8, cw)).T[:, 0:1]
    v = (ft[...] - mean) * scale * gain_col
    yall[:, pl.ds(pl.multiple_of(placed * cw, 128), cw)] = (v * jax.nn.sigmoid(v)).T.astype(bf16)
    mail.tag = "begun"
    yg.start()
    mail.tag = "share"
    mg.second()
    eg.second()
    for g in (mg, eg):
        for i in range(g.half):
            g.third(i)
    mail.tag = "last"
    mail.finish("gather")
    for i in range(yg.half):
        yg.first(i)
    for k in range(2, last):
        for p in parts:
            ol.relay(k, p)
    mg.last(pieces)
    eg.last(pieces)
    mail.finish("share")
    rest_at = 8 * (cw + major)

    @pl.loop(0, SEGMENTS // 2)
    def _(i):
        values = yrest[pl.ds(pl.multiple_of(i * seg, 16), seg)]
        low = [values[:, j * 2 * minor : j * 2 * minor + minor] for j in range(8)]
        high = [values[:, j * 2 * minor + minor : (j + 1) * 2 * minor] for j in range(8)]
        for begin, chosen in ((0, low), (length // 2, high)):
            here = pl.ds(pl.multiple_of(begin + i * seg, 16), seg)
            yall[here, pl.ds(rest_at, 8 * minor)] = jnp.concatenate(chosen, axis=1)

    yg.second()
    yg.third(0)
    for k in range(1, last):
        for p in parts:
            ol.settle(k, p)

    cols = wz.shape[2]
    upward = me.z < part

    def lanes_of(h):
        return pl.ds(0, cols) if h is None else pl.ds(h * half_cols, half_cols)

    def summed(q, k, h, low, high):
        here = pl.ds(pl.multiple_of(q * 2 * rows, 16), 2 * rows)
        total = jnp.zeros((2 * rows, cols if h is None else half_cols), f32)
        for c, block in ((me.c, wz.at[me.c * part + k]), (1 - me.c, wp.at[k])):
            begin = 0
            for at, lanes in ((0, 4 * cw), (8 * cw, 4 * major), (rest_at, 4 * minor)):
                first, end = max(begin, low), min(begin + lanes, high)
                if first < end:
                    spot = pl.multiple_of(at + c * lanes + first - begin, 128)
                    right = block[pl.ds(first, end - first), lanes_of(h)]
                    left_part = yall[here, pl.ds(spot, end - first)]
                    total = total + jnp.dot(left_part, right, preferred_element_type=f32)
                begin = begin + lanes
        return here, total

    def multiply(q, k, h):
        here, total = summed(q, k, h, tall if h == 1 else 0, 2 * tall)
        if h == 1:
            total = total + cacc[here, pl.ds(0, half_cols)]
        total = total.astype(bf16)
        for c in range(2):
            cbuf[q * 2 + c, k, :, lanes_of(h)] = total[c * rows : (c + 1) * rows]

    def place(q, c, k, h):
        at = ((c * part + k) * 4 + q) * cols + (0 if h is None else h * half_cols)
        return out.at[:, pl.ds(pl.multiple_of(at, 128), cols if h is None else half_cols)]

    def mate_of(i):
        flip = 3 - i
        return (me.q // 2 + flip // 2) % 2 * 2 + (me.q % 2 + flip % 2) % 2

    mail.finish("begun")

    def left(d, k, h):
        return rvq.at[k, d // 2, d % 2 * 2 + (h or 0)]

    def landed(d, k, h):
        return zrc.at[k, d // 2, d % 2 * 2 + (h or 0)]

    def parcel(q, c, k, h):
        return pltpu.make_async_remote_copy(
            src_ref=cbuf.at[q * 2 + c, k, :, lanes_of(h)], dst_ref=place(me.q, me.c, k, h),
            send_sem=left(q * 2 + c, k, h), recv_sem=landed(mine, k, h),
            device_id=me.at(me.z * 4 + q, c), device_id_type=MESH,
        )

    def kept(k, h):
        src = cbuf.at[mine, k, :, lanes_of(h)]
        return pltpu.make_async_copy(src, place(me.q, me.c, k, h), left(mine, k, h))

    def serve(q, k, h):
        multiply(q, k, h)
        pl.when(q != me.q)(lambda: parcel(q, me.c, k, h).start())
        parcel(q, 1 - me.c, k, h).start()
        pl.when(q == me.q)(lambda: kept(k, h).start())

    def ready(k, ps):
        for p in ps:
            mail.arrived(wp.at[(k, *cut(p))], rw.at[k, p], me.partner)

    order = [jnp.where(upward, n, part - 1 - n) for n in range(part)]
    ready(order[0], parts)
    for i in range(yg.half):
        if i:
            yg.third(i)
        for q in pieces:
            for row_part in ((me.qx, me.qy), (me.q, me.qd))[i]:
                yg.paired(q, row_part)

        @pl.loop(0, 2)
        def _(n):
            serve(mate_of(3 - 3 * (1 - n) if i else 2 - n), order[0], None)

    for n in range(1, part - 1):
        ready(order[n], parts)
        pl.loop(0, 4)(lambda i: serve(mate_of(i), order[n], None))
    k_far = order[-1]
    for p in parts[:2]:
        ol.settle(last, p)
    ready(k_far, parts[:2])
    pl.loop(0, 4)(lambda i: serve(mate_of(i), k_far, 0))
    ol.settle(last, 2)
    ready(k_far, parts[2:3])

    @pl.loop(0, 4)
    def _(q):
        here, total = summed(q, k_far, 1, 0, tall)
        cacc[here, pl.ds(0, half_cols)] = total

    ol.settle(last, 3)
    ready(k_far, parts[3:])
    pl.loop(0, 4)(lambda i: serve(mate_of(i), k_far, 1))
    rounds = [(k, None) for k in order[:-1]] + [(order[-1], 0), (order[-1], 1)]

    @pl.loop(0, 4)
    def _(i):
        q = mate_of(i)
        for k, h in rounds:
            mail.arrived(place(q, 1 - me.c, k, h), landed(q * 2 + 1 - me.c, k, h), me.partner)
            parcel(q, 1 - me.c, k, h).wait_send()

    @pl.loop(0, 3)
    def _(i):
        q = mate_of(i)
        for k, h in rounds:
            mail.arrived(place(q, me.c, k, h), landed(q * 2 + me.c, k, h), me.partner)
            parcel(q, me.c, k, h).wait_send()

    for k, h in rounds:
        kept(k, h).wait()
    mail.finish()


def handed_out_kernel(src, dst, held, got, sent):
    count = got.shape[0]
    tall = src.shape[0] // count
    spots = [pl.ds(i * tall, tall) for i in range(count)]
    taken = [pltpu.make_async_copy(src.at[s], held.at[s], got.at[i]) for i, s in enumerate(spots)]
    given = [pltpu.make_async_copy(held.at[s], dst.at[s], sent.at[i]) for i, s in enumerate(spots)]
    for copy in taken:
        copy.start()
    for came, goes in zip(taken, given):
        came.wait()
        goes.start()
    for copy in given:
        copy.wait()


def handed_out(result):
    dma = pltpu.SemaphoreType.DMA
    return pl.pallas_call(
        handed_out_kernel,
        out_shape=jax.ShapeDtypeStruct(result.shape, result.dtype),
        in_specs=[ANY],
        out_specs=ANY,
        scratch_shapes=[pltpu.VMEM(result.shape, result.dtype), dma((6,)), dma((6,))],
    )(result)


def layer(planes, lags, tokens, norm_gain, val_w, gate_w, rgate_w, rin_w, taps, bias, cgain, staps, dmap, imap, rbase, jump, ocw, orw):
    rows, width_in = tokens.shape
    length = 8 * rows
    depth = rin_w.shape[0]
    cw, rwid = val_w.shape[1] // 4, rin_w.shape[1] // 4
    used, cols = cw + rwid, ocw.shape[1]
    minor = rwid % 128
    fold = (rwid + 127) // 128
    f32, bf16 = jnp.float32, jnp.bfloat16
    dma = pltpu.SemaphoreType.DMA
    top = lags[0] + -lags[0] % 16
    rtop = lags[1] + -lags[1] % 16
    part = planes // 2
    deep = planes * 4 * depth

    def vmem(*shape, dtype=bf16):
        return pltpu.VMEM(shape, dtype)

    def wide(*shape):
        return pltpu.VMEM(shape, f32)

    return pl.pallas_call(
        functools.partial(layer_kernel, planes, lags),
        out_shape=jax.ShapeDtypeStruct((rows, planes * 4 * cols), bf16),
        in_specs=[ANY] * 16,
        out_specs=ANY,
        scratch_shapes=[
            vmem(rows, width_in), wide(1, width_in), vmem(*rin_w.shape), vmem(*rgate_w.shape),
            vmem(4, depth, 2 * rwid), vmem(4, depth, 2 * cw),
            vmem(*taps.shape), wide(1, 4 * cw), wide(1, 4 * cw), vmem(*staps.shape),
            vmem(*dmap.shape), vmem(*imap.shape), wide(4 * rwid), wide(*jump.shape),
            vmem(4, jump.shape[0] // 2, 2 * rwid), wide(lags[0] + 3 + -(lags[0] + 3) % 8, cw), wide(8, rwid),
            vmem(length, width_in),
            vmem(deep, 2 * rwid),
            vmem(deep, 2 * cw),
            vmem(length, 2 * rwid),
            vmem(4, jump.shape[0] // 2, 2 * rwid),
            vmem(planes, 4 * used, cols),
            vmem(part, 4 * used, cols),
            vmem(length, 8 * used),
            vmem(length // 2, 16 * minor),
            wide(length, 2 * cw),
            vmem(8, part, rows, cols),
            wide(top + length, cw),
            wide(rtop + length, rwid),
            wide(length, cw),
            wide(fold, length + 8 * SEGMENTS, 128),
            wide(fold, length + 8 * SEGMENTS, 128),
            vmem(rwid, 2 * fold * 128),
            wide(cw, length),
            wide(8, 2, length),
            wide(8, 128),
            wide(planes, 8, 128),
            dma((POOL,)), dma((4, 4)), dma((4, 4)), dma((4,)), dma((4,)),
            dma((part, planes, 4)), dma((planes, OUT_PARTS)), dma((4,)),
            dma((part, 4, 4)), dma((4, 2)), dma((4, 2)), dma((part, OUT_PARTS)),
            dma((2,)), dma((8,)), dma((planes,)),
        ],
        compiler_params=pltpu.CompilerParams(
            collective_id=0, has_side_effects=True, vmem_limit_bytes=60 * 1024 * 1024
        ),
    )(
        tokens, norm_gain[None], val_w, gate_w, rgate_w, rin_w, taps, bias[None], cgain[None], staps,
        dmap, imap, rbase, jump, ocw, orw,
    )


def plane_shards(
    planes,
    tokens,
    norm_gain,
    conv_val_w,
    conv_gate_w,
    rec_gate_w,
    rec_in_w,
    conv_taps,
    conv_bias,
    conv_gain,
    short_taps,
    decay_map,
    input_map,
    decay_base,
    decay_jump,
    out_conv_w,
    out_rec_w,
):
    lags = (conv_taps.shape[0] - 1, short_taps.shape[0] - 1)
    return handed_out(layer(
        planes, lags, tokens, norm_gain, conv_val_w, conv_gate_w, rec_gate_w, rec_in_w, conv_taps, conv_bias,
        conv_gain, short_taps, decay_map, input_map, decay_base, decay_jump, out_conv_w, out_rec_w,
    ))


def solution(mesh):
    in_specs = (
        P(("sp", "tp"), None),
        P(),
        P("sp", "tp"),
        P("sp", "tp"),
        P("sp", "tp"),
        P("sp", "tp"),
        P(None, "tp"),
        P("tp"),
        P("tp"),
        P(None, "tp"),
        P("tp", None, None),
        P("tp", None, None),
        P("tp"),
        P("sp", "tp"),
        P("tp", "sp"),
        P("tp", "sp"),
    )
    out_specs = P(("sp", "tp"), None)
    count = mesh.shape["sp"]
    planar = mesh.shape["tp"] == 2 and count % 8 == 0 and count >= 16
    body = functools.partial(plane_shards, count // 4) if planar else shards
    return jax.shard_map(body, mesh=mesh, in_specs=in_specs, out_specs=out_specs, check_vma=False)
```
